32 devices in a mesh: sp: 16 (over z, y, core), tp: 2 (over x).
Axes of the slice: x: 2, y: 2, z: 4, core: 2. Of those that a mesh axis runs over, the one named last changes fastest.
Arguments:
- tokens: bfloat16 [6144, 2048], P('sp', 'tp'), may hold values from -60 to 60
- pre_gain: bfloat16 [2048], P('tp'), may hold values from 0.099609375 to 1.8984375
- w_query: bfloat16 [2048, 1024], P('sp', 'tp'), may hold values from -1 to 1
- w_key: bfloat16 [2048, 1024], P('sp', 'tp'), may hold values from -1 to 1
- w_value: bfloat16 [2048, 1024], P('sp', 'tp'), may hold values from -0.125 to 0.125
- w_pool: bfloat16 [2048, 1024], P('sp', 'tp'), may hold values from -0.125 to 0.125
- lambdas: float32 [8], P('tp'), may hold values from 0.3 to 0.8
- sub_gain: float32 [128], replicated, may hold values from 0.1 to 1.9
- group_weight: bfloat16 [8, 128, 128], P('tp'), may hold values from -0.5 to 0.5
- pool_scale: float32 [1024], P('tp'), may hold values from 0.1 to 1.9
- w_out: bfloat16 [2048, 2048], P('tp', 'sp'), may hold values from -0.125 to 0.125
Outputs:
- mixed_out: bfloat16 [6144, 2048], P(('sp', 'tp'))
The draws below stay inside these ranges and needn't reach their ends.
All inputs are finite; a program needn't handle non-finite values.
Results may differ from the reference program's by a relative error of at most 0.015.
Values may be sent and summed in bfloat16 or wider, within the bound.
A program may use at most 128 MiB of HBM per device.

```python
import math
import jax
import jax.numpy as jnp
import numpy as np
from jax import lax

D = 2048
HEADS = 8
HDIM = 64
VDIM = 128
GROUPS = 8
GDIM = 128
TOKENS = 6144


def draw_tokens(key, part):
    noise = jax.random.normal(jax.random.fold_in(key, 11), (TOKENS, D), jnp.float32)
    row_scale = jnp.exp(jax.random.uniform(jax.random.fold_in(key, 12), (TOKENS, 1), jnp.float32, 0.0, math.log(10.0)))
    column_rise = 1.1 * jnp.arange(D, dtype=jnp.float32)[None, :] / D
    column_scale = jnp.exp(jax.random.uniform(jax.random.fold_in(key, 13), (1, D), jnp.float32, -0.7, 0.7) + column_rise)
    result = noise * row_scale * column_scale
    return jnp.clip(result, -60.0, 60.0).astype(jnp.bfloat16)


def query_key_pair(key):
    columns = HEADS * 2 * HDIM
    spread = math.sqrt(2.0 / D)
    first = jax.random.normal(jax.random.fold_in(key, 21), (D, columns), jnp.float32) * spread
    second = jax.random.normal(jax.random.fold_in(key, 22), (D, columns), jnp.float32) * spread
    return (jnp.clip(first, -1.0, 1.0), jnp.clip(second, -1.0, 1.0))


def draw_w_query(key, part):
    return query_key_pair(key)[0].astype(jnp.bfloat16)


def draw_w_key(key, part):
    return query_key_pair(key)[1].astype(jnp.bfloat16)


def level_of(rng, shape, split, least, high):
    factor_of, own = 1.0, jax.random.fold_in(rng, 6)
    for dim, shards_of in split:
        heights = jnp.exp(jax.random.uniform(jax.random.fold_in(own, dim), (shards_of,), jnp.float32, least / len(split), high / len(split)))
        factor_of = factor_of * jnp.repeat(heights, shape[dim] // shards_of).reshape([-1 if axis == dim else 1 for axis in range(len(shape))])
    return factor_of


def bell_draw(stream_key, extent, width, reach, shards=(), held_as=jnp.bfloat16):
    values = jax.random.normal(stream_key, extent, jnp.float32) * width
    if len(shards) > 0:
        values = level_of(stream_key, extent, shards, -0.22, 0.18) * values
    return jnp.clip(values, min=-reach, max=reach).astype(held_as)


def setup_inputs(seed: int = 0) -> dict:
    splits = jax.random.split(jax.random.key(seed), 12)
    tokens = draw_tokens(jax.random.fold_in(splits[11], 71), 0)
    pre_gain = jnp.clip(1.0 + 0.18 * jax.random.normal(splits[1], (D,), jnp.float32), 0.099609375, 1.8984375).astype(jnp.bfloat16)
    w_query = draw_w_query(jax.random.fold_in(splits[11], 71), 0)
    w_key = draw_w_key(jax.random.fold_in(splits[11], 71), 0)
    w_value = bell_draw(splits[4], (D, HEADS * VDIM), D ** -0.5, 0.125, ((0, 16), (1, 2)))
    w_pool = bell_draw(splits[5], (D, GROUPS * GDIM), D ** -0.5, 0.125, ((0, 16), (1, 2)))
    lambdas = jnp.clip(0.3 + 0.5 * jax.random.uniform(splits[6], (HEADS,), jnp.float32) ** level_of(splits[6], (HEADS,), ((0, 2),), -0.2, 0.2), 0.3, 0.8)
    sub_gain = jnp.clip(1.0 + 0.18 * jax.random.normal(splits[7], (VDIM,), jnp.float32), 0.1, 1.9)
    group_weight = bell_draw(splits[8], (GROUPS, GDIM, GDIM), GDIM ** -0.5, 0.5, ((0, 2),))
    pool_scale = jnp.clip(1.0 + 0.18 * jax.random.normal(splits[9], (GROUPS * GDIM,), jnp.float32), 0.1, 1.9)
    w_out = bell_draw(splits[10], (HEADS * (VDIM + GDIM), D), (HEADS * (VDIM + GDIM)) ** -0.5, 0.125, ((0, 2), (1, 16)))
    return {"tokens": tokens, "pre_gain": pre_gain, "w_query": w_query, "w_key": w_key, "w_value": w_value, "w_pool": w_pool, "lambdas": lambdas, "sub_gain": sub_gain, "group_weight": group_weight, "pool_scale": pool_scale, "w_out": w_out}


EPSILON = 1e-06
WINDOWS = (2, 4, 8, 16)
RIM_ROWS = 15

def head_block(query_head, key_head, value_head, weight_two, first_row):
    block_len = query_head.shape[0]
    key_len = key_head.shape[0]
    score_scale = 1.0 / math.sqrt(HDIM)
    scores = jnp.einsum('qmd,kmd->mqk', query_head.astype(jnp.float32), key_head.astype(jnp.float32)) * score_scale
    allowed = jnp.arange(key_len, dtype=jnp.int32)[None, :] <= (first_row + jnp.arange(block_len, dtype=jnp.int32))[:, None]
    scores = jnp.where(allowed[None], scores, -jnp.inf)
    row_max = lax.optimization_barrier(jnp.max(scores, axis=-1, keepdims=True))
    expo = jnp.where(allowed[None], jnp.exp(scores - row_max), 0.0)
    row_sum = lax.optimization_barrier(jnp.sum(expo, axis=-1))
    rounded = lax.optimization_barrier(expo.astype(jnp.bfloat16)).astype(jnp.float32)
    weighted = jnp.einsum('mqk,kd->mqd', rounded, value_head.astype(jnp.float32))
    head_mix = weighted[0] / row_sum[0][:, None] - weight_two * weighted[1] / row_sum[1][:, None]
    return head_mix

def reference(tokens, pre_gain, w_query, w_key, w_value, w_pool, lambdas, sub_gain, group_weight, pool_scale, w_out):
    features = tokens.astype(jnp.float32)
    inverse = lax.rsqrt(lax.optimization_barrier(jnp.mean(features * features, axis=1, keepdims=True)) + EPSILON)
    scaled = (features * pre_gain.astype(jnp.float32)).astype(jnp.bfloat16)

    def project(weight):
        return (jnp.dot(scaled, weight, preferred_element_type=jnp.float32) * inverse).astype(jnp.bfloat16)
    queries = project(w_query).reshape(TOKENS, HEADS, 2, HDIM)
    key_rows = project(w_key).reshape(TOKENS, HEADS, 2, HDIM)
    values = project(w_value).reshape(TOKENS, HEADS, VDIM)
    pool_in = project(w_pool)
    block_len = math.gcd(TOKENS, 512)
    pieces = []
    for block_index in range(TOKENS // block_len):
        first_row = block_index * block_len
        key_len = first_row + block_len
        query_heads = jnp.transpose(queries[first_row:key_len], (1, 0, 2, 3))
        key_heads = jnp.transpose(key_rows[:key_len], (1, 0, 2, 3))
        value_heads = jnp.transpose(values[:key_len], (1, 0, 2))

        def one_head(packed):
            return head_block(packed[0], packed[1], packed[2], packed[3], first_row)
        mixed_heads = lax.map(one_head, (query_heads, key_heads, value_heads, lambdas))
        mean_sq = lax.optimization_barrier(jnp.mean(mixed_heads * mixed_heads, axis=-1, keepdims=True))
        normed = mixed_heads * lax.rsqrt(mean_sq + EPSILON) * sub_gain
        pieces.append(jnp.transpose(normed, (1, 0, 2)).astype(jnp.bfloat16))
    attention = jnp.concatenate(pieces, axis=0)
    pool_float = pool_in.astype(jnp.float32)
    extended = jnp.concatenate([jnp.zeros((RIM_ROWS, GROUPS * GDIM), jnp.float32), pool_float], axis=0)
    running = jnp.concatenate([jnp.zeros((1, GROUPS * GDIM), jnp.float32), jnp.cumsum(extended, axis=0)], axis=0)
    running_top = running[RIM_ROWS + 1:]
    positions = jnp.arange(TOKENS, dtype=jnp.int32)
    window_of_column = np.repeat(np.arange(GROUPS) % len(WINDOWS), GDIM)
    average = jnp.zeros_like(running_top)
    for window_slot, window_span in enumerate(WINDOWS):
        running_low = running[RIM_ROWS + 1 - window_span:RIM_ROWS + 1 - window_span + TOKENS]
        window_count = jnp.minimum(positions + 1, window_span).astype(jnp.float32)
        average = average + jnp.where(window_of_column[None, :] == window_slot, (running_top - running_low) / window_count[:, None], 0.0)
    differ = (average - pool_float).astype(jnp.bfloat16).reshape(TOKENS, GROUPS, GDIM)
    pooled = jnp.einsum('tgc,gcd->tgd', differ.astype(jnp.float32), group_weight.astype(jnp.float32))
    pooled = (pooled * pool_scale.reshape(GROUPS, GDIM)).astype(jnp.bfloat16)
    branch = jnp.concatenate([attention, pooled], axis=2).reshape(TOKENS, HEADS * (VDIM + GDIM))
    return jnp.dot(branch, w_out, preferred_element_type=jnp.float32).astype(jnp.bfloat16)
```

```python
import functools
import math

import jax
import jax.numpy as jnp
from jax import lax
from jax.experimental import pallas as pl
from jax.experimental.pallas import tpu as pltpu
from jax.sharding import PartitionSpec as P

EPSILON = 1e-06
NEG_LARGE = -1e30
WINDOWS = (2, 4, 8, 16)
RIM_ROWS = 15


def passed_along(block, axis, distance):
    devices = range(lax.axis_size(axis))
    route = [(i - distance, i) for i in devices if i - distance in devices]
    return lax.ppermute(block, axis, route)


def attend(inner, vdim, hdim, member_ref, lam_ref, q_ref, kv_ref, gain_ref, out_ref, acc_ref, max_ref):
    rows = q_ref.shape[1]
    block = pl.program_id(0)
    last = block * inner + member_ref[0]
    scale = 1.0 / math.sqrt(hdim)
    queries = (q_ref[0].astype(jnp.float32) * scale).astype(jnp.bfloat16)
    maps = (queries[:, :hdim], queries[:, hdim:])
    ones = jnp.ones((rows, vdim), jnp.bfloat16)
    acc_ref[...] = jnp.zeros_like(acc_ref)
    max_ref[...] = jnp.full_like(max_ref, NEG_LARGE)

    def step(g, masked):
        keys_values = kv_ref[lax.rem(g, inner), lax.div(g, inner)]
        values = jnp.concatenate([keys_values[:, 2 * hdim :], ones], axis=1)
        for m in range(2):
            keys = keys_values[:, m * hdim : (m + 1) * hdim]
            scores = lax.dot_general(
                maps[m], keys, (((1,), (1,)), ((), ())), preferred_element_type=jnp.float32
            )
            if masked:
                row = lax.broadcasted_iota(jnp.int32, scores.shape, 0)
                col = lax.broadcasted_iota(jnp.int32, scores.shape, 1)
                scores = jnp.where(col <= row, scores, NEG_LARGE)
            old_max = max_ref[m]
            new_max = jnp.maximum(old_max, jnp.max(scores, axis=1, keepdims=True))
            factor = jnp.exp(old_max - new_max)
            expo = jnp.exp(scores - new_max[:, :1])
            acc_ref[m] = acc_ref[m] * factor[:, :1] + jnp.dot(
                expo.astype(jnp.bfloat16), values, preferred_element_type=jnp.float32
            )
            max_ref[m] = new_max

    def body(g, carry):
        step(g, False)
        return carry

    lax.fori_loop(0, last, body, 0)
    step(last, True)
    first = acc_ref[0]
    second = acc_ref[1]
    mix = first[:, :vdim] / first[:, vdim:] - lam_ref[0] * (second[:, :vdim] / second[:, vdim:])
    mean_sq = jnp.mean(mix * mix, axis=1, keepdims=True)
    out_ref[0] = (mix * lax.rsqrt(mean_sq + EPSILON) * gain_ref[...]).astype(jnp.bfloat16)


def flash(q, kv, member, lam, sub_gain):
    inner, outer, rows, width = kv.shape
    qdim = q.shape[-1]
    vdim = width - qdim
    smem = pl.BlockSpec(memory_space=pltpu.SMEM)
    work = outer * rows * outer * rows * inner
    return pl.pallas_call(
        functools.partial(attend, inner, vdim, qdim // 2),
        grid=(outer,),
        out_shape=jax.ShapeDtypeStruct((outer, rows, vdim), jnp.bfloat16),
        in_specs=[
            smem,
            smem,
            pl.BlockSpec((1, rows, qdim), lambda b: (b, 0, 0)),
            pl.BlockSpec(memory_space=pltpu.VMEM),
            pl.BlockSpec(memory_space=pltpu.VMEM),
        ],
        out_specs=pl.BlockSpec((1, rows, vdim), lambda b: (b, 0, 0)),
        scratch_shapes=[
            pltpu.VMEM((2, rows, 2 * vdim), jnp.float32),
            pltpu.VMEM((2, rows, 128), jnp.float32),
        ],
        compiler_params=pltpu.CompilerParams(vmem_limit_bytes=56 * 2**20),
        cost_estimate=pl.CostEstimate(
            flops=4 * work * vdim, bytes_accessed=kv.size * 2, transcendentals=work
        ),
    )(member, lam, q, kv, sub_gain.reshape(1, -1))


def attend_members(hdim, lam_ref, q_ref, own_ref, gain_ref, out_ref, held, acc_ref, max_ref, send, recv):
    outer, rows, _ = q_ref.shape
    vdim = own_ref.shape[2] - 2 * hdim
    sp = lax.axis_index("sp")
    member = lax.rem(sp, 4)
    y = lax.div(member, 2)
    c = lax.rem(member, 2)
    y_peer = sp + 2 - 4 * y
    c_peer = sp + 1 - 2 * c
    barrier = pltpu.get_barrier_semaphore()
    for peer in (y_peer, c_peer):
        pl.semaphore_signal(
            barrier, 1, device_id={"sp": peer}, device_id_type=pl.DeviceIdType.MESH
        )
    pl.semaphore_wait(barrier, 2)

    def remote(src, index, peer):
        return pltpu.make_async_remote_copy(
            src_ref=src,
            dst_ref=held.at[index],
            send_sem=send.at[index],
            recv_sem=recv.at[index],
            device_id={"sp": peer},
            device_id_type=pl.DeviceIdType.MESH,
        )

    across = remote(own_ref, 1, y_peer)
    beside = remote(own_ref, 0, c_peer)
    onward = remote(held.at[1], 2, c_peer)
    across.start()
    beside.start()
    acc_ref[...] = jnp.zeros_like(acc_ref)
    max_ref[...] = jnp.full_like(max_ref, NEG_LARGE)
    scale = 1.0 / math.sqrt(hdim)

    def visit(ref, other):
        shift = (member - other) * rows
        for block in range(outer):
            queries = (q_ref[block].astype(jnp.float32) * scale).astype(jnp.bfloat16)
            length = (block + 1) * rows
            keys_values = ref[: block + 1].reshape(length, 2 * hdim + vdim)
            values = jnp.concatenate(
                [keys_values[:, 2 * hdim :], jnp.ones((length, vdim), jnp.bfloat16)], axis=1
            )
            for m in range(2):
                scores = lax.dot_general(
                    queries[:, m * hdim : (m + 1) * hdim],
                    keys_values[:, m * hdim : (m + 1) * hdim],
                    (((1,), (1,)), ((), ())),
                    preferred_element_type=jnp.float32,
                )
                edge = scores[:, block * rows :]
                row = lax.broadcasted_iota(jnp.int32, edge.shape, 0)
                col = lax.broadcasted_iota(jnp.int32, edge.shape, 1)
                edge = jnp.where(col <= row + shift, edge, NEG_LARGE)
                if block > 0:
                    scores = jnp.concatenate([scores[:, : block * rows], edge], axis=1)
                else:
                    scores = edge
                old_max = max_ref[block, m]
                new_max = jnp.maximum(old_max, jnp.max(scores, axis=1, keepdims=True))
                factor = jnp.exp(old_max - new_max)
                expo = jnp.exp(scores - new_max[:, :1])
                acc_ref[block, m] = acc_ref[block, m] * factor[:, :1] + jnp.dot(
                    expo.astype(jnp.bfloat16), values, preferred_element_type=jnp.float32
                )
                max_ref[block, m] = new_max

    visit(own_ref, member)

    def arrived(j, carry):
        @pl.when(j == 0)
        def _():
            beside.wait_recv()

        @pl.when(j == 1)
        def _():
            across.wait_recv()
            onward.start()

        @pl.when(j == 2)
        def _():
            onward.wait_recv()

        other_y = jnp.where(j >= 1, 1 - y, y)
        other_c = jnp.where(j == 1, c, 1 - c)
        visit(held.at[j], 2 * other_y + other_c)
        return carry

    lax.fori_loop(0, 3, arrived, 0)
    for copy in (across, beside, onward):
        copy.wait_send()
    for block in range(outer):
        first = acc_ref[block, 0]
        second = acc_ref[block, 1]
        mix = first[:, :vdim] / first[:, vdim:]
        mix = mix - lam_ref[0] * (second[:, :vdim] / second[:, vdim:])
        mean_sq = jnp.mean(mix * mix, axis=1, keepdims=True)
        normed = mix * lax.rsqrt(mean_sq + EPSILON) * gain_ref[...]
        out_ref[block] = normed.astype(jnp.bfloat16)


def flash_members(q, kv, lam, sub_gain):
    outer, rows, width = kv.shape
    qdim = q.shape[-1]
    vdim = width - qdim
    vmem = pl.BlockSpec(memory_space=pltpu.VMEM)
    work = 4 * outer * rows * outer * rows
    return pl.pallas_call(
        functools.partial(attend_members, qdim // 2),
        out_shape=jax.ShapeDtypeStruct((outer, rows, vdim), jnp.bfloat16),
        in_specs=[pl.BlockSpec(memory_space=pltpu.SMEM), vmem, vmem, vmem],
        out_specs=vmem,
        scratch_shapes=[
            pltpu.VMEM((3, outer, rows, width), jnp.bfloat16),
            pltpu.VMEM((outer, 2, rows, 2 * vdim), jnp.float32),
            pltpu.VMEM((outer, 2, rows, 128), jnp.float32),
            pltpu.SemaphoreType.DMA((3,)),
            pltpu.SemaphoreType.DMA((3,)),
        ],
        compiler_params=pltpu.CompilerParams(
            vmem_limit_bytes=56 * 2**20, collective_id=1, has_side_effects=True
        ),
        cost_estimate=pl.CostEstimate(
            flops=4 * work * vdim, bytes_accessed=4 * kv.size * 2, transcendentals=work
        ),
    )(lam, q, kv, sub_gain.reshape(1, -1))


def spread(n_sp, count, with_swap, *refs):
    weights, refs = refs[:count], refs[count:]
    mine, refs = refs[0], refs[1:]
    fulls, refs = refs[:count], refs[count:]
    theirs, refs = refs[0], refs[1:]
    up_send, up_recv, down_send, down_recv, y_send, y_recv, c_send, c_recv, own_sem, swap_sem = refs
    depth = n_sp // 4
    rows = weights[0].shape[0]
    sp = lax.axis_index("sp")
    z = lax.div(sp, 4)
    y = lax.rem(lax.div(sp, 2), 2)
    c = lax.rem(sp, 2)
    y_peer = z * 4 + (1 - y) * 2 + c
    c_peer = z * 4 + y * 2 + (1 - c)
    barrier = pltpu.get_barrier_semaphore()

    def greet(device):
        pl.semaphore_signal(barrier, 1, device_id=device, device_id_type=pl.DeviceIdType.MESH)

    greet({"sp": y_peer})
    greet({"sp": c_peer})
    greeted = 2
    if with_swap:
        greet({"tp": 1 - lax.axis_index("tp")})
        greeted = 3

    @pl.when(z > 0)
    def _():
        greet({"sp": sp - 4})

    @pl.when(z < depth - 1)
    def _():
        greet({"sp": sp + 4})

    in_line = jnp.where(z > 0, 1, 0) + jnp.where(z < depth - 1, 1, 0)
    pl.semaphore_wait(barrier, greeted + in_line)

    def slot(a, zz, yy, cc):
        start = pl.multiple_of((zz * 4 + yy * 2 + cc) * rows, rows)
        return fulls[a].at[pl.ds(start, rows), :]

    def remote(src, dst, send, recv, device):
        return pltpu.make_async_remote_copy(
            src_ref=src,
            dst_ref=dst,
            send_sem=send,
            recv_sem=recv,
            device_id=device,
            device_id_type=pl.DeviceIdType.MESH,
        )

    def line_copy(side, k, a, src):
        sends, recvs = (up_send, up_recv) if side > 0 else (down_send, down_recv)
        there = slot(a, z - side * k, y, c)
        return remote(
            there if src is None else src,
            there,
            sends.at[k, a],
            recvs.at[k + 1, a],
            {"sp": sp + 4 * side},
        )

    def y_copy(zz, yy, a, src):
        there = slot(a, zz, yy, c)
        src = there if src is None else src
        return remote(src, there, y_send.at[zz, a], y_recv.at[zz, a], {"sp": y_peer})

    def c_copy(zz, yy, cc, a, src):
        there = slot(a, zz, yy, cc)
        src = there if src is None else src
        return remote(src, there, c_send.at[zz, yy, a], c_recv.at[zz, yy, a], {"sp": c_peer})

    def can_go(side):
        return z < depth - 1 if side > 0 else z > 0

    def came(side, k):
        return z >= k if side > 0 else z + k <= depth - 1

    if with_swap:
        swap = remote(
            mine, theirs, swap_sem.at[0], swap_sem.at[1], {"tp": 1 - lax.axis_index("tp")}
        )
        swap.start()
    for a in range(count):
        for side in (1, -1):

            @pl.when(can_go(side))
            def _():
                line_copy(side, 0, a, weights[a]).start()

        y_copy(z, y, a, weights[a]).start()
    for a in range(count):
        c_copy(z, y, c, a, weights[a]).start()
        pltpu.make_async_copy(weights[a], slot(a, z, y, c), own_sem.at[a]).start()

    def from_pair(zz):
        for a in range(count):
            y_copy(zz, 1 - y, a, None).wait_recv()
            c_copy(zz, 1 - y, c, a, None).start()

    def relay(k, carry):
        for side in (1, -1):
            recvs = up_recv if side > 0 else down_recv

            @pl.when(came(side, k))
            def _():
                zz = z - side * k
                for a in range(count):
                    there = slot(a, zz, y, c)
                    remote(there, there, up_send.at[0, a], recvs.at[k, a], {"sp": y_peer}).wait_recv()

                    @pl.when(can_go(side))
                    def _():
                        line_copy(side, k, a, None).start()

                    y_copy(zz, y, a, None).start()
                    c_copy(zz, y, c, a, None).start()

        @pl.when(k == 1)
        def _():
            from_pair(z)

        for side in (1, -1):

            @pl.when((k > 1) & came(side, k - 1))
            def _():
                from_pair(z - side * (k - 1))

        return carry

    lax.fori_loop(1, depth, relay, 0)
    if depth == 1:
        from_pair(z)
    for side in (1, -1):
        if depth > 1:

            @pl.when(came(side, depth - 1))
            def _():
                from_pair(z - side * (depth - 1))

    def drain(zz, carry):
        for a in range(count):
            y_copy(zz, y, a, None).wait_send()
            for yy in range(2):
                c_copy(zz, yy, 1 - c, a, None).wait_recv()
                c_copy(zz, yy, c, a, None).wait_send()
        return carry

    lax.fori_loop(0, depth, drain, 0)

    def drain_line(k, carry):
        for side in (1, -1):

            @pl.when(came(side, k) & can_go(side))
            def _():
                for a in range(count):
                    line_copy(side, k, a, None).wait_send()

        return carry

    lax.fori_loop(0, depth, drain_line, 0)
    for a in range(count):
        pltpu.make_async_copy(weights[a], slot(a, z, y, c), own_sem.at[a]).wait()
    if with_swap:
        swap.wait()


def gather_weights(weights, mine, with_swap):
    n_sp = lax.axis_size("sp")
    count = len(weights)
    depth = n_sp // 4
    sems = pltpu.SemaphoreType.DMA
    any_spec = pl.BlockSpec(memory_space=pl.ANY)
    vmem_spec = pl.BlockSpec(memory_space=pltpu.VMEM)
    shapes = [jax.ShapeDtypeStruct((n_sp * w.shape[0], w.shape[1]), w.dtype) for w in weights]
    shapes.append(jax.ShapeDtypeStruct(mine.shape, mine.dtype))
    moved = sum(w.size for w in weights) * 2 * n_sp
    return pl.pallas_call(
        functools.partial(spread, n_sp, count, with_swap),
        out_shape=shapes,
        in_specs=[vmem_spec] * (count + 1),
        out_specs=[any_spec] * (count + 1),
        scratch_shapes=[
            sems((depth + 1, count)),
            sems((depth + 1, count)),
            sems((depth + 1, count)),
            sems((depth + 1, count)),
            sems((depth, count)),
            sems((depth, count)),
            sems((depth, 2, count)),
            sems((depth, 2, count)),
            sems((count,)),
            sems((2,)),
        ],
        compiler_params=pltpu.CompilerParams(collective_id=0, has_side_effects=True),
        cost_estimate=pl.CostEstimate(flops=10**10, bytes_accessed=moved, transcendentals=0),
    )(*weights, mine)


def arrival(z, i):
    half = z // 2
    return (z, 1 + 4 * half - z, 2 - half, 3 - 3 * half)[i]


def mix(hdim, lam_ref, q_ref, k_ref, v_ref, gain_ref, out_ref, q_in, k_all, v_all, acc, top, total, done, *sems):
    (z_send, z_recv, in_send, in_recv, back_send, back_recv) = sems
    planes, rows, _ = q_ref.shape
    vdim = v_ref.shape[1]
    members = k_all.shape[1]
    sp = lax.axis_index("sp")
    z = sp // members
    m = sp % members
    y_member = (m + 2) % members
    c_member = m + 1 - 2 * (m % 2)
    turned = members - 1 - m

    def at(plane, member):
        return {"sp": plane * members + member}

    def holder(block, member):
        return member + (block % 2) * (members - 1 - 2 * member)

    barrier = pltpu.get_barrier_semaphore()

    def greet(device):
        pl.semaphore_signal(barrier, 1, device_id=device, device_id_type=pl.DeviceIdType.MESH)

    order = [arrival(z, i) for i in range(planes)]
    for plane in order[1:]:
        greet(at(plane, m))
        greet(at(plane, turned))
    for member in (turned, y_member, c_member):
        greet(at(z, member))
    pl.semaphore_wait(barrier, 2 * planes + 1)

    def remote(src, dst, send, recv, device):
        return pltpu.make_async_remote_copy(
            src_ref=src,
            dst_ref=dst,
            send_sem=send,
            recv_sem=recv,
            device_id=device,
            device_id_type=pl.DeviceIdType.MESH,
        )

    def k_out(plane):
        return remote(k_ref.at[plane], k_all.at[z, m], z_send.at[0, plane], z_recv.at[0, z], at(plane, m))

    def v_out(plane):
        return remote(v_ref.at[plane], v_all.at[z, m], z_send.at[1, plane], z_recv.at[1, z], at(plane, m))

    def q_out(plane):
        return remote(
            q_ref.at[plane], q_in.at[z], z_send.at[2, plane], z_recv.at[2, z], at(plane, holder(z, m))
        )

    def came(kind, plane, dst):
        remote(dst, dst, z_send.at[kind, plane], z_recv.at[kind, plane], at(z, c_member)).wait_recv()

    def in_plane(plane, own):
        copies = []
        for t, (mine, everyone) in enumerate(((k_ref, k_all), (v_ref, v_all))):
            src = mine.at[plane] if own else everyone.at[plane, m]
            there = everyone.at[plane, m]
            passed = everyone.at[plane, y_member]
            copies.append(
                [
                    remote(src, there, in_send.at[plane, 0, t], in_recv.at[plane, 0, t], at(z, y_member)),
                    remote(src, there, in_send.at[plane, 1, t], in_recv.at[plane, 1, t], at(z, c_member)),
                    remote(passed, passed, in_send.at[plane, 2, t], in_recv.at[plane, 2, t], at(z, c_member)),
                ]
            )
        return copies

    def share(plane, own):
        for copies in in_plane(plane, own):
            copies[0].start()
            copies[1].start()

    def hand_on(plane, own):
        for copies in in_plane(plane, own):
            copies[0].wait_recv()
            copies[2].start()

    def shared(plane, own):
        for copies in in_plane(plane, own):
            copies[1].wait_recv()
            copies[2].wait_recv()

    share(z, True)

    @pl.when(z % 2 == 1)
    def _():
        q_out(z).start()

    for plane in order[1:]:
        k_out(plane).start()
        v_out(plane).start()
        q_out(plane).start()
    k_all[z, m] = k_ref[z]
    v_all[z, m] = v_ref[z]

    @pl.when(z % 2 == 0)
    def _():
        q_in[z] = q_ref[z]

    acc[...] = jnp.zeros_like(acc)
    total[...] = jnp.zeros_like(total)
    top[...] = jnp.full_like(top, NEG_LARGE)

    def visit(block, plane, first, count, masked):
        query = q_in[block]
        lane = lax.broadcasted_iota(jnp.int32, query.shape, 1)
        none = jnp.zeros_like(query)
        both = jnp.concatenate(
            [jnp.where(lane < hdim, query, none), jnp.where(lane < hdim, none, query)], axis=0
        )
        keys = k_all[plane, pl.ds(first, count)].reshape(count * rows, 2 * hdim)
        values = jnp.concatenate([v_all[plane, first + i] for i in range(count)], axis=1)
        scores = lax.dot_general(
            keys, both, (((1,), (1,)), ((), ())), preferred_element_type=jnp.float32
        )
        if masked:
            shift = (first - holder(block, m)) * rows
            key = lax.broadcasted_iota(jnp.int32, scores.shape, 0)
            col = lax.broadcasted_iota(jnp.int32, scores.shape, 1)
            col = jnp.where(col < rows, col, col - rows)
            scores = jnp.where(key + shift <= col, scores, NEG_LARGE)
        old = top[block]
        new = jnp.maximum(old, jnp.max(scores, axis=0, keepdims=True))
        factor = jnp.exp(old - new)
        expo = jnp.exp(scores - new)
        acc[block] = acc[block] * factor + jnp.dot(
            values, expo.astype(jnp.bfloat16), preferred_element_type=jnp.float32
        )
        partial = jnp.sum(expo.reshape(count * rows // 8, 8, 2 * rows), axis=0)
        total[block] = total[block] * factor + partial
        top[block] = new

    def diagonal(block):
        pair = holder(block, m) // 2

        @pl.when(pair > 0)
        def _():
            visit(block, block, 0, members // 2, False)

        visit(block, block, pair * (members // 2), members // 2, True)

    def across(a, b):
        visit(jnp.maximum(a, b), jnp.minimum(a, b), 0, members, False)

    def result_copy(block):
        return remote(
            done.at[block], out_ref.at[z], back_send.at[block], back_recv.at[z], at(block, holder(block, m))
        )

    def at_home(block):
        return (block == z) & (z % 2 == 0)

    def finish(block):
        both = acc[block] / jnp.sum(total[block], axis=0, keepdims=True)
        mixed = both[:, :rows] - lam_ref[z] * both[:, rows:]
        mean_sq = jnp.mean(mixed * mixed, axis=0, keepdims=True)
        normed = (mixed * lax.rsqrt(mean_sq + EPSILON)).T * gain_ref[...]
        done[block] = normed.astype(jnp.bfloat16)

        @pl.when(at_home(block))
        def _():
            out_ref[z] = done[block]

        @pl.when(jnp.logical_not(at_home(block)))
        def _():
            result_copy(block).start()

    def landed(i):
        plane = order[i]
        came(0, plane, k_all.at[plane, m])
        came(1, plane, v_all.at[plane, m])
        share(plane, False)

    hand_on(z, True)
    shared(z, True)

    @pl.when(z % 2 == 1)
    def _():
        came(2, z, q_in.at[z])

    for i in range(planes - 1):
        landed(i + 1)
        diagonal(order[i])
        hand_on(order[i + 1], False)
        for j in range(i):
            across(order[i], order[j])
        came(2, order[i + 1], q_in.at[order[i + 1]])
        shared(order[i + 1], False)
    late = order[planes - 1]
    diagonal(late)
    finish(0)
    half = z // 2

    def last(s, carry):
        across(late, s - 1 + half)
        finish(s)
        return carry

    lax.fori_loop(1, planes, last, 0)

    for plane in order[1:]:
        k_out(plane).wait_send()
        v_out(plane).wait_send()
        q_out(plane).wait_send()

    @pl.when(z % 2 == 1)
    def _():
        q_out(z).wait_send()

    for i in range(planes):
        for copies in in_plane(order[i], i == 0):
            for copy in copies:
                copy.wait_send()
    for block in range(planes):

        @pl.when(jnp.logical_not(at_home(block)))
        def _():
            result_copy(block).wait_send()
            here = out_ref.at[block]
            remote(here, here, back_send.at[block], back_recv.at[block], at(z, c_member)).wait_recv()


def attend_and_return(queries, keys, values, lambdas, sub_gain):
    planes, rows, width = queries.shape
    vdim = values.shape[1]
    members = lax.axis_size("sp") // planes
    vmem = pl.BlockSpec(memory_space=pltpu.VMEM)
    dma = pltpu.SemaphoreType.DMA
    work = planes * rows * members * planes * rows
    return pl.pallas_call(
        functools.partial(mix, width // 2),
        out_shape=jax.ShapeDtypeStruct((planes, rows, vdim), jnp.bfloat16),
        in_specs=[pl.BlockSpec(memory_space=pltpu.SMEM), vmem, vmem, vmem, vmem],
        out_specs=vmem,
        scratch_shapes=[
            pltpu.VMEM((planes, rows, width), jnp.bfloat16),
            pltpu.VMEM((planes, members, rows, width), jnp.bfloat16),
            pltpu.VMEM((planes, members, vdim, rows), jnp.bfloat16),
            pltpu.VMEM((planes, vdim, 2 * rows), jnp.float32),
            pltpu.VMEM((planes, 1, 2 * rows), jnp.float32),
            pltpu.VMEM((planes, 8, 2 * rows), jnp.float32),
            pltpu.VMEM((planes, rows, vdim), jnp.bfloat16),
            dma((3, planes)),
            dma((3, planes)),
            dma((planes, 3, 2)),
            dma((planes, 3, 2)),
            dma((planes,)),
            dma((planes,)),
        ],
        compiler_params=pltpu.CompilerParams(
            vmem_limit_bytes=56 * 2**20, collective_id=2, has_side_effects=True
        ),
        cost_estimate=pl.CostEstimate(
            flops=4 * work * vdim, bytes_accessed=keys.size * 8, transcendentals=work
        ),
    )(lambdas, queries, keys, values, sub_gain.reshape(1, -1))


def trailing(x, window_ids, group_dim):
    column_window = jnp.repeat(window_ids, group_dim)[None, :]
    running = x
    picked = jnp.zeros_like(x)
    for slot, span in enumerate(WINDOWS):
        half = span // 2
        running = running + jnp.pad(running[:-half], ((half, 0), (0, 0)))
        picked = jnp.where(column_window == slot, running, picked)
    return picked


def general_attention(queries, key_rows, values, lambdas, sub_gain):
    n_sp = lax.axis_size("sp")
    sp = lax.axis_index("sp")
    tok_rows = queries.shape[0]
    heads = lambdas.shape[0]
    qdim = queries.shape[1] // heads
    vdim = values.shape[1] // heads
    head_width = 2 * qdim + vdim
    outer = math.gcd(n_sp, heads)
    inner = n_sp // outer
    per_device = heads // outer
    by_head = jnp.concatenate(
        [
            x.reshape(tok_rows, heads, -1).swapaxes(0, 1)
            for x in (queries, key_rows, values)
        ],
        axis=2,
    )
    across = [[o * inner + i for o in range(outer)] for i in range(inner)]
    within = [[o * inner + i for i in range(inner)] for o in range(outer)]
    by_head = by_head.reshape(outer, per_device, tok_rows, head_width)
    if outer > 1:
        by_head = lax.all_to_all(by_head, "sp", 0, 0, axis_index_groups=across)
    first_head = lax.div(sp, inner) * per_device
    attended = []
    if inner == 4 and per_device == 1:
        lam = lax.dynamic_slice_in_dim(lambdas, first_head, 1)
        attended.append(
            flash_members(by_head[:, 0, :, :qdim], by_head[:, 0, :, qdim:], lam, sub_gain)
        )
    else:
        kv = lax.all_gather(by_head[..., qdim:], "sp", axis=0, axis_index_groups=within)
        member = lax.rem(sp, inner).reshape(1)
        for p in range(per_device):
            lam = lax.dynamic_slice_in_dim(lambdas, first_head + p, 1)
            attended.append(flash(by_head[:, p, :, :qdim], kv[:, :, p], member, lam, sub_gain))
    attended = jnp.stack(attended, axis=1)
    if outer > 1:
        attended = lax.all_to_all(attended, "sp", 0, 0, axis_index_groups=across)
    return attended.reshape(heads, tok_rows, vdim)


def local(
    tokens,
    pre_gain,
    w_query,
    w_key,
    w_value,
    w_pool,
    lambdas,
    sub_gain,
    group_weight,
    pool_scale,
    w_out,
):
    n_tp = lax.axis_size("tp")
    n_sp = lax.axis_size("sp")
    tp = lax.axis_index("tp")
    sp = lax.axis_index("sp")
    tok_rows = tokens.shape[0]
    model_width = tokens.shape[1] * n_tp
    heads = lambdas.shape[0]
    qdim = w_query.shape[1] // heads
    vdim = w_value.shape[1] // heads
    groups = group_weight.shape[0]
    group_dim = group_weight.shape[1]

    features = tokens.astype(jnp.float32)
    mine = (features * pre_gain.astype(jnp.float32)[None, :]).astype(jnp.bfloat16)
    squares = jnp.sum(features * features, axis=1, keepdims=True)
    swap = [(0, 1), (1, 0)]
    weights = [w_query, w_key, w_value, w_pool]
    if n_sp % 4 == 0:
        *weights, theirs = gather_weights(weights, mine, n_tp == 2)
    else:
        weights = [lax.all_gather(w, "sp", axis=0, tiled=True) for w in weights]
        theirs = lax.ppermute(mine, "tp", swap) if n_tp == 2 else mine
    w_sorted = w_out.reshape(heads, 2, vdim, -1).swapaxes(0, 1).reshape(w_out.shape)
    w_sorted, weights = lax.optimization_barrier((w_sorted, weights))
    w_out_rows = lax.all_gather(w_sorted, "sp", axis=1, tiled=True)
    if n_tp == 2:
        squares = squares + lax.ppermute(squares, "tp", swap)
        scaled = jnp.concatenate(
            [jnp.where(tp == 0, mine, theirs), jnp.where(tp == 0, theirs, mine)], axis=1
        )
    else:
        scaled = lax.all_gather(mine, "tp", axis=1, tiled=True)
        squares = lax.psum(squares, "tp")
    inverse = lax.rsqrt(squares / model_width + EPSILON)
    queries, key_rows, values, pool_in = [
        (jnp.dot(scaled, w, preferred_element_type=jnp.float32) * inverse).astype(jnp.bfloat16)
        for w in weights
    ]
    shaped_for_mix = n_tp == 2 and heads == 4 and n_sp == 4 * heads and qdim == vdim
    if shaped_for_mix:
        scale = 1.0 / math.sqrt(qdim // 2)
        by_head = [x.reshape(tok_rows, heads, -1) for x in (queries * scale, key_rows, values)]
        attended = attend_and_return(
            by_head[0].swapaxes(0, 1),
            by_head[1].swapaxes(0, 1),
            by_head[2].transpose(1, 2, 0),
            lambdas,
            sub_gain,
        )
    else:
        attended = general_attention(queries, key_rows, values, lambdas, sub_gain)

    halo = passed_along(pool_in[tok_rows - RIM_ROWS - 1 :], "sp", 1)
    extended = jnp.concatenate([halo, pool_in], axis=0).astype(jnp.float32)
    window_ids = (tp * groups + jnp.arange(groups, dtype=jnp.int32)) % len(WINDOWS)
    sums = trailing(extended, window_ids, group_dim)[RIM_ROWS + 1 :]
    spans = jnp.repeat(jnp.left_shift(2, window_ids), group_dim)
    positions = sp * tok_rows + jnp.arange(tok_rows, dtype=jnp.int32)
    count = jnp.minimum(positions[:, None] + 1, spans[None, :]).astype(jnp.float32)
    differ = (sums / count - pool_in.astype(jnp.float32)).astype(jnp.bfloat16)
    pooled = jnp.einsum(
        "tgc,gcd->tgd",
        differ.reshape(tok_rows, groups, group_dim),
        group_weight,
        preferred_element_type=jnp.float32,
    )
    pooled = (pooled * pool_scale.reshape(groups, group_dim)).astype(jnp.bfloat16)
    branch = jnp.concatenate(
        [attended.swapaxes(0, 1).reshape(tok_rows, -1), pooled.reshape(tok_rows, -1)], axis=1
    )
    if n_tp == 2:
        half = tok_rows // 2
        send = lax.dynamic_slice_in_dim(branch, (1 - tp) * half, half, 0)
        send = jnp.dot(send, w_out_rows, preferred_element_type=jnp.float32).astype(jnp.bfloat16)
        got = lax.ppermute(send, "tp", swap)
        keep = lax.dynamic_slice_in_dim(branch, tp * half, half, 0)
        keep = jnp.dot(keep, w_out_rows, preferred_element_type=jnp.float32)
        return (keep + got.astype(jnp.float32)).astype(jnp.bfloat16)
    partial = jnp.dot(branch, w_out_rows, preferred_element_type=jnp.float32)
    return lax.psum_scatter(partial.astype(jnp.bfloat16), "tp", scatter_dimension=0, tiled=True)


def solution(mesh):
    placed = (
        P("sp", "tp"),
        P("tp"),
        P("sp", "tp"),
        P("sp", "tp"),
        P("sp", "tp"),
        P("sp", "tp"),
        P("tp"),
        P(),
        P("tp", None, None),
        P("tp"),
        P("tp", "sp"),
    )
    return jax.shard_map(
        local, mesh=mesh, in_specs=placed, out_specs=P(("sp", "tp"), None), check_vma=False
    )
```

```python
import functools
import math

import jax
import jax.numpy as jnp
from jax import lax
from jax.experimental import pallas as pl
from jax.experimental.pallas import tpu as pltpu
from jax.sharding import PartitionSpec as P

EPSILON = 1e-06
NEG_LARGE = -1e30
WINDOWS = (2, 4, 8, 16)
RIM_ROWS = 15


def passed_along(block, axis, distance):
    devices = range(lax.axis_size(axis))
    route = [(i - distance, i) for i in devices if i - distance in devices]
    return lax.ppermute(block, axis, route)


def attend(inner, vdim, hdim, member_ref, lam_ref, q_ref, kv_ref, gain_ref, out_ref, acc_ref, max_ref):
    rows = q_ref.shape[1]
    block = pl.program_id(0)
    last = block * inner + member_ref[0]
    scale = 1.0 / math.sqrt(hdim)
    queries = (q_ref[0].astype(jnp.float32) * scale).astype(jnp.bfloat16)
    maps = (queries[:, :hdim], queries[:, hdim:])
    ones = jnp.ones((rows, vdim), jnp.bfloat16)
    acc_ref[...] = jnp.zeros_like(acc_ref)
    max_ref[...] = jnp.full_like(max_ref, NEG_LARGE)

    def step(g, masked):
        keys_values = kv_ref[lax.rem(g, inner), lax.div(g, inner)]
        values = jnp.concatenate([keys_values[:, 2 * hdim :], ones], axis=1)
        for m in range(2):
            keys = keys_values[:, m * hdim : (m + 1) * hdim]
            scores = lax.dot_general(
                maps[m], keys, (((1,), (1,)), ((), ())), preferred_element_type=jnp.float32
            )
            if masked:
                row = lax.broadcasted_iota(jnp.int32, scores.shape, 0)
                col = lax.broadcasted_iota(jnp.int32, scores.shape, 1)
                scores = jnp.where(col <= row, scores, NEG_LARGE)
            old_max = max_ref[m]
            new_max = jnp.maximum(old_max, jnp.max(scores, axis=1, keepdims=True))
            factor = jnp.exp(old_max - new_max)
            expo = jnp.exp(scores - new_max[:, :1])
            acc_ref[m] = acc_ref[m] * factor[:, :1] + jnp.dot(
                expo.astype(jnp.bfloat16), values, preferred_element_type=jnp.float32
            )
            max_ref[m] = new_max

    def body(g, carry):
        step(g, False)
        return carry

    lax.fori_loop(0, last, body, 0)
    step(last, True)
    first = acc_ref[0]
    second = acc_ref[1]
    mix = first[:, :vdim] / first[:, vdim:] - lam_ref[0] * (second[:, :vdim] / second[:, vdim:])
    mean_sq = jnp.mean(mix * mix, axis=1, keepdims=True)
    out_ref[0] = (mix * lax.rsqrt(mean_sq + EPSILON) * gain_ref[...]).astype(jnp.bfloat16)


def flash(q, kv, member, lam, sub_gain):
    inner, outer, rows, width = kv.shape
    qdim = q.shape[-1]
    vdim = width - qdim
    smem = pl.BlockSpec(memory_space=pltpu.SMEM)
    work = outer * rows * outer * rows * inner
    return pl.pallas_call(
        functools.partial(attend, inner, vdim, qdim // 2),
        grid=(outer,),
        out_shape=jax.ShapeDtypeStruct((outer, rows, vdim), jnp.bfloat16),
        in_specs=[
            smem,
            smem,
            pl.BlockSpec((1, rows, qdim), lambda b: (b, 0, 0)),
            pl.BlockSpec(memory_space=pltpu.VMEM),
            pl.BlockSpec(memory_space=pltpu.VMEM),
        ],
        out_specs=pl.BlockSpec((1, rows, vdim), lambda b: (b, 0, 0)),
        scratch_shapes=[
            pltpu.VMEM((2, rows, 2 * vdim), jnp.float32),
            pltpu.VMEM((2, rows, 128), jnp.float32),
        ],
        compiler_params=pltpu.CompilerParams(vmem_limit_bytes=56 * 2**20),
        cost_estimate=pl.CostEstimate(
            flops=4 * work * vdim, bytes_accessed=kv.size * 2, transcendentals=work
        ),
    )(member, lam, q, kv, sub_gain.reshape(1, -1))


def attend_members(hdim, lam_ref, q_ref, own_ref, gain_ref, out_ref, held, acc_ref, max_ref, send, recv):
    outer, rows, _ = q_ref.shape
    vdim = own_ref.shape[2] - 2 * hdim
    sp = lax.axis_index("sp")
    member = lax.rem(sp, 4)
    y = lax.div(member, 2)
    c = lax.rem(member, 2)
    y_peer = sp + 2 - 4 * y
    c_peer = sp + 1 - 2 * c
    barrier = pltpu.get_barrier_semaphore()
    for peer in (y_peer, c_peer):
        pl.semaphore_signal(
            barrier, 1, device_id={"sp": peer}, device_id_type=pl.DeviceIdType.MESH
        )
    pl.semaphore_wait(barrier, 2)

    def remote(src, index, peer):
        return pltpu.make_async_remote_copy(
            src_ref=src,
            dst_ref=held.at[index],
            send_sem=send.at[index],
            recv_sem=recv.at[index],
            device_id={"sp": peer},
            device_id_type=pl.DeviceIdType.MESH,
        )

    across = remote(own_ref, 1, y_peer)
    beside = remote(own_ref, 0, c_peer)
    onward = remote(held.at[1], 2, c_peer)
    across.start()
    beside.start()
    acc_ref[...] = jnp.zeros_like(acc_ref)
    max_ref[...] = jnp.full_like(max_ref, NEG_LARGE)
    scale = 1.0 / math.sqrt(hdim)

    def visit(ref, other):
        shift = (member - other) * rows
        for block in range(outer):
            queries = (q_ref[block].astype(jnp.float32) * scale).astype(jnp.bfloat16)
            length = (block + 1) * rows
            keys_values = ref[: block + 1].reshape(length, 2 * hdim + vdim)
            values = jnp.concatenate(
                [keys_values[:, 2 * hdim :], jnp.ones((length, vdim), jnp.bfloat16)], axis=1
            )
            for m in range(2):
                scores = lax.dot_general(
                    queries[:, m * hdim : (m + 1) * hdim],
                    keys_values[:, m * hdim : (m + 1) * hdim],
                    (((1,), (1,)), ((), ())),
                    preferred_element_type=jnp.float32,
                )
                edge = scores[:, block * rows :]
                row = lax.broadcasted_iota(jnp.int32, edge.shape, 0)
                col = lax.broadcasted_iota(jnp.int32, edge.shape, 1)
                edge = jnp.where(col <= row + shift, edge, NEG_LARGE)
                if block > 0:
                    scores = jnp.concatenate([scores[:, : block * rows], edge], axis=1)
                else:
                    scores = edge
                old_max = max_ref[block, m]
                new_max = jnp.maximum(old_max, jnp.max(scores, axis=1, keepdims=True))
                factor = jnp.exp(old_max - new_max)
                expo = jnp.exp(scores - new_max[:, :1])
                acc_ref[block, m] = acc_ref[block, m] * factor[:, :1] + jnp.dot(
                    expo.astype(jnp.bfloat16), values, preferred_element_type=jnp.float32
                )
                max_ref[block, m] = new_max

    visit(own_ref, member)

    def arrived(j, carry):
        @pl.when(j == 0)
        def _():
            beside.wait_recv()

        @pl.when(j == 1)
        def _():
            across.wait_recv()
            onward.start()

        @pl.when(j == 2)
        def _():
            onward.wait_recv()

        other_y = jnp.where(j >= 1, 1 - y, y)
        other_c = jnp.where(j == 1, c, 1 - c)
        visit(held.at[j], 2 * other_y + other_c)
        return carry

    lax.fori_loop(0, 3, arrived, 0)
    for copy in (across, beside, onward):
        copy.wait_send()
    for block in range(outer):
        first = acc_ref[block, 0]
        second = acc_ref[block, 1]
        mix = first[:, :vdim] / first[:, vdim:]
        mix = mix - lam_ref[0] * (second[:, :vdim] / second[:, vdim:])
        mean_sq = jnp.mean(mix * mix, axis=1, keepdims=True)
        normed = mix * lax.rsqrt(mean_sq + EPSILON) * gain_ref[...]
        out_ref[block] = normed.astype(jnp.bfloat16)


def flash_members(q, kv, lam, sub_gain):
    outer, rows, width = kv.shape
    qdim = q.shape[-1]
    vdim = width - qdim
    vmem = pl.BlockSpec(memory_space=pltpu.VMEM)
    work = 4 * outer * rows * outer * rows
    return pl.pallas_call(
        functools.partial(attend_members, qdim // 2),
        out_shape=jax.ShapeDtypeStruct((outer, rows, vdim), jnp.bfloat16),
        in_specs=[pl.BlockSpec(memory_space=pltpu.SMEM), vmem, vmem, vmem],
        out_specs=vmem,
        scratch_shapes=[
            pltpu.VMEM((3, outer, rows, width), jnp.bfloat16),
            pltpu.VMEM((outer, 2, rows, 2 * vdim), jnp.float32),
            pltpu.VMEM((outer, 2, rows, 128), jnp.float32),
            pltpu.SemaphoreType.DMA((3,)),
            pltpu.SemaphoreType.DMA((3,)),
        ],
        compiler_params=pltpu.CompilerParams(
            vmem_limit_bytes=56 * 2**20, collective_id=1, has_side_effects=True
        ),
        cost_estimate=pl.CostEstimate(
            flops=4 * work * vdim, bytes_accessed=4 * kv.size * 2, transcendentals=work
        ),
    )(lam, q, kv, sub_gain.reshape(1, -1))


def spread(n_sp, count, with_swap, *refs):
    weights, refs = refs[:count], refs[count:]
    mine, refs = refs[0], refs[1:]
    fulls, refs = refs[:count], refs[count:]
    theirs, refs = refs[0], refs[1:]
    up_send, up_recv, down_send, down_recv, y_send, y_recv, c_send, c_recv, own_sem, swap_sem = refs
    depth = n_sp // 4
    rows = weights[0].shape[0]
    sp = lax.axis_index("sp")
    z = lax.div(sp, 4)
    y = lax.rem(lax.div(sp, 2), 2)
    c = lax.rem(sp, 2)
    y_peer = z * 4 + (1 - y) * 2 + c
    c_peer = z * 4 + y * 2 + (1 - c)
    barrier = pltpu.get_barrier_semaphore()

    def greet(device):
        pl.semaphore_signal(barrier, 1, device_id=device, device_id_type=pl.DeviceIdType.MESH)

    greet({"sp": y_peer})
    greet({"sp": c_peer})
    greeted = 2
    if with_swap:
        greet({"tp": 1 - lax.axis_index("tp")})
        greeted = 3

    @pl.when(z > 0)
    def _():
        greet({"sp": sp - 4})

    @pl.when(z < depth - 1)
    def _():
        greet({"sp": sp + 4})

    in_line = jnp.where(z > 0, 1, 0) + jnp.where(z < depth - 1, 1, 0)
    pl.semaphore_wait(barrier, greeted + in_line)

    def slot(a, zz, yy, cc):
        start = pl.multiple_of((zz * 4 + yy * 2 + cc) * rows, rows)
        return fulls[a].at[pl.ds(start, rows), :]

    def remote(src, dst, send, recv, device):
        return pltpu.make_async_remote_copy(
            src_ref=src,
            dst_ref=dst,
            send_sem=send,
            recv_sem=recv,
            device_id=device,
            device_id_type=pl.DeviceIdType.MESH,
        )

    def line_copy(side, k, a, src):
        sends, recvs = (up_send, up_recv) if side > 0 else (down_send, down_recv)
        there = slot(a, z - side * k, y, c)
        return remote(
            there if src is None else src,
            there,
            sends.at[k, a],
            recvs.at[k + 1, a],
            {"sp": sp + 4 * side},
        )

    def y_copy(zz, yy, a, src):
        there = slot(a, zz, yy, c)
        src = there if src is None else src
        return remote(src, there, y_send.at[zz, a], y_recv.at[zz, a], {"sp": y_peer})

    def c_copy(zz, yy, cc, a, src):
        there = slot(a, zz, yy, cc)
        src = there if src is None else src
        return remote(src, there, c_send.at[zz, yy, a], c_recv.at[zz, yy, a], {"sp": c_peer})

    def can_go(side):
        return z < depth - 1 if side > 0 else z > 0

    def came(side, k):
        return z >= k if side > 0 else z + k <= depth - 1

    if with_swap:
        swap = remote(
            mine, theirs, swap_sem.at[0], swap_sem.at[1], {"tp": 1 - lax.axis_index("tp")}
        )
        swap.start()
    for a in range(count):
        for side in (1, -1):

            @pl.when(can_go(side))
            def _():
                line_copy(side, 0, a, weights[a]).start()

        y_copy(z, y, a, weights[a]).start()
    for a in range(count):
        c_copy(z, y, c, a, weights[a]).start()
        pltpu.make_async_copy(weights[a], slot(a, z, y, c), own_sem.at[a]).start()

    def from_pair(zz):
        for a in range(count):
            y_copy(zz, 1 - y, a, None).wait_recv()
            c_copy(zz, 1 - y, c, a, None).start()

    def relay(k, carry):
        for side in (1, -1):
            recvs = up_recv if side > 0 else down_recv

            @pl.when(came(side, k))
            def _():
                zz = z - side * k
                for a in range(count):
                    there = slot(a, zz, y, c)
                    remote(there, there, up_send.at[0, a], recvs.at[k, a], {"sp": y_peer}).wait_recv()

                    @pl.when(can_go(side))
                    def _():
                        line_copy(side, k, a, None).start()

                    y_copy(zz, y, a, None).start()
                    c_copy(zz, y, c, a, None).start()

        @pl.when(k == 1)
        def _():
            from_pair(z)

        for side in (1, -1):

            @pl.when((k > 1) & came(side, k - 1))
            def _():
                from_pair(z - side * (k - 1))

        return carry

    lax.fori_loop(1, depth, relay, 0)
    if depth == 1:
        from_pair(z)
    for side in (1, -1):
        if depth > 1:

            @pl.when(came(side, depth - 1))
            def _():
                from_pair(z - side * (depth - 1))

    def drain(zz, carry):
        for a in range(count):
            y_copy(zz, y, a, None).wait_send()
            for yy in range(2):
                c_copy(zz, yy, 1 - c, a, None).wait_recv()
                c_copy(zz, yy, c, a, None).wait_send()
        return carry

    lax.fori_loop(0, depth, drain, 0)

    def drain_line(k, carry):
        for side in (1, -1):

            @pl.when(came(side, k) & can_go(side))
            def _():
                for a in range(count):
                    line_copy(side, k, a, None).wait_send()

        return carry

    lax.fori_loop(0, depth, drain_line, 0)
    for a in range(count):
        pltpu.make_async_copy(weights[a], slot(a, z, y, c), own_sem.at[a]).wait()
    if with_swap:
        swap.wait()


def gather_weights(weights, mine, with_swap):
    n_sp = lax.axis_size("sp")
    count = len(weights)
    depth = n_sp // 4
    sems = pltpu.SemaphoreType.DMA
    any_spec = pl.BlockSpec(memory_space=pl.ANY)
    vmem_spec = pl.BlockSpec(memory_space=pltpu.VMEM)
    shapes = [jax.ShapeDtypeStruct((n_sp * w.shape[0], w.shape[1]), w.dtype) for w in weights]
    shapes.append(jax.ShapeDtypeStruct(mine.shape, mine.dtype))
    moved = sum(w.size for w in weights) * 2 * n_sp
    return pl.pallas_call(
        functools.partial(spread, n_sp, count, with_swap),
        out_shape=shapes,
        in_specs=[vmem_spec] * (count + 1),
        out_specs=[any_spec] * (count + 1),
        scratch_shapes=[
            sems((depth + 1, count)),
            sems((depth + 1, count)),
            sems((depth + 1, count)),
            sems((depth + 1, count)),
            sems((depth, count)),
            sems((depth, count)),
            sems((depth, 2, count)),
            sems((depth, 2, count)),
            sems((count,)),
            sems((2,)),
        ],
        compiler_params=pltpu.CompilerParams(collective_id=0, has_side_effects=True),
        cost_estimate=pl.CostEstimate(flops=10**10, bytes_accessed=moved, transcendentals=0),
    )(*weights, mine)


def arrival(z, i):
    half = z // 2
    return (z, 1 + 4 * half - z, 2 - half, 3 - 3 * half)[i]


def project(
    hdim,
    model_width,
    tok_ref,
    gain_ref,
    wq_ref,
    wk_ref,
    wv_ref,
    q_out,
    k_out,
    v_out,
    scaled_out,
    inverse_out,
    full,
    theirs,
    their_gain,
    pieces,
    acc,
    *sems,
):
    (line_send, line_recv, y_send, y_recv, c_send, c_recv, turn_send, turn_recv, swap_sem) = sems
    weights = (wq_ref, wk_ref, wv_ref)
    arrays = range(len(weights))
    rows, columns = wq_ref.shape
    tok_rows, half_width = tok_ref.shape
    planes = q_out.shape[0]
    members = lax.axis_size("sp") // planes
    sp = lax.axis_index("sp")
    tp = lax.axis_index("tp")
    z = sp // members
    y = (sp % members) // 2
    c = sp % 2
    y_peer = {"sp": sp + 2 - 4 * y}
    c_peer = {"sp": sp + 1 - 2 * c}
    x_peer = {"tp": 1 - tp}
    order = [arrival(z, i) for i in range(planes)]
    partner = {"sp": order[1] * members + sp % members}

    barrier = pltpu.get_barrier_semaphore()

    def greet(device):
        pl.semaphore_signal(barrier, 1, device_id=device, device_id_type=pl.DeviceIdType.MESH)

    for device in (y_peer, c_peer, x_peer):
        greet(device)

    @pl.when(z > 0)
    def _():
        greet({"sp": sp - members})

    @pl.when(z < planes - 1)
    def _():
        greet({"sp": sp + members})

    pl.semaphore_wait(barrier, 3 + jnp.where(z > 0, 1, 0) + jnp.where(z < planes - 1, 1, 0))

    def remote(src, dst, send, recv, device):
        return pltpu.make_async_remote_copy(
            src_ref=src,
            dst_ref=dst,
            send_sem=send,
            recv_sem=recv,
            device_id=device,
            device_id_type=pl.DeviceIdType.MESH,
        )

    def slot(a, zz, yy, cc, first=0, count=rows):
        start = pl.multiple_of((zz * members + yy * 2 + cc) * rows + first, count)
        return full.at[a, pl.ds(start, count), :]

    def line(a, zz, up, own):
        there = slot(a, zz, y, c)
        side = 1 if up else 0
        return remote(
            weights[a] if own else there,
            there,
            line_send.at[zz, side, a],
            line_recv.at[zz, a],
            {"sp": sp + (members if up else -members)},
        )

    def y_copy(a, i, own):
        if i == 1:
            there = slot(a, order[i], y, c, rows // 2, rows // 2)
            src = there
        else:
            there = slot(a, order[i], y, c)
            src = weights[a] if own else there
        return remote(src, there, y_send.at[order[i], a], y_recv.at[order[i], a], y_peer)

    def y_came(a, i):
        there = slot(a, order[i], 1 - y, c, *((rows // 2, rows // 2) if i == 1 else ()))
        return remote(there, there, y_send.at[order[i], a], y_recv.at[order[i], a], y_peer)

    def turn(a):
        there = slot(a, z, 1 - y, c, 0, rows // 2)
        return remote(there, there, turn_send.at[a], turn_recv.at[a], partner)

    def turned(a):
        there = slot(a, order[1], 1 - y, c, 0, rows // 2)
        return remote(there, there, turn_send.at[a], turn_recv.at[a], partner)

    def c_copy(a, zz, yy, own):
        there = slot(a, zz, yy, c)
        src = weights[a] if own else there
        return remote(src, there, c_send.at[zz, yy, a], c_recv.at[zz, yy, a], c_peer)

    def c_came(a, zz, yy):
        there = slot(a, zz, yy, 1 - c)
        return remote(there, there, c_send.at[zz, yy, a], c_recv.at[zz, yy, a], c_peer)

    swaps = (
        remote(tok_ref, theirs, swap_sem.at[0], swap_sem.at[1], x_peer),
        remote(gain_ref, their_gain, swap_sem.at[2], swap_sem.at[3], x_peer),
    )
    for a in arrays:

        @pl.when(z < planes - 1)
        def _():
            line(a, z, True, True).start()

        @pl.when(z > 0)
        def _():
            line(a, z, False, True).start()

        y_copy(a, 0, True).start()
        if a == 0:
            for swap in swaps:
                swap.start()
    for a in arrays:
        c_copy(a, z, y, True).start()
        full[a, pl.ds(pl.multiple_of(sp * rows, rows), rows), :] = weights[a][...]

    def from_line(i):
        zz = order[i]
        for a in arrays:
            there = slot(a, zz, y, c)
            remote(there, there, line_send.at[zz, 0, a], line_recv.at[zz, a], c_peer).wait_recv()

            @pl.when((zz < z) & (z < planes - 1))
            def _():
                line(a, zz, True, False).start()

            @pl.when((zz > z) & (z > 0))
            def _():
                line(a, zz, False, False).start()

            y_copy(a, i, False).start()
            c_copy(a, zz, y, False).start()

    def from_pair(i):
        zz = order[i]
        for a in arrays:
            y_came(a, i).wait_recv()
            if i == 0:
                turn(a).start()
            if i == 1:
                turned(a).wait_recv()
            c_copy(a, zz, 1 - y, False).start()

    def multiply(zz, yy, first=False):
        for a in arrays:
            c_came(a, zz, yy).wait_recv()
        piece = zz * 2 + yy
        start = pl.multiple_of(piece * 2 * rows, 2 * rows)
        for a in arrays:
            part = jnp.dot(
                pieces[piece], full[a, pl.ds(start, 2 * rows), :], preferred_element_type=jnp.float32
            )
            if first:
                acc[a] = part
            else:
                acc[a] += part

    from_line(1)
    from_pair(0)
    from_line(2)
    for swap in swaps:
        swap.wait()
    squares = jnp.zeros((tok_rows, 1), jnp.float32)
    per_half = half_width // (2 * rows)
    for ref, gains, owner in ((tok_ref, gain_ref, tp), (theirs, their_gain, 1 - tp)):
        for j in range(per_half):
            chunk = pl.ds(j * 2 * rows, 2 * rows)
            features = ref[:, chunk].astype(jnp.float32)
            squares += jnp.sum(features * features, axis=1, keepdims=True)
            scaled = (features * gains[:, chunk].astype(jnp.float32)).astype(jnp.bfloat16)
            pieces[owner * per_half + j] = scaled
    inverse = lax.rsqrt(squares / model_width + EPSILON)
    inverse_out[...] = jnp.broadcast_to(inverse, inverse_out.shape)
    multiply(order[0], y, True)
    multiply(order[0], 1 - y)
    from_line(3)
    from_pair(1)
    multiply(order[1], y)
    from_pair(2)
    multiply(order[1], 1 - y)
    for j in range(2 * per_half):
        scaled_out[:, j * 2 * rows : (j + 1) * 2 * rows] = pieces[j]
    multiply(order[2], y)
    multiply(order[2], 1 - y)
    from_pair(3)
    multiply(order[3], y)
    multiply(order[3], 1 - y)
    width = columns // planes
    scale = 1.0 / math.sqrt(hdim)
    for p in range(planes):
        part = slice(p * width, (p + 1) * width)
        q_out[p] = (acc[0, :, part] * inverse).astype(jnp.bfloat16) * scale
        k_out[p] = (acc[1, :, part] * inverse).astype(jnp.bfloat16)
        v_out[p] = (acc[2, :, part] * inverse).T.astype(jnp.bfloat16)

    for a in arrays:
        for i in range(planes):
            zz = order[i]
            y_copy(a, i, i == 0).wait_send()
            c_copy(a, zz, y, i == 0).wait_send()
            c_copy(a, zz, 1 - y, False).wait_send()

            @pl.when((zz <= z) & (z < planes - 1))
            def _():
                line(a, zz, True, i == 0).wait_send()

            @pl.when((zz >= z) & (z > 0))
            def _():
                line(a, zz, False, i == 0).wait_send()

        turn(a).wait_send()


def gather_and_project(tokens, pre_gain, w_query, w_key, w_value, heads):
    tok_rows, half_width = tokens.shape
    n_sp = lax.axis_size("sp")
    rows, columns = w_query.shape
    width = columns // heads
    full_width = n_sp * rows
    vmem = pl.BlockSpec(memory_space=pltpu.VMEM)
    dma = pltpu.SemaphoreType.DMA
    by_head = jax.ShapeDtypeStruct((heads, tok_rows, width), jnp.bfloat16)
    return pl.pallas_call(
        functools.partial(project, width // 2, full_width),
        out_shape=[
            by_head,
            by_head,
            jax.ShapeDtypeStruct((heads, width, tok_rows), jnp.bfloat16),
            jax.ShapeDtypeStruct((tok_rows, full_width), jnp.bfloat16),
            jax.ShapeDtypeStruct((tok_rows, 128), jnp.float32),
        ],
        in_specs=[vmem] * 5,
        out_specs=[vmem] * 5,
        scratch_shapes=[
            pltpu.VMEM((3, full_width, columns), jnp.bfloat16),
            pltpu.VMEM((tok_rows, half_width), jnp.bfloat16),
            pltpu.VMEM((1, half_width), jnp.bfloat16),
            pltpu.VMEM((full_width // (2 * rows), tok_rows, 2 * rows), jnp.bfloat16),
            pltpu.VMEM((3, tok_rows, columns), jnp.float32),
            dma((heads, 2, 3)),
            dma((heads, 3)),
            dma((heads, 3)),
            dma((heads, 3)),
            dma((heads, 2, 3)),
            dma((heads, 2, 3)),
            dma((3,)),
            dma((3,)),
            dma((4,)),
        ],
        compiler_params=pltpu.CompilerParams(
            vmem_limit_bytes=56 * 2**20, collective_id=3, has_side_effects=True
        ),
        cost_estimate=pl.CostEstimate(
            flops=6 * tok_rows * full_width * columns, bytes_accessed=2**23, transcendentals=0
        ),
    )(tokens, pre_gain.reshape(1, -1), w_query, w_key, w_value)


def mix(hdim, lam_ref, q_ref, k_ref, v_ref, gain_ref, out_ref, q_in, k_all, v_all, acc, top, total, done, *sems):
    (z_send, z_recv, in_send, in_recv, back_send, back_recv) = sems
    planes, rows, _ = q_ref.shape
    vdim = v_ref.shape[1]
    members = k_all.shape[1]
    sp = lax.axis_index("sp")
    z = sp // members
    m = sp % members
    y_member = (m + 2) % members
    c_member = m + 1 - 2 * (m % 2)
    turned = members - 1 - m

    def at(plane, member):
        return {"sp": plane * members + member}

    def holder(block, member):
        return member + (block % 2) * (members - 1 - 2 * member)

    barrier = pltpu.get_barrier_semaphore()

    def greet(device):
        pl.semaphore_signal(barrier, 1, device_id=device, device_id_type=pl.DeviceIdType.MESH)

    order = [arrival(z, i) for i in range(planes)]
    for plane in order[1:]:
        greet(at(plane, m))
        greet(at(plane, turned))
    for member in (turned, y_member, c_member):
        greet(at(z, member))
    pl.semaphore_wait(barrier, 2 * planes + 1)

    def remote(src, dst, send, recv, device):
        return pltpu.make_async_remote_copy(
            src_ref=src,
            dst_ref=dst,
            send_sem=send,
            recv_sem=recv,
            device_id=device,
            device_id_type=pl.DeviceIdType.MESH,
        )

    def k_out(plane):
        return remote(k_ref.at[plane], k_all.at[z, m], z_send.at[0, plane], z_recv.at[0, z], at(plane, m))

    def v_out(plane):
        return remote(v_ref.at[plane], v_all.at[z, m], z_send.at[1, plane], z_recv.at[1, z], at(plane, m))

    def q_out(plane):
        return remote(
            q_ref.at[plane], q_in.at[z], z_send.at[2, plane], z_recv.at[2, z], at(plane, holder(z, m))
        )

    def came(kind, plane, dst):
        remote(dst, dst, z_send.at[kind, plane], z_recv.at[kind, plane], at(z, c_member)).wait_recv()

    def in_plane(plane, own):
        copies = []
        for t, (mine, everyone) in enumerate(((k_ref, k_all), (v_ref, v_all))):
            src = mine.at[plane] if own else everyone.at[plane, m]
            there = everyone.at[plane, m]
            passed = everyone.at[plane, y_member]
            copies.append(
                [
                    remote(src, there, in_send.at[plane, 0, t], in_recv.at[plane, 0, t], at(z, y_member)),
                    remote(src, there, in_send.at[plane, 1, t], in_recv.at[plane, 1, t], at(z, c_member)),
                    remote(passed, passed, in_send.at[plane, 2, t], in_recv.at[plane, 2, t], at(z, c_member)),
                ]
            )
        return copies

    def share(plane, own):
        for copies in in_plane(plane, own):
            copies[0].start()
            copies[1].start()

    def hand_on(plane, own):
        for copies in in_plane(plane, own):
            copies[0].wait_recv()
            copies[2].start()

    def shared(plane, own):
        for copies in in_plane(plane, own):
            copies[1].wait_recv()
            copies[2].wait_recv()

    share(z, True)

    @pl.when(z % 2 == 1)
    def _():
        q_out(z).start()

    for plane in order[1:]:
        k_out(plane).start()
        v_out(plane).start()
        q_out(plane).start()
    k_all[z, m] = k_ref[z]
    v_all[z, m] = v_ref[z]

    @pl.when(z % 2 == 0)
    def _():
        q_in[z] = q_ref[z]

    acc[...] = jnp.zeros_like(acc)
    total[...] = jnp.zeros_like(total)
    top[...] = jnp.full_like(top, NEG_LARGE)

    def visit(block, plane, first, count, masked):
        query = q_in[block]
        lane = lax.broadcasted_iota(jnp.int32, query.shape, 1)
        none = jnp.zeros_like(query)
        both = jnp.concatenate(
            [jnp.where(lane < hdim, query, none), jnp.where(lane < hdim, none, query)], axis=0
        )
        keys = k_all[plane, pl.ds(first, count)].reshape(count * rows, 2 * hdim)
        values = jnp.concatenate([v_all[plane, first + i] for i in range(count)], axis=1)
        scores = lax.dot_general(
            keys, both, (((1,), (1,)), ((), ())), preferred_element_type=jnp.float32
        )
        if masked:
            shift = (first - holder(block, m)) * rows
            key = lax.broadcasted_iota(jnp.int32, scores.shape, 0)
            col = lax.broadcasted_iota(jnp.int32, scores.shape, 1)
            col = jnp.where(col < rows, col, col - rows)
            scores = jnp.where(key + shift <= col, scores, NEG_LARGE)
        old = top[block]
        new = jnp.maximum(old, jnp.max(scores, axis=0, keepdims=True))
        factor = jnp.exp(old - new)
        expo = jnp.exp(scores - new)
        acc[block] = acc[block] * factor + jnp.dot(
            values, expo.astype(jnp.bfloat16), preferred_element_type=jnp.float32
        )
        partial = jnp.sum(expo.reshape(count * rows // 8, 8, 2 * rows), axis=0)
        total[block] = total[block] * factor + partial
        top[block] = new

    def diagonal(block):
        pair = holder(block, m) // 2

        @pl.when(pair > 0)
        def _():
            visit(block, block, 0, members // 2, False)

        visit(block, block, pair * (members // 2), members // 2, True)

    def across(a, b):
        visit(jnp.maximum(a, b), jnp.minimum(a, b), 0, members, False)

    def result_copy(block):
        return remote(
            done.at[block], out_ref.at[z], back_send.at[block], back_recv.at[z], at(block, holder(block, m))
        )

    def at_home(block):
        return (block == z) & (z % 2 == 0)

    def finish(block):
        both = acc[block] / jnp.sum(total[block], axis=0, keepdims=True)
        mixed = both[:, :rows] - lam_ref[z] * both[:, rows:]
        mean_sq = jnp.mean(mixed * mixed, axis=0, keepdims=True)
        normed = (mixed * lax.rsqrt(mean_sq + EPSILON)).T * gain_ref[...]
        done[block] = normed.astype(jnp.bfloat16)

        @pl.when(at_home(block))
        def _():
            out_ref[z] = done[block]

        @pl.when(jnp.logical_not(at_home(block)))
        def _():
            result_copy(block).start()

    def landed(i):
        plane = order[i]
        came(0, plane, k_all.at[plane, m])
        came(1, plane, v_all.at[plane, m])
        share(plane, False)

    hand_on(z, True)
    shared(z, True)

    @pl.when(z % 2 == 1)
    def _():
        came(2, z, q_in.at[z])

    for i in range(planes - 1):
        landed(i + 1)
        diagonal(order[i])
        hand_on(order[i + 1], False)
        for j in range(i):
            across(order[i], order[j])
        came(2, order[i + 1], q_in.at[order[i + 1]])
        shared(order[i + 1], False)
    late = order[planes - 1]
    diagonal(late)
    finish(0)
    half = z // 2

    def last(s, carry):
        across(late, s - 1 + half)
        finish(s)
        return carry

    lax.fori_loop(1, planes, last, 0)

    for plane in order[1:]:
        k_out(plane).wait_send()
        v_out(plane).wait_send()
        q_out(plane).wait_send()

    @pl.when(z % 2 == 1)
    def _():
        q_out(z).wait_send()

    for i in range(planes):
        for copies in in_plane(order[i], i == 0):
            for copy in copies:
                copy.wait_send()
    for block in range(planes):

        @pl.when(jnp.logical_not(at_home(block)))
        def _():
            result_copy(block).wait_send()
            here = out_ref.at[block]
            remote(here, here, back_send.at[block], back_recv.at[block], at(z, c_member)).wait_recv()


def attend_and_return(queries, keys, values, lambdas, sub_gain):
    planes, rows, width = queries.shape
    vdim = values.shape[1]
    members = lax.axis_size("sp") // planes
    vmem = pl.BlockSpec(memory_space=pltpu.VMEM)
    dma = pltpu.SemaphoreType.DMA
    work = planes * rows * members * planes * rows
    return pl.pallas_call(
        functools.partial(mix, width // 2),
        out_shape=jax.ShapeDtypeStruct((planes, rows, vdim), jnp.bfloat16),
        in_specs=[pl.BlockSpec(memory_space=pltpu.SMEM), vmem, vmem, vmem, vmem],
        out_specs=vmem,
        scratch_shapes=[
            pltpu.VMEM((planes, rows, width), jnp.bfloat16),
            pltpu.VMEM((planes, members, rows, width), jnp.bfloat16),
            pltpu.VMEM((planes, members, vdim, rows), jnp.bfloat16),
            pltpu.VMEM((planes, vdim, 2 * rows), jnp.float32),
            pltpu.VMEM((planes, 1, 2 * rows), jnp.float32),
            pltpu.VMEM((planes, 8, 2 * rows), jnp.float32),
            pltpu.VMEM((planes, rows, vdim), jnp.bfloat16),
            dma((3, planes)),
            dma((3, planes)),
            dma((planes, 3, 2)),
            dma((planes, 3, 2)),
            dma((planes,)),
            dma((planes,)),
        ],
        compiler_params=pltpu.CompilerParams(
            vmem_limit_bytes=56 * 2**20, collective_id=2, has_side_effects=True
        ),
        cost_estimate=pl.CostEstimate(
            flops=4 * work * vdim, bytes_accessed=keys.size * 8, transcendentals=work
        ),
    )(lambdas, queries, keys, values, sub_gain.reshape(1, -1))


def trailing(x, window_ids, group_dim):
    column_window = jnp.repeat(window_ids, group_dim)[None, :]
    running = x
    picked = jnp.zeros_like(x)
    for slot, span in enumerate(WINDOWS):
        half = span // 2
        running = running + jnp.pad(running[:-half], ((half, 0), (0, 0)))
        picked = jnp.where(column_window == slot, running, picked)
    return picked


def general_attention(queries, key_rows, values, lambdas, sub_gain):
    n_sp = lax.axis_size("sp")
    sp = lax.axis_index("sp")
    tok_rows = queries.shape[0]
    heads = lambdas.shape[0]
    qdim = queries.shape[1] // heads
    vdim = values.shape[1] // heads
    head_width = 2 * qdim + vdim
    outer = math.gcd(n_sp, heads)
    inner = n_sp // outer
    per_device = heads // outer
    by_head = jnp.concatenate(
        [
            x.reshape(tok_rows, heads, -1).swapaxes(0, 1)
            for x in (queries, key_rows, values)
        ],
        axis=2,
    )
    across = [[o * inner + i for o in range(outer)] for i in range(inner)]
    within = [[o * inner + i for i in range(inner)] for o in range(outer)]
    by_head = by_head.reshape(outer, per_device, tok_rows, head_width)
    if outer > 1:
        by_head = lax.all_to_all(by_head, "sp", 0, 0, axis_index_groups=across)
    first_head = lax.div(sp, inner) * per_device
    attended = []
    if inner == 4 and per_device == 1:
        lam = lax.dynamic_slice_in_dim(lambdas, first_head, 1)
        attended.append(
            flash_members(by_head[:, 0, :, :qdim], by_head[:, 0, :, qdim:], lam, sub_gain)
        )
    else:
        kv = lax.all_gather(by_head[..., qdim:], "sp", axis=0, axis_index_groups=within)
        member = lax.rem(sp, inner).reshape(1)
        for p in range(per_device):
            lam = lax.dynamic_slice_in_dim(lambdas, first_head + p, 1)
            attended.append(flash(by_head[:, p, :, :qdim], kv[:, :, p], member, lam, sub_gain))
    attended = jnp.stack(attended, axis=1)
    if outer > 1:
        attended = lax.all_to_all(attended, "sp", 0, 0, axis_index_groups=across)
    return attended.reshape(heads, tok_rows, vdim)


def local(
    tokens,
    pre_gain,
    w_query,
    w_key,
    w_value,
    w_pool,
    lambdas,
    sub_gain,
    group_weight,
    pool_scale,
    w_out,
):
    n_tp = lax.axis_size("tp")
    n_sp = lax.axis_size("sp")
    tp = lax.axis_index("tp")
    sp = lax.axis_index("sp")
    tok_rows = tokens.shape[0]
    model_width = tokens.shape[1] * n_tp
    heads = lambdas.shape[0]
    qdim = w_query.shape[1] // heads
    vdim = w_value.shape[1] // heads
    groups = group_weight.shape[0]
    group_dim = group_weight.shape[1]

    swap = [(0, 1), (1, 0)]
    shaped_for_mix = n_tp == 2 and heads == 4 and n_sp == 4 * heads and qdim == vdim
    w_sorted = w_out.reshape(heads, 2, vdim, -1).swapaxes(0, 1).reshape(w_out.shape)
    if shaped_for_mix:
        w_pool_rows = lax.all_gather(w_pool, "sp", axis=0, tiled=True)
        w_out_rows = lax.all_gather(w_sorted, "sp", axis=1, tiled=True)
        queries, key_rows, values, scaled, inverse = gather_and_project(
            tokens, pre_gain, w_query, w_key, w_value, heads
        )
        attended = attend_and_return(queries, key_rows, values, lambdas, sub_gain)
        pool_in = jnp.dot(scaled, w_pool_rows, preferred_element_type=jnp.float32)
        pool_in = (pool_in * inverse[:, :1]).astype(jnp.bfloat16)
    else:
        features = tokens.astype(jnp.float32)
        mine = (features * pre_gain.astype(jnp.float32)[None, :]).astype(jnp.bfloat16)
        squares = jnp.sum(features * features, axis=1, keepdims=True)
        weights = [w_query, w_key, w_value, w_pool]
        if n_sp % 4 == 0:
            *weights, theirs = gather_weights(weights, mine, n_tp == 2)
        else:
            weights = [lax.all_gather(w, "sp", axis=0, tiled=True) for w in weights]
            theirs = lax.ppermute(mine, "tp", swap) if n_tp == 2 else mine
        w_sorted, weights = lax.optimization_barrier((w_sorted, weights))
        w_out_rows = lax.all_gather(w_sorted, "sp", axis=1, tiled=True)
        if n_tp == 2:
            squares = squares + lax.ppermute(squares, "tp", swap)
            scaled = jnp.concatenate(
                [jnp.where(tp == 0, mine, theirs), jnp.where(tp == 0, theirs, mine)], axis=1
            )
        else:
            scaled = lax.all_gather(mine, "tp", axis=1, tiled=True)
            squares = lax.psum(squares, "tp")
        inverse = lax.rsqrt(squares / model_width + EPSILON)
        queries, key_rows, values, pool_in = [
            (jnp.dot(scaled, w, preferred_element_type=jnp.float32) * inverse).astype(jnp.bfloat16)
            for w in weights
        ]
        attended = general_attention(queries, key_rows, values, lambdas, sub_gain)

    halo = passed_along(pool_in[tok_rows - RIM_ROWS - 1 :], "sp", 1)
    extended = jnp.concatenate([halo, pool_in], axis=0).astype(jnp.float32)
    window_ids = (tp * groups + jnp.arange(groups, dtype=jnp.int32)) % len(WINDOWS)
    sums = trailing(extended, window_ids, group_dim)[RIM_ROWS + 1 :]
    spans = jnp.repeat(jnp.left_shift(2, window_ids), group_dim)
    positions = sp * tok_rows + jnp.arange(tok_rows, dtype=jnp.int32)
    count = jnp.minimum(positions[:, None] + 1, spans[None, :]).astype(jnp.float32)
    differ = (sums / count - pool_in.astype(jnp.float32)).astype(jnp.bfloat16)
    pooled = jnp.einsum(
        "tgc,gcd->tgd",
        differ.reshape(tok_rows, groups, group_dim),
        group_weight,
        preferred_element_type=jnp.float32,
    )
    pooled = (pooled * pool_scale.reshape(groups, group_dim)).astype(jnp.bfloat16)
    branch = jnp.concatenate(
        [attended.swapaxes(0, 1).reshape(tok_rows, -1), pooled.reshape(tok_rows, -1)], axis=1
    )
    if n_tp == 2:
        half = tok_rows // 2
        send = lax.dynamic_slice_in_dim(branch, (1 - tp) * half, half, 0)
        send = jnp.dot(send, w_out_rows, preferred_element_type=jnp.float32).astype(jnp.bfloat16)
        got = lax.ppermute(send, "tp", swap)
        keep = lax.dynamic_slice_in_dim(branch, tp * half, half, 0)
        keep = jnp.dot(keep, w_out_rows, preferred_element_type=jnp.float32)
        return (keep + got.astype(jnp.float32)).astype(jnp.bfloat16)
    partial = jnp.dot(branch, w_out_rows, preferred_element_type=jnp.float32)
    return lax.psum_scatter(partial.astype(jnp.bfloat16), "tp", scatter_dimension=0, tiled=True)


def solution(mesh):
    placed = (
        P("sp", "tp"),
        P("tp"),
        P("sp", "tp"),
        P("sp", "tp"),
        P("sp", "tp"),
        P("sp", "tp"),
        P("tp"),
        P(),
        P("tp", None, None),
        P("tp"),
        P("tp", "sp"),
    )
    return jax.shard_map(
        local, mesh=mesh, in_specs=placed, out_specs=P(("sp", "tp"), None), check_vma=False
    )
```

```python
import functools
import math

import jax
import jax.numpy as jnp
from jax import lax
from jax.experimental import pallas as pl
from jax.experimental.pallas import tpu as pltpu
from jax.sharding import PartitionSpec as P

EPSILON = 1e-06
NEG_LARGE = -1e30
WINDOWS = (2, 4, 8, 16)
RIM_ROWS = 15
LINE_STAGE = 2


def passed_along(block, axis, distance):
    devices = range(lax.axis_size(axis))
    route = [(i - distance, i) for i in devices if i - distance in devices]
    return lax.ppermute(block, axis, route)


def attend(inner, vdim, hdim, member_ref, lam_ref, q_ref, kv_ref, gain_ref, out_ref, acc_ref, max_ref):
    rows = q_ref.shape[1]
    block = pl.program_id(0)
    last = block * inner + member_ref[0]
    scale = 1.0 / math.sqrt(hdim)
    queries = (q_ref[0].astype(jnp.float32) * scale).astype(jnp.bfloat16)
    maps = (queries[:, :hdim], queries[:, hdim:])
    ones = jnp.ones((rows, vdim), jnp.bfloat16)
    acc_ref[...] = jnp.zeros_like(acc_ref)
    max_ref[...] = jnp.full_like(max_ref, NEG_LARGE)

    def step(g, masked):
        keys_values = kv_ref[lax.rem(g, inner), lax.div(g, inner)]
        values = jnp.concatenate([keys_values[:, 2 * hdim :], ones], axis=1)
        for m in range(2):
            keys = keys_values[:, m * hdim : (m + 1) * hdim]
            scores = lax.dot_general(
                maps[m], keys, (((1,), (1,)), ((), ())), preferred_element_type=jnp.float32
            )
            if masked:
                row = lax.broadcasted_iota(jnp.int32, scores.shape, 0)
                col = lax.broadcasted_iota(jnp.int32, scores.shape, 1)
                scores = jnp.where(col <= row, scores, NEG_LARGE)
            old_max = max_ref[m]
            new_max = jnp.maximum(old_max, jnp.max(scores, axis=1, keepdims=True))
            factor = jnp.exp(old_max - new_max)
            expo = jnp.exp(scores - new_max[:, :1])
            acc_ref[m] = acc_ref[m] * factor[:, :1] + jnp.dot(
                expo.astype(jnp.bfloat16), values, preferred_element_type=jnp.float32
            )
            max_ref[m] = new_max

    def body(g, carry):
        step(g, False)
        return carry

    lax.fori_loop(0, last, body, 0)
    step(last, True)
    first = acc_ref[0]
    second = acc_ref[1]
    mix = first[:, :vdim] / first[:, vdim:] - lam_ref[0] * (second[:, :vdim] / second[:, vdim:])
    mean_sq = jnp.mean(mix * mix, axis=1, keepdims=True)
    out_ref[0] = (mix * lax.rsqrt(mean_sq + EPSILON) * gain_ref[...]).astype(jnp.bfloat16)


def flash(q, kv, member, lam, sub_gain):
    inner, outer, rows, width = kv.shape
    qdim = q.shape[-1]
    vdim = width - qdim
    smem = pl.BlockSpec(memory_space=pltpu.SMEM)
    work = outer * rows * outer * rows * inner
    return pl.pallas_call(
        functools.partial(attend, inner, vdim, qdim // 2),
        grid=(outer,),
        out_shape=jax.ShapeDtypeStruct((outer, rows, vdim), jnp.bfloat16),
        in_specs=[
            smem,
            smem,
            pl.BlockSpec((1, rows, qdim), lambda b: (b, 0, 0)),
            pl.BlockSpec(memory_space=pltpu.VMEM),
            pl.BlockSpec(memory_space=pltpu.VMEM),
        ],
        out_specs=pl.BlockSpec((1, rows, vdim), lambda b: (b, 0, 0)),
        scratch_shapes=[
            pltpu.VMEM((2, rows, 2 * vdim), jnp.float32),
            pltpu.VMEM((2, rows, 128), jnp.float32),
        ],
        compiler_params=pltpu.CompilerParams(vmem_limit_bytes=56 * 2**20),
        cost_estimate=pl.CostEstimate(
            flops=4 * work * vdim, bytes_accessed=kv.size * 2, transcendentals=work
        ),
    )(member, lam, q, kv, sub_gain.reshape(1, -1))


def attend_members(hdim, lam_ref, q_ref, own_ref, gain_ref, out_ref, held, acc_ref, max_ref, send, recv):
    outer, rows, _ = q_ref.shape
    vdim = own_ref.shape[2] - 2 * hdim
    sp = lax.axis_index("sp")
    member = lax.rem(sp, 4)
    y = lax.div(member, 2)
    c = lax.rem(member, 2)
    y_peer = sp + 2 - 4 * y
    c_peer = sp + 1 - 2 * c
    barrier = pltpu.get_barrier_semaphore()
    for peer in (y_peer, c_peer):
        pl.semaphore_signal(
            barrier, 1, device_id={"sp": peer}, device_id_type=pl.DeviceIdType.MESH
        )
    pl.semaphore_wait(barrier, 2)

    def remote(src, index, peer):
        return pltpu.make_async_remote_copy(
            src_ref=src,
            dst_ref=held.at[index],
            send_sem=send.at[index],
            recv_sem=recv.at[index],
            device_id={"sp": peer},
            device_id_type=pl.DeviceIdType.MESH,
        )

    across = remote(own_ref, 1, y_peer)
    beside = remote(own_ref, 0, c_peer)
    onward = remote(held.at[1], 2, c_peer)
    across.start()
    beside.start()
    acc_ref[...] = jnp.zeros_like(acc_ref)
    max_ref[...] = jnp.full_like(max_ref, NEG_LARGE)
    scale = 1.0 / math.sqrt(hdim)

    def visit(ref, other):
        shift = (member - other) * rows
        for block in range(outer):
            queries = (q_ref[block].astype(jnp.float32) * scale).astype(jnp.bfloat16)
            length = (block + 1) * rows
            keys_values = ref[: block + 1].reshape(length, 2 * hdim + vdim)
            values = jnp.concatenate(
                [keys_values[:, 2 * hdim :], jnp.ones((length, vdim), jnp.bfloat16)], axis=1
            )
            for m in range(2):
                scores = lax.dot_general(
                    queries[:, m * hdim : (m + 1) * hdim],
                    keys_values[:, m * hdim : (m + 1) * hdim],
                    (((1,), (1,)), ((), ())),
                    preferred_element_type=jnp.float32,
                )
                edge = scores[:, block * rows :]
                row = lax.broadcasted_iota(jnp.int32, edge.shape, 0)
                col = lax.broadcasted_iota(jnp.int32, edge.shape, 1)
                edge = jnp.where(col <= row + shift, edge, NEG_LARGE)
                if block > 0:
                    scores = jnp.concatenate([scores[:, : block * rows], edge], axis=1)
                else:
                    scores = edge
                old_max = max_ref[block, m]
                new_max = jnp.maximum(old_max, jnp.max(scores, axis=1, keepdims=True))
                factor = jnp.exp(old_max - new_max)
                expo = jnp.exp(scores - new_max[:, :1])
                acc_ref[block, m] = acc_ref[block, m] * factor[:, :1] + jnp.dot(
                    expo.astype(jnp.bfloat16), values, preferred_element_type=jnp.float32
                )
                max_ref[block, m] = new_max

    visit(own_ref, member)

    def arrived(j, carry):
        @pl.when(j == 0)
        def _():
            beside.wait_recv()

        @pl.when(j == 1)
        def _():
            across.wait_recv()
            onward.start()

        @pl.when(j == 2)
        def _():
            onward.wait_recv()

        other_y = jnp.where(j >= 1, 1 - y, y)
        other_c = jnp.where(j == 1, c, 1 - c)
        visit(held.at[j], 2 * other_y + other_c)
        return carry

    lax.fori_loop(0, 3, arrived, 0)
    for copy in (across, beside, onward):
        copy.wait_send()
    for block in range(outer):
        first = acc_ref[block, 0]
        second = acc_ref[block, 1]
        mix = first[:, :vdim] / first[:, vdim:]
        mix = mix - lam_ref[0] * (second[:, :vdim] / second[:, vdim:])
        mean_sq = jnp.mean(mix * mix, axis=1, keepdims=True)
        normed = mix * lax.rsqrt(mean_sq + EPSILON) * gain_ref[...]
        out_ref[block] = normed.astype(jnp.bfloat16)


def flash_members(q, kv, lam, sub_gain):
    outer, rows, width = kv.shape
    qdim = q.shape[-1]
    vdim = width - qdim
    vmem = pl.BlockSpec(memory_space=pltpu.VMEM)
    work = 4 * outer * rows * outer * rows
    return pl.pallas_call(
        functools.partial(attend_members, qdim // 2),
        out_shape=jax.ShapeDtypeStruct((outer, rows, vdim), jnp.bfloat16),
        in_specs=[pl.BlockSpec(memory_space=pltpu.SMEM), vmem, vmem, vmem],
        out_specs=vmem,
        scratch_shapes=[
            pltpu.VMEM((3, outer, rows, width), jnp.bfloat16),
            pltpu.VMEM((outer, 2, rows, 2 * vdim), jnp.float32),
            pltpu.VMEM((outer, 2, rows, 128), jnp.float32),
            pltpu.SemaphoreType.DMA((3,)),
            pltpu.SemaphoreType.DMA((3,)),
        ],
        compiler_params=pltpu.CompilerParams(
            vmem_limit_bytes=56 * 2**20, collective_id=1, has_side_effects=True
        ),
        cost_estimate=pl.CostEstimate(
            flops=4 * work * vdim, bytes_accessed=4 * kv.size * 2, transcendentals=work
        ),
    )(lam, q, kv, sub_gain.reshape(1, -1))


def spread(n_sp, count, with_swap, *refs):
    weights, refs = refs[:count], refs[count:]
    mine, refs = refs[0], refs[1:]
    fulls, refs = refs[:count], refs[count:]
    theirs, refs = refs[0], refs[1:]
    up_send, up_recv, down_send, down_recv, y_send, y_recv, c_send, c_recv, own_sem, swap_sem = refs
    depth = n_sp // 4
    rows = weights[0].shape[0]
    sp = lax.axis_index("sp")
    z = lax.div(sp, 4)
    y = lax.rem(lax.div(sp, 2), 2)
    c = lax.rem(sp, 2)
    y_peer = z * 4 + (1 - y) * 2 + c
    c_peer = z * 4 + y * 2 + (1 - c)
    barrier = pltpu.get_barrier_semaphore()

    def greet(device):
        pl.semaphore_signal(barrier, 1, device_id=device, device_id_type=pl.DeviceIdType.MESH)

    greet({"sp": y_peer})
    greet({"sp": c_peer})
    greeted = 2
    if with_swap:
        greet({"tp": 1 - lax.axis_index("tp")})
        greeted = 3

    @pl.when(z > 0)
    def _():
        greet({"sp": sp - 4})

    @pl.when(z < depth - 1)
    def _():
        greet({"sp": sp + 4})

    in_line = jnp.where(z > 0, 1, 0) + jnp.where(z < depth - 1, 1, 0)
    pl.semaphore_wait(barrier, greeted + in_line)

    def slot(a, zz, yy, cc):
        start = pl.multiple_of((zz * 4 + yy * 2 + cc) * rows, rows)
        return fulls[a].at[pl.ds(start, rows), :]

    def remote(src, dst, send, recv, device):
        return pltpu.make_async_remote_copy(
            src_ref=src,
            dst_ref=dst,
            send_sem=send,
            recv_sem=recv,
            device_id=device,
            device_id_type=pl.DeviceIdType.MESH,
        )

    def line_copy(side, k, a, src):
        sends, recvs = (up_send, up_recv) if side > 0 else (down_send, down_recv)
        there = slot(a, z - side * k, y, c)
        return remote(
            there if src is None else src,
            there,
            sends.at[k, a],
            recvs.at[k + 1, a],
            {"sp": sp + 4 * side},
        )

    def y_copy(zz, yy, a, src):
        there = slot(a, zz, yy, c)
        src = there if src is None else src
        return remote(src, there, y_send.at[zz, a], y_recv.at[zz, a], {"sp": y_peer})

    def c_copy(zz, yy, cc, a, src):
        there = slot(a, zz, yy, cc)
        src = there if src is None else src
        return remote(src, there, c_send.at[zz, yy, a], c_recv.at[zz, yy, a], {"sp": c_peer})

    def can_go(side):
        return z < depth - 1 if side > 0 else z > 0

    def came(side, k):
        return z >= k if side > 0 else z + k <= depth - 1

    if with_swap:
        swap = remote(
            mine, theirs, swap_sem.at[0], swap_sem.at[1], {"tp": 1 - lax.axis_index("tp")}
        )
        swap.start()
    for a in range(count):
        for side in (1, -1):

            @pl.when(can_go(side))
            def _():
                line_copy(side, 0, a, weights[a]).start()

        y_copy(z, y, a, weights[a]).start()
    for a in range(count):
        c_copy(z, y, c, a, weights[a]).start()
        pltpu.make_async_copy(weights[a], slot(a, z, y, c), own_sem.at[a]).start()

    def from_pair(zz):
        for a in range(count):
            y_copy(zz, 1 - y, a, None).wait_recv()
            c_copy(zz, 1 - y, c, a, None).start()

    def relay(k, carry):
        for side in (1, -1):
            recvs = up_recv if side > 0 else down_recv

            @pl.when(came(side, k))
            def _():
                zz = z - side * k
                for a in range(count):
                    there = slot(a, zz, y, c)
                    remote(there, there, up_send.at[0, a], recvs.at[k, a], {"sp": y_peer}).wait_recv()

                    @pl.when(can_go(side))
                    def _():
                        line_copy(side, k, a, None).start()

                    y_copy(zz, y, a, None).start()
                    c_copy(zz, y, c, a, None).start()

        @pl.when(k == 1)
        def _():
            from_pair(z)

        for side in (1, -1):

            @pl.when((k > 1) & came(side, k - 1))
            def _():
                from_pair(z - side * (k - 1))

        return carry

    lax.fori_loop(1, depth, relay, 0)
    if depth == 1:
        from_pair(z)
    for side in (1, -1):
        if depth > 1:

            @pl.when(came(side, depth - 1))
            def _():
                from_pair(z - side * (depth - 1))

    def drain(zz, carry):
        for a in range(count):
            y_copy(zz, y, a, None).wait_send()
            for yy in range(2):
                c_copy(zz, yy, 1 - c, a, None).wait_recv()
                c_copy(zz, yy, c, a, None).wait_send()
        return carry

    lax.fori_loop(0, depth, drain, 0)

    def drain_line(k, carry):
        for side in (1, -1):

            @pl.when(came(side, k) & can_go(side))
            def _():
                for a in range(count):
                    line_copy(side, k, a, None).wait_send()

        return carry

    lax.fori_loop(0, depth, drain_line, 0)
    for a in range(count):
        pltpu.make_async_copy(weights[a], slot(a, z, y, c), own_sem.at[a]).wait()
    if with_swap:
        swap.wait()


def gather_weights(weights, mine, with_swap):
    n_sp = lax.axis_size("sp")
    count = len(weights)
    depth = n_sp // 4
    sems = pltpu.SemaphoreType.DMA
    any_spec = pl.BlockSpec(memory_space=pl.ANY)
    vmem_spec = pl.BlockSpec(memory_space=pltpu.VMEM)
    shapes = [jax.ShapeDtypeStruct((n_sp * w.shape[0], w.shape[1]), w.dtype) for w in weights]
    shapes.append(jax.ShapeDtypeStruct(mine.shape, mine.dtype))
    moved = sum(w.size for w in weights) * 2 * n_sp
    return pl.pallas_call(
        functools.partial(spread, n_sp, count, with_swap),
        out_shape=shapes,
        in_specs=[vmem_spec] * (count + 1),
        out_specs=[any_spec] * (count + 1),
        scratch_shapes=[
            sems((depth + 1, count)),
            sems((depth + 1, count)),
            sems((depth + 1, count)),
            sems((depth + 1, count)),
            sems((depth, count)),
            sems((depth, count)),
            sems((depth, 2, count)),
            sems((depth, 2, count)),
            sems((count,)),
            sems((2,)),
        ],
        compiler_params=pltpu.CompilerParams(collective_id=0, has_side_effects=True),
        cost_estimate=pl.CostEstimate(flops=10**10, bytes_accessed=moved, transcendentals=0),
    )(*weights, mine)


def arrival(z, i):
    half = z // 2
    later = jnp.where(i == 2, 2 - half, 3 - 3 * half)
    return jnp.where(i == 0, z, jnp.where(i == 1, 1 + 4 * half - z, later))


def project(
    hdim,
    model_width,
    tok_ref,
    gain_ref,
    wq_ref,
    wk_ref,
    wv_ref,
    wp_ref,
    q_out,
    k_out,
    v_out,
    scaled_out,
    inverse_out,
    pool_out,
    full,
    theirs,
    their_gain,
    pieces,
    acc,
    *sems,
):
    (line_send, line_recv, y_send, y_recv, c_send, c_recv, turn_send, turn_recv, swap_sem, pool_send, pool_recv) = sems
    weights = (wq_ref, wk_ref, wv_ref)
    arrays = range(len(weights))
    rows, columns = wq_ref.shape
    tok_rows, half_width = tok_ref.shape
    planes = q_out.shape[0]
    members = lax.axis_size("sp") // planes
    sp = lax.axis_index("sp")
    tp = lax.axis_index("tp")
    z = sp // members
    y = (sp % members) // 2
    c = sp % 2
    y_peer = {"sp": sp + 2 - 4 * y}
    c_peer = {"sp": sp + 1 - 2 * c}
    x_peer = {"tp": 1 - tp}
    order = [arrival(z, i) for i in range(planes)]
    partner = {"sp": order[1] * members + sp % members}

    barrier = pltpu.get_barrier_semaphore()

    def greet(device):
        pl.semaphore_signal(barrier, 1, device_id=device, device_id_type=pl.DeviceIdType.MESH)

    for device in (y_peer, c_peer, x_peer):
        greet(device)

    @pl.when(z > 0)
    def _():
        greet({"sp": sp - members})

    @pl.when(z < planes - 1)
    def _():
        greet({"sp": sp + members})

    pl.semaphore_wait(barrier, 3 + jnp.where(z > 0, 1, 0) + jnp.where(z < planes - 1, 1, 0))

    def remote(src, dst, send, recv, device):
        return pltpu.make_async_remote_copy(
            src_ref=src,
            dst_ref=dst,
            send_sem=send,
            recv_sem=recv,
            device_id=device,
            device_id_type=pl.DeviceIdType.MESH,
        )

    def slot(a, zz, yy, cc, first=0, count=rows):
        start = pl.multiple_of((zz * members + yy * 2 + cc) * rows + first, count)
        return full.at[a, pl.ds(start, count), :]

    def line(a, zz, up, own):
        there = slot(a, zz, y, c)
        side = 1 if up else 0
        return remote(
            weights[a] if own else there,
            there,
            line_send.at[zz, side, a],
            line_recv.at[zz, a],
            {"sp": sp + (members if up else -members)},
        )

    def y_copy(a, i, own):
        if i == 1:
            there = slot(a, order[i], y, c, rows // 2, rows // 2)
            src = there
        else:
            there = slot(a, order[i], y, c)
            src = weights[a] if own else there
        return remote(src, there, y_send.at[order[i], a], y_recv.at[order[i], a], y_peer)

    def y_came(a, i):
        there = slot(a, order[i], 1 - y, c, *((rows // 2, rows // 2) if i == 1 else ()))
        return remote(there, there, y_send.at[order[i], a], y_recv.at[order[i], a], y_peer)

    def turn(a):
        there = slot(a, z, 1 - y, c, 0, rows // 2)
        return remote(there, there, turn_send.at[a], turn_recv.at[a], partner)

    def turned(a):
        there = slot(a, order[1], 1 - y, c, 0, rows // 2)
        return remote(there, there, turn_send.at[a], turn_recv.at[a], partner)

    def c_copy(a, zz, yy, own):
        there = slot(a, zz, yy, c)
        src = weights[a] if own else there
        return remote(src, there, c_send.at[zz, yy, a], c_recv.at[zz, yy, a], c_peer)

    def c_came(a, zz, yy):
        there = slot(a, zz, yy, 1 - c)
        return remote(there, there, c_send.at[zz, yy, a], c_recv.at[zz, yy, a], c_peer)

    swaps = (
        remote(tok_ref, theirs, swap_sem.at[0], swap_sem.at[1], x_peer),
        remote(gain_ref, their_gain, swap_sem.at[2], swap_sem.at[3], x_peer),
    )
    for a in arrays:

        @pl.when(z < planes - 1)
        def _():
            line(a, z, True, True).start()

        @pl.when(z > 0)
        def _():
            line(a, z, False, True).start()

        y_copy(a, 0, True).start()
        if a == 0:
            for swap in swaps:
                swap.start()
    for a in arrays:
        c_copy(a, z, y, True).start()
        full[a, pl.ds(pl.multiple_of(sp * rows, rows), rows), :] = weights[a][...]

    def from_line(i):
        zz = order[i]
        for a in arrays:
            there = slot(a, zz, y, c)
            remote(there, there, line_send.at[zz, 0, a], line_recv.at[zz, a], c_peer).wait_recv()

            @pl.when((zz < z) & (z < planes - 1))
            def _():
                line(a, zz, True, False).start()

            @pl.when((zz > z) & (z > 0))
            def _():
                line(a, zz, False, False).start()

            y_copy(a, i, False).start()
            c_copy(a, zz, y, False).start()

    def from_pair(i):
        zz = order[i]
        for a in arrays:
            y_came(a, i).wait_recv()
            if i == 0:
                turn(a).start()
            if i == 1:
                turned(a).wait_recv()
            c_copy(a, zz, 1 - y, False).start()

    def multiply(zz, yy, first=False):
        for a in arrays:
            c_came(a, zz, yy).wait_recv()
        piece = zz * 2 + yy
        start = pl.multiple_of(piece * 2 * rows, 2 * rows)
        for a in arrays:
            part = jnp.dot(
                pieces[piece], full[a, pl.ds(start, 2 * rows), :], preferred_element_type=jnp.float32
            )
            if first:
                acc[a] = part
            else:
                acc[a] += part

    def pool_line(zz, up, own):
        there = pool_out.at[zz]
        side = 1 if up else 0
        return remote(
            wp_ref if own else there,
            there,
            pool_send.at[zz, side],
            pool_recv.at[zz],
            {"sp": sp + (members if up else -members)},
        )

    def pool_start():
        @pl.when(z < planes - 1)
        def _():
            pool_line(z, True, True).start()

        @pl.when(z > 0)
        def _():
            pool_line(z, False, True).start()

        pool_out[z] = wp_ref[...]

    def pool_from(i):
        zz = order[i]
        there = pool_out.at[zz]
        remote(there, there, pool_send.at[zz, 0], pool_recv.at[zz], c_peer).wait_recv()

        @pl.when((zz < z) & (z < planes - 1))
        def _():
            pool_line(zz, True, False).start()

        @pl.when((zz > z) & (z > 0))
        def _():
            pool_line(zz, False, False).start()

    from_line(1)
    from_pair(0)
    from_line(2)
    for swap in swaps:
        swap.wait()
    squares = jnp.zeros((tok_rows, 1), jnp.float32)
    per_half = half_width // (2 * rows)
    for ref, gains, owner in ((tok_ref, gain_ref, tp), (theirs, their_gain, 1 - tp)):
        for j in range(per_half):
            chunk = pl.ds(j * 2 * rows, 2 * rows)
            features = ref[:, chunk].astype(jnp.float32)
            squares += jnp.sum(features * features, axis=1, keepdims=True)
            scaled = (features * gains[:, chunk].astype(jnp.float32)).astype(jnp.bfloat16)
            pieces[owner * per_half + j] = scaled
    inverse = lax.rsqrt(squares / model_width + EPSILON)
    inverse_out[...] = jnp.broadcast_to(inverse, inverse_out.shape)
    multiply(order[0], y, True)
    multiply(order[0], 1 - y)
    from_line(3)
    pool_start()
    from_pair(1)
    multiply(order[1], y)
    from_pair(2)
    multiply(order[1], 1 - y)
    for j in range(2 * per_half):
        scaled_out[:, j * 2 * rows : (j + 1) * 2 * rows] = pieces[j]
    multiply(order[2], y)
    pool_from(1)
    multiply(order[2], 1 - y)
    from_pair(3)
    multiply(order[3], y)
    multiply(order[3], 1 - y)
    pool_from(2)
    width = columns // planes
    scale = 1.0 / math.sqrt(hdim)
    for p in range(planes):
        part = slice(p * width, (p + 1) * width)
        q_out[p] = (acc[0, :, part] * inverse).astype(jnp.bfloat16) * scale
        k_out[p] = (acc[1, :, part] * inverse).astype(jnp.bfloat16)
        v_out[p] = (acc[2, :, part] * inverse).T.astype(jnp.bfloat16)

    pool_from(3)
    for i in range(planes):
        zz = order[i]

        @pl.when((zz <= z) & (z < planes - 1))
        def _():
            pool_line(zz, True, i == 0).wait_send()

        @pl.when((zz >= z) & (z > 0))
        def _():
            pool_line(zz, False, i == 0).wait_send()

    for a in arrays:
        for i in range(planes):
            zz = order[i]
            y_copy(a, i, i == 0).wait_send()
            c_copy(a, zz, y, i == 0).wait_send()
            c_copy(a, zz, 1 - y, False).wait_send()

            @pl.when((zz <= z) & (z < planes - 1))
            def _():
                line(a, zz, True, i == 0).wait_send()

            @pl.when((zz >= z) & (z > 0))
            def _():
                line(a, zz, False, i == 0).wait_send()

        turn(a).wait_send()


def gather_and_project(tokens, pre_gain, w_query, w_key, w_value, w_pool, heads):
    tok_rows, half_width = tokens.shape
    n_sp = lax.axis_size("sp")
    rows, columns = w_query.shape
    width = columns // heads
    full_width = n_sp * rows
    vmem = pl.BlockSpec(memory_space=pltpu.VMEM)
    dma = pltpu.SemaphoreType.DMA
    by_head = jax.ShapeDtypeStruct((heads, tok_rows, width), jnp.bfloat16)
    return pl.pallas_call(
        functools.partial(project, width // 2, full_width),
        out_shape=[
            by_head,
            by_head,
            jax.ShapeDtypeStruct((heads, width, tok_rows), jnp.bfloat16),
            jax.ShapeDtypeStruct((tok_rows, full_width), jnp.bfloat16),
            jax.ShapeDtypeStruct((tok_rows, 128), jnp.float32),
            jax.ShapeDtypeStruct((heads,) + w_pool.shape, jnp.bfloat16),
        ],
        in_specs=[vmem] * 6,
        out_specs=[vmem] * 6,
        scratch_shapes=[
            pltpu.VMEM((3, full_width, columns), jnp.bfloat16),
            pltpu.VMEM((tok_rows, half_width), jnp.bfloat16),
            pltpu.VMEM((1, half_width), jnp.bfloat16),
            pltpu.VMEM((full_width // (2 * rows), tok_rows, 2 * rows), jnp.bfloat16),
            pltpu.VMEM((3, tok_rows, columns), jnp.float32),
            dma((heads, 2, 3)),
            dma((heads, 3)),
            dma((heads, 3)),
            dma((heads, 3)),
            dma((heads, 2, 3)),
            dma((heads, 2, 3)),
            dma((3,)),
            dma((3,)),
            dma((4,)),
            dma((heads, 2)),
            dma((heads,)),
        ],
        compiler_params=pltpu.CompilerParams(
            vmem_limit_bytes=56 * 2**20, collective_id=3, has_side_effects=True
        ),
        cost_estimate=pl.CostEstimate(
            flops=6 * tok_rows * full_width * columns, bytes_accessed=2**23, transcendentals=0
        ),
    )(tokens, pre_gain.reshape(1, -1), w_query, w_key, w_value, w_pool)


def mix(
    hdim,
    lam_ref,
    q_ref,
    k_ref,
    v_ref,
    gain_ref,
    scaled_ref,
    inverse_ref,
    pool_ref,
    group_ref,
    pscale_ref,
    wo_ref,
    out_ref,
    q_in,
    k_all,
    v_all,
    acc,
    top,
    total,
    done,
    w_pool,
    w_full,
    branch,
    pool_sc,
    halo,
    pooled_sc,
    *sems,
):
    (z_send, z_recv, in_send, in_recv, back_send, back_recv) = sems[:6]
    (py_send, py_recv, pc_send, pc_recv, edge_sem, half_sem) = sems[6:12]
    (wl_send, wl_recv, wy_send, wy_recv, wx_send, wx_recv, wc_send, wc_recv) = sems[12:]
    planes, rows, _ = q_ref.shape
    vdim = v_ref.shape[1]
    members = k_all.shape[1]
    groups = group_ref.shape[0]
    half_rows = rows // 2
    sp = lax.axis_index("sp")
    tp = lax.axis_index("tp")
    n_sp = lax.axis_size("sp")
    z = sp // members
    m = sp % members
    y = m // 2
    c = m % 2
    y_member = (m + 2) % members
    c_member = m + 1 - 2 * c
    turned = members - 1 - m
    upper = z // 2

    def at(plane, member, half=None):
        device = {"sp": plane * members + member}
        if half is not None:
            device["tp"] = half
        return device

    y_peer = at(z, y_member)
    c_peer = at(z, c_member)
    x_peer = {"tp": 1 - tp}

    def holder(block, member):
        return member + (block % 2) * (members - 1 - 2 * member)

    def order(i):
        return arrival(z, i)

    barrier = pltpu.get_barrier_semaphore()

    def greet(device):
        pl.semaphore_signal(barrier, 1, device_id=device, device_id_type=pl.DeviceIdType.MESH)

    for i in range(1, planes):
        greet(at(order(i), m))
        greet(at(order(i), turned))
    for member in (turned, y_member, c_member):
        greet(at(z, member))
    for plane in range(planes):
        greet(at(plane, m, 1 - tp))
        greet(at(plane, turned, 1 - tp))
    pl.semaphore_wait(barrier, 4 * planes + 1)

    def remote(src, dst, send, recv, device):
        return pltpu.make_async_remote_copy(
            src_ref=src,
            dst_ref=dst,
            send_sem=send,
            recv_sem=recv,
            device_id=device,
            device_id_type=pl.DeviceIdType.MESH,
        )

    def arrived(ref, recv):
        remote(ref, ref, recv, recv, c_peer).wait_recv()

    def k_out(plane):
        return remote(k_ref.at[plane], k_all.at[z, m], z_send.at[0, plane], z_recv.at[0, z], at(plane, m))

    def v_out(plane):
        return remote(v_ref.at[plane], v_all.at[z, m], z_send.at[1, plane], z_recv.at[1, z], at(plane, m))

    def q_out(plane):
        return remote(
            q_ref.at[plane], q_in.at[z], z_send.at[2, plane], z_recv.at[2, z], at(plane, holder(z, m))
        )

    def in_plane(plane, own):
        copies = []
        for t, (mine, everyone) in enumerate(((k_ref, k_all), (v_ref, v_all))):
            src = mine.at[plane] if own else everyone.at[plane, m]
            there = everyone.at[plane, m]
            passed = everyone.at[plane, y_member]
            copies.append(
                [
                    remote(src, there, in_send.at[plane, 0, t], in_recv.at[plane, 0, t], y_peer),
                    remote(src, there, in_send.at[plane, 1, t], in_recv.at[plane, 1, t], c_peer),
                    remote(passed, passed, in_send.at[plane, 2, t], in_recv.at[plane, 2, t], c_peer),
                ]
            )
        return copies

    def share(plane, own):
        for copies in in_plane(plane, own):
            copies[0].start()
            copies[1].start()

    def hand_on(plane, own):
        for copies in in_plane(plane, own):
            copies[0].wait_recv()
            copies[2].start()

    def shared(plane, own):
        for copies in in_plane(plane, own):
            copies[1].wait_recv()
            copies[2].wait_recv()

    def landed(i):
        plane = order(i)
        arrived(k_all.at[plane, m], z_recv.at[0, plane])
        arrived(v_all.at[plane, m], z_recv.at[1, plane])
        share(plane, False)

    pool_rows = pool_ref.shape[1]

    def pool_slot(plane, member):
        start = pl.multiple_of((plane * members + member) * pool_rows, pool_rows)
        return w_pool.at[pl.ds(start, pool_rows), :]

    def pool_across(plane):
        return remote(pool_ref.at[plane], pool_slot(plane, m), py_send.at[plane], py_recv.at[plane], y_peer)

    def pool_beside(plane):
        return remote(pool_ref.at[plane], pool_slot(plane, m), pc_send.at[plane, 0], pc_recv.at[plane, 0], c_peer)

    def pool_onward(plane):
        passed = pool_slot(plane, y_member)
        return remote(passed, passed, pc_send.at[plane, 1], pc_recv.at[plane, 1], c_peer)

    out_rows, out_columns = wo_ref.shape

    def out_slot(half, plane, yy, cc):
        first = pl.multiple_of(half * out_rows, out_rows)
        column = pl.multiple_of((plane * members + yy * 2 + cc) * out_columns, out_columns)
        return w_full.at[pl.ds(first, out_rows), pl.ds(column, out_columns)]

    def w_line(plane, up, own):
        there = out_slot(tp, plane, y, c)
        side = 1 if up else 0
        return remote(
            wo_ref if own else there,
            there,
            wl_send.at[plane, side],
            wl_recv.at[plane],
            {"sp": sp + (members if up else -members)},
        )

    def w_across(plane, own):
        there = out_slot(tp, plane, y, c)
        return remote(wo_ref if own else there, there, wy_send.at[plane], wy_recv.at[plane], y_peer)

    def w_swap(plane, yy, own):
        there = out_slot(tp, plane, yy, c)
        return remote(wo_ref if own else there, there, wx_send.at[plane, yy], wx_recv.at[plane, yy], x_peer)

    def w_beside(half, plane, yy, own):
        there = out_slot(half, plane, yy, c)
        return remote(
            wo_ref if own else there, there, wc_send.at[half, plane, yy], wc_recv.at[half, plane, yy], c_peer
        )

    def w_spread(plane, own):
        w_across(plane, own).start()
        w_swap(plane, y, own).start()
        w_beside(tp, plane, y, own).start()

    def w_line_start():
        @pl.when(z < planes - 1)
        def _():
            w_line(z, True, True).start()

        @pl.when(z > 0)
        def _():
            w_line(z, False, True).start()

    def w_from_line(i):
        plane = order(i)
        arrived(out_slot(tp, plane, y, c), wl_recv.at[plane])

        @pl.when((plane < z) & (z < planes - 1))
        def _():
            w_line(plane, True, False).start()

        @pl.when((plane > z) & (z > 0))
        def _():
            w_line(plane, False, False).start()

        w_spread(plane, False)

    def w_from_pair(i):
        plane = order(i)
        arrived(out_slot(tp, plane, 1 - y, c), wy_recv.at[plane])
        w_swap(plane, 1 - y, False).start()
        w_beside(tp, plane, 1 - y, False).start()

    def w_from_swap(i):
        plane = order(i)
        for yy in (y, 1 - y):
            arrived(out_slot(1 - tp, plane, yy, c), wx_recv.at[plane, yy])
            w_beside(1 - tp, plane, yy, False).start()

    share(z, True)

    @pl.when(z % 2 == 1)
    def _():
        q_out(z).start()

    for i in range(1, planes):
        k_out(order(i)).start()
        v_out(order(i)).start()
        q_out(order(i)).start()
    for plane in range(planes):
        pool_across(plane).start()
        pool_beside(plane).start()
    w_spread(z, True)
    k_all[z, m] = k_ref[z]
    v_all[z, m] = v_ref[z]
    for plane in range(planes):
        start = pl.multiple_of((plane * members + m) * pool_rows, pool_rows)
        w_pool[pl.ds(start, pool_rows), :] = pool_ref[plane]
    w_full[
        pl.ds(pl.multiple_of(tp * out_rows, out_rows), out_rows),
        pl.ds(pl.multiple_of(sp * out_columns, out_columns), out_columns),
    ] = wo_ref[...]

    @pl.when(z % 2 == 0)
    def _():
        q_in[z] = q_ref[z]

    acc[...] = jnp.zeros_like(acc)
    total[...] = jnp.zeros_like(total)
    top[...] = jnp.full_like(top, NEG_LARGE)

    def visit(block, plane, first, count, masked):
        query = q_in[block]
        lane = lax.broadcasted_iota(jnp.int32, query.shape, 1)
        none = jnp.zeros_like(query)
        both = jnp.concatenate(
            [jnp.where(lane < hdim, query, none), jnp.where(lane < hdim, none, query)], axis=0
        )
        keys = k_all[plane, pl.ds(first, count)].reshape(count * rows, 2 * hdim)
        values = jnp.concatenate([v_all[plane, first + i] for i in range(count)], axis=1)
        scores = lax.dot_general(
            keys, both, (((1,), (1,)), ((), ())), preferred_element_type=jnp.float32
        )
        if masked:
            shift = (first - holder(block, m)) * rows
            key = lax.broadcasted_iota(jnp.int32, scores.shape, 0)
            col = lax.broadcasted_iota(jnp.int32, scores.shape, 1)
            col = jnp.where(col < rows, col, col - rows)
            scores = jnp.where(key + shift <= col, scores, NEG_LARGE)
        old = top[block]
        new = jnp.maximum(old, jnp.max(scores, axis=0, keepdims=True))
        factor = jnp.exp(old - new)
        expo = jnp.exp(scores - new)
        acc[block] = acc[block] * factor + jnp.dot(
            values, expo.astype(jnp.bfloat16), preferred_element_type=jnp.float32
        )
        partial = jnp.sum(expo.reshape(count * rows // 8, 8, 2 * rows), axis=0)
        total[block] = total[block] * factor + partial
        top[block] = new

    def diagonal(block):
        pair = holder(block, m) // 2

        @pl.when(pair > 0)
        def _():
            visit(block, block, 0, members // 2, False)

        visit(block, block, pair * (members // 2), members // 2, True)

    def result_copy(block, half):
        return remote(
            done.at[block, pl.ds(pl.multiple_of(half * half_rows, half_rows), half_rows)],
            branch.at[tp * planes + z, :, pl.ds(0, vdim)],
            back_send.at[block, half],
            back_recv.at[tp * planes + z],
            at(block, holder(block, m), half),
        )

    def at_home(block):
        return (block == z) & (z % 2 == 0)

    def finish(block):
        both = acc[block] / jnp.sum(total[block], axis=0, keepdims=True)
        mixed = both[:, :rows] - lam_ref[z] * both[:, rows:]
        mean_sq = jnp.mean(mixed * mixed, axis=0, keepdims=True)
        normed = (mixed * lax.rsqrt(mean_sq + EPSILON)).T * gain_ref[...]
        done[block] = normed.astype(jnp.bfloat16)

        @pl.when(at_home(block))
        def _():
            kept = pl.ds(pl.multiple_of(tp * half_rows, half_rows), half_rows)
            branch[tp * planes + z, :, :vdim] = done[block, kept]

        @pl.when(jnp.logical_not(at_home(block)))
        def _():
            result_copy(block, tp).start()

        result_copy(block, 1 - tp).start()

    edge_rows = halo.shape[0]

    def edge_out():
        return remote(
            pool_sc.at[pl.ds(rows - edge_rows, edge_rows)], halo, edge_sem.at[0], edge_sem.at[1], {"sp": sp + 1}
        )

    def half_out():
        mine = pl.ds(pl.multiple_of(tp * groups, groups), groups)
        return remote(
            pooled_sc, branch.at[mine, :, pl.ds(vdim, vdim)], half_sem.at[0], half_sem.at[1], x_peer
        )

    def pool_project():
        for plane in range(planes):
            arrived(pool_slot(plane, c_member), pc_recv.at[plane, 0])
            arrived(pool_slot(plane, members - 1 - m), pc_recv.at[plane, 1])
        product = jnp.dot(scaled_ref[...], w_pool[...], preferred_element_type=jnp.float32)
        pool_sc[...] = (product * inverse_ref[:, :1]).astype(jnp.bfloat16)

        @pl.when(sp < n_sp - 1)
        def _():
            edge_out().start()

        @pl.when(sp == 0)
        def _():
            halo[...] = jnp.zeros_like(halo)

    def pool_mix():
        @pl.when(sp > 0)
        def _():
            arrived(halo, edge_sem.at[1])

        for g in range(groups):
            part = slice(g * vdim, (g + 1) * vdim)
            own = pool_sc[:, part].astype(jnp.float32)
            running = jnp.concatenate([halo[:, part].astype(jnp.float32), own], axis=0)
            span = WINDOWS[g % len(WINDOWS)]
            step = 1
            while step < span:
                running = running + pltpu.roll(running, step, 0)
                step *= 2
            position = sp * rows + lax.broadcasted_iota(jnp.int32, own.shape, 0)
            count = jnp.minimum(position + 1, span).astype(jnp.float32)
            differ = (running[edge_rows:] / count - own).astype(jnp.bfloat16)
            pooled = jnp.dot(differ, group_ref[g], preferred_element_type=jnp.float32)
            pooled = (pooled * pscale_ref[:, part]).astype(jnp.bfloat16)
            low, high = pooled[:half_rows], pooled[half_rows:]
            branch[tp * groups + g, :, vdim:] = jnp.where(tp == 0, low, high)
            pooled_sc[g] = jnp.where(tp == 0, high, low)
        half_out().start()

    hand_on(z, True)
    shared(z, True)

    @pl.when(z % 2 == 1)
    def _():
        arrived(q_in.at[z], z_recv.at[2, z])

    for plane in range(planes):
        arrived(pool_slot(plane, y_member), py_recv.at[plane])
        pool_onward(plane).start()

    def stage(i, carry):
        block = order(i)

        @pl.when(i < planes - 1)
        def _():
            landed(i + 1)

        @pl.when(i == LINE_STAGE)
        def _():
            w_line_start()

        diagonal(block)

        @pl.when(i < planes - 1)
        def _():
            hand_on(order(i + 1), False)

        @pl.when(i == 0)
        def _():
            pool_project()
            w_from_pair(0)

        @pl.when(i == 1)
        def _():
            pool_mix()
            w_from_swap(0)

        @pl.when(i == planes - 1)
        def _():
            w_from_line(1)
            finish(0)

        def pair(j, carry):
            other = jnp.where(i < planes - 1, order(j), j + upper)
            visit(jnp.maximum(block, other), jnp.minimum(block, other), 0, members, False)

            @pl.when(i == planes - 1)
            def _():
                finish(j + 1)

                @pl.when(j == 0)
                def _():
                    w_from_pair(1)
                    w_from_line(2)

                @pl.when(j == 1)
                def _():
                    w_from_pair(2)
                    w_from_line(3)

            return carry

        lax.fori_loop(0, i, pair, 0)

        @pl.when(i < planes - 1)
        def _():
            arrived(q_in.at[order(i + 1)], z_recv.at[2, order(i + 1)])
            shared(order(i + 1), False)

        return carry

    lax.fori_loop(0, planes, stage, 0)
    w_from_pair(3)
    for i in range(1, planes):
        w_from_swap(i)

    for head in range(2 * planes):
        own_head = tp * planes + z == head

        @pl.when(jnp.logical_not(own_head & at_home(z)))
        def _():
            arrived(branch.at[head, :, pl.ds(0, vdim)], back_recv.at[head])

    theirs = pl.ds(pl.multiple_of((1 - tp) * groups, groups), groups)
    arrived(branch.at[theirs, :, pl.ds(vdim, vdim)], half_sem.at[1])
    for half in range(2):
        for plane in range(planes):
            for yy in range(2):
                arrived(out_slot(half, plane, yy, 1 - c), wc_recv.at[half, plane, yy])
    left = jnp.concatenate([branch[head] for head in range(2 * planes)], axis=1)
    width = out_ref.shape[1] // planes

    def column(n, carry):
        part = pl.ds(pl.multiple_of(n * width, width), width)
        out_ref[:, part] = jnp.dot(
            left, w_full[:, part], preferred_element_type=jnp.float32
        ).astype(jnp.bfloat16)
        return carry

    lax.fori_loop(0, planes, column, 0)

    for i in range(1, planes):
        k_out(order(i)).wait_send()
        v_out(order(i)).wait_send()
        q_out(order(i)).wait_send()

    @pl.when(z % 2 == 1)
    def _():
        q_out(z).wait_send()

    for i in range(planes):
        plane = order(i)
        for copies in in_plane(plane, i == 0):
            for copy in copies:
                copy.wait_send()
        w_across(plane, i == 0).wait_send()
        for yy in (y, 1 - y):
            w_swap(plane, yy, False).wait_send()
            w_beside(0, plane, yy, False).wait_send()
            w_beside(1, plane, yy, False).wait_send()

        @pl.when((plane <= z) & (z < planes - 1))
        def _():
            w_line(plane, True, False).wait_send()

        @pl.when((plane >= z) & (z > 0))
        def _():
            w_line(plane, False, False).wait_send()

    for plane in range(planes):
        pool_across(plane).wait_send()
        pool_beside(plane).wait_send()
        pool_onward(plane).wait_send()
        result_copy(plane, 1 - tp).wait_send()

        @pl.when(jnp.logical_not(at_home(plane)))
        def _():
            result_copy(plane, tp).wait_send()

    half_out().wait_send()

    @pl.when(sp < n_sp - 1)
    def _():
        edge_out().wait_send()


def attend_and_project(
    queries, keys, values, lambdas, sub_gain, scaled, inverse, pool_lines, group_weight, pool_scale, w_out
):
    planes, rows, width = queries.shape
    vdim = values.shape[1]
    n_sp = lax.axis_size("sp")
    members = n_sp // planes
    groups, group_dim, _ = group_weight.shape
    out_rows, out_columns = w_out.shape
    vmem = pl.BlockSpec(memory_space=pltpu.VMEM)
    dma = pltpu.SemaphoreType.DMA
    work = planes * rows * members * planes * rows
    return pl.pallas_call(
        functools.partial(mix, width // 2),
        out_shape=jax.ShapeDtypeStruct((rows // 2, n_sp * out_columns), jnp.bfloat16),
        in_specs=[pl.BlockSpec(memory_space=pltpu.SMEM)] + [vmem] * 10,
        out_specs=vmem,
        scratch_shapes=[
            pltpu.VMEM((planes, rows, width), jnp.bfloat16),
            pltpu.VMEM((planes, members, rows, width), jnp.bfloat16),
            pltpu.VMEM((planes, members, vdim, rows), jnp.bfloat16),
            pltpu.VMEM((planes, vdim, 2 * rows), jnp.float32),
            pltpu.VMEM((planes, 1, 2 * rows), jnp.float32),
            pltpu.VMEM((planes, 8, 2 * rows), jnp.float32),
            pltpu.VMEM((planes, rows, vdim), jnp.bfloat16),
            pltpu.VMEM((scaled.shape[1], groups * group_dim), jnp.bfloat16),
            pltpu.VMEM((2 * out_rows, n_sp * out_columns), jnp.bfloat16),
            pltpu.VMEM((2 * planes, rows // 2, 2 * vdim), jnp.bfloat16),
            pltpu.VMEM((rows, groups * group_dim), jnp.bfloat16),
            pltpu.VMEM((RIM_ROWS + 1, groups * group_dim), jnp.bfloat16),
            pltpu.VMEM((groups, rows // 2, group_dim), jnp.bfloat16),
            dma((3, planes)),
            dma((3, planes)),
            dma((planes, 3, 2)),
            dma((planes, 3, 2)),
            dma((planes, 2)),
            dma((2 * planes,)),
            dma((planes,)),
            dma((planes,)),
            dma((planes, 2)),
            dma((planes, 2)),
            dma((2,)),
            dma((2,)),
            dma((planes, 2)),
            dma((planes,)),
            dma((planes,)),
            dma((planes,)),
            dma((planes, 2)),
            dma((planes, 2)),
            dma((2, planes, 2)),
            dma((2, planes, 2)),
        ],
        compiler_params=pltpu.CompilerParams(
            vmem_limit_bytes=60 * 2**20, collective_id=2, has_side_effects=True
        ),
        cost_estimate=pl.CostEstimate(
            flops=4 * work * vdim, bytes_accessed=keys.size * 8, transcendentals=work
        ),
    )(
        lambdas,
        queries,
        keys,
        values,
        sub_gain.reshape(1, -1),
        scaled,
        inverse,
        pool_lines,
        group_weight,
        pool_scale.reshape(1, -1),
        w_out,
    )


def trailing(x, window_ids, group_dim):
    column_window = jnp.repeat(window_ids, group_dim)[None, :]
    running = x
    picked = jnp.zeros_like(x)
    for slot, span in enumerate(WINDOWS):
        half = span // 2
        running = running + jnp.pad(running[:-half], ((half, 0), (0, 0)))
        picked = jnp.where(column_window == slot, running, picked)
    return picked


def general_attention(queries, key_rows, values, lambdas, sub_gain):
    n_sp = lax.axis_size("sp")
    sp = lax.axis_index("sp")
    tok_rows = queries.shape[0]
    heads = lambdas.shape[0]
    qdim = queries.shape[1] // heads
    vdim = values.shape[1] // heads
    head_width = 2 * qdim + vdim
    outer = math.gcd(n_sp, heads)
    inner = n_sp // outer
    per_device = heads // outer
    by_head = jnp.concatenate(
        [
            x.reshape(tok_rows, heads, -1).swapaxes(0, 1)
            for x in (queries, key_rows, values)
        ],
        axis=2,
    )
    across = [[o * inner + i for o in range(outer)] for i in range(inner)]
    within = [[o * inner + i for i in range(inner)] for o in range(outer)]
    by_head = by_head.reshape(outer, per_device, tok_rows, head_width)
    if outer > 1:
        by_head = lax.all_to_all(by_head, "sp", 0, 0, axis_index_groups=across)
    first_head = lax.div(sp, inner) * per_device
    attended = []
    if inner == 4 and per_device == 1:
        lam = lax.dynamic_slice_in_dim(lambdas, first_head, 1)
        attended.append(
            flash_members(by_head[:, 0, :, :qdim], by_head[:, 0, :, qdim:], lam, sub_gain)
        )
    else:
        kv = lax.all_gather(by_head[..., qdim:], "sp", axis=0, axis_index_groups=within)
        member = lax.rem(sp, inner).reshape(1)
        for p in range(per_device):
            lam = lax.dynamic_slice_in_dim(lambdas, first_head + p, 1)
            attended.append(flash(by_head[:, p, :, :qdim], kv[:, :, p], member, lam, sub_gain))
    attended = jnp.stack(attended, axis=1)
    if outer > 1:
        attended = lax.all_to_all(attended, "sp", 0, 0, axis_index_groups=across)
    return attended.reshape(heads, tok_rows, vdim)


def local(
    tokens,
    pre_gain,
    w_query,
    w_key,
    w_value,
    w_pool,
    lambdas,
    sub_gain,
    group_weight,
    pool_scale,
    w_out,
):
    n_tp = lax.axis_size("tp")
    n_sp = lax.axis_size("sp")
    tp = lax.axis_index("tp")
    sp = lax.axis_index("sp")
    tok_rows = tokens.shape[0]
    model_width = tokens.shape[1] * n_tp
    heads = lambdas.shape[0]
    qdim = w_query.shape[1] // heads
    vdim = w_value.shape[1] // heads
    groups = group_weight.shape[0]
    group_dim = group_weight.shape[1]

    shaped_for_mix = n_tp == 2 and heads == 4 and n_sp == 4 * heads and tok_rows % 32 == 0
    if shaped_for_mix and qdim == vdim == group_dim and groups == heads:
        queries, key_rows, values, scaled, inverse, pool_lines = gather_and_project(
            tokens, pre_gain, w_query, w_key, w_value, w_pool, heads
        )
        return attend_and_project(
            queries,
            key_rows,
            values,
            lambdas,
            sub_gain,
            scaled,
            inverse,
            pool_lines,
            group_weight,
            pool_scale,
            w_out,
        )
    swap = [(0, 1), (1, 0)]
    w_sorted = w_out.reshape(heads, 2, vdim, -1).swapaxes(0, 1).reshape(w_out.shape)
    features = tokens.astype(jnp.float32)
    mine = (features * pre_gain.astype(jnp.float32)[None, :]).astype(jnp.bfloat16)
    squares = jnp.sum(features * features, axis=1, keepdims=True)
    weights = [w_query, w_key, w_value, w_pool]
    if n_sp % 4 == 0:
        *weights, theirs = gather_weights(weights, mine, n_tp == 2)
    else:
        weights = [lax.all_gather(w, "sp", axis=0, tiled=True) for w in weights]
        theirs = lax.ppermute(mine, "tp", swap) if n_tp == 2 else mine
    w_sorted, weights = lax.optimization_barrier((w_sorted, weights))
    w_out_rows = lax.all_gather(w_sorted, "sp", axis=1, tiled=True)
    if n_tp == 2:
        squares = squares + lax.ppermute(squares, "tp", swap)
        scaled = jnp.concatenate(
            [jnp.where(tp == 0, mine, theirs), jnp.where(tp == 0, theirs, mine)], axis=1
        )
    else:
        scaled = lax.all_gather(mine, "tp", axis=1, tiled=True)
        squares = lax.psum(squares, "tp")
    inverse = lax.rsqrt(squares / model_width + EPSILON)
    queries, key_rows, values, pool_in = [
        (jnp.dot(scaled, w, preferred_element_type=jnp.float32) * inverse).astype(jnp.bfloat16)
        for w in weights
    ]
    attended = general_attention(queries, key_rows, values, lambdas, sub_gain)

    halo = passed_along(pool_in[tok_rows - RIM_ROWS - 1 :], "sp", 1)
    extended = jnp.concatenate([halo, pool_in], axis=0).astype(jnp.float32)
    window_ids = (tp * groups + jnp.arange(groups, dtype=jnp.int32)) % len(WINDOWS)
    sums = trailing(extended, window_ids, group_dim)[RIM_ROWS + 1 :]
    spans = jnp.repeat(jnp.left_shift(2, window_ids), group_dim)
    positions = sp * tok_rows + jnp.arange(tok_rows, dtype=jnp.int32)
    count = jnp.minimum(positions[:, None] + 1, spans[None, :]).astype(jnp.float32)
    differ = (sums / count - pool_in.astype(jnp.float32)).astype(jnp.bfloat16)
    pooled = jnp.einsum(
        "tgc,gcd->tgd",
        differ.reshape(tok_rows, groups, group_dim),
        group_weight,
        preferred_element_type=jnp.float32,
    )
    pooled = (pooled * pool_scale.reshape(groups, group_dim)).astype(jnp.bfloat16)
    branch = jnp.concatenate(
        [attended.swapaxes(0, 1).reshape(tok_rows, -1), pooled.reshape(tok_rows, -1)], axis=1
    )
    if n_tp == 2:
        half = tok_rows // 2
        send = lax.dynamic_slice_in_dim(branch, (1 - tp) * half, half, 0)
        send = jnp.dot(send, w_out_rows, preferred_element_type=jnp.float32).astype(jnp.bfloat16)
        got = lax.ppermute(send, "tp", swap)
        keep = lax.dynamic_slice_in_dim(branch, tp * half, half, 0)
        keep = jnp.dot(keep, w_out_rows, preferred_element_type=jnp.float32)
        return (keep + got.astype(jnp.float32)).astype(jnp.bfloat16)
    partial = jnp.dot(branch, w_out_rows, preferred_element_type=jnp.float32)
    return lax.psum_scatter(partial.astype(jnp.bfloat16), "tp", scatter_dimension=0, tiled=True)


def solution(mesh):
    placed = (
        P("sp", "tp"),
        P("tp"),
        P("sp", "tp"),
        P("sp", "tp"),
        P("sp", "tp"),
        P("sp", "tp"),
        P("tp"),
        P(),
        P("tp", None, None),
        P("tp"),
        P("tp", "sp"),
    )
    return jax.shard_map(
        local, mesh=mesh, in_specs=placed, out_specs=P(("sp", "tp"), None), check_vma=False
    )
```

```python
import functools
import math

import jax
import jax.numpy as jnp
from jax import lax
from jax.experimental import pallas as pl
from jax.experimental.pallas import tpu as pltpu
from jax.sharding import PartitionSpec as P

EPSILON = 1e-06
NEG_LARGE = -1e30
WINDOWS = (2, 4, 8, 16)
RIM_ROWS = 15


def passed_along(block, axis, distance):
    devices = range(lax.axis_size(axis))
    route = [(i - distance, i) for i in devices if i - distance in devices]
    return lax.ppermute(block, axis, route)


def attend(inner, vdim, hdim, member_ref, lam_ref, q_ref, kv_ref, gain_ref, out_ref, acc_ref, max_ref):
    rows = q_ref.shape[1]
    block = pl.program_id(0)
    last = block * inner + member_ref[0]
    scale = 1.0 / math.sqrt(hdim)
    queries = (q_ref[0].astype(jnp.float32) * scale).astype(jnp.bfloat16)
    maps = (queries[:, :hdim], queries[:, hdim:])
    ones = jnp.ones((rows, vdim), jnp.bfloat16)
    acc_ref[...] = jnp.zeros_like(acc_ref)
    max_ref[...] = jnp.full_like(max_ref, NEG_LARGE)

    def step(g, masked):
        keys_values = kv_ref[lax.rem(g, inner), lax.div(g, inner)]
        values = jnp.concatenate([keys_values[:, 2 * hdim :], ones], axis=1)
        for m in range(2):
            keys = keys_values[:, m * hdim : (m + 1) * hdim]
            scores = lax.dot_general(
                maps[m], keys, (((1,), (1,)), ((), ())), preferred_element_type=jnp.float32
            )
            if masked:
                row = lax.broadcasted_iota(jnp.int32, scores.shape, 0)
                col = lax.broadcasted_iota(jnp.int32, scores.shape, 1)
                scores = jnp.where(col <= row, scores, NEG_LARGE)
            old_max = max_ref[m]
            new_max = jnp.maximum(old_max, jnp.max(scores, axis=1, keepdims=True))
            factor = jnp.exp(old_max - new_max)
            expo = jnp.exp(scores - new_max[:, :1])
            acc_ref[m] = acc_ref[m] * factor[:, :1] + jnp.dot(
                expo.astype(jnp.bfloat16), values, preferred_element_type=jnp.float32
            )
            max_ref[m] = new_max

    def body(g, carry):
        step(g, False)
        return carry

    lax.fori_loop(0, last, body, 0)
    step(last, True)
    first = acc_ref[0]
    second = acc_ref[1]
    mix = first[:, :vdim] / first[:, vdim:] - lam_ref[0] * (second[:, :vdim] / second[:, vdim:])
    mean_sq = jnp.mean(mix * mix, axis=1, keepdims=True)
    out_ref[0] = (mix * lax.rsqrt(mean_sq + EPSILON) * gain_ref[...]).astype(jnp.bfloat16)


def flash(q, kv, member, lam, sub_gain):
    inner, outer, rows, width = kv.shape
    qdim = q.shape[-1]
    vdim = width - qdim
    smem = pl.BlockSpec(memory_space=pltpu.SMEM)
    work = outer * rows * outer * rows * inner
    return pl.pallas_call(
        functools.partial(attend, inner, vdim, qdim // 2),
        grid=(outer,),
        out_shape=jax.ShapeDtypeStruct((outer, rows, vdim), jnp.bfloat16),
        in_specs=[
            smem,
            smem,
            pl.BlockSpec((1, rows, qdim), lambda b: (b, 0, 0)),
            pl.BlockSpec(memory_space=pltpu.VMEM),
            pl.BlockSpec(memory_space=pltpu.VMEM),
        ],
        out_specs=pl.BlockSpec((1, rows, vdim), lambda b: (b, 0, 0)),
        scratch_shapes=[
            pltpu.VMEM((2, rows, 2 * vdim), jnp.float32),
            pltpu.VMEM((2, rows, 128), jnp.float32),
        ],
        compiler_params=pltpu.CompilerParams(vmem_limit_bytes=56 * 2**20),
        cost_estimate=pl.CostEstimate(
            flops=4 * work * vdim, bytes_accessed=kv.size * 2, transcendentals=work
        ),
    )(member, lam, q, kv, sub_gain.reshape(1, -1))


def attend_members(hdim, lam_ref, q_ref, own_ref, gain_ref, out_ref, held, acc_ref, max_ref, send, recv):
    outer, rows, _ = q_ref.shape
    vdim = own_ref.shape[2] - 2 * hdim
    sp = lax.axis_index("sp")
    member = lax.rem(sp, 4)
    y = lax.div(member, 2)
    c = lax.rem(member, 2)
    y_peer = sp + 2 - 4 * y
    c_peer = sp + 1 - 2 * c
    barrier = pltpu.get_barrier_semaphore()
    for peer in (y_peer, c_peer):
        pl.semaphore_signal(
            barrier, 1, device_id={"sp": peer}, device_id_type=pl.DeviceIdType.MESH
        )
    pl.semaphore_wait(barrier, 2)

    def remote(src, index, peer):
        return pltpu.make_async_remote_copy(
            src_ref=src,
            dst_ref=held.at[index],
            send_sem=send.at[index],
            recv_sem=recv.at[index],
            device_id={"sp": peer},
            device_id_type=pl.DeviceIdType.MESH,
        )

    across = remote(own_ref, 1, y_peer)
    beside = remote(own_ref, 0, c_peer)
    onward = remote(held.at[1], 2, c_peer)
    across.start()
    beside.start()
    acc_ref[...] = jnp.zeros_like(acc_ref)
    max_ref[...] = jnp.full_like(max_ref, NEG_LARGE)
    scale = 1.0 / math.sqrt(hdim)

    def visit(ref, other):
        shift = (member - other) * rows
        for block in range(outer):
            queries = (q_ref[block].astype(jnp.float32) * scale).astype(jnp.bfloat16)
            length = (block + 1) * rows
            keys_values = ref[: block + 1].reshape(length, 2 * hdim + vdim)
            values = jnp.concatenate(
                [keys_values[:, 2 * hdim :], jnp.ones((length, vdim), jnp.bfloat16)], axis=1
            )
            for m in range(2):
                scores = lax.dot_general(
                    queries[:, m * hdim : (m + 1) * hdim],
                    keys_values[:, m * hdim : (m + 1) * hdim],
                    (((1,), (1,)), ((), ())),
                    preferred_element_type=jnp.float32,
                )
                edge = scores[:, block * rows :]
                row = lax.broadcasted_iota(jnp.int32, edge.shape, 0)
                col = lax.broadcasted_iota(jnp.int32, edge.shape, 1)
                edge = jnp.where(col <= row + shift, edge, NEG_LARGE)
                if block > 0:
                    scores = jnp.concatenate([scores[:, : block * rows], edge], axis=1)
                else:
                    scores = edge
                old_max = max_ref[block, m]
                new_max = jnp.maximum(old_max, jnp.max(scores, axis=1, keepdims=True))
                factor = jnp.exp(old_max - new_max)
                expo = jnp.exp(scores - new_max[:, :1])
                acc_ref[block, m] = acc_ref[block, m] * factor[:, :1] + jnp.dot(
                    expo.astype(jnp.bfloat16), values, preferred_element_type=jnp.float32
                )
                max_ref[block, m] = new_max

    visit(own_ref, member)

    def arrived(j, carry):
        @pl.when(j == 0)
        def _():
            beside.wait_recv()

        @pl.when(j == 1)
        def _():
            across.wait_recv()
            onward.start()

        @pl.when(j == 2)
        def _():
            onward.wait_recv()

        other_y = jnp.where(j >= 1, 1 - y, y)
        other_c = jnp.where(j == 1, c, 1 - c)
        visit(held.at[j], 2 * other_y + other_c)
        return carry

    lax.fori_loop(0, 3, arrived, 0)
    for copy in (across, beside, onward):
        copy.wait_send()
    for block in range(outer):
        first = acc_ref[block, 0]
        second = acc_ref[block, 1]
        mix = first[:, :vdim] / first[:, vdim:]
        mix = mix - lam_ref[0] * (second[:, :vdim] / second[:, vdim:])
        mean_sq = jnp.mean(mix * mix, axis=1, keepdims=True)
        normed = mix * lax.rsqrt(mean_sq + EPSILON) * gain_ref[...]
        out_ref[block] = normed.astype(jnp.bfloat16)


def flash_members(q, kv, lam, sub_gain):
    outer, rows, width = kv.shape
    qdim = q.shape[-1]
    vdim = width - qdim
    vmem = pl.BlockSpec(memory_space=pltpu.VMEM)
    work = 4 * outer * rows * outer * rows
    return pl.pallas_call(
        functools.partial(attend_members, qdim // 2),
        out_shape=jax.ShapeDtypeStruct((outer, rows, vdim), jnp.bfloat16),
        in_specs=[pl.BlockSpec(memory_space=pltpu.SMEM), vmem, vmem, vmem],
        out_specs=vmem,
        scratch_shapes=[
            pltpu.VMEM((3, outer, rows, width), jnp.bfloat16),
            pltpu.VMEM((outer, 2, rows, 2 * vdim), jnp.float32),
            pltpu.VMEM((outer, 2, rows, 128), jnp.float32),
            pltpu.SemaphoreType.DMA((3,)),
            pltpu.SemaphoreType.DMA((3,)),
        ],
        compiler_params=pltpu.CompilerParams(
            vmem_limit_bytes=56 * 2**20, collective_id=1, has_side_effects=True
        ),
        cost_estimate=pl.CostEstimate(
            flops=4 * work * vdim, bytes_accessed=4 * kv.size * 2, transcendentals=work
        ),
    )(lam, q, kv, sub_gain.reshape(1, -1))


def spread(n_sp, count, with_swap, *refs):
    weights, refs = refs[:count], refs[count:]
    mine, refs = refs[0], refs[1:]
    fulls, refs = refs[:count], refs[count:]
    theirs, refs = refs[0], refs[1:]
    up_send, up_recv, down_send, down_recv, y_send, y_recv, c_send, c_recv, own_sem, swap_sem = refs
    depth = n_sp // 4
    rows = weights[0].shape[0]
    sp = lax.axis_index("sp")
    z = lax.div(sp, 4)
    y = lax.rem(lax.div(sp, 2), 2)
    c = lax.rem(sp, 2)
    y_peer = z * 4 + (1 - y) * 2 + c
    c_peer = z * 4 + y * 2 + (1 - c)
    barrier = pltpu.get_barrier_semaphore()

    def greet(device):
        pl.semaphore_signal(barrier, 1, device_id=device, device_id_type=pl.DeviceIdType.MESH)

    greet({"sp": y_peer})
    greet({"sp": c_peer})
    greeted = 2
    if with_swap:
        greet({"tp": 1 - lax.axis_index("tp")})
        greeted = 3

    @pl.when(z > 0)
    def _():
        greet({"sp": sp - 4})

    @pl.when(z < depth - 1)
    def _():
        greet({"sp": sp + 4})

    in_line = jnp.where(z > 0, 1, 0) + jnp.where(z < depth - 1, 1, 0)
    pl.semaphore_wait(barrier, greeted + in_line)

    def slot(a, zz, yy, cc):
        start = pl.multiple_of((zz * 4 + yy * 2 + cc) * rows, rows)
        return fulls[a].at[pl.ds(start, rows), :]

    def remote(src, dst, send, recv, device):
        return pltpu.make_async_remote_copy(
            src_ref=src,
            dst_ref=dst,
            send_sem=send,
            recv_sem=recv,
            device_id=device,
            device_id_type=pl.DeviceIdType.MESH,
        )

    def line_copy(side, k, a, src):
        sends, recvs = (up_send, up_recv) if side > 0 else (down_send, down_recv)
        there = slot(a, z - side * k, y, c)
        return remote(
            there if src is None else src,
            there,
            sends.at[k, a],
            recvs.at[k + 1, a],
            {"sp": sp + 4 * side},
        )

    def y_copy(zz, yy, a, src):
        there = slot(a, zz, yy, c)
        src = there if src is None else src
        return remote(src, there, y_send.at[zz, a], y_recv.at[zz, a], {"sp": y_peer})

    def c_copy(zz, yy, cc, a, src):
        there = slot(a, zz, yy, cc)
        src = there if src is None else src
        return remote(src, there, c_send.at[zz, yy, a], c_recv.at[zz, yy, a], {"sp": c_peer})

    def can_go(side):
        return z < depth - 1 if side > 0 else z > 0

    def came(side, k):
        return z >= k if side > 0 else z + k <= depth - 1

    if with_swap:
        swap = remote(
            mine, theirs, swap_sem.at[0], swap_sem.at[1], {"tp": 1 - lax.axis_index("tp")}
        )
        swap.start()
    for a in range(count):
        for side in (1, -1):

            @pl.when(can_go(side))
            def _():
                line_copy(side, 0, a, weights[a]).start()

        y_copy(z, y, a, weights[a]).start()
    for a in range(count):
        c_copy(z, y, c, a, weights[a]).start()
        pltpu.make_async_copy(weights[a], slot(a, z, y, c), own_sem.at[a]).start()

    def from_pair(zz):
        for a in range(count):
            y_copy(zz, 1 - y, a, None).wait_recv()
            c_copy(zz, 1 - y, c, a, None).start()

    def relay(k, carry):
        for side in (1, -1):
            recvs = up_recv if side > 0 else down_recv

            @pl.when(came(side, k))
            def _():
                zz = z - side * k
                for a in range(count):
                    there = slot(a, zz, y, c)
                    remote(there, there, up_send.at[0, a], recvs.at[k, a], {"sp": y_peer}).wait_recv()

                    @pl.when(can_go(side))
                    def _():
                        line_copy(side, k, a, None).start()

                    y_copy(zz, y, a, None).start()
                    c_copy(zz, y, c, a, None).start()

        @pl.when(k == 1)
        def _():
            from_pair(z)

        for side in (1, -1):

            @pl.when((k > 1) & came(side, k - 1))
            def _():
                from_pair(z - side * (k - 1))

        return carry

    lax.fori_loop(1, depth, relay, 0)
    if depth == 1:
        from_pair(z)
    for side in (1, -1):
        if depth > 1:

            @pl.when(came(side, depth - 1))
            def _():
                from_pair(z - side * (depth - 1))

    def drain(zz, carry):
        for a in range(count):
            y_copy(zz, y, a, None).wait_send()
            for yy in range(2):
                c_copy(zz, yy, 1 - c, a, None).wait_recv()
                c_copy(zz, yy, c, a, None).wait_send()
        return carry

    lax.fori_loop(0, depth, drain, 0)

    def drain_line(k, carry):
        for side in (1, -1):

            @pl.when(came(side, k) & can_go(side))
            def _():
                for a in range(count):
                    line_copy(side, k, a, None).wait_send()

        return carry

    lax.fori_loop(0, depth, drain_line, 0)
    for a in range(count):
        pltpu.make_async_copy(weights[a], slot(a, z, y, c), own_sem.at[a]).wait()
    if with_swap:
        swap.wait()


def gather_weights(weights, mine, with_swap):
    n_sp = lax.axis_size("sp")
    count = len(weights)
    depth = n_sp // 4
    sems = pltpu.SemaphoreType.DMA
    any_spec = pl.BlockSpec(memory_space=pl.ANY)
    vmem_spec = pl.BlockSpec(memory_space=pltpu.VMEM)
    shapes = [jax.ShapeDtypeStruct((n_sp * w.shape[0], w.shape[1]), w.dtype) for w in weights]
    shapes.append(jax.ShapeDtypeStruct(mine.shape, mine.dtype))
    moved = sum(w.size for w in weights) * 2 * n_sp
    return pl.pallas_call(
        functools.partial(spread, n_sp, count, with_swap),
        out_shape=shapes,
        in_specs=[vmem_spec] * (count + 1),
        out_specs=[any_spec] * (count + 1),
        scratch_shapes=[
            sems((depth + 1, count)),
            sems((depth + 1, count)),
            sems((depth + 1, count)),
            sems((depth + 1, count)),
            sems((depth, count)),
            sems((depth, count)),
            sems((depth, 2, count)),
            sems((depth, 2, count)),
            sems((count,)),
            sems((2,)),
        ],
        compiler_params=pltpu.CompilerParams(collective_id=0, has_side_effects=True),
        cost_estimate=pl.CostEstimate(flops=10**10, bytes_accessed=moved, transcendentals=0),
    )(*weights, mine)


def arrival(z, i):
    half = z // 2
    later = jnp.where(i == 2, 2 - half, 3 - 3 * half)
    return jnp.where(i == 0, z, jnp.where(i == 1, 1 + 4 * half - z, later))


def layer(
    hdim,
    model_width,
    lam_ref,
    tok_ref,
    gain_in,
    wk_ref,
    wv_ref,
    wq_ref,
    wp_ref,
    gain_ref,
    group_ref,
    pscale_ref,
    wo_ref,
    out_ref,
    full,
    theirs,
    their_gain,
    pieces,
    product,
    inverse_sc,
    k_src,
    v_src,
    q_src,
    q_in,
    k_all,
    v_all,
    acc,
    top,
    total,
    done,
    w_pool,
    w_full,
    branch,
    pool_sc,
    halo,
    pooled_sc,
    *sems,
):
    (line_send, line_recv, y_send, y_recv, c_send, c_recv, turn_send, turn_recv, swap_sem) = sems[:9]
    (z_send, z_recv, in_send, in_recv, back_send, back_recv) = sems[9:15]
    (py_send, py_recv, pc_send, pc_recv, edge_sem, half_sem, pool_send, pool_recv) = sems[15:23]
    (wl_send, wl_recv, wy_send, wy_recv, wx_send, wx_recv, wc_send, wc_recv) = sems[23:]
    weights = (wk_ref, wv_ref, wq_ref)
    first_pair, last_one = (0, 1), (2,)
    planes, rows, _ = q_src.shape
    vdim = v_src.shape[1]
    members = k_all.shape[1]
    w_rows, columns = wq_ref.shape
    half_width = tok_ref.shape[1]
    groups = group_ref.shape[0]
    half_rows = rows // 2
    sp = lax.axis_index("sp")
    tp = lax.axis_index("tp")
    n_sp = lax.axis_size("sp")
    z = sp // members
    m = sp % members
    y = m // 2
    c = m % 2
    y_member = (m + 2) % members
    c_member = m + 1 - 2 * c
    turned = members - 1 - m
    upper = z // 2

    def at(plane, member, half=None):
        device = {"sp": plane * members + member}
        if half is not None:
            device["tp"] = half
        return device

    y_peer = at(z, y_member)
    c_peer = at(z, c_member)
    x_peer = {"tp": 1 - tp}

    def holder(block, member):
        return member + (block % 2) * (members - 1 - 2 * member)

    def order(i):
        return arrival(z, i)

    barrier = pltpu.get_barrier_semaphore()

    def greet(device):
        pl.semaphore_signal(barrier, 1, device_id=device, device_id_type=pl.DeviceIdType.MESH)

    for i in range(1, planes):
        greet(at(order(i), m))
        greet(at(order(i), turned))
    for member in (turned, y_member, c_member):
        greet(at(z, member))
    for plane in range(planes):
        greet(at(plane, m, 1 - tp))
        greet(at(plane, turned, 1 - tp))
    pl.semaphore_wait(barrier, 4 * planes + 1)

    def remote(src, dst, send, recv, device):
        return pltpu.make_async_remote_copy(
            src_ref=src,
            dst_ref=dst,
            send_sem=send,
            recv_sem=recv,
            device_id=device,
            device_id_type=pl.DeviceIdType.MESH,
        )

    def arrived(ref, recv):
        remote(ref, ref, recv, recv, c_peer).wait_recv()

    def k_out(plane):
        return remote(k_src.at[plane], k_all.at[z, m], z_send.at[0, plane], z_recv.at[0, z], at(plane, m))

    def v_out(plane):
        return remote(v_src.at[plane], v_all.at[z, m], z_send.at[1, plane], z_recv.at[1, z], at(plane, m))

    def q_out(plane):
        return remote(
            q_src.at[plane], q_in.at[z], z_send.at[2, plane], z_recv.at[2, z], at(plane, holder(z, m))
        )

    def in_plane(plane, own):
        copies = []
        for t, (mine, everyone) in enumerate(((k_src, k_all), (v_src, v_all))):
            src = mine.at[plane] if own else everyone.at[plane, m]
            there = everyone.at[plane, m]
            passed = everyone.at[plane, y_member]
            copies.append(
                [
                    remote(src, there, in_send.at[plane, 0, t], in_recv.at[plane, 0, t], y_peer),
                    remote(src, there, in_send.at[plane, 1, t], in_recv.at[plane, 1, t], c_peer),
                    remote(passed, passed, in_send.at[plane, 2, t], in_recv.at[plane, 2, t], c_peer),
                ]
            )
        return copies

    def share(plane, own):
        for copies in in_plane(plane, own):
            copies[0].start()
            copies[1].start()

    def hand_on(plane, own):
        for copies in in_plane(plane, own):
            copies[0].wait_recv()
            copies[2].start()

    def shared(plane, own):
        for copies in in_plane(plane, own):
            copies[1].wait_recv()
            copies[2].wait_recv()

    def landed(i):
        plane = order(i)
        arrived(k_all.at[plane, m], z_recv.at[0, plane])
        arrived(v_all.at[plane, m], z_recv.at[1, plane])
        share(plane, False)

    pool_rows = wp_ref.shape[0]

    def pool_slot(plane, member):
        start = pl.multiple_of((plane * members + member) * pool_rows, pool_rows)
        return w_pool.at[pl.ds(start, pool_rows), :]

    def pool_line(plane, up, own):
        there = pool_slot(plane, m)
        side = 1 if up else 0
        return remote(
            wp_ref if own else there,
            there,
            pool_send.at[plane, side],
            pool_recv.at[plane],
            {"sp": sp + (members if up else -members)},
        )

    def pool_across(plane, own):
        there = pool_slot(plane, m)
        return remote(wp_ref if own else there, there, py_send.at[plane], py_recv.at[plane], y_peer)

    def pool_beside(plane, own):
        there = pool_slot(plane, m)
        return remote(wp_ref if own else there, there, pc_send.at[plane, 0], pc_recv.at[plane, 0], c_peer)

    def pool_onward(plane):
        passed = pool_slot(plane, y_member)
        return remote(passed, passed, pc_send.at[plane, 1], pc_recv.at[plane, 1], c_peer)

    def pool_start():
        @pl.when(z < planes - 1)
        def _():
            pool_line(z, True, True).start()

        @pl.when(z > 0)
        def _():
            pool_line(z, False, True).start()

        pool_across(z, True).start()
        pool_beside(z, True).start()

    def pool_from_line(i):
        plane = order(i)
        arrived(pool_slot(plane, m), pool_recv.at[plane])

        @pl.when((plane < z) & (z < planes - 1))
        def _():
            pool_line(plane, True, False).start()

        @pl.when((plane > z) & (z > 0))
        def _():
            pool_line(plane, False, False).start()

        pool_across(plane, False).start()
        pool_beside(plane, False).start()

    def pool_from_pair(i):
        arrived(pool_slot(order(i), y_member), py_recv.at[order(i)])
        pool_onward(order(i)).start()

    out_rows, out_columns = wo_ref.shape

    def out_slot(half, plane, yy, cc):
        first = pl.multiple_of(half * out_rows, out_rows)
        column = pl.multiple_of((plane * members + yy * 2 + cc) * out_columns, out_columns)
        return w_full.at[pl.ds(first, out_rows), pl.ds(column, out_columns)]

    def w_line(plane, up, own):
        there = out_slot(tp, plane, y, c)
        side = 1 if up else 0
        return remote(
            wo_ref if own else there,
            there,
            wl_send.at[plane, side],
            wl_recv.at[plane],
            {"sp": sp + (members if up else -members)},
        )

    def w_across(plane, own):
        there = out_slot(tp, plane, y, c)
        return remote(wo_ref if own else there, there, wy_send.at[plane], wy_recv.at[plane], y_peer)

    def w_swap(plane, yy, own):
        there = out_slot(tp, plane, yy, c)
        return remote(wo_ref if own else there, there, wx_send.at[plane, yy], wx_recv.at[plane, yy], x_peer)

    def w_beside(half, plane, yy, own):
        there = out_slot(half, plane, yy, c)
        return remote(
            wo_ref if own else there, there, wc_send.at[half, plane, yy], wc_recv.at[half, plane, yy], c_peer
        )

    def w_spread(plane):
        w_across(plane, False).start()
        w_swap(plane, y, False).start()
        w_beside(tp, plane, y, False).start()

    def w_line_start():
        @pl.when(z < planes - 1)
        def _():
            w_line(z, True, True).start()

        @pl.when(z > 0)
        def _():
            w_line(z, False, True).start()

    def w_from_line(i):
        plane = order(i)
        arrived(out_slot(tp, plane, y, c), wl_recv.at[plane])

        @pl.when((plane < z) & (z < planes - 1))
        def _():
            w_line(plane, True, False).start()

        @pl.when((plane > z) & (z > 0))
        def _():
            w_line(plane, False, False).start()

        w_spread(plane)

    def w_from_pair(i):
        plane = order(i)
        arrived(out_slot(tp, plane, 1 - y, c), wy_recv.at[plane])
        w_swap(plane, 1 - y, False).start()
        w_beside(tp, plane, 1 - y, False).start()

    def w_from_swap(i):
        plane = order(i)
        for yy in (y, 1 - y):
            arrived(out_slot(1 - tp, plane, yy, c), wx_recv.at[plane, yy])
            w_beside(1 - tp, plane, yy, False).start()

    def slot(a, zz, yy, cc, first=0, count=w_rows):
        start = pl.multiple_of((zz * members + yy * 2 + cc) * w_rows + first, count)
        return full.at[a, pl.ds(start, count), :]

    def line(a, zz, up, own):
        there = slot(a, zz, y, c)
        side = 1 if up else 0
        return remote(
            weights[a] if own else there,
            there,
            line_send.at[zz, side, a],
            line_recv.at[zz, a],
            {"sp": sp + (members if up else -members)},
        )

    def y_copy(a, i, own):
        if i == 1:
            there = slot(a, order(i), y, c, w_rows // 2, w_rows // 2)
            src = there
        else:
            there = slot(a, order(i), y, c)
            src = weights[a] if own else there
        return remote(src, there, y_send.at[order(i), a], y_recv.at[order(i), a], y_peer)

    def y_came(a, i):
        there = slot(a, order(i), 1 - y, c, *((w_rows // 2, w_rows // 2) if i == 1 else ()))
        return remote(there, there, y_send.at[order(i), a], y_recv.at[order(i), a], y_peer)

    def turn(a):
        there = slot(a, z, 1 - y, c, 0, w_rows // 2)
        return remote(there, there, turn_send.at[a], turn_recv.at[a], at(order(1), m))

    def turn_came(a):
        there = slot(a, order(1), 1 - y, c, 0, w_rows // 2)
        return remote(there, there, turn_send.at[a], turn_recv.at[a], at(order(1), m))

    def c_copy(a, zz, yy, own):
        there = slot(a, zz, yy, c)
        src = weights[a] if own else there
        return remote(src, there, c_send.at[zz, yy, a], c_recv.at[zz, yy, a], c_peer)

    def c_came(a, zz, yy):
        there = slot(a, zz, yy, 1 - c)
        return remote(there, there, c_send.at[zz, yy, a], c_recv.at[zz, yy, a], c_peer)

    def from_line(i, arrays):
        zz = order(i)
        for a in arrays:
            there = slot(a, zz, y, c)
            remote(there, there, line_send.at[zz, 0, a], line_recv.at[zz, a], c_peer).wait_recv()

            @pl.when((zz < z) & (z < planes - 1))
            def _():
                line(a, zz, True, False).start()

            @pl.when((zz > z) & (z > 0))
            def _():
                line(a, zz, False, False).start()

            y_copy(a, i, False).start()
            c_copy(a, zz, y, False).start()

    def from_pair(i, arrays):
        zz = order(i)
        for a in arrays:
            y_came(a, i).wait_recv()
            if i == 0:
                turn(a).start()
            if i == 1:
                turn_came(a).wait_recv()
            c_copy(a, zz, 1 - y, False).start()

    def multiply(i, yy, arrays):
        zz = order(i)
        for a in arrays:
            c_came(a, zz, yy).wait_recv()
        piece = zz * 2 + yy
        start = pl.multiple_of(piece * 2 * w_rows, 2 * w_rows)
        for a in arrays:
            part = jnp.dot(
                pieces[piece], full[a, pl.ds(start, 2 * w_rows), :], preferred_element_type=jnp.float32
            )
            product[a] += part

    def own_weights(arrays):
        for a in arrays:

            @pl.when(z < planes - 1)
            def _():
                line(a, z, True, True).start()

            @pl.when(z > 0)
            def _():
                line(a, z, False, True).start()

            y_copy(a, 0, True).start()
            c_copy(a, z, y, True).start()
            full[a, pl.ds(pl.multiple_of(sp * w_rows, w_rows), w_rows), :] = weights[a][...]

    swaps = (
        remote(tok_ref, theirs, swap_sem.at[0], swap_sem.at[1], x_peer),
        remote(gain_in, their_gain, swap_sem.at[2], swap_sem.at[3], x_peer),
    )
    own_weights(first_pair)
    for swap in swaps:
        swap.start()
    w_swap(z, y, True).start()
    w_beside(tp, z, y, True).start()
    product[...] = jnp.zeros_like(product)
    acc[...] = jnp.zeros_like(acc)
    total[...] = jnp.zeros_like(total)
    top[...] = jnp.full_like(top, NEG_LARGE)
    own_pool = pl.ds(pl.multiple_of(sp * pool_rows, pool_rows), pool_rows)
    w_pool[own_pool, :] = wp_ref[...]
    w_full[
        pl.ds(pl.multiple_of(tp * out_rows, out_rows), out_rows),
        pl.ds(pl.multiple_of(sp * out_columns, out_columns), out_columns),
    ] = wo_ref[...]

    from_line(1, first_pair)
    from_pair(0, first_pair)
    from_line(2, first_pair)
    for swap in swaps:
        swap.wait()
    squares = jnp.zeros((rows, 1), jnp.float32)
    per_half = half_width // (2 * w_rows)
    for ref, gains, owner in ((tok_ref, gain_in, tp), (theirs, their_gain, 1 - tp)):
        for j in range(per_half):
            chunk = pl.ds(j * 2 * w_rows, 2 * w_rows)
            features = ref[:, chunk].astype(jnp.float32)
            squares += jnp.sum(features * features, axis=1, keepdims=True)
            scaled = (features * gains[:, chunk].astype(jnp.float32)).astype(jnp.bfloat16)
            pieces[owner * per_half + j] = scaled
    inverse = lax.rsqrt(squares / model_width + EPSILON)
    inverse_sc[...] = jnp.broadcast_to(inverse, inverse_sc.shape)
    multiply(0, y, first_pair)
    multiply(0, 1 - y, first_pair)
    from_line(3, first_pair)
    own_weights(last_one)
    from_pair(1, first_pair)
    multiply(1, y, first_pair)
    from_pair(2, first_pair)
    multiply(1, 1 - y, first_pair)
    multiply(2, y, first_pair)
    from_line(1, last_one)
    from_pair(0, last_one)
    multiply(2, 1 - y, first_pair)
    from_pair(3, first_pair)
    multiply(3, y, first_pair)
    multiply(3, 1 - y, first_pair)
    width = columns // planes
    for p in range(planes):
        part = slice(p * width, (p + 1) * width)
        k_src[p] = (product[0, :, part] * inverse_sc[:, :1]).astype(jnp.bfloat16)
        v_src[p] = (product[1, :, part] * inverse_sc[:, :1]).T.astype(jnp.bfloat16)
    k_all[z, m] = k_src[z]
    v_all[z, m] = v_src[z]
    share(z, True)
    k_out(order(1)).start()
    v_out(order(1)).start()
    from_line(2, last_one)
    k_out(order(2)).start()
    v_out(order(2)).start()
    from_pair(1, last_one)
    multiply(0, y, last_one)
    multiply(0, 1 - y, last_one)
    from_line(3, last_one)
    k_out(order(3)).start()
    v_out(order(3)).start()
    from_pair(2, last_one)
    hand_on(z, True)
    multiply(1, y, last_one)
    multiply(1, 1 - y, last_one)
    multiply(2, y, last_one)
    multiply(2, 1 - y, last_one)
    from_pair(3, last_one)
    multiply(3, y, last_one)
    multiply(3, 1 - y, last_one)
    for p in range(planes):
        part = slice(p * width, (p + 1) * width)
        query = (product[2, :, part] * inverse_sc[:, :1]).astype(jnp.bfloat16)
        q_src[p] = query * (1.0 / math.sqrt(hdim))

    @pl.when(z % 2 == 0)
    def _():
        q_in[z] = q_src[z]

    @pl.when(z % 2 == 1)
    def _():
        q_out(z).start()

    for i in range(1, planes):
        q_out(order(i)).start()
    w_across(z, True).start()
    w_line_start()
    pool_start()

    def visit(block, plane, first, count, masked):
        query = q_in[block]
        lane = lax.broadcasted_iota(jnp.int32, query.shape, 1)
        none = jnp.zeros_like(query)
        both = jnp.concatenate(
            [jnp.where(lane < hdim, query, none), jnp.where(lane < hdim, none, query)], axis=0
        )
        keys = k_all[plane, pl.ds(first, count)].reshape(count * rows, 2 * hdim)
        values = jnp.concatenate([v_all[plane, first + i] for i in range(count)], axis=1)
        scores = lax.dot_general(
            keys, both, (((1,), (1,)), ((), ())), preferred_element_type=jnp.float32
        )
        if masked:
            shift = (first - holder(block, m)) * rows
            key = lax.broadcasted_iota(jnp.int32, scores.shape, 0)
            col = lax.broadcasted_iota(jnp.int32, scores.shape, 1)
            col = jnp.where(col < rows, col, col - rows)
            scores = jnp.where(key + shift <= col, scores, NEG_LARGE)
        old = top[block]
        new = jnp.maximum(old, jnp.max(scores, axis=0, keepdims=True))
        factor = jnp.exp(old - new)
        expo = jnp.exp(scores - new)
        acc[block] = acc[block] * factor + jnp.dot(
            values, expo.astype(jnp.bfloat16), preferred_element_type=jnp.float32
        )
        partial = jnp.sum(expo.reshape(count * rows // 8, 8, 2 * rows), axis=0)
        total[block] = total[block] * factor + partial
        top[block] = new

    def diagonal(block):
        pair = holder(block, m) // 2

        @pl.when(pair > 0)
        def _():
            visit(block, block, 0, members // 2, False)

        visit(block, block, pair * (members // 2), members // 2, True)

    def result_copy(block, half):
        return remote(
            done.at[block, pl.ds(pl.multiple_of(half * half_rows, half_rows), half_rows)],
            branch.at[tp * planes + z, :, pl.ds(0, vdim)],
            back_send.at[block, half],
            back_recv.at[tp * planes + z],
            at(block, holder(block, m), half),
        )

    def at_home(block):
        return (block == z) & (z % 2 == 0)

    def finish(block):
        both = acc[block] / jnp.sum(total[block], axis=0, keepdims=True)
        mixed = both[:, :rows] - lam_ref[z] * both[:, rows:]
        mean_sq = jnp.mean(mixed * mixed, axis=0, keepdims=True)
        normed = (mixed * lax.rsqrt(mean_sq + EPSILON)).T * gain_ref[...]
        done[block] = normed.astype(jnp.bfloat16)

        @pl.when(at_home(block))
        def _():
            kept = pl.ds(pl.multiple_of(tp * half_rows, half_rows), half_rows)
            branch[tp * planes + z, :, :vdim] = done[block, kept]

        @pl.when(jnp.logical_not(at_home(block)))
        def _():
            result_copy(block, tp).start()

        result_copy(block, 1 - tp).start()

    edge_rows = halo.shape[0]

    def edge_out():
        return remote(
            pool_sc.at[pl.ds(rows - edge_rows, edge_rows)], halo, edge_sem.at[0], edge_sem.at[1], {"sp": sp + 1}
        )

    def half_out():
        mine = pl.ds(pl.multiple_of(tp * groups, groups), groups)
        return remote(
            pooled_sc, branch.at[mine, :, pl.ds(vdim, vdim)], half_sem.at[0], half_sem.at[1], x_peer
        )

    def pool_project():
        for plane in range(planes):
            arrived(pool_slot(plane, c_member), pc_recv.at[plane, 0])
            arrived(pool_slot(plane, turned), pc_recv.at[plane, 1])
        scaled = jnp.concatenate([pieces[j] for j in range(pieces.shape[0])], axis=1)
        pool_in = jnp.dot(scaled, w_pool[...], preferred_element_type=jnp.float32)
        pool_sc[...] = (pool_in * inverse_sc[:, :1]).astype(jnp.bfloat16)

        @pl.when(sp < n_sp - 1)
        def _():
            edge_out().start()

        @pl.when(sp == 0)
        def _():
            halo[...] = jnp.zeros_like(halo)

    def pool_mix():
        @pl.when(sp > 0)
        def _():
            arrived(halo, edge_sem.at[1])

        for g in range(groups):
            part = slice(g * vdim, (g + 1) * vdim)
            own = pool_sc[:, part].astype(jnp.float32)
            running = jnp.concatenate([halo[:, part].astype(jnp.float32), own], axis=0)
            span = WINDOWS[g % len(WINDOWS)]
            step = 1
            while step < span:
                running = running + pltpu.roll(running, step, 0)
                step *= 2
            position = sp * rows + lax.broadcasted_iota(jnp.int32, own.shape, 0)
            count = jnp.minimum(position + 1, span).astype(jnp.float32)
            differ = (running[edge_rows:] / count - own).astype(jnp.bfloat16)
            pooled = jnp.dot(differ, group_ref[g], preferred_element_type=jnp.float32)
            pooled = (pooled * pscale_ref[:, part]).astype(jnp.bfloat16)
            low, high = pooled[:half_rows], pooled[half_rows:]
            branch[tp * groups + g, :, vdim:] = jnp.where(tp == 0, low, high)
            pooled_sc[g] = jnp.where(tp == 0, high, low)
        half_out().start()

    shared(z, True)

    @pl.when(z % 2 == 1)
    def _():
        arrived(q_in.at[z], z_recv.at[2, z])

    def stage(i, carry):
        block = order(i)

        @pl.when(i < planes - 1)
        def _():
            landed(i + 1)

        diagonal(block)

        @pl.when(i < planes - 1)
        def _():
            hand_on(order(i + 1), False)

        @pl.when(i == 0)
        def _():
            w_from_pair(0)

        @pl.when(i == 1)
        def _():
            pool_from_pair(0)

        @pl.when(i == planes - 1)
        def _():
            finish(0)

        def pair(j, carry):
            other = jnp.where(i < planes - 1, order(j), j + upper)
            visit(jnp.maximum(block, other), jnp.minimum(block, other), 0, members, False)

            @pl.when((i == planes - 2) & (j == i - 1))
            def _():
                w_from_line(1)
                pool_from_line(1)

            @pl.when(i == planes - 1)
            def _():
                finish(j + 1)

                @pl.when(j == 0)
                def _():
                    w_from_pair(1)
                    w_from_line(2)
                    pool_from_line(2)

                @pl.when(j == 1)
                def _():
                    w_from_pair(2)
                    w_from_line(3)
                    pool_from_line(3)

            return carry

        lax.fori_loop(0, i, pair, 0)

        @pl.when(i < planes - 1)
        def _():
            arrived(q_in.at[order(i + 1)], z_recv.at[2, order(i + 1)])
            shared(order(i + 1), False)

        return carry

    lax.fori_loop(0, planes, stage, 0)
    w_from_swap(0)
    pool_from_pair(1)
    pool_from_pair(2)
    w_from_pair(3)
    pool_from_pair(3)
    pool_project()
    w_from_swap(1)
    pool_mix()
    w_from_swap(2)
    w_from_swap(3)

    for head in range(2 * planes):
        own_head = tp * planes + z == head

        @pl.when(jnp.logical_not(own_head & at_home(z)))
        def _():
            arrived(branch.at[head, :, pl.ds(0, vdim)], back_recv.at[head])

    theirs = pl.ds(pl.multiple_of((1 - tp) * groups, groups), groups)
    arrived(branch.at[theirs, :, pl.ds(vdim, vdim)], half_sem.at[1])
    for half in range(2):
        for plane in range(planes):
            for yy in range(2):
                arrived(out_slot(half, plane, yy, 1 - c), wc_recv.at[half, plane, yy])
    left = jnp.concatenate([branch[head] for head in range(2 * planes)], axis=1)
    out_width = out_ref.shape[1] // planes

    def column(n, carry):
        part = pl.ds(pl.multiple_of(n * out_width, out_width), out_width)
        out_ref[:, part] = jnp.dot(
            left, w_full[:, part], preferred_element_type=jnp.float32
        ).astype(jnp.bfloat16)
        return carry

    lax.fori_loop(0, planes, column, 0)

    for i in range(1, planes):
        k_out(order(i)).wait_send()
        v_out(order(i)).wait_send()
        q_out(order(i)).wait_send()

    @pl.when(z % 2 == 1)
    def _():
        q_out(z).wait_send()

    for i in range(planes):
        plane = order(i)
        for copies in in_plane(plane, i == 0):
            for copy in copies:
                copy.wait_send()
        w_across(plane, False).wait_send()
        for a in first_pair + last_one:
            y_copy(a, i, False).wait_send()
            c_copy(a, plane, y, False).wait_send()
            c_copy(a, plane, 1 - y, False).wait_send()
            if i == 0:
                turn(a).wait_send()
        for yy in (y, 1 - y):
            w_swap(plane, yy, False).wait_send()
            w_beside(0, plane, yy, False).wait_send()
            w_beside(1, plane, yy, False).wait_send()

        @pl.when((plane <= z) & (z < planes - 1))
        def _():
            w_line(plane, True, False).wait_send()
            pool_line(plane, True, False).wait_send()
            for a in first_pair + last_one:
                line(a, plane, True, False).wait_send()

        @pl.when((plane >= z) & (z > 0))
        def _():
            w_line(plane, False, False).wait_send()
            pool_line(plane, False, False).wait_send()
            for a in first_pair + last_one:
                line(a, plane, False, False).wait_send()

    for plane in range(planes):
        pool_across(plane, False).wait_send()
        pool_beside(plane, False).wait_send()
        pool_onward(plane).wait_send()
        result_copy(plane, 1 - tp).wait_send()

        @pl.when(jnp.logical_not(at_home(plane)))
        def _():
            result_copy(plane, tp).wait_send()

    half_out().wait_send()

    @pl.when(sp < n_sp - 1)
    def _():
        edge_out().wait_send()


def whole_layer(
    tokens,
    pre_gain,
    w_query,
    w_key,
    w_value,
    w_pool,
    lambdas,
    sub_gain,
    group_weight,
    pool_scale,
    w_out,
):
    planes = lambdas.shape[0]
    rows, half_width = tokens.shape
    n_sp = lax.axis_size("sp")
    members = n_sp // planes
    w_rows, columns = w_query.shape
    model_width = n_sp * w_rows
    width = columns // planes
    groups, vdim, _ = group_weight.shape
    out_rows, out_columns = w_out.shape
    vmem = pl.BlockSpec(memory_space=pltpu.VMEM)
    dma = pltpu.SemaphoreType.DMA
    bf16, f32 = jnp.bfloat16, jnp.float32
    work = planes * rows * members * planes * rows
    return pl.pallas_call(
        functools.partial(layer, width // 2, model_width),
        out_shape=jax.ShapeDtypeStruct((rows // 2, n_sp * out_columns), bf16),
        in_specs=[pl.BlockSpec(memory_space=pltpu.SMEM)] + [vmem] * 10,
        out_specs=vmem,
        scratch_shapes=[
            pltpu.VMEM((3, model_width, columns), bf16),
            pltpu.VMEM((rows, half_width), bf16),
            pltpu.VMEM((1, half_width), bf16),
            pltpu.VMEM((model_width // (2 * w_rows), rows, 2 * w_rows), bf16),
            pltpu.VMEM((3, rows, columns), f32),
            pltpu.VMEM((rows, 128), f32),
            pltpu.VMEM((planes, rows, width), bf16),
            pltpu.VMEM((planes, vdim, rows), bf16),
            pltpu.VMEM((planes, rows, width), bf16),
            pltpu.VMEM((planes, rows, width), bf16),
            pltpu.VMEM((planes, members, rows, width), bf16),
            pltpu.VMEM((planes, members, vdim, rows), bf16),
            pltpu.VMEM((planes, vdim, 2 * rows), f32),
            pltpu.VMEM((planes, 1, 2 * rows), f32),
            pltpu.VMEM((planes, 8, 2 * rows), f32),
            pltpu.VMEM((planes, rows, vdim), bf16),
            pltpu.VMEM((model_width, groups * vdim), bf16),
            pltpu.VMEM((2 * out_rows, n_sp * out_columns), bf16),
            pltpu.VMEM((2 * planes, rows // 2, 2 * vdim), bf16),
            pltpu.VMEM((rows, groups * vdim), bf16),
            pltpu.VMEM((RIM_ROWS + 1, groups * vdim), bf16),
            pltpu.VMEM((groups, rows // 2, vdim), bf16),
            dma((planes, 2, 3)),
            dma((planes, 3)),
            dma((planes, 3)),
            dma((planes, 3)),
            dma((planes, 2, 3)),
            dma((planes, 2, 3)),
            dma((3,)),
            dma((3,)),
            dma((4,)),
            dma((3, planes)),
            dma((3, planes)),
            dma((planes, 3, 2)),
            dma((planes, 3, 2)),
            dma((planes, 2)),
            dma((2 * planes,)),
            dma((planes,)),
            dma((planes,)),
            dma((planes, 2)),
            dma((planes, 2)),
            dma((2,)),
            dma((2,)),
            dma((planes, 2)),
            dma((planes,)),
            dma((planes, 2)),
            dma((planes,)),
            dma((planes,)),
            dma((planes,)),
            dma((planes, 2)),
            dma((planes, 2)),
            dma((2, planes, 2)),
            dma((2, planes, 2)),
        ],
        compiler_params=pltpu.CompilerParams(
            vmem_limit_bytes=60 * 2**20, collective_id=2, has_side_effects=True
        ),
        cost_estimate=pl.CostEstimate(
            flops=4 * work * vdim, bytes_accessed=2**24, transcendentals=work
        ),
    )(
        lambdas,
        tokens,
        pre_gain.reshape(1, -1),
        w_key,
        w_value,
        w_query,
        w_pool,
        sub_gain.reshape(1, -1),
        group_weight,
        pool_scale.reshape(1, -1),
        w_out,
    )


def trailing(x, window_ids, group_dim):
    column_window = jnp.repeat(window_ids, group_dim)[None, :]
    running = x
    picked = jnp.zeros_like(x)
    for slot, span in enumerate(WINDOWS):
        half = span // 2
        running = running + jnp.pad(running[:-half], ((half, 0), (0, 0)))
        picked = jnp.where(column_window == slot, running, picked)
    return picked


def general_attention(queries, key_rows, values, lambdas, sub_gain):
    n_sp = lax.axis_size("sp")
    sp = lax.axis_index("sp")
    tok_rows = queries.shape[0]
    heads = lambdas.shape[0]
    qdim = queries.shape[1] // heads
    vdim = values.shape[1] // heads
    head_width = 2 * qdim + vdim
    outer = math.gcd(n_sp, heads)
    inner = n_sp // outer
    per_device = heads // outer
    by_head = jnp.concatenate(
        [
            x.reshape(tok_rows, heads, -1).swapaxes(0, 1)
            for x in (queries, key_rows, values)
        ],
        axis=2,
    )
    across = [[o * inner + i for o in range(outer)] for i in range(inner)]
    within = [[o * inner + i for i in range(inner)] for o in range(outer)]
    by_head = by_head.reshape(outer, per_device, tok_rows, head_width)
    if outer > 1:
        by_head = lax.all_to_all(by_head, "sp", 0, 0, axis_index_groups=across)
    first_head = lax.div(sp, inner) * per_device
    attended = []
    if inner == 4 and per_device == 1:
        lam = lax.dynamic_slice_in_dim(lambdas, first_head, 1)
        attended.append(
            flash_members(by_head[:, 0, :, :qdim], by_head[:, 0, :, qdim:], lam, sub_gain)
        )
    else:
        kv = lax.all_gather(by_head[..., qdim:], "sp", axis=0, axis_index_groups=within)
        member = lax.rem(sp, inner).reshape(1)
        for p in range(per_device):
            lam = lax.dynamic_slice_in_dim(lambdas, first_head + p, 1)
            attended.append(flash(by_head[:, p, :, :qdim], kv[:, :, p], member, lam, sub_gain))
    attended = jnp.stack(attended, axis=1)
    if outer > 1:
        attended = lax.all_to_all(attended, "sp", 0, 0, axis_index_groups=across)
    return attended.reshape(heads, tok_rows, vdim)


def local(
    tokens,
    pre_gain,
    w_query,
    w_key,
    w_value,
    w_pool,
    lambdas,
    sub_gain,
    group_weight,
    pool_scale,
    w_out,
):
    n_tp = lax.axis_size("tp")
    n_sp = lax.axis_size("sp")
    tp = lax.axis_index("tp")
    sp = lax.axis_index("sp")
    tok_rows = tokens.shape[0]
    model_width = tokens.shape[1] * n_tp
    heads = lambdas.shape[0]
    qdim = w_query.shape[1] // heads
    vdim = w_value.shape[1] // heads
    groups = group_weight.shape[0]
    group_dim = group_weight.shape[1]

    shaped_for_mix = n_tp == 2 and heads == 4 and n_sp == 4 * heads and tok_rows % 32 == 0
    if shaped_for_mix and qdim == vdim == group_dim and groups == heads:
        return whole_layer(
            tokens,
            pre_gain,
            w_query,
            w_key,
            w_value,
            w_pool,
            lambdas,
            sub_gain,
            group_weight,
            pool_scale,
            w_out,
        )
    swap = [(0, 1), (1, 0)]
    w_sorted = w_out.reshape(heads, 2, vdim, -1).swapaxes(0, 1).reshape(w_out.shape)
    features = tokens.astype(jnp.float32)
    mine = (features * pre_gain.astype(jnp.float32)[None, :]).astype(jnp.bfloat16)
    squares = jnp.sum(features * features, axis=1, keepdims=True)
    weights = [w_query, w_key, w_value, w_pool]
    if n_sp % 4 == 0:
        *weights, theirs = gather_weights(weights, mine, n_tp == 2)
    else:
        weights = [lax.all_gather(w, "sp", axis=0, tiled=True) for w in weights]
        theirs = lax.ppermute(mine, "tp", swap) if n_tp == 2 else mine
    w_sorted, weights = lax.optimization_barrier((w_sorted, weights))
    w_out_rows = lax.all_gather(w_sorted, "sp", axis=1, tiled=True)
    if n_tp == 2:
        squares = squares + lax.ppermute(squares, "tp", swap)
        scaled = jnp.concatenate(
            [jnp.where(tp == 0, mine, theirs), jnp.where(tp == 0, theirs, mine)], axis=1
        )
    else:
        scaled = lax.all_gather(mine, "tp", axis=1, tiled=True)
        squares = lax.psum(squares, "tp")
    inverse = lax.rsqrt(squares / model_width + EPSILON)
    queries, key_rows, values, pool_in = [
        (jnp.dot(scaled, w, preferred_element_type=jnp.float32) * inverse).astype(jnp.bfloat16)
        for w in weights
    ]
    attended = general_attention(queries, key_rows, values, lambdas, sub_gain)

    halo = passed_along(pool_in[tok_rows - RIM_ROWS - 1 :], "sp", 1)
    extended = jnp.concatenate([halo, pool_in], axis=0).astype(jnp.float32)
    window_ids = (tp * groups + jnp.arange(groups, dtype=jnp.int32)) % len(WINDOWS)
    sums = trailing(extended, window_ids, group_dim)[RIM_ROWS + 1 :]
    spans = jnp.repeat(jnp.left_shift(2, window_ids), group_dim)
    positions = sp * tok_rows + jnp.arange(tok_rows, dtype=jnp.int32)
    count = jnp.minimum(positions[:, None] + 1, spans[None, :]).astype(jnp.float32)
    differ = (sums / count - pool_in.astype(jnp.float32)).astype(jnp.bfloat16)
    pooled = jnp.einsum(
        "tgc,gcd->tgd",
        differ.reshape(tok_rows, groups, group_dim),
        group_weight,
        preferred_element_type=jnp.float32,
    )
    pooled = (pooled * pool_scale.reshape(groups, group_dim)).astype(jnp.bfloat16)
    branch = jnp.concatenate(
        [attended.swapaxes(0, 1).reshape(tok_rows, -1), pooled.reshape(tok_rows, -1)], axis=1
    )
    if n_tp == 2:
        half = tok_rows // 2
        send = lax.dynamic_slice_in_dim(branch, (1 - tp) * half, half, 0)
        send = jnp.dot(send, w_out_rows, preferred_element_type=jnp.float32).astype(jnp.bfloat16)
        got = lax.ppermute(send, "tp", swap)
        keep = lax.dynamic_slice_in_dim(branch, tp * half, half, 0)
        keep = jnp.dot(keep, w_out_rows, preferred_element_type=jnp.float32)
        return (keep + got.astype(jnp.float32)).astype(jnp.bfloat16)
    partial = jnp.dot(branch, w_out_rows, preferred_element_type=jnp.float32)
    return lax.psum_scatter(partial.astype(jnp.bfloat16), "tp", scatter_dimension=0, tiled=True)


def solution(mesh):
    placed = (
        P("sp", "tp"),
        P("tp"),
        P("sp", "tp"),
        P("sp", "tp"),
        P("sp", "tp"),
        P("sp", "tp"),
        P("tp"),
        P(),
        P("tp", None, None),
        P("tp"),
        P("tp", "sp"),
    )
    return jax.shard_map(
        local, mesh=mesh, in_specs=placed, out_specs=P(("sp", "tp"), None), check_vma=False
    )
```

```python
import functools
import math

import jax
import jax.numpy as jnp
from jax import lax
from jax.experimental import pallas as pl
from jax.experimental.pallas import tpu as pltpu
from jax.sharding import PartitionSpec as P

EPSILON = 1e-06
NEG_LARGE = -1e30
WINDOWS = (2, 4, 8, 16)
RIM_ROWS = 15


def passed_along(block, axis, distance):
    devices = range(lax.axis_size(axis))
    route = [(i - distance, i) for i in devices if i - distance in devices]
    return lax.ppermute(block, axis, route)


def attend(inner, vdim, hdim, member_ref, lam_ref, q_ref, kv_ref, gain_ref, out_ref, acc_ref, max_ref):
    rows = q_ref.shape[1]
    block = pl.program_id(0)
    last = block * inner + member_ref[0]
    scale = 1.0 / math.sqrt(hdim)
    queries = (q_ref[0].astype(jnp.float32) * scale).astype(jnp.bfloat16)
    maps = (queries[:, :hdim], queries[:, hdim:])
    ones = jnp.ones((rows, vdim), jnp.bfloat16)
    acc_ref[...] = jnp.zeros_like(acc_ref)
    max_ref[...] = jnp.full_like(max_ref, NEG_LARGE)

    def step(g, masked):
        keys_values = kv_ref[lax.rem(g, inner), lax.div(g, inner)]
        values = jnp.concatenate([keys_values[:, 2 * hdim :], ones], axis=1)
        for m in range(2):
            keys = keys_values[:, m * hdim : (m + 1) * hdim]
            scores = lax.dot_general(
                maps[m], keys, (((1,), (1,)), ((), ())), preferred_element_type=jnp.float32
            )
            if masked:
                row = lax.broadcasted_iota(jnp.int32, scores.shape, 0)
                col = lax.broadcasted_iota(jnp.int32, scores.shape, 1)
                scores = jnp.where(col <= row, scores, NEG_LARGE)
            old_max = max_ref[m]
            new_max = jnp.maximum(old_max, jnp.max(scores, axis=1, keepdims=True))
            factor = jnp.exp(old_max - new_max)
            expo = jnp.exp(scores - new_max[:, :1])
            acc_ref[m] = acc_ref[m] * factor[:, :1] + jnp.dot(
                expo.astype(jnp.bfloat16), values, preferred_element_type=jnp.float32
            )
            max_ref[m] = new_max

    def body(g, carry):
        step(g, False)
        return carry

    lax.fori_loop(0, last, body, 0)
    step(last, True)
    first = acc_ref[0]
    second = acc_ref[1]
    mix = first[:, :vdim] / first[:, vdim:] - lam_ref[0] * (second[:, :vdim] / second[:, vdim:])
    mean_sq = jnp.mean(mix * mix, axis=1, keepdims=True)
    out_ref[0] = (mix * lax.rsqrt(mean_sq + EPSILON) * gain_ref[...]).astype(jnp.bfloat16)


def flash(q, kv, member, lam, sub_gain):
    inner, outer, rows, width = kv.shape
    qdim = q.shape[-1]
    vdim = width - qdim
    smem = pl.BlockSpec(memory_space=pltpu.SMEM)
    work = outer * rows * outer * rows * inner
    return pl.pallas_call(
        functools.partial(attend, inner, vdim, qdim // 2),
        grid=(outer,),
        out_shape=jax.ShapeDtypeStruct((outer, rows, vdim), jnp.bfloat16),
        in_specs=[
            smem,
            smem,
            pl.BlockSpec((1, rows, qdim), lambda b: (b, 0, 0)),
            pl.BlockSpec(memory_space=pltpu.VMEM),
            pl.BlockSpec(memory_space=pltpu.VMEM),
        ],
        out_specs=pl.BlockSpec((1, rows, vdim), lambda b: (b, 0, 0)),
        scratch_shapes=[
            pltpu.VMEM((2, rows, 2 * vdim), jnp.float32),
            pltpu.VMEM((2, rows, 128), jnp.float32),
        ],
        compiler_params=pltpu.CompilerParams(vmem_limit_bytes=56 * 2**20),
        cost_estimate=pl.CostEstimate(
            flops=4 * work * vdim, bytes_accessed=kv.size * 2, transcendentals=work
        ),
    )(member, lam, q, kv, sub_gain.reshape(1, -1))


def attend_members(hdim, lam_ref, q_ref, own_ref, gain_ref, out_ref, held, acc_ref, max_ref, send, recv):
    outer, rows, _ = q_ref.shape
    vdim = own_ref.shape[2] - 2 * hdim
    sp = lax.axis_index("sp")
    member = lax.rem(sp, 4)
    y = lax.div(member, 2)
    c = lax.rem(member, 2)
    y_peer = sp + 2 - 4 * y
    c_peer = sp + 1 - 2 * c
    barrier = pltpu.get_barrier_semaphore()
    for peer in (y_peer, c_peer):
        pl.semaphore_signal(
            barrier, 1, device_id={"sp": peer}, device_id_type=pl.DeviceIdType.MESH
        )
    pl.semaphore_wait(barrier, 2)

    def remote(src, index, peer):
        return pltpu.make_async_remote_copy(
            src_ref=src,
            dst_ref=held.at[index],
            send_sem=send.at[index],
            recv_sem=recv.at[index],
            device_id={"sp": peer},
            device_id_type=pl.DeviceIdType.MESH,
        )

    across = remote(own_ref, 1, y_peer)
    beside = remote(own_ref, 0, c_peer)
    onward = remote(held.at[1], 2, c_peer)
    across.start()
    beside.start()
    acc_ref[...] = jnp.zeros_like(acc_ref)
    max_ref[...] = jnp.full_like(max_ref, NEG_LARGE)
    scale = 1.0 / math.sqrt(hdim)

    def visit(ref, other):
        shift = (member - other) * rows
        for block in range(outer):
            queries = (q_ref[block].astype(jnp.float32) * scale).astype(jnp.bfloat16)
            length = (block + 1) * rows
            keys_values = ref[: block + 1].reshape(length, 2 * hdim + vdim)
            values = jnp.concatenate(
                [keys_values[:, 2 * hdim :], jnp.ones((length, vdim), jnp.bfloat16)], axis=1
            )
            for m in range(2):
                scores = lax.dot_general(
                    queries[:, m * hdim : (m + 1) * hdim],
                    keys_values[:, m * hdim : (m + 1) * hdim],
                    (((1,), (1,)), ((), ())),
                    preferred_element_type=jnp.float32,
                )
                edge = scores[:, block * rows :]
                row = lax.broadcasted_iota(jnp.int32, edge.shape, 0)
                col = lax.broadcasted_iota(jnp.int32, edge.shape, 1)
                edge = jnp.where(col <= row + shift, edge, NEG_LARGE)
                if block > 0:
                    scores = jnp.concatenate([scores[:, : block * rows], edge], axis=1)
                else:
                    scores = edge
                old_max = max_ref[block, m]
                new_max = jnp.maximum(old_max, jnp.max(scores, axis=1, keepdims=True))
                factor = jnp.exp(old_max - new_max)
                expo = jnp.exp(scores - new_max[:, :1])
                acc_ref[block, m] = acc_ref[block, m] * factor[:, :1] + jnp.dot(
                    expo.astype(jnp.bfloat16), values, preferred_element_type=jnp.float32
                )
                max_ref[block, m] = new_max

    visit(own_ref, member)

    def arrived(j, carry):
        @pl.when(j == 0)
        def _():
            beside.wait_recv()

        @pl.when(j == 1)
        def _():
            across.wait_recv()
            onward.start()

        @pl.when(j == 2)
        def _():
            onward.wait_recv()

        other_y = jnp.where(j >= 1, 1 - y, y)
        other_c = jnp.where(j == 1, c, 1 - c)
        visit(held.at[j], 2 * other_y + other_c)
        return carry

    lax.fori_loop(0, 3, arrived, 0)
    for copy in (across, beside, onward):
        copy.wait_send()
    for block in range(outer):
        first = acc_ref[block, 0]
        second = acc_ref[block, 1]
        mix = first[:, :vdim] / first[:, vdim:]
        mix = mix - lam_ref[0] * (second[:, :vdim] / second[:, vdim:])
        mean_sq = jnp.mean(mix * mix, axis=1, keepdims=True)
        normed = mix * lax.rsqrt(mean_sq + EPSILON) * gain_ref[...]
        out_ref[block] = normed.astype(jnp.bfloat16)


def flash_members(q, kv, lam, sub_gain):
    outer, rows, width = kv.shape
    qdim = q.shape[-1]
    vdim = width - qdim
    vmem = pl.BlockSpec(memory_space=pltpu.VMEM)
    work = 4 * outer * rows * outer * rows
    return pl.pallas_call(
        functools.partial(attend_members, qdim // 2),
        out_shape=jax.ShapeDtypeStruct((outer, rows, vdim), jnp.bfloat16),
        in_specs=[pl.BlockSpec(memory_space=pltpu.SMEM), vmem, vmem, vmem],
        out_specs=vmem,
        scratch_shapes=[
            pltpu.VMEM((3, outer, rows, width), jnp.bfloat16),
            pltpu.VMEM((outer, 2, rows, 2 * vdim), jnp.float32),
            pltpu.VMEM((outer, 2, rows, 128), jnp.float32),
            pltpu.SemaphoreType.DMA((3,)),
            pltpu.SemaphoreType.DMA((3,)),
        ],
        compiler_params=pltpu.CompilerParams(
            vmem_limit_bytes=56 * 2**20, collective_id=1, has_side_effects=True
        ),
        cost_estimate=pl.CostEstimate(
            flops=4 * work * vdim, bytes_accessed=4 * kv.size * 2, transcendentals=work
        ),
    )(lam, q, kv, sub_gain.reshape(1, -1))


def spread(n_sp, count, with_swap, *refs):
    weights, refs = refs[:count], refs[count:]
    mine, refs = refs[0], refs[1:]
    fulls, refs = refs[:count], refs[count:]
    theirs, refs = refs[0], refs[1:]
    up_send, up_recv, down_send, down_recv, y_send, y_recv, c_send, c_recv, own_sem, swap_sem = refs
    depth = n_sp // 4
    rows = weights[0].shape[0]
    sp = lax.axis_index("sp")
    z = lax.div(sp, 4)
    y = lax.rem(lax.div(sp, 2), 2)
    c = lax.rem(sp, 2)
    y_peer = z * 4 + (1 - y) * 2 + c
    c_peer = z * 4 + y * 2 + (1 - c)
    barrier = pltpu.get_barrier_semaphore()

    def greet(device):
        pl.semaphore_signal(barrier, 1, device_id=device, device_id_type=pl.DeviceIdType.MESH)

    greet({"sp": y_peer})
    greet({"sp": c_peer})
    greeted = 2
    if with_swap:
        greet({"tp": 1 - lax.axis_index("tp")})
        greeted = 3

    @pl.when(z > 0)
    def _():
        greet({"sp": sp - 4})

    @pl.when(z < depth - 1)
    def _():
        greet({"sp": sp + 4})

    in_line = jnp.where(z > 0, 1, 0) + jnp.where(z < depth - 1, 1, 0)
    pl.semaphore_wait(barrier, greeted + in_line)

    def slot(a, zz, yy, cc):
        start = pl.multiple_of((zz * 4 + yy * 2 + cc) * rows, rows)
        return fulls[a].at[pl.ds(start, rows), :]

    def remote(src, dst, send, recv, device):
        return pltpu.make_async_remote_copy(
            src_ref=src,
            dst_ref=dst,
            send_sem=send,
            recv_sem=recv,
            device_id=device,
            device_id_type=pl.DeviceIdType.MESH,
        )

    def line_copy(side, k, a, src):
        sends, recvs = (up_send, up_recv) if side > 0 else (down_send, down_recv)
        there = slot(a, z - side * k, y, c)
        return remote(
            there if src is None else src,
            there,
            sends.at[k, a],
            recvs.at[k + 1, a],
            {"sp": sp + 4 * side},
        )

    def y_copy(zz, yy, a, src):
        there = slot(a, zz, yy, c)
        src = there if src is None else src
        return remote(src, there, y_send.at[zz, a], y_recv.at[zz, a], {"sp": y_peer})

    def c_copy(zz, yy, cc, a, src):
        there = slot(a, zz, yy, cc)
        src = there if src is None else src
        return remote(src, there, c_send.at[zz, yy, a], c_recv.at[zz, yy, a], {"sp": c_peer})

    def can_go(side):
        return z < depth - 1 if side > 0 else z > 0

    def came(side, k):
        return z >= k if side > 0 else z + k <= depth - 1

    if with_swap:
        swap = remote(
            mine, theirs, swap_sem.at[0], swap_sem.at[1], {"tp": 1 - lax.axis_index("tp")}
        )
        swap.start()
    for a in range(count):
        for side in (1, -1):

            @pl.when(can_go(side))
            def _():
                line_copy(side, 0, a, weights[a]).start()

        y_copy(z, y, a, weights[a]).start()
    for a in range(count):
        c_copy(z, y, c, a, weights[a]).start()
        pltpu.make_async_copy(weights[a], slot(a, z, y, c), own_sem.at[a]).start()

    def from_pair(zz):
        for a in range(count):
            y_copy(zz, 1 - y, a, None).wait_recv()
            c_copy(zz, 1 - y, c, a, None).start()

    def relay(k, carry):
        for side in (1, -1):
            recvs = up_recv if side > 0 else down_recv

            @pl.when(came(side, k))
            def _():
                zz = z - side * k
                for a in range(count):
                    there = slot(a, zz, y, c)
                    remote(there, there, up_send.at[0, a], recvs.at[k, a], {"sp": y_peer}).wait_recv()

                    @pl.when(can_go(side))
                    def _():
                        line_copy(side, k, a, None).start()

                    y_copy(zz, y, a, None).start()
                    c_copy(zz, y, c, a, None).start()

        @pl.when(k == 1)
        def _():
            from_pair(z)

        for side in (1, -1):

            @pl.when((k > 1) & came(side, k - 1))
            def _():
                from_pair(z - side * (k - 1))

        return carry

    lax.fori_loop(1, depth, relay, 0)
    if depth == 1:
        from_pair(z)
    for side in (1, -1):
        if depth > 1:

            @pl.when(came(side, depth - 1))
            def _():
                from_pair(z - side * (depth - 1))

    def drain(zz, carry):
        for a in range(count):
            y_copy(zz, y, a, None).wait_send()
            for yy in range(2):
                c_copy(zz, yy, 1 - c, a, None).wait_recv()
                c_copy(zz, yy, c, a, None).wait_send()
        return carry

    lax.fori_loop(0, depth, drain, 0)

    def drain_line(k, carry):
        for side in (1, -1):

            @pl.when(came(side, k) & can_go(side))
            def _():
                for a in range(count):
                    line_copy(side, k, a, None).wait_send()

        return carry

    lax.fori_loop(0, depth, drain_line, 0)
    for a in range(count):
        pltpu.make_async_copy(weights[a], slot(a, z, y, c), own_sem.at[a]).wait()
    if with_swap:
        swap.wait()


def gather_weights(weights, mine, with_swap):
    n_sp = lax.axis_size("sp")
    count = len(weights)
    depth = n_sp // 4
    sems = pltpu.SemaphoreType.DMA
    any_spec = pl.BlockSpec(memory_space=pl.ANY)
    vmem_spec = pl.BlockSpec(memory_space=pltpu.VMEM)
    shapes = [jax.ShapeDtypeStruct((n_sp * w.shape[0], w.shape[1]), w.dtype) for w in weights]
    shapes.append(jax.ShapeDtypeStruct(mine.shape, mine.dtype))
    moved = sum(w.size for w in weights) * 2 * n_sp
    return pl.pallas_call(
        functools.partial(spread, n_sp, count, with_swap),
        out_shape=shapes,
        in_specs=[vmem_spec] * (count + 1),
        out_specs=[any_spec] * (count + 1),
        scratch_shapes=[
            sems((depth + 1, count)),
            sems((depth + 1, count)),
            sems((depth + 1, count)),
            sems((depth + 1, count)),
            sems((depth, count)),
            sems((depth, count)),
            sems((depth, 2, count)),
            sems((depth, 2, count)),
            sems((count,)),
            sems((2,)),
        ],
        compiler_params=pltpu.CompilerParams(collective_id=0, has_side_effects=True),
        cost_estimate=pl.CostEstimate(flops=10**10, bytes_accessed=moved, transcendentals=0),
    )(*weights, mine)


def arrival(z, i):
    half = z // 2
    later = jnp.where(i == 2, 2 - half, 3 - 3 * half)
    return jnp.where(i == 0, z, jnp.where(i == 1, 1 + 4 * half - z, later))


def layer(
    hdim,
    model_width,
    lam_ref,
    tok_ref,
    gain_in,
    wk_ref,
    wv_ref,
    wq_ref,
    wp_ref,
    gain_ref,
    group_ref,
    pscale_ref,
    wo_ref,
    out_ref,
    full,
    theirs,
    their_gain,
    pieces,
    product,
    inverse_sc,
    k_src,
    v_src,
    q_src,
    q_in,
    k_all,
    v_all,
    acc,
    top,
    total,
    done,
    w_pool,
    w_full,
    branch,
    pool_sc,
    halo,
    pooled_sc,
    *sems,
):
    (line_send, line_recv, y_send, y_recv, c_send, c_recv, swap_sem) = sems[:7]
    (z_send, z_recv, in_send, in_recv, back_send, back_recv) = sems[7:13]
    (py_send, py_recv, pc_send, pc_recv, edge_sem, half_sem, pool_send, pool_recv) = sems[13:21]
    (wl_send, wl_recv, wy_send, wy_recv, wx_send, wx_recv, wc_send, wc_recv) = sems[21:]
    weights = (wk_ref, wv_ref, wq_ref)
    first_pair, last_one = (0, 1), (2,)
    planes, rows, _ = q_src.shape
    vdim = v_src.shape[1]
    members = k_all.shape[1]
    w_rows, columns = wq_ref.shape
    half_width = tok_ref.shape[1]
    groups = group_ref.shape[0]
    half_rows = rows // 2
    sp = lax.axis_index("sp")
    tp = lax.axis_index("tp")
    n_sp = lax.axis_size("sp")
    z = sp // members
    m = sp % members
    y = m // 2
    c = m % 2
    y_member = (m + 2) % members
    c_member = m + 1 - 2 * c
    turned = members - 1 - m
    upper = z // 2
    between = (z > 0) & (z < planes - 1)
    turn = [jnp.where(between, 1 + i % 3, i) for i in range(planes)]
    turn[0] = 0

    def at(plane, member, half=None):
        device = {"sp": plane * members + member}
        if half is not None:
            device["tp"] = half
        return device

    y_peer = at(z, y_member)
    c_peer = at(z, c_member)
    x_peer = {"tp": 1 - tp}

    def holder(block, member):
        return member + (block % 2) * (members - 1 - 2 * member)

    def order(i):
        return arrival(z, i)

    barrier = pltpu.get_barrier_semaphore()

    def greet(device):
        pl.semaphore_signal(barrier, 1, device_id=device, device_id_type=pl.DeviceIdType.MESH)

    for i in range(1, planes):
        greet(at(order(i), m))
        greet(at(order(i), turned))
    for member in (turned, y_member, c_member):
        greet(at(z, member))
    for plane in range(planes):
        greet(at(plane, m, 1 - tp))
        greet(at(plane, turned, 1 - tp))
    pl.semaphore_wait(barrier, 4 * planes + 1)

    def remote(src, dst, send, recv, device):
        return pltpu.make_async_remote_copy(
            src_ref=src,
            dst_ref=dst,
            send_sem=send,
            recv_sem=recv,
            device_id=device,
            device_id_type=pl.DeviceIdType.MESH,
        )

    def arrived(ref, recv):
        remote(ref, ref, recv, recv, c_peer).wait_recv()

    def k_out(plane):
        return remote(k_src.at[plane], k_all.at[z, m], z_send.at[0, plane], z_recv.at[0, z], at(plane, m))

    def v_out(plane):
        return remote(v_src.at[plane], v_all.at[z, m], z_send.at[1, plane], z_recv.at[1, z], at(plane, m))

    def q_out(plane):
        return remote(
            q_src.at[plane], q_in.at[z], z_send.at[2, plane], z_recv.at[2, z], at(plane, holder(z, m))
        )

    def in_plane(plane, own):
        copies = []
        for t, (mine, everyone) in enumerate(((k_src, k_all), (v_src, v_all))):
            src = mine.at[plane] if own else everyone.at[plane, m]
            there = everyone.at[plane, m]
            passed = everyone.at[plane, y_member]
            copies.append(
                [
                    remote(src, there, in_send.at[plane, 0, t], in_recv.at[plane, 0, t], y_peer),
                    remote(src, there, in_send.at[plane, 1, t], in_recv.at[plane, 1, t], c_peer),
                    remote(passed, passed, in_send.at[plane, 2, t], in_recv.at[plane, 2, t], c_peer),
                ]
            )
        return copies

    def share(plane, own):
        for copies in in_plane(plane, own):
            copies[0].start()
            copies[1].start()

    def hand_on(plane, own):
        for copies in in_plane(plane, own):
            copies[0].wait_recv()
            copies[2].start()

    def shared(plane, own):
        for copies in in_plane(plane, own):
            copies[1].wait_recv()
            copies[2].wait_recv()

    def landed(i):
        plane = order(i)
        arrived(k_all.at[plane, m], z_recv.at[0, plane])
        arrived(v_all.at[plane, m], z_recv.at[1, plane])
        share(plane, False)

    pool_rows = wp_ref.shape[0]

    def pool_slot(plane, member):
        start = pl.multiple_of((plane * members + member) * pool_rows, pool_rows)
        return w_pool.at[pl.ds(start, pool_rows), :]

    def pool_line(i):
        return remote(wp_ref, pool_slot(z, m), pool_send.at[i - 1], pool_recv.at[z], at(order(i), m))

    def pool_line_on(i):
        there = pool_slot(order(i), m)
        return remote(there, there, pool_send.at[i], pool_recv.at[order(i)], at(order(1), m))

    def pool_across(plane, own):
        there = pool_slot(plane, m)
        return remote(wp_ref if own else there, there, py_send.at[plane], py_recv.at[plane], y_peer)

    def pool_beside(plane, own):
        there = pool_slot(plane, m)
        return remote(wp_ref if own else there, there, pc_send.at[plane, 0], pc_recv.at[plane, 0], c_peer)

    def pool_onward(plane):
        passed = pool_slot(plane, y_member)
        return remote(passed, passed, pc_send.at[plane, 1], pc_recv.at[plane, 1], c_peer)

    def pool_start():
        pool_line(1).start()
        pool_line(2).start()

    def pool_from_line(i):
        plane = order(i)
        arrived(pool_slot(plane, m), pool_recv.at[plane])
        if i > 1:

            @pl.when(between)
            def _():
                pool_line_on(i).start()

        pool_across(plane, False).start()
        pool_beside(plane, False).start()

    def pool_from_pair(i):
        arrived(pool_slot(order(i), y_member), py_recv.at[order(i)])
        pool_onward(order(i)).start()

    out_rows, out_columns = wo_ref.shape

    def out_slot(half, plane, yy, cc):
        first = pl.multiple_of(half * out_rows, out_rows)
        column = pl.multiple_of((plane * members + yy * 2 + cc) * out_columns, out_columns)
        return w_full.at[pl.ds(first, out_rows), pl.ds(column, out_columns)]

    def w_line(i):
        return remote(wo_ref, out_slot(tp, z, y, c), wl_send.at[i - 1], wl_recv.at[z], at(order(i), m))

    def w_line_on(i):
        there = out_slot(tp, order(i), y, c)
        return remote(there, there, wl_send.at[i], wl_recv.at[order(i)], at(order(1), m))

    def w_across(plane, own):
        there = out_slot(tp, plane, y, c)
        return remote(wo_ref if own else there, there, wy_send.at[plane], wy_recv.at[plane], y_peer)

    def w_swap(plane, yy, own):
        there = out_slot(tp, plane, yy, c)
        return remote(wo_ref if own else there, there, wx_send.at[plane, yy], wx_recv.at[plane, yy], x_peer)

    def w_beside(half, plane, yy, own):
        there = out_slot(half, plane, yy, c)
        return remote(
            wo_ref if own else there, there, wc_send.at[half, plane, yy], wc_recv.at[half, plane, yy], c_peer
        )

    def w_line_start():
        w_line(1).start()
        w_line(2).start()

    def w_from_line(i):
        plane = order(i)
        arrived(out_slot(tp, plane, y, c), wl_recv.at[plane])
        if i > 1:

            @pl.when(between)
            def _():
                w_line_on(i).start()

        w_swap(plane, y, False).start()
        w_beside(tp, plane, y, False).start()

    def w_from_pair(i):
        plane = order(i)
        arrived(out_slot(tp, plane, 1 - y, c), wy_recv.at[plane])
        w_swap(plane, 1 - y, False).start()
        w_beside(tp, plane, 1 - y, False).start()

    def w_from_swap(i):
        plane = order(i)
        for yy in (y, 1 - y):
            arrived(out_slot(1 - tp, plane, yy, c), wx_recv.at[plane, yy])
            w_beside(1 - tp, plane, yy, False).start()

    def slot(a, zz, yy, cc):
        start = pl.multiple_of((zz * members + yy * 2 + cc) * w_rows, w_rows)
        return full.at[a, pl.ds(start, w_rows), :]

    def line(a, i):
        there = slot(a, z, y, c)
        return remote(weights[a], there, line_send.at[i - 1, a], line_recv.at[z, a], at(order(i), m))

    def line_on(a, i):
        there = slot(a, order(i), y, c)
        return remote(there, there, line_send.at[i, a], line_recv.at[order(i), a], at(order(1), m))

    def y_copy(a, i, own):
        there = slot(a, order(i), y, c)
        src = weights[a] if own else there
        return remote(src, there, y_send.at[order(i), a], y_recv.at[order(i), a], y_peer)

    def c_copy(a, zz, yy, own):
        there = slot(a, zz, yy, c)
        src = weights[a] if own else there
        return remote(src, there, c_send.at[zz, yy, a], c_recv.at[zz, yy, a], c_peer)

    def c_came(a, zz, yy):
        there = slot(a, zz, yy, 1 - c)
        return remote(there, there, c_send.at[zz, yy, a], c_recv.at[zz, yy, a], c_peer)

    def from_line(i, arrays):
        zz = order(i)
        for a in arrays:
            arrived(slot(a, zz, y, c), line_recv.at[zz, a])

            @pl.when(between & (i > 1))
            def _():
                line_on(a, i).start()

            y_copy(a, i, False).start()
            c_copy(a, zz, y, False).start()

    def from_pair(i, arrays):
        zz = order(i)
        for a in arrays:
            arrived(slot(a, zz, 1 - y, c), y_recv.at[zz, a])
            c_copy(a, zz, 1 - y, False).start()

    def multiply(i, yy, arrays):
        zz = order(i)
        for a in arrays:
            c_came(a, zz, yy).wait_recv()
        piece = zz * 2 + yy
        start = pl.multiple_of(piece * 2 * w_rows, 2 * w_rows)
        for a in arrays:
            part = jnp.dot(
                pieces[piece], full[a, pl.ds(start, 2 * w_rows), :], preferred_element_type=jnp.float32
            )
            product[a] += part

    def own_weights(arrays):
        for a in arrays:
            line(a, 2).start()
            line(a, 1).start()
            y_copy(a, 0, True).start()
            c_copy(a, z, y, True).start()
            full[a, pl.ds(pl.multiple_of(sp * w_rows, w_rows), w_rows), :] = weights[a][...]

    swaps = (
        remote(tok_ref, theirs, swap_sem.at[0], swap_sem.at[1], x_peer),
        remote(gain_in, their_gain, swap_sem.at[2], swap_sem.at[3], x_peer),
    )
    own_weights(first_pair)
    for swap in swaps:
        swap.start()
    own_weights(last_one)
    w_swap(z, y, True).start()
    w_beside(tp, z, y, True).start()
    product[...] = jnp.zeros_like(product)
    acc[...] = jnp.zeros_like(acc)
    total[...] = jnp.zeros_like(total)
    top[...] = jnp.full_like(top, NEG_LARGE)
    own_pool = pl.ds(pl.multiple_of(sp * pool_rows, pool_rows), pool_rows)
    w_pool[own_pool, :] = wp_ref[...]
    w_full[
        pl.ds(pl.multiple_of(tp * out_rows, out_rows), out_rows),
        pl.ds(pl.multiple_of(sp * out_columns, out_columns), out_columns),
    ] = wo_ref[...]

    from_line(turn[1], first_pair)
    from_line(turn[2], first_pair)
    from_pair(0, first_pair)
    from_line(turn[1], last_one)
    from_line(turn[2], last_one)
    from_pair(0, last_one)
    from_line(turn[3], first_pair)
    from_pair(turn[1], first_pair)
    for swap in swaps:
        swap.wait()
    squares = jnp.zeros((rows, 1), jnp.float32)
    per_half = half_width // (2 * w_rows)
    for ref, gains, owner in ((tok_ref, gain_in, tp), (theirs, their_gain, 1 - tp)):
        for j in range(per_half):
            chunk = pl.ds(j * 2 * w_rows, 2 * w_rows)
            features = ref[:, chunk].astype(jnp.float32)
            squares += jnp.sum(features * features, axis=1, keepdims=True)
            scaled = (features * gains[:, chunk].astype(jnp.float32)).astype(jnp.bfloat16)
            pieces[owner * per_half + j] = scaled
    inverse = lax.rsqrt(squares / model_width + EPSILON)
    inverse_sc[...] = jnp.broadcast_to(inverse, inverse_sc.shape)
    every = first_pair + last_one
    multiply(0, y, every)
    multiply(0, 1 - y, every)
    from_line(turn[3], last_one)
    w_line_start()
    from_pair(turn[1], last_one)
    multiply(turn[1], y, every)
    from_pair(turn[2], first_pair)
    multiply(turn[1], 1 - y, every)
    from_pair(turn[2], last_one)
    multiply(turn[2], y, every)
    multiply(turn[2], 1 - y, every)
    multiply(turn[3], y, first_pair)
    from_pair(turn[3], first_pair)
    multiply(turn[3], 1 - y, first_pair)
    width = columns // planes
    for p in range(planes):
        part = slice(p * width, (p + 1) * width)
        k_src[p] = (product[0, :, part] * inverse_sc[:, :1]).astype(jnp.bfloat16)
        v_src[p] = (product[1, :, part] * inverse_sc[:, :1]).T.astype(jnp.bfloat16)
    k_all[z, m] = k_src[z]
    v_all[z, m] = v_src[z]
    share(z, True)
    w_across(z, True).start()
    for i in range(1, planes):
        k_out(order(i)).start()
        v_out(order(i)).start()
    from_pair(turn[3], last_one)
    multiply(turn[3], y, last_one)
    multiply(turn[3], 1 - y, last_one)
    for p in range(planes):
        part = slice(p * width, (p + 1) * width)
        query = (product[2, :, part] * inverse_sc[:, :1]).astype(jnp.bfloat16)
        q_src[p] = query * (1.0 / math.sqrt(hdim))

    @pl.when(z % 2 == 0)
    def _():
        q_in[z] = q_src[z]

    @pl.when(z % 2 == 1)
    def _():
        q_out(z).start()

    for i in range(1, planes):
        q_out(order(i)).start()
    pool_start()
    w_from_line(1)

    @pl.when(between)
    def _():
        w_from_line(2)
        w_from_line(3)

    def visit(block, plane, first, count, masked):
        query = q_in[block]
        lane = lax.broadcasted_iota(jnp.int32, query.shape, 1)
        none = jnp.zeros_like(query)
        both = jnp.concatenate(
            [jnp.where(lane < hdim, query, none), jnp.where(lane < hdim, none, query)], axis=0
        )
        keys = k_all[plane, pl.ds(first, count)].reshape(count * rows, 2 * hdim)
        values = jnp.concatenate([v_all[plane, first + i] for i in range(count)], axis=1)
        scores = lax.dot_general(
            keys, both, (((1,), (1,)), ((), ())), preferred_element_type=jnp.float32
        )
        if masked:
            shift = (first - holder(block, m)) * rows
            key = lax.broadcasted_iota(jnp.int32, scores.shape, 0)
            col = lax.broadcasted_iota(jnp.int32, scores.shape, 1)
            col = jnp.where(col < rows, col, col - rows)
            scores = jnp.where(key + shift <= col, scores, NEG_LARGE)
        old = top[block]
        new = jnp.maximum(old, jnp.max(scores, axis=0, keepdims=True))
        factor = jnp.exp(old - new)
        expo = jnp.exp(scores - new)
        acc[block] = acc[block] * factor + jnp.dot(
            values, expo.astype(jnp.bfloat16), preferred_element_type=jnp.float32
        )
        partial = jnp.sum(expo.reshape(count * rows // 8, 8, 2 * rows), axis=0)
        total[block] = total[block] * factor + partial
        top[block] = new

    def diagonal(block):
        pair = holder(block, m) // 2

        @pl.when(pair > 0)
        def _():
            visit(block, block, 0, members // 2, False)

        visit(block, block, pair * (members // 2), members // 2, True)

    def result_copy(block, half):
        return remote(
            done.at[block, pl.ds(pl.multiple_of(half * half_rows, half_rows), half_rows)],
            branch.at[tp * planes + z, :, pl.ds(0, vdim)],
            back_send.at[block, half],
            back_recv.at[tp * planes + z],
            at(block, holder(block, m), half),
        )

    def at_home(block):
        return (block == z) & (z % 2 == 0)

    def finish(block):
        both = acc[block] / jnp.sum(total[block], axis=0, keepdims=True)
        mixed = both[:, :rows] - lam_ref[z] * both[:, rows:]
        mean_sq = jnp.mean(mixed * mixed, axis=0, keepdims=True)
        normed = (mixed * lax.rsqrt(mean_sq + EPSILON)).T * gain_ref[...]
        done[block] = normed.astype(jnp.bfloat16)

        @pl.when(at_home(block))
        def _():
            kept = pl.ds(pl.multiple_of(tp * half_rows, half_rows), half_rows)
            branch[tp * planes + z, :, :vdim] = done[block, kept]

        @pl.when(jnp.logical_not(at_home(block)))
        def _():
            result_copy(block, tp).start()

        result_copy(block, 1 - tp).start()

    edge_rows = halo.shape[0]

    def edge_out():
        return remote(
            pool_sc.at[pl.ds(rows - edge_rows, edge_rows)], halo, edge_sem.at[0], edge_sem.at[1], {"sp": sp + 1}
        )

    def half_out():
        mine = pl.ds(pl.multiple_of(tp * groups, groups), groups)
        return remote(
            pooled_sc, branch.at[mine, :, pl.ds(vdim, vdim)], half_sem.at[0], half_sem.at[1], x_peer
        )

    def pool_project():
        for plane in range(planes):
            arrived(pool_slot(plane, c_member), pc_recv.at[plane, 0])
            arrived(pool_slot(plane, turned), pc_recv.at[plane, 1])
        scaled = jnp.concatenate([pieces[j] for j in range(pieces.shape[0])], axis=1)
        pool_in = jnp.dot(scaled, w_pool[...], preferred_element_type=jnp.float32)
        pool_sc[...] = (pool_in * inverse_sc[:, :1]).astype(jnp.bfloat16)

        @pl.when(sp < n_sp - 1)
        def _():
            edge_out().start()

        @pl.when(sp == 0)
        def _():
            halo[...] = jnp.zeros_like(halo)

    def pool_mix():
        @pl.when(sp > 0)
        def _():
            arrived(halo, edge_sem.at[1])

        for g in range(groups):
            part = slice(g * vdim, (g + 1) * vdim)
            own = pool_sc[:, part].astype(jnp.float32)
            running = jnp.concatenate([halo[:, part].astype(jnp.float32), own], axis=0)
            span = WINDOWS[g % len(WINDOWS)]
            step = 1
            while step < span:
                running = running + pltpu.roll(running, step, 0)
                step *= 2
            position = sp * rows + lax.broadcasted_iota(jnp.int32, own.shape, 0)
            count = jnp.minimum(position + 1, span).astype(jnp.float32)
            differ = (running[edge_rows:] / count - own).astype(jnp.bfloat16)
            pooled = jnp.dot(differ, group_ref[g], preferred_element_type=jnp.float32)
            pooled = (pooled * pscale_ref[:, part]).astype(jnp.bfloat16)
            low, high = pooled[:half_rows], pooled[half_rows:]
            branch[tp * groups + g, :, vdim:] = jnp.where(tp == 0, low, high)
            pooled_sc[g] = jnp.where(tp == 0, high, low)
        half_out().start()

    hand_on(z, True)
    landed(1)
    shared(z, True)

    @pl.when(z % 2 == 1)
    def _():
        arrived(q_in.at[z], z_recv.at[2, z])

    def stage(i, carry):
        block = order(i)

        @pl.when(i < planes - 2)
        def _():
            landed(i + 2)

        @pl.when(i == planes - 3)
        def _():
            w_across(order(1), False).start()

            @pl.when(between)
            def _():
                w_across(order(2), False).start()
                w_across(order(3), False).start()

            pool_across(z, True).start()
            pool_beside(z, True).start()

        @pl.when(i == planes - 2)
        def _():
            w_from_pair(0)

            @pl.when(jnp.logical_not(between))
            def _():
                w_from_line(2)
                w_across(order(2), False).start()

        diagonal(block)

        @pl.when(i < planes - 1)
        def _():
            hand_on(order(i + 1), False)

        @pl.when(i == planes - 1)
        def _():
            finish(0)

        def pair(j, carry):
            other = jnp.where(i < planes - 1, order(j), j + upper)
            visit(jnp.maximum(block, other), jnp.minimum(block, other), 0, members, False)

            @pl.when(i == planes - 1)
            def _():
                finish(j + 1)

                @pl.when(j == 0)
                def _():
                    @pl.when(jnp.logical_not(between))
                    def _():
                        w_from_line(3)
                        w_across(order(3), False).start()

                    pool_from_line(1)

                @pl.when(j == 1)
                def _():
                    w_from_pair(1)
                    pool_from_line(2)

            return carry

        lax.fori_loop(0, i, pair, 0)

        @pl.when(i < planes - 1)
        def _():
            arrived(q_in.at[order(i + 1)], z_recv.at[2, order(i + 1)])
            shared(order(i + 1), False)

        return carry

    lax.fori_loop(0, planes, stage, 0)

    w_from_pair(2)
    pool_from_line(3)
    w_from_swap(0)
    w_from_pair(3)
    w_from_swap(1)
    for i in range(planes):
        pool_from_pair(i)
    pool_project()
    w_from_swap(2)
    pool_mix()
    w_from_swap(3)

    for head in range(2 * planes):
        own_head = tp * planes + z == head

        @pl.when(jnp.logical_not(own_head & at_home(z)))
        def _():
            arrived(branch.at[head, :, pl.ds(0, vdim)], back_recv.at[head])

    theirs = pl.ds(pl.multiple_of((1 - tp) * groups, groups), groups)
    arrived(branch.at[theirs, :, pl.ds(vdim, vdim)], half_sem.at[1])
    for half in range(2):
        for plane in range(planes):
            for yy in range(2):
                arrived(out_slot(half, plane, yy, 1 - c), wc_recv.at[half, plane, yy])
    left = jnp.concatenate([branch[head] for head in range(2 * planes)], axis=1)
    out_width = out_ref.shape[1] // planes

    def column(n, carry):
        part = pl.ds(pl.multiple_of(n * out_width, out_width), out_width)
        out_ref[:, part] = jnp.dot(
            left, w_full[:, part], preferred_element_type=jnp.float32
        ).astype(jnp.bfloat16)
        return carry

    lax.fori_loop(0, planes, column, 0)

    for i in range(1, planes):
        k_out(order(i)).wait_send()
        v_out(order(i)).wait_send()
        q_out(order(i)).wait_send()

    @pl.when(z % 2 == 1)
    def _():
        q_out(z).wait_send()

    for i in range(planes):
        plane = order(i)
        for copies in in_plane(plane, i == 0):
            for copy in copies:
                copy.wait_send()
        w_across(plane, False).wait_send()
        for a in first_pair + last_one:
            y_copy(a, i, False).wait_send()
            c_copy(a, plane, y, False).wait_send()
            c_copy(a, plane, 1 - y, False).wait_send()
        for yy in (y, 1 - y):
            w_swap(plane, yy, False).wait_send()
            w_beside(0, plane, yy, False).wait_send()
            w_beside(1, plane, yy, False).wait_send()

    for i in (1, 2):
        w_line(i).wait_send()
        pool_line(i).wait_send()
        for a in first_pair + last_one:
            line(a, i).wait_send()

    @pl.when(between)
    def _():
        for i in (2, 3):
            w_line_on(i).wait_send()
            pool_line_on(i).wait_send()
            for a in first_pair + last_one:
                line_on(a, i).wait_send()

    for plane in range(planes):
        pool_across(plane, False).wait_send()
        pool_beside(plane, False).wait_send()
        pool_onward(plane).wait_send()
        result_copy(plane, 1 - tp).wait_send()

        @pl.when(jnp.logical_not(at_home(plane)))
        def _():
            result_copy(plane, tp).wait_send()

    half_out().wait_send()

    @pl.when(sp < n_sp - 1)
    def _():
        edge_out().wait_send()


def whole_layer(
    tokens,
    pre_gain,
    w_query,
    w_key,
    w_value,
    w_pool,
    lambdas,
    sub_gain,
    group_weight,
    pool_scale,
    w_out,
):
    planes = lambdas.shape[0]
    rows, half_width = tokens.shape
    n_sp = lax.axis_size("sp")
    members = n_sp // planes
    w_rows, columns = w_query.shape
    model_width = n_sp * w_rows
    width = columns // planes
    groups, vdim, _ = group_weight.shape
    out_rows, out_columns = w_out.shape
    vmem = pl.BlockSpec(memory_space=pltpu.VMEM)
    dma = pltpu.SemaphoreType.DMA
    bf16, f32 = jnp.bfloat16, jnp.float32
    work = planes * rows * members * planes * rows
    return pl.pallas_call(
        functools.partial(layer, width // 2, model_width),
        out_shape=jax.ShapeDtypeStruct((rows // 2, n_sp * out_columns), bf16),
        in_specs=[pl.BlockSpec(memory_space=pltpu.SMEM)] + [vmem] * 10,
        out_specs=vmem,
        scratch_shapes=[
            pltpu.VMEM((3, model_width, columns), bf16),
            pltpu.VMEM((rows, half_width), bf16),
            pltpu.VMEM((1, half_width), bf16),
            pltpu.VMEM((model_width // (2 * w_rows), rows, 2 * w_rows), bf16),
            pltpu.VMEM((3, rows, columns), f32),
            pltpu.VMEM((rows, 128), f32),
            pltpu.VMEM((planes, rows, width), bf16),
            pltpu.VMEM((planes, vdim, rows), bf16),
            pltpu.VMEM((planes, rows, width), bf16),
            pltpu.VMEM((planes, rows, width), bf16),
            pltpu.VMEM((planes, members, rows, width), bf16),
            pltpu.VMEM((planes, members, vdim, rows), bf16),
            pltpu.VMEM((planes, vdim, 2 * rows), f32),
            pltpu.VMEM((planes, 1, 2 * rows), f32),
            pltpu.VMEM((planes, 8, 2 * rows), f32),
            pltpu.VMEM((planes, rows, vdim), bf16),
            pltpu.VMEM((model_width, groups * vdim), bf16),
            pltpu.VMEM((2 * out_rows, n_sp * out_columns), bf16),
            pltpu.VMEM((2 * planes, rows // 2, 2 * vdim), bf16),
            pltpu.VMEM((rows, groups * vdim), bf16),
            pltpu.VMEM((RIM_ROWS + 1, groups * vdim), bf16),
            pltpu.VMEM((groups, rows // 2, vdim), bf16),
            dma((planes, 3)),
            dma((planes, 3)),
            dma((planes, 3)),
            dma((planes, 3)),
            dma((planes, 2, 3)),
            dma((planes, 2, 3)),
            dma((4,)),
            dma((3, planes)),
            dma((3, planes)),
            dma((planes, 3, 2)),
            dma((planes, 3, 2)),
            dma((planes, 2)),
            dma((2 * planes,)),
            dma((planes,)),
            dma((planes,)),
            dma((planes, 2)),
            dma((planes, 2)),
            dma((2,)),
            dma((2,)),
            dma((planes,)),
            dma((planes,)),
            dma((planes,)),
            dma((planes,)),
            dma((planes,)),
            dma((planes,)),
            dma((planes, 2)),
            dma((planes, 2)),
            dma((2, planes, 2)),
            dma((2, planes, 2)),
        ],
        compiler_params=pltpu.CompilerParams(
            vmem_limit_bytes=60 * 2**20, collective_id=2, has_side_effects=True
        ),
        cost_estimate=pl.CostEstimate(
            flops=4 * work * vdim, bytes_accessed=2**24, transcendentals=work
        ),
    )(
        lambdas,
        tokens,
        pre_gain.reshape(1, -1),
        w_key,
        w_value,
        w_query,
        w_pool,
        sub_gain.reshape(1, -1),
        group_weight,
        pool_scale.reshape(1, -1),
        w_out,
    )


def trailing(x, window_ids, group_dim):
    column_window = jnp.repeat(window_ids, group_dim)[None, :]
    running = x
    picked = jnp.zeros_like(x)
    for slot, span in enumerate(WINDOWS):
        half = span // 2
        running = running + jnp.pad(running[:-half], ((half, 0), (0, 0)))
        picked = jnp.where(column_window == slot, running, picked)
    return picked


def general_attention(queries, key_rows, values, lambdas, sub_gain):
    n_sp = lax.axis_size("sp")
    sp = lax.axis_index("sp")
    tok_rows = queries.shape[0]
    heads = lambdas.shape[0]
    qdim = queries.shape[1] // heads
    vdim = values.shape[1] // heads
    head_width = 2 * qdim + vdim
    outer = math.gcd(n_sp, heads)
    inner = n_sp // outer
    per_device = heads // outer
    by_head = jnp.concatenate(
        [
            x.reshape(tok_rows, heads, -1).swapaxes(0, 1)
            for x in (queries, key_rows, values)
        ],
        axis=2,
    )
    across = [[o * inner + i for o in range(outer)] for i in range(inner)]
    within = [[o * inner + i for i in range(inner)] for o in range(outer)]
    by_head = by_head.reshape(outer, per_device, tok_rows, head_width)
    if outer > 1:
        by_head = lax.all_to_all(by_head, "sp", 0, 0, axis_index_groups=across)
    first_head = lax.div(sp, inner) * per_device
    attended = []
    if inner == 4 and per_device == 1:
        lam = lax.dynamic_slice_in_dim(lambdas, first_head, 1)
        attended.append(
            flash_members(by_head[:, 0, :, :qdim], by_head[:, 0, :, qdim:], lam, sub_gain)
        )
    else:
        kv = lax.all_gather(by_head[..., qdim:], "sp", axis=0, axis_index_groups=within)
        member = lax.rem(sp, inner).reshape(1)
        for p in range(per_device):
            lam = lax.dynamic_slice_in_dim(lambdas, first_head + p, 1)
            attended.append(flash(by_head[:, p, :, :qdim], kv[:, :, p], member, lam, sub_gain))
    attended = jnp.stack(attended, axis=1)
    if outer > 1:
        attended = lax.all_to_all(attended, "sp", 0, 0, axis_index_groups=across)
    return attended.reshape(heads, tok_rows, vdim)


def local(
    tokens,
    pre_gain,
    w_query,
    w_key,
    w_value,
    w_pool,
    lambdas,
    sub_gain,
    group_weight,
    pool_scale,
    w_out,
):
    n_tp = lax.axis_size("tp")
    n_sp = lax.axis_size("sp")
    tp = lax.axis_index("tp")
    sp = lax.axis_index("sp")
    tok_rows = tokens.shape[0]
    model_width = tokens.shape[1] * n_tp
    heads = lambdas.shape[0]
    qdim = w_query.shape[1] // heads
    vdim = w_value.shape[1] // heads
    groups = group_weight.shape[0]
    group_dim = group_weight.shape[1]

    shaped_for_mix = n_tp == 2 and heads == 4 and n_sp == 4 * heads and tok_rows % 32 == 0
    if shaped_for_mix and qdim == vdim == group_dim and groups == heads:
        return whole_layer(
            tokens,
            pre_gain,
            w_query,
            w_key,
            w_value,
            w_pool,
            lambdas,
            sub_gain,
            group_weight,
            pool_scale,
            w_out,
        )
    swap = [(0, 1), (1, 0)]
    w_sorted = w_out.reshape(heads, 2, vdim, -1).swapaxes(0, 1).reshape(w_out.shape)
    features = tokens.astype(jnp.float32)
    mine = (features * pre_gain.astype(jnp.float32)[None, :]).astype(jnp.bfloat16)
    squares = jnp.sum(features * features, axis=1, keepdims=True)
    weights = [w_query, w_key, w_value, w_pool]
    if n_sp % 4 == 0:
        *weights, theirs = gather_weights(weights, mine, n_tp == 2)
    else:
        weights = [lax.all_gather(w, "sp", axis=0, tiled=True) for w in weights]
        theirs = lax.ppermute(mine, "tp", swap) if n_tp == 2 else mine
    w_sorted, weights = lax.optimization_barrier((w_sorted, weights))
    w_out_rows = lax.all_gather(w_sorted, "sp", axis=1, tiled=True)
    if n_tp == 2:
        squares = squares + lax.ppermute(squares, "tp", swap)
        scaled = jnp.concatenate(
            [jnp.where(tp == 0, mine, theirs), jnp.where(tp == 0, theirs, mine)], axis=1
        )
    else:
        scaled = lax.all_gather(mine, "tp", axis=1, tiled=True)
        squares = lax.psum(squares, "tp")
    inverse = lax.rsqrt(squares / model_width + EPSILON)
    queries, key_rows, values, pool_in = [
        (jnp.dot(scaled, w, preferred_element_type=jnp.float32) * inverse).astype(jnp.bfloat16)
        for w in weights
    ]
    attended = general_attention(queries, key_rows, values, lambdas, sub_gain)

    halo = passed_along(pool_in[tok_rows - RIM_ROWS - 1 :], "sp", 1)
    extended = jnp.concatenate([halo, pool_in], axis=0).astype(jnp.float32)
    window_ids = (tp * groups + jnp.arange(groups, dtype=jnp.int32)) % len(WINDOWS)
    sums = trailing(extended, window_ids, group_dim)[RIM_ROWS + 1 :]
    spans = jnp.repeat(jnp.left_shift(2, window_ids), group_dim)
    positions = sp * tok_rows + jnp.arange(tok_rows, dtype=jnp.int32)
    count = jnp.minimum(positions[:, None] + 1, spans[None, :]).astype(jnp.float32)
    differ = (sums / count - pool_in.astype(jnp.float32)).astype(jnp.bfloat16)
    pooled = jnp.einsum(
        "tgc,gcd->tgd",
        differ.reshape(tok_rows, groups, group_dim),
        group_weight,
        preferred_element_type=jnp.float32,
    )
    pooled = (pooled * pool_scale.reshape(groups, group_dim)).astype(jnp.bfloat16)
    branch = jnp.concatenate(
        [attended.swapaxes(0, 1).reshape(tok_rows, -1), pooled.reshape(tok_rows, -1)], axis=1
    )
    if n_tp == 2:
        half = tok_rows // 2
        send = lax.dynamic_slice_in_dim(branch, (1 - tp) * half, half, 0)
        send = jnp.dot(send, w_out_rows, preferred_element_type=jnp.float32).astype(jnp.bfloat16)
        got = lax.ppermute(send, "tp", swap)
        keep = lax.dynamic_slice_in_dim(branch, tp * half, half, 0)
        keep = jnp.dot(keep, w_out_rows, preferred_element_type=jnp.float32)
        return (keep + got.astype(jnp.float32)).astype(jnp.bfloat16)
    partial = jnp.dot(branch, w_out_rows, preferred_element_type=jnp.float32)
    return lax.psum_scatter(partial.astype(jnp.bfloat16), "tp", scatter_dimension=0, tiled=True)


def solution(mesh):
    placed = (
        P("sp", "tp"),
        P("tp"),
        P("sp", "tp"),
        P("sp", "tp"),
        P("sp", "tp"),
        P("sp", "tp"),
        P("tp"),
        P(),
        P("tp", None, None),
        P("tp"),
        P("tp", "sp"),
    )
    return jax.shard_map(
        local, mesh=mesh, in_specs=placed, out_specs=P(("sp", "tp"), None), check_vma=False
    )
```

```python
import functools
import math

import jax
import jax.numpy as jnp
from jax import lax
from jax.experimental import pallas as pl
from jax.experimental.pallas import tpu as pltpu
from jax.sharding import PartitionSpec as P

EPSILON = 1e-06
NEG_LARGE = -1e30
WINDOWS = (2, 4, 8, 16)
RIM_ROWS = 15


def passed_along(block, axis, distance):
    devices = range(lax.axis_size(axis))
    route = [(i - distance, i) for i in devices if i - distance in devices]
    return lax.ppermute(block, axis, route)


def attend(inner, vdim, hdim, member_ref, lam_ref, q_ref, kv_ref, gain_ref, out_ref, acc_ref, max_ref):
    rows = q_ref.shape[1]
    block = pl.program_id(0)
    last = block * inner + member_ref[0]
    scale = 1.0 / math.sqrt(hdim)
    queries = (q_ref[0].astype(jnp.float32) * scale).astype(jnp.bfloat16)
    maps = (queries[:, :hdim], queries[:, hdim:])
    ones = jnp.ones((rows, vdim), jnp.bfloat16)
    acc_ref[...] = jnp.zeros_like(acc_ref)
    max_ref[...] = jnp.full_like(max_ref, NEG_LARGE)

    def step(g, masked):
        keys_values = kv_ref[lax.rem(g, inner), lax.div(g, inner)]
        values = jnp.concatenate([keys_values[:, 2 * hdim :], ones], axis=1)
        for m in range(2):
            keys = keys_values[:, m * hdim : (m + 1) * hdim]
            scores = lax.dot_general(
                maps[m], keys, (((1,), (1,)), ((), ())), preferred_element_type=jnp.float32
            )
            if masked:
                row = lax.broadcasted_iota(jnp.int32, scores.shape, 0)
                col = lax.broadcasted_iota(jnp.int32, scores.shape, 1)
                scores = jnp.where(col <= row, scores, NEG_LARGE)
            old_max = max_ref[m]
            new_max = jnp.maximum(old_max, jnp.max(scores, axis=1, keepdims=True))
            factor = jnp.exp(old_max - new_max)
            expo = jnp.exp(scores - new_max[:, :1])
            acc_ref[m] = acc_ref[m] * factor[:, :1] + jnp.dot(
                expo.astype(jnp.bfloat16), values, preferred_element_type=jnp.float32
            )
            max_ref[m] = new_max

    def body(g, carry):
        step(g, False)
        return carry

    lax.fori_loop(0, last, body, 0)
    step(last, True)
    first = acc_ref[0]
    second = acc_ref[1]
    mix = first[:, :vdim] / first[:, vdim:] - lam_ref[0] * (second[:, :vdim] / second[:, vdim:])
    mean_sq = jnp.mean(mix * mix, axis=1, keepdims=True)
    out_ref[0] = (mix * lax.rsqrt(mean_sq + EPSILON) * gain_ref[...]).astype(jnp.bfloat16)


def flash(q, kv, member, lam, sub_gain):
    inner, outer, rows, width = kv.shape
    qdim = q.shape[-1]
    vdim = width - qdim
    smem = pl.BlockSpec(memory_space=pltpu.SMEM)
    work = outer * rows * outer * rows * inner
    return pl.pallas_call(
        functools.partial(attend, inner, vdim, qdim // 2),
        grid=(outer,),
        out_shape=jax.ShapeDtypeStruct((outer, rows, vdim), jnp.bfloat16),
        in_specs=[
            smem,
            smem,
            pl.BlockSpec((1, rows, qdim), lambda b: (b, 0, 0)),
            pl.BlockSpec(memory_space=pltpu.VMEM),
            pl.BlockSpec(memory_space=pltpu.VMEM),
        ],
        out_specs=pl.BlockSpec((1, rows, vdim), lambda b: (b, 0, 0)),
        scratch_shapes=[
            pltpu.VMEM((2, rows, 2 * vdim), jnp.float32),
            pltpu.VMEM((2, rows, 128), jnp.float32),
        ],
        compiler_params=pltpu.CompilerParams(vmem_limit_bytes=56 * 2**20),
        cost_estimate=pl.CostEstimate(
            flops=4 * work * vdim, bytes_accessed=kv.size * 2, transcendentals=work
        ),
    )(member, lam, q, kv, sub_gain.reshape(1, -1))


def attend_members(hdim, lam_ref, q_ref, own_ref, gain_ref, out_ref, held, acc_ref, max_ref, send, recv):
    outer, rows, _ = q_ref.shape
    vdim = own_ref.shape[2] - 2 * hdim
    sp = lax.axis_index("sp")
    member = lax.rem(sp, 4)
    y = lax.div(member, 2)
    c = lax.rem(member, 2)
    y_peer = sp + 2 - 4 * y
    c_peer = sp + 1 - 2 * c
    barrier = pltpu.get_barrier_semaphore()
    for peer in (y_peer, c_peer):
        pl.semaphore_signal(
            barrier, 1, device_id={"sp": peer}, device_id_type=pl.DeviceIdType.MESH
        )
    pl.semaphore_wait(barrier, 2)

    def remote(src, index, peer):
        return pltpu.make_async_remote_copy(
            src_ref=src,
            dst_ref=held.at[index],
            send_sem=send.at[index],
            recv_sem=recv.at[index],
            device_id={"sp": peer},
            device_id_type=pl.DeviceIdType.MESH,
        )

    across = remote(own_ref, 1, y_peer)
    beside = remote(own_ref, 0, c_peer)
    onward = remote(held.at[1], 2, c_peer)
    across.start()
    beside.start()
    acc_ref[...] = jnp.zeros_like(acc_ref)
    max_ref[...] = jnp.full_like(max_ref, NEG_LARGE)
    scale = 1.0 / math.sqrt(hdim)

    def visit(ref, other):
        shift = (member - other) * rows
        for block in range(outer):
            queries = (q_ref[block].astype(jnp.float32) * scale).astype(jnp.bfloat16)
            length = (block + 1) * rows
            keys_values = ref[: block + 1].reshape(length, 2 * hdim + vdim)
            values = jnp.concatenate(
                [keys_values[:, 2 * hdim :], jnp.ones((length, vdim), jnp.bfloat16)], axis=1
            )
            for m in range(2):
                scores = lax.dot_general(
                    queries[:, m * hdim : (m + 1) * hdim],
                    keys_values[:, m * hdim : (m + 1) * hdim],
                    (((1,), (1,)), ((), ())),
                    preferred_element_type=jnp.float32,
                )
                edge = scores[:, block * rows :]
                row = lax.broadcasted_iota(jnp.int32, edge.shape, 0)
                col = lax.broadcasted_iota(jnp.int32, edge.shape, 1)
                edge = jnp.where(col <= row + shift, edge, NEG_LARGE)
                if block > 0:
                    scores = jnp.concatenate([scores[:, : block * rows], edge], axis=1)
                else:
                    scores = edge
                old_max = max_ref[block, m]
                new_max = jnp.maximum(old_max, jnp.max(scores, axis=1, keepdims=True))
                factor = jnp.exp(old_max - new_max)
                expo = jnp.exp(scores - new_max[:, :1])
                acc_ref[block, m] = acc_ref[block, m] * factor[:, :1] + jnp.dot(
                    expo.astype(jnp.bfloat16), values, preferred_element_type=jnp.float32
                )
                max_ref[block, m] = new_max

    visit(own_ref, member)

    def arrived(j, carry):
        @pl.when(j == 0)
        def _():
            beside.wait_recv()

        @pl.when(j == 1)
        def _():
            across.wait_recv()
            onward.start()

        @pl.when(j == 2)
        def _():
            onward.wait_recv()

        other_y = jnp.where(j >= 1, 1 - y, y)
        other_c = jnp.where(j == 1, c, 1 - c)
        visit(held.at[j], 2 * other_y + other_c)
        return carry

    lax.fori_loop(0, 3, arrived, 0)
    for copy in (across, beside, onward):
        copy.wait_send()
    for block in range(outer):
        first = acc_ref[block, 0]
        second = acc_ref[block, 1]
        mix = first[:, :vdim] / first[:, vdim:]
        mix = mix - lam_ref[0] * (second[:, :vdim] / second[:, vdim:])
        mean_sq = jnp.mean(mix * mix, axis=1, keepdims=True)
        normed = mix * lax.rsqrt(mean_sq + EPSILON) * gain_ref[...]
        out_ref[block] = normed.astype(jnp.bfloat16)


def flash_members(q, kv, lam, sub_gain):
    outer, rows, width = kv.shape
    qdim = q.shape[-1]
    vdim = width - qdim
    vmem = pl.BlockSpec(memory_space=pltpu.VMEM)
    work = 4 * outer * rows * outer * rows
    return pl.pallas_call(
        functools.partial(attend_members, qdim // 2),
        out_shape=jax.ShapeDtypeStruct((outer, rows, vdim), jnp.bfloat16),
        in_specs=[pl.BlockSpec(memory_space=pltpu.SMEM), vmem, vmem, vmem],
        out_specs=vmem,
        scratch_shapes=[
            pltpu.VMEM((3, outer, rows, width), jnp.bfloat16),
            pltpu.VMEM((outer, 2, rows, 2 * vdim), jnp.float32),
            pltpu.VMEM((outer, 2, rows, 128), jnp.float32),
            pltpu.SemaphoreType.DMA((3,)),
            pltpu.SemaphoreType.DMA((3,)),
        ],
        compiler_params=pltpu.CompilerParams(
            vmem_limit_bytes=56 * 2**20, collective_id=1, has_side_effects=True
        ),
        cost_estimate=pl.CostEstimate(
            flops=4 * work * vdim, bytes_accessed=4 * kv.size * 2, transcendentals=work
        ),
    )(lam, q, kv, sub_gain.reshape(1, -1))


def spread(n_sp, count, with_swap, *refs):
    weights, refs = refs[:count], refs[count:]
    mine, refs = refs[0], refs[1:]
    fulls, refs = refs[:count], refs[count:]
    theirs, refs = refs[0], refs[1:]
    up_send, up_recv, down_send, down_recv, y_send, y_recv, c_send, c_recv, own_sem, swap_sem = refs
    depth = n_sp // 4
    rows = weights[0].shape[0]
    sp = lax.axis_index("sp")
    z = lax.div(sp, 4)
    y = lax.rem(lax.div(sp, 2), 2)
    c = lax.rem(sp, 2)
    y_peer = z * 4 + (1 - y) * 2 + c
    c_peer = z * 4 + y * 2 + (1 - c)
    barrier = pltpu.get_barrier_semaphore()

    def greet(device):
        pl.semaphore_signal(barrier, 1, device_id=device, device_id_type=pl.DeviceIdType.MESH)

    greet({"sp": y_peer})
    greet({"sp": c_peer})
    greeted = 2
    if with_swap:
        greet({"tp": 1 - lax.axis_index("tp")})
        greeted = 3

    @pl.when(z > 0)
    def _():
        greet({"sp": sp - 4})

    @pl.when(z < depth - 1)
    def _():
        greet({"sp": sp + 4})

    in_line = jnp.where(z > 0, 1, 0) + jnp.where(z < depth - 1, 1, 0)
    pl.semaphore_wait(barrier, greeted + in_line)

    def slot(a, zz, yy, cc):
        start = pl.multiple_of((zz * 4 + yy * 2 + cc) * rows, rows)
        return fulls[a].at[pl.ds(start, rows), :]

    def remote(src, dst, send, recv, device):
        return pltpu.make_async_remote_copy(
            src_ref=src,
            dst_ref=dst,
            send_sem=send,
            recv_sem=recv,
            device_id=device,
            device_id_type=pl.DeviceIdType.MESH,
        )

    def line_copy(side, k, a, src):
        sends, recvs = (up_send, up_recv) if side > 0 else (down_send, down_recv)
        there = slot(a, z - side * k, y, c)
        return remote(
            there if src is None else src,
            there,
            sends.at[k, a],
            recvs.at[k + 1, a],
            {"sp": sp + 4 * side},
        )

    def y_copy(zz, yy, a, src):
        there = slot(a, zz, yy, c)
        src = there if src is None else src
        return remote(src, there, y_send.at[zz, a], y_recv.at[zz, a], {"sp": y_peer})

    def c_copy(zz, yy, cc, a, src):
        there = slot(a, zz, yy, cc)
        src = there if src is None else src
        return remote(src, there, c_send.at[zz, yy, a], c_recv.at[zz, yy, a], {"sp": c_peer})

    def can_go(side):
        return z < depth - 1 if side > 0 else z > 0

    def came(side, k):
        return z >= k if side > 0 else z + k <= depth - 1

    if with_swap:
        swap = remote(
            mine, theirs, swap_sem.at[0], swap_sem.at[1], {"tp": 1 - lax.axis_index("tp")}
        )
        swap.start()
    for a in range(count):
        for side in (1, -1):

            @pl.when(can_go(side))
            def _():
                line_copy(side, 0, a, weights[a]).start()

        y_copy(z, y, a, weights[a]).start()
    for a in range(count):
        c_copy(z, y, c, a, weights[a]).start()
        pltpu.make_async_copy(weights[a], slot(a, z, y, c), own_sem.at[a]).start()

    def from_pair(zz):
        for a in range(count):
            y_copy(zz, 1 - y, a, None).wait_recv()
            c_copy(zz, 1 - y, c, a, None).start()

    def relay(k, carry):
        for side in (1, -1):
            recvs = up_recv if side > 0 else down_recv

            @pl.when(came(side, k))
            def _():
                zz = z - side * k
                for a in range(count):
                    there = slot(a, zz, y, c)
                    remote(there, there, up_send.at[0, a], recvs.at[k, a], {"sp": y_peer}).wait_recv()

                    @pl.when(can_go(side))
                    def _():
                        line_copy(side, k, a, None).start()

                    y_copy(zz, y, a, None).start()
                    c_copy(zz, y, c, a, None).start()

        @pl.when(k == 1)
        def _():
            from_pair(z)

        for side in (1, -1):

            @pl.when((k > 1) & came(side, k - 1))
            def _():
                from_pair(z - side * (k - 1))

        return carry

    lax.fori_loop(1, depth, relay, 0)
    if depth == 1:
        from_pair(z)
    for side in (1, -1):
        if depth > 1:

            @pl.when(came(side, depth - 1))
            def _():
                from_pair(z - side * (depth - 1))

    def drain(zz, carry):
        for a in range(count):
            y_copy(zz, y, a, None).wait_send()
            for yy in range(2):
                c_copy(zz, yy, 1 - c, a, None).wait_recv()
                c_copy(zz, yy, c, a, None).wait_send()
        return carry

    lax.fori_loop(0, depth, drain, 0)

    def drain_line(k, carry):
        for side in (1, -1):

            @pl.when(came(side, k) & can_go(side))
            def _():
                for a in range(count):
                    line_copy(side, k, a, None).wait_send()

        return carry

    lax.fori_loop(0, depth, drain_line, 0)
    for a in range(count):
        pltpu.make_async_copy(weights[a], slot(a, z, y, c), own_sem.at[a]).wait()
    if with_swap:
        swap.wait()


def gather_weights(weights, mine, with_swap):
    n_sp = lax.axis_size("sp")
    count = len(weights)
    depth = n_sp // 4
    sems = pltpu.SemaphoreType.DMA
    any_spec = pl.BlockSpec(memory_space=pl.ANY)
    vmem_spec = pl.BlockSpec(memory_space=pltpu.VMEM)
    shapes = [jax.ShapeDtypeStruct((n_sp * w.shape[0], w.shape[1]), w.dtype) for w in weights]
    shapes.append(jax.ShapeDtypeStruct(mine.shape, mine.dtype))
    moved = sum(w.size for w in weights) * 2 * n_sp
    return pl.pallas_call(
        functools.partial(spread, n_sp, count, with_swap),
        out_shape=shapes,
        in_specs=[vmem_spec] * (count + 1),
        out_specs=[any_spec] * (count + 1),
        scratch_shapes=[
            sems((depth + 1, count)),
            sems((depth + 1, count)),
            sems((depth + 1, count)),
            sems((depth + 1, count)),
            sems((depth, count)),
            sems((depth, count)),
            sems((depth, 2, count)),
            sems((depth, 2, count)),
            sems((count,)),
            sems((2,)),
        ],
        compiler_params=pltpu.CompilerParams(collective_id=0, has_side_effects=True),
        cost_estimate=pl.CostEstimate(flops=10**10, bytes_accessed=moved, transcendentals=0),
    )(*weights, mine)


def arrival(z, i):
    half = z // 2
    later = jnp.where(i == 2, 2 - half, 3 - 3 * half)
    return jnp.where(i == 0, z, jnp.where(i == 1, 1 + 4 * half - z, later))


def layer(
    hdim,
    model_width,
    lam_ref,
    tok_ref,
    gain_in,
    wk_ref,
    wv_ref,
    wq_ref,
    wp_ref,
    gain_ref,
    group_ref,
    pscale_ref,
    wo_ref,
    out_ref,
    full,
    theirs,
    their_gain,
    pieces,
    product,
    inverse_sc,
    k_src,
    v_src,
    q_src,
    q_in,
    k_all,
    v_all,
    acc,
    top,
    total,
    done,
    w_pool,
    w_full,
    branch,
    pool_sc,
    halo,
    pooled_sc,
    *sems,
):
    (line_send, line_recv, y_send, y_recv, c_send, c_recv, swap_sem) = sems[:7]
    (z_send, z_recv, in_send, in_recv, back_send, back_recv) = sems[7:13]
    (py_send, py_recv, pc_send, pc_recv, edge_sem, half_sem, pool_send, pool_recv) = sems[13:21]
    (wl_send, wl_recv, wy_send, wy_recv, wx_send, wx_recv, wc_send, wc_recv) = sems[21:]
    weights = (wk_ref, wv_ref, wq_ref)
    first_pair, last_one = (0, 1), (2,)
    planes, rows, _ = q_src.shape
    vdim = v_src.shape[1]
    members = k_all.shape[1]
    w_rows, columns = wq_ref.shape
    half_width = tok_ref.shape[1]
    groups = group_ref.shape[0]
    half_rows = rows // 2
    sp = lax.axis_index("sp")
    tp = lax.axis_index("tp")
    n_sp = lax.axis_size("sp")
    z = sp // members
    m = sp % members
    y = m // 2
    c = m % 2
    y_member = (m + 2) % members
    c_member = m + 1 - 2 * c
    turned = members - 1 - m
    upper = z // 2
    between = (z > 0) & (z < planes - 1)
    turn = [jnp.where(between, 1 + i % 3, i) for i in range(planes)]
    turn[0] = 0

    def at(plane, member, half=None):
        device = {"sp": plane * members + member}
        if half is not None:
            device["tp"] = half
        return device

    y_peer = at(z, y_member)
    c_peer = at(z, c_member)
    x_peer = {"tp": 1 - tp}

    def order(i):
        return arrival(z, i)

    barrier = pltpu.get_barrier_semaphore()

    def greet(device):
        pl.semaphore_signal(barrier, 1, device_id=device, device_id_type=pl.DeviceIdType.MESH)

    for i in range(1, planes):
        greet(at(order(i), m))
    for member in range(1, members):
        greet(at(z, (m + member) % members))
    for plane in range(planes):
        greet(at(plane, m, 1 - tp))

    @pl.when((m == 0) & (z > 0))
    def _():
        greet({"sp": sp - 1})

    @pl.when((m == members - 1) & (z < planes - 1))
    def _():
        greet({"sp": sp + 1})

    beyond = jnp.where((m == 0) & (z > 0), 1, 0)
    beyond += jnp.where((m == members - 1) & (z < planes - 1), 1, 0)
    pl.semaphore_wait(barrier, 2 * planes + members - 2 + beyond)

    def remote(src, dst, send, recv, device):
        return pltpu.make_async_remote_copy(
            src_ref=src,
            dst_ref=dst,
            send_sem=send,
            recv_sem=recv,
            device_id=device,
            device_id_type=pl.DeviceIdType.MESH,
        )

    def arrived(ref, recv):
        remote(ref, ref, recv, recv, c_peer).wait_recv()

    def k_out(plane):
        return remote(k_src.at[plane], k_all.at[z, m], z_send.at[0, plane], z_recv.at[0, z], at(plane, m))

    def v_out(plane):
        return remote(v_src.at[plane], v_all.at[z, m], z_send.at[1, plane], z_recv.at[1, z], at(plane, m))

    def q_out(plane):
        return remote(
            q_src.at[plane], q_in.at[z], z_send.at[2, plane], z_recv.at[2, z], at(plane, m)
        )

    def in_plane(plane, own):
        copies = []
        for t, (mine, everyone) in enumerate(((k_src, k_all), (v_src, v_all))):
            src = mine.at[plane] if own else everyone.at[plane, m]
            there = everyone.at[plane, m]
            passed = everyone.at[plane, y_member]
            copies.append(
                [
                    remote(src, there, in_send.at[plane, 0, t], in_recv.at[plane, 0, t], y_peer),
                    remote(src, there, in_send.at[plane, 1, t], in_recv.at[plane, 1, t], c_peer),
                    remote(passed, passed, in_send.at[plane, 2, t], in_recv.at[plane, 2, t], c_peer),
                ]
            )
        return copies

    def share(plane, own):
        for copies in in_plane(plane, own):
            copies[0].start()
            copies[1].start()

    def hand_on(plane, own):
        for copies in in_plane(plane, own):
            copies[0].wait_recv()
            copies[2].start()

    def shared(plane, own):
        for copies in in_plane(plane, own):
            copies[1].wait_recv()
            copies[2].wait_recv()

    def landed(i):
        plane = order(i)
        arrived(k_all.at[plane, m], z_recv.at[0, plane])
        arrived(v_all.at[plane, m], z_recv.at[1, plane])
        share(plane, False)

    pool_rows = wp_ref.shape[0]

    def pool_slot(plane, member):
        start = pl.multiple_of((plane * members + member) * pool_rows, pool_rows)
        return w_pool.at[pl.ds(start, pool_rows), :]

    def pool_line(i):
        return remote(wp_ref, pool_slot(z, m), pool_send.at[i - 1], pool_recv.at[z], at(order(i), m))

    def pool_line_on(i):
        there = pool_slot(order(i), m)
        return remote(there, there, pool_send.at[i], pool_recv.at[order(i)], at(order(1), m))

    def pool_across(plane, own):
        there = pool_slot(plane, m)
        return remote(wp_ref if own else there, there, py_send.at[plane], py_recv.at[plane], y_peer)

    def pool_beside(plane, own):
        there = pool_slot(plane, m)
        return remote(wp_ref if own else there, there, pc_send.at[plane, 0], pc_recv.at[plane, 0], c_peer)

    def pool_onward(plane):
        passed = pool_slot(plane, y_member)
        return remote(passed, passed, pc_send.at[plane, 1], pc_recv.at[plane, 1], c_peer)

    def pool_from_line(i):
        plane = order(i)
        arrived(pool_slot(plane, m), pool_recv.at[plane])
        pool_beside(plane, False).start()

    def pool_from_pair(i):
        arrived(pool_slot(order(i), y_member), py_recv.at[order(i)])
        pool_onward(order(i)).start()

    out_rows, out_columns = wo_ref.shape

    def out_slot(half, plane, yy, cc):
        first = pl.multiple_of(half * out_rows, out_rows)
        column = pl.multiple_of((plane * members + yy * 2 + cc) * out_columns, out_columns)
        return w_full.at[pl.ds(first, out_rows), pl.ds(column, out_columns)]

    def w_line(i):
        return remote(wo_ref, out_slot(tp, z, y, c), wl_send.at[i - 1], wl_recv.at[z], at(order(i), m))

    def w_line_on(i):
        there = out_slot(tp, order(i), y, c)
        return remote(there, there, wl_send.at[i], wl_recv.at[order(i)], at(order(1), m))

    def w_across(plane, own):
        there = out_slot(tp, plane, y, c)
        return remote(wo_ref if own else there, there, wy_send.at[plane], wy_recv.at[plane], y_peer)

    def w_swap(plane, yy, own):
        there = out_slot(tp, plane, yy, c)
        return remote(wo_ref if own else there, there, wx_send.at[plane, yy], wx_recv.at[plane, yy], x_peer)

    def w_beside(half, plane, yy, own):
        there = out_slot(half, plane, yy, c)
        return remote(
            wo_ref if own else there, there, wc_send.at[half, plane, yy], wc_recv.at[half, plane, yy], c_peer
        )

    def w_from_line(i):
        plane = order(i)
        arrived(out_slot(tp, plane, y, c), wl_recv.at[plane])
        w_swap(plane, y, False).start()
        w_beside(tp, plane, y, False).start()

    def w_from_pair(i):
        plane = order(i)
        arrived(out_slot(tp, plane, 1 - y, c), wy_recv.at[plane])
        w_swap(plane, 1 - y, False).start()
        w_beside(tp, plane, 1 - y, False).start()

    def w_from_swap(i):
        plane = order(i)
        for yy in (y, 1 - y):
            arrived(out_slot(1 - tp, plane, yy, c), wx_recv.at[plane, yy])
            w_beside(1 - tp, plane, yy, False).start()

    def slot(a, zz, yy, cc):
        start = pl.multiple_of((zz * members + yy * 2 + cc) * w_rows, w_rows)
        return full.at[a, pl.ds(start, w_rows), :]

    def line(a, i):
        there = slot(a, z, y, c)
        return remote(weights[a], there, line_send.at[i - 1, a], line_recv.at[z, a], at(order(i), m))

    def line_on(a, i):
        there = slot(a, order(i), y, c)
        return remote(there, there, line_send.at[i, a], line_recv.at[order(i), a], at(order(1), m))

    def y_copy(a, i, own):
        there = slot(a, order(i), y, c)
        src = weights[a] if own else there
        return remote(src, there, y_send.at[order(i), a], y_recv.at[order(i), a], y_peer)

    def c_copy(a, zz, yy, own):
        there = slot(a, zz, yy, c)
        src = weights[a] if own else there
        return remote(src, there, c_send.at[zz, yy, a], c_recv.at[zz, yy, a], c_peer)

    def c_came(a, zz, yy):
        there = slot(a, zz, yy, 1 - c)
        return remote(there, there, c_send.at[zz, yy, a], c_recv.at[zz, yy, a], c_peer)

    def from_line(i, arrays):
        zz = order(i)
        for a in arrays:
            arrived(slot(a, zz, y, c), line_recv.at[zz, a])

            @pl.when(between & (i > 1))
            def _():
                line_on(a, i).start()

            y_copy(a, i, False).start()
            c_copy(a, zz, y, False).start()

    def from_pair(i, arrays):
        zz = order(i)
        for a in arrays:
            arrived(slot(a, zz, 1 - y, c), y_recv.at[zz, a])
            c_copy(a, zz, 1 - y, False).start()

    def multiply(i, yy, arrays):
        zz = order(i)
        for a in arrays:
            c_came(a, zz, yy).wait_recv()
        piece = zz * 2 + yy
        start = pl.multiple_of(piece * 2 * w_rows, 2 * w_rows)
        for a in arrays:
            part = jnp.dot(
                pieces[piece], full[a, pl.ds(start, 2 * w_rows), :], preferred_element_type=jnp.float32
            )
            product[a] += part

    def own_weights(arrays):
        for a in arrays:
            line(a, 2).start()
            line(a, 1).start()
            y_copy(a, 0, True).start()
            c_copy(a, z, y, True).start()
            full[a, pl.ds(pl.multiple_of(sp * w_rows, w_rows), w_rows), :] = weights[a][...]

    swaps = (
        remote(tok_ref, theirs, swap_sem.at[0], swap_sem.at[1], x_peer),
        remote(gain_in, their_gain, swap_sem.at[2], swap_sem.at[3], x_peer),
    )
    own_weights(first_pair)
    for swap in swaps:
        swap.start()
    own_weights(last_one)
    w_swap(z, y, True).start()
    w_beside(tp, z, y, True).start()
    pool_beside(z, True).start()
    w_line(2).start()
    pool_line(2).start()

    @pl.when(jnp.logical_not(between))
    def _():
        w_line(1).start()
        pool_line(1).start()

    product[...] = jnp.zeros_like(product)
    acc[...] = jnp.zeros_like(acc)
    total[...] = jnp.zeros_like(total)
    top[...] = jnp.full_like(top, NEG_LARGE)
    own_pool = pl.ds(pl.multiple_of(sp * pool_rows, pool_rows), pool_rows)
    w_pool[own_pool, :] = wp_ref[...]
    w_full[
        pl.ds(pl.multiple_of(tp * out_rows, out_rows), out_rows),
        pl.ds(pl.multiple_of(sp * out_columns, out_columns), out_columns),
    ] = wo_ref[...]

    from_line(turn[1], first_pair)
    from_line(turn[2], first_pair)
    from_pair(0, first_pair)
    from_line(turn[1], last_one)
    from_line(turn[2], last_one)
    from_pair(0, last_one)
    from_line(turn[3], first_pair)
    from_pair(turn[1], first_pair)
    for swap in swaps:
        swap.wait()
    squares = jnp.zeros((rows, 1), jnp.float32)
    per_half = half_width // (2 * w_rows)
    for ref, gains, owner in ((tok_ref, gain_in, tp), (theirs, their_gain, 1 - tp)):
        for j in range(per_half):
            chunk = pl.ds(j * 2 * w_rows, 2 * w_rows)
            features = ref[:, chunk].astype(jnp.float32)
            squares += jnp.sum(features * features, axis=1, keepdims=True)
            scaled = (features * gains[:, chunk].astype(jnp.float32)).astype(jnp.bfloat16)
            pieces[owner * per_half + j] = scaled
    inverse = lax.rsqrt(squares / model_width + EPSILON)
    inverse_sc[...] = jnp.broadcast_to(inverse, inverse_sc.shape)
    every = first_pair + last_one
    multiply(0, y, every)
    multiply(0, 1 - y, every)
    from_line(turn[3], last_one)

    @pl.when(between)
    def _():
        w_line(1).start()
        pool_line(1).start()

    from_pair(turn[1], last_one)
    multiply(turn[1], y, every)
    from_pair(turn[2], first_pair)
    multiply(turn[1], 1 - y, every)
    from_pair(turn[2], last_one)
    multiply(turn[2], y, every)
    multiply(turn[2], 1 - y, every)
    multiply(turn[3], y, first_pair)
    from_pair(turn[3], first_pair)
    multiply(turn[3], 1 - y, first_pair)
    width = columns // planes
    for p in range(planes):
        part = slice(p * width, (p + 1) * width)
        k_src[p] = (product[0, :, part] * inverse_sc[:, :1]).astype(jnp.bfloat16)
        v_src[p] = (product[1, :, part] * inverse_sc[:, :1]).T.astype(jnp.bfloat16)
    k_all[z, m] = k_src[z]
    v_all[z, m] = v_src[z]
    share(z, True)
    w_across(z, True).start()
    for i in range(1, planes):
        k_out(order(i)).start()
        v_out(order(i)).start()
    from_pair(turn[3], last_one)
    multiply(turn[3], y, last_one)
    multiply(turn[3], 1 - y, last_one)
    for p in range(planes):
        part = slice(p * width, (p + 1) * width)
        query = (product[2, :, part] * inverse_sc[:, :1]).astype(jnp.bfloat16)
        q_src[p] = query * (1.0 / math.sqrt(hdim))

    q_in[z] = q_src[z]
    for i in range(1, planes):
        q_out(order(i)).start()
    w_from_line(1)
    pool_from_line(1)

    @pl.when(between)
    def _():
        for i in (2, 3):
            w_from_line(i)
            pool_from_line(i)

    def visit(block, plane, first, count, masked):
        query = q_in[block]
        lane = lax.broadcasted_iota(jnp.int32, query.shape, 1)
        none = jnp.zeros_like(query)
        both = jnp.concatenate(
            [jnp.where(lane < hdim, query, none), jnp.where(lane < hdim, none, query)], axis=0
        )
        keys = k_all[plane, pl.ds(first, count)].reshape(count * rows, 2 * hdim)
        values = jnp.concatenate([v_all[plane, first + i] for i in range(count)], axis=1)
        scores = lax.dot_general(
            keys, both, (((1,), (1,)), ((), ())), preferred_element_type=jnp.float32
        )
        if masked:
            shift = (first - m) * rows
            key = lax.broadcasted_iota(jnp.int32, scores.shape, 0)
            col = lax.broadcasted_iota(jnp.int32, scores.shape, 1)
            col = jnp.where(col < rows, col, col - rows)
            scores = jnp.where(key + shift <= col, scores, NEG_LARGE)
        old = top[block]
        new = jnp.maximum(old, jnp.max(scores, axis=0, keepdims=True))
        factor = jnp.exp(old - new)
        expo = jnp.exp(scores - new)
        acc[block] = acc[block] * factor + jnp.dot(
            values, expo.astype(jnp.bfloat16), preferred_element_type=jnp.float32
        )
        partial = jnp.sum(expo.reshape(count * rows // 8, 8, 2 * rows), axis=0)
        total[block] = total[block] * factor + partial
        top[block] = new

    def diagonal(block):
        pair = m // 2

        @pl.when(pair > 0)
        def _():
            visit(block, block, 0, members // 2, False)

        visit(block, block, pair * (members // 2), members // 2, True)

    def result_copy(block, half):
        return remote(
            done.at[block, pl.ds(pl.multiple_of(half * half_rows, half_rows), half_rows)],
            branch.at[tp * planes + z, :, pl.ds(0, vdim)],
            back_send.at[block, half],
            back_recv.at[tp * planes + z],
            at(block, m, half),
        )

    def at_home(block):
        return block == z

    def finish(block):
        both = acc[block] / jnp.sum(total[block], axis=0, keepdims=True)
        mixed = both[:, :rows] - lam_ref[z] * both[:, rows:]
        mean_sq = jnp.mean(mixed * mixed, axis=0, keepdims=True)
        normed = (mixed * lax.rsqrt(mean_sq + EPSILON)).T * gain_ref[...]
        done[block] = normed.astype(jnp.bfloat16)

        @pl.when(at_home(block))
        def _():
            kept = pl.ds(pl.multiple_of(tp * half_rows, half_rows), half_rows)
            branch[tp * planes + z, :, :vdim] = done[block, kept]

        @pl.when(jnp.logical_not(at_home(block)))
        def _():
            result_copy(block, tp).start()

        result_copy(block, 1 - tp).start()

    edge_rows = halo.shape[0]

    def edge_out():
        return remote(
            pool_sc.at[pl.ds(rows - edge_rows, edge_rows)], halo, edge_sem.at[0], edge_sem.at[1], {"sp": sp + 1}
        )

    def half_out():
        mine = pl.ds(pl.multiple_of(tp * groups, groups), groups)
        return remote(
            pooled_sc, branch.at[mine, :, pl.ds(vdim, vdim)], half_sem.at[0], half_sem.at[1], x_peer
        )

    def pool_project():
        for plane in range(planes):
            arrived(pool_slot(plane, c_member), pc_recv.at[plane, 0])
            arrived(pool_slot(plane, turned), pc_recv.at[plane, 1])
        scaled = jnp.concatenate([pieces[j] for j in range(pieces.shape[0])], axis=1)
        pool_in = jnp.dot(scaled, w_pool[...], preferred_element_type=jnp.float32)
        pool_sc[...] = (pool_in * inverse_sc[:, :1]).astype(jnp.bfloat16)

        @pl.when(sp < n_sp - 1)
        def _():
            edge_out().start()

        @pl.when(sp == 0)
        def _():
            halo[...] = jnp.zeros_like(halo)

    def pool_mix():
        @pl.when(sp > 0)
        def _():
            arrived(halo, edge_sem.at[1])

        for g in range(groups):
            part = slice(g * vdim, (g + 1) * vdim)
            own = pool_sc[:, part].astype(jnp.float32)
            running = jnp.concatenate([halo[:, part].astype(jnp.float32), own], axis=0)
            span = WINDOWS[g % len(WINDOWS)]
            step = 1
            while step < span:
                running = running + pltpu.roll(running, step, 0)
                step *= 2
            position = sp * rows + lax.broadcasted_iota(jnp.int32, own.shape, 0)
            count = jnp.minimum(position + 1, span).astype(jnp.float32)
            differ = (running[edge_rows:] / count - own).astype(jnp.bfloat16)
            pooled = jnp.dot(differ, group_ref[g], preferred_element_type=jnp.float32)
            pooled = (pooled * pscale_ref[:, part]).astype(jnp.bfloat16)
            low, high = pooled[:half_rows], pooled[half_rows:]
            branch[tp * groups + g, :, vdim:] = jnp.where(tp == 0, low, high)
            pooled_sc[g] = jnp.where(tp == 0, high, low)
        half_out().start()

    hand_on(z, True)
    landed(1)
    shared(z, True)

    def stage(i, carry):
        block = order(i)

        diagonal(block)

        @pl.when(i < planes - 2)
        def _():
            landed(i + 2)

        @pl.when(i == 0)
        def _():
            w_from_pair(0)

        @pl.when(i == 1)
        def _():
            w_across(order(1), False).start()

            @pl.when(between)
            def _():
                for j in (2, 3):
                    w_line_on(j).start()
                    w_across(order(j), False).start()
                for j in (2, 3):
                    pool_line_on(j).start()

            pool_across(z, True).start()
            pool_across(order(1), False).start()

            @pl.when(between)
            def _():
                for j in (2, 3):
                    pool_across(order(j), False).start()

        for j in (2, 3):

            @pl.when((i == j) & jnp.logical_not(between))
            def _():
                w_from_line(j)
                w_across(order(j), False).start()

        @pl.when(i == 2)
        def _():
            w_from_pair(1)

        @pl.when((i == 3) & between)
        def _():
            w_from_pair(2)

        @pl.when(i < planes - 1)
        def _():
            hand_on(order(i + 1), False)

        @pl.when(i == planes - 1)
        def _():
            finish(0)

        def pair(j, carry):
            other = jnp.where(i < planes - 1, order(j), j + upper)
            visit(jnp.maximum(block, other), jnp.minimum(block, other), 0, members, False)

            @pl.when(i == planes - 1)
            def _():
                finish(j + 1)

                @pl.when((j == 1) & between)
                def _():
                    w_from_pair(3)

                @pl.when((j == 1) & jnp.logical_not(between))
                def _():
                    w_from_pair(2)

            return carry

        lax.fori_loop(0, i, pair, 0)

        @pl.when(i < planes - 1)
        def _():
            arrived(q_in.at[order(i + 1)], z_recv.at[2, order(i + 1)])
            shared(order(i + 1), False)

        return carry

    lax.fori_loop(0, planes, stage, 0)


    @pl.when(jnp.logical_not(between))
    def _():
        for i in (2, 3):
            pool_from_line(i)
            pool_across(order(i), False).start()
        w_from_pair(3)

    for i in range(planes):
        pool_from_pair(i)
    pool_project()
    w_from_swap(0)
    pool_mix()

    for head in range(2 * planes):
        own_head = tp * planes + z == head

        @pl.when(jnp.logical_not(own_head & at_home(z)))
        def _():
            arrived(branch.at[head, :, pl.ds(0, vdim)], back_recv.at[head])

    theirs = pl.ds(pl.multiple_of((1 - tp) * groups, groups), groups)
    arrived(branch.at[theirs, :, pl.ds(vdim, vdim)], half_sem.at[1])
    left = jnp.concatenate([branch[head] for head in range(2 * planes)], axis=1)
    out_width = members * out_columns

    def column(i, carry):
        plane = order(i)

        @pl.when(i > 0)
        def _():
            w_from_swap(i)

        for half in range(2):
            for yy in range(2):
                arrived(out_slot(half, plane, yy, 1 - c), wc_recv.at[half, plane, yy])
        part = pl.ds(pl.multiple_of(plane * out_width, out_width), out_width)
        out_ref[:, part] = jnp.dot(
            left, w_full[:, part], preferred_element_type=jnp.float32
        ).astype(jnp.bfloat16)
        return carry

    lax.fori_loop(0, planes, column, 0)

    for i in range(1, planes):
        k_out(order(i)).wait_send()
        v_out(order(i)).wait_send()
        q_out(order(i)).wait_send()

    for i in range(planes):
        plane = order(i)
        for copies in in_plane(plane, i == 0):
            for copy in copies:
                copy.wait_send()
        w_across(plane, False).wait_send()
        for a in first_pair + last_one:
            y_copy(a, i, False).wait_send()
            c_copy(a, plane, y, False).wait_send()
            c_copy(a, plane, 1 - y, False).wait_send()
        for yy in (y, 1 - y):
            w_swap(plane, yy, False).wait_send()
            w_beside(0, plane, yy, False).wait_send()
            w_beside(1, plane, yy, False).wait_send()

    for i in (1, 2):
        w_line(i).wait_send()
        pool_line(i).wait_send()
        for a in first_pair + last_one:
            line(a, i).wait_send()

    @pl.when(between)
    def _():
        for i in (2, 3):
            w_line_on(i).wait_send()
            pool_line_on(i).wait_send()
            for a in first_pair + last_one:
                line_on(a, i).wait_send()

    for plane in range(planes):
        pool_across(plane, False).wait_send()
        pool_beside(plane, False).wait_send()
        pool_onward(plane).wait_send()
        result_copy(plane, 1 - tp).wait_send()

        @pl.when(jnp.logical_not(at_home(plane)))
        def _():
            result_copy(plane, tp).wait_send()

    half_out().wait_send()

    @pl.when(sp < n_sp - 1)
    def _():
        edge_out().wait_send()


def whole_layer(
    tokens,
    pre_gain,
    w_query,
    w_key,
    w_value,
    w_pool,
    lambdas,
    sub_gain,
    group_weight,
    pool_scale,
    w_out,
):
    planes = lambdas.shape[0]
    rows, half_width = tokens.shape
    n_sp = lax.axis_size("sp")
    members = n_sp // planes
    w_rows, columns = w_query.shape
    model_width = n_sp * w_rows
    width = columns // planes
    groups, vdim, _ = group_weight.shape
    out_rows, out_columns = w_out.shape
    vmem = pl.BlockSpec(memory_space=pltpu.VMEM)
    dma = pltpu.SemaphoreType.DMA
    bf16, f32 = jnp.bfloat16, jnp.float32
    work = planes * rows * members * planes * rows
    return pl.pallas_call(
        functools.partial(layer, width // 2, model_width),
        out_shape=jax.ShapeDtypeStruct((rows // 2, n_sp * out_columns), bf16),
        in_specs=[pl.BlockSpec(memory_space=pltpu.SMEM)] + [vmem] * 10,
        out_specs=vmem,
        scratch_shapes=[
            pltpu.VMEM((3, model_width, columns), bf16),
            pltpu.VMEM((rows, half_width), bf16),
            pltpu.VMEM((1, half_width), bf16),
            pltpu.VMEM((model_width // (2 * w_rows), rows, 2 * w_rows), bf16),
            pltpu.VMEM((3, rows, columns), f32),
            pltpu.VMEM((rows, 128), f32),
            pltpu.VMEM((planes, rows, width), bf16),
            pltpu.VMEM((planes, vdim, rows), bf16),
            pltpu.VMEM((planes, rows, width), bf16),
            pltpu.VMEM((planes, rows, width), bf16),
            pltpu.VMEM((planes, members, rows, width), bf16),
            pltpu.VMEM((planes, members, vdim, rows), bf16),
            pltpu.VMEM((planes, vdim, 2 * rows), f32),
            pltpu.VMEM((planes, 1, 2 * rows), f32),
            pltpu.VMEM((planes, 8, 2 * rows), f32),
            pltpu.VMEM((planes, rows, vdim), bf16),
            pltpu.VMEM((model_width, groups * vdim), bf16),
            pltpu.VMEM((2 * out_rows, n_sp * out_columns), bf16),
            pltpu.VMEM((2 * planes, rows // 2, 2 * vdim), bf16),
            pltpu.VMEM((rows, groups * vdim), bf16),
            pltpu.VMEM((RIM_ROWS + 1, groups * vdim), bf16),
            pltpu.VMEM((groups, rows // 2, vdim), bf16),
            dma((planes, 3)),
            dma((planes, 3)),
            dma((planes, 3)),
            dma((planes, 3)),
            dma((planes, 2, 3)),
            dma((planes, 2, 3)),
            dma((4,)),
            dma((3, planes)),
            dma((3, planes)),
            dma((planes, 3, 2)),
            dma((planes, 3, 2)),
            dma((planes, 2)),
            dma((2 * planes,)),
            dma((planes,)),
            dma((planes,)),
            dma((planes, 2)),
            dma((planes, 2)),
            dma((2,)),
            dma((2,)),
            dma((planes,)),
            dma((planes,)),
            dma((planes,)),
            dma((planes,)),
            dma((planes,)),
            dma((planes,)),
            dma((planes, 2)),
            dma((planes, 2)),
            dma((2, planes, 2)),
            dma((2, planes, 2)),
        ],
        compiler_params=pltpu.CompilerParams(
            vmem_limit_bytes=60 * 2**20, collective_id=2, has_side_effects=True
        ),
        cost_estimate=pl.CostEstimate(
            flops=4 * work * vdim, bytes_accessed=2**24, transcendentals=work
        ),
    )(
        lambdas,
        tokens,
        pre_gain.reshape(1, -1),
        w_key,
        w_value,
        w_query,
        w_pool,
        sub_gain.reshape(1, -1),
        group_weight,
        pool_scale.reshape(1, -1),
        w_out,
    )


def trailing(x, window_ids, group_dim):
    column_window = jnp.repeat(window_ids, group_dim)[None, :]
    running = x
    picked = jnp.zeros_like(x)
    for slot, span in enumerate(WINDOWS):
        half = span // 2
        running = running + jnp.pad(running[:-half], ((half, 0), (0, 0)))
        picked = jnp.where(column_window == slot, running, picked)
    return picked


def general_attention(queries, key_rows, values, lambdas, sub_gain):
    n_sp = lax.axis_size("sp")
    sp = lax.axis_index("sp")
    tok_rows = queries.shape[0]
    heads = lambdas.shape[0]
    qdim = queries.shape[1] // heads
    vdim = values.shape[1] // heads
    head_width = 2 * qdim + vdim
    outer = math.gcd(n_sp, heads)
    inner = n_sp // outer
    per_device = heads // outer
    by_head = jnp.concatenate(
        [
            x.reshape(tok_rows, heads, -1).swapaxes(0, 1)
            for x in (queries, key_rows, values)
        ],
        axis=2,
    )
    across = [[o * inner + i for o in range(outer)] for i in range(inner)]
    within = [[o * inner + i for i in range(inner)] for o in range(outer)]
    by_head = by_head.reshape(outer, per_device, tok_rows, head_width)
    if outer > 1:
        by_head = lax.all_to_all(by_head, "sp", 0, 0, axis_index_groups=across)
    first_head = lax.div(sp, inner) * per_device
    attended = []
    if inner == 4 and per_device == 1:
        lam = lax.dynamic_slice_in_dim(lambdas, first_head, 1)
        attended.append(
            flash_members(by_head[:, 0, :, :qdim], by_head[:, 0, :, qdim:], lam, sub_gain)
        )
    else:
        kv = lax.all_gather(by_head[..., qdim:], "sp", axis=0, axis_index_groups=within)
        member = lax.rem(sp, inner).reshape(1)
        for p in range(per_device):
            lam = lax.dynamic_slice_in_dim(lambdas, first_head + p, 1)
            attended.append(flash(by_head[:, p, :, :qdim], kv[:, :, p], member, lam, sub_gain))
    attended = jnp.stack(attended, axis=1)
    if outer > 1:
        attended = lax.all_to_all(attended, "sp", 0, 0, axis_index_groups=across)
    return attended.reshape(heads, tok_rows, vdim)


def local(
    tokens,
    pre_gain,
    w_query,
    w_key,
    w_value,
    w_pool,
    lambdas,
    sub_gain,
    group_weight,
    pool_scale,
    w_out,
):
    n_tp = lax.axis_size("tp")
    n_sp = lax.axis_size("sp")
    tp = lax.axis_index("tp")
    sp = lax.axis_index("sp")
    tok_rows = tokens.shape[0]
    model_width = tokens.shape[1] * n_tp
    heads = lambdas.shape[0]
    qdim = w_query.shape[1] // heads
    vdim = w_value.shape[1] // heads
    groups = group_weight.shape[0]
    group_dim = group_weight.shape[1]

    shaped_for_mix = n_tp == 2 and heads == 4 and n_sp == 4 * heads and tok_rows % 32 == 0
    if shaped_for_mix and qdim == vdim == group_dim and groups == heads:
        return whole_layer(
            tokens,
            pre_gain,
            w_query,
            w_key,
            w_value,
            w_pool,
            lambdas,
            sub_gain,
            group_weight,
            pool_scale,
            w_out,
        )
    swap = [(0, 1), (1, 0)]
    w_sorted = w_out.reshape(heads, 2, vdim, -1).swapaxes(0, 1).reshape(w_out.shape)
    features = tokens.astype(jnp.float32)
    mine = (features * pre_gain.astype(jnp.float32)[None, :]).astype(jnp.bfloat16)
    squares = jnp.sum(features * features, axis=1, keepdims=True)
    weights = [w_query, w_key, w_value, w_pool]
    if n_sp % 4 == 0:
        *weights, theirs = gather_weights(weights, mine, n_tp == 2)
    else:
        weights = [lax.all_gather(w, "sp", axis=0, tiled=True) for w in weights]
        theirs = lax.ppermute(mine, "tp", swap) if n_tp == 2 else mine
    w_sorted, weights = lax.optimization_barrier((w_sorted, weights))
    w_out_rows = lax.all_gather(w_sorted, "sp", axis=1, tiled=True)
    if n_tp == 2:
        squares = squares + lax.ppermute(squares, "tp", swap)
        scaled = jnp.concatenate(
            [jnp.where(tp == 0, mine, theirs), jnp.where(tp == 0, theirs, mine)], axis=1
        )
    else:
        scaled = lax.all_gather(mine, "tp", axis=1, tiled=True)
        squares = lax.psum(squares, "tp")
    inverse = lax.rsqrt(squares / model_width + EPSILON)
    queries, key_rows, values, pool_in = [
        (jnp.dot(scaled, w, preferred_element_type=jnp.float32) * inverse).astype(jnp.bfloat16)
        for w in weights
    ]
    attended = general_attention(queries, key_rows, values, lambdas, sub_gain)

    halo = passed_along(pool_in[tok_rows - RIM_ROWS - 1 :], "sp", 1)
    extended = jnp.concatenate([halo, pool_in], axis=0).astype(jnp.float32)
    window_ids = (tp * groups + jnp.arange(groups, dtype=jnp.int32)) % len(WINDOWS)
    sums = trailing(extended, window_ids, group_dim)[RIM_ROWS + 1 :]
    spans = jnp.repeat(jnp.left_shift(2, window_ids), group_dim)
    positions = sp * tok_rows + jnp.arange(tok_rows, dtype=jnp.int32)
    count = jnp.minimum(positions[:, None] + 1, spans[None, :]).astype(jnp.float32)
    differ = (sums / count - pool_in.astype(jnp.float32)).astype(jnp.bfloat16)
    pooled = jnp.einsum(
        "tgc,gcd->tgd",
        differ.reshape(tok_rows, groups, group_dim),
        group_weight,
        preferred_element_type=jnp.float32,
    )
    pooled = (pooled * pool_scale.reshape(groups, group_dim)).astype(jnp.bfloat16)
    branch = jnp.concatenate(
        [attended.swapaxes(0, 1).reshape(tok_rows, -1), pooled.reshape(tok_rows, -1)], axis=1
    )
    if n_tp == 2:
        half = tok_rows // 2
        send = lax.dynamic_slice_in_dim(branch, (1 - tp) * half, half, 0)
        send = jnp.dot(send, w_out_rows, preferred_element_type=jnp.float32).astype(jnp.bfloat16)
        got = lax.ppermute(send, "tp", swap)
        keep = lax.dynamic_slice_in_dim(branch, tp * half, half, 0)
        keep = jnp.dot(keep, w_out_rows, preferred_element_type=jnp.float32)
        return (keep + got.astype(jnp.float32)).astype(jnp.bfloat16)
    partial = jnp.dot(branch, w_out_rows, preferred_element_type=jnp.float32)
    return lax.psum_scatter(partial.astype(jnp.bfloat16), "tp", scatter_dimension=0, tiled=True)


def solution(mesh):
    placed = (
        P("sp", "tp"),
        P("tp"),
        P("sp", "tp"),
        P("sp", "tp"),
        P("sp", "tp"),
        P("sp", "tp"),
        P("tp"),
        P(),
        P("tp", None, None),
        P("tp"),
        P("tp", "sp"),
    )
    return jax.shard_map(
        local, mesh=mesh, in_specs=placed, out_specs=P(("sp", "tp"), None), check_vma=False
    )
```

```python
import functools
import math

import jax
import jax.numpy as jnp
from jax import lax
from jax.experimental import pallas as pl
from jax.experimental.pallas import tpu as pltpu
from jax.sharding import PartitionSpec as P

EPSILON = 1e-06
NEG_LARGE = -1e30
WINDOWS = (2, 4, 8, 16)
RIM_ROWS = 15


def passed_along(block, axis, distance):
    devices = range(lax.axis_size(axis))
    route = [(i - distance, i) for i in devices if i - distance in devices]
    return lax.ppermute(block, axis, route)


def attend(inner, vdim, hdim, member_ref, lam_ref, q_ref, kv_ref, gain_ref, out_ref, acc_ref, max_ref):
    rows = q_ref.shape[1]
    block = pl.program_id(0)
    last = block * inner + member_ref[0]
    scale = 1.0 / math.sqrt(hdim)
    queries = (q_ref[0].astype(jnp.float32) * scale).astype(jnp.bfloat16)
    maps = (queries[:, :hdim], queries[:, hdim:])
    ones = jnp.ones((rows, vdim), jnp.bfloat16)
    acc_ref[...] = jnp.zeros_like(acc_ref)
    max_ref[...] = jnp.full_like(max_ref, NEG_LARGE)

    def step(g, masked):
        keys_values = kv_ref[lax.rem(g, inner), lax.div(g, inner)]
        values = jnp.concatenate([keys_values[:, 2 * hdim :], ones], axis=1)
        for m in range(2):
            keys = keys_values[:, m * hdim : (m + 1) * hdim]
            scores = lax.dot_general(
                maps[m], keys, (((1,), (1,)), ((), ())), preferred_element_type=jnp.float32
            )
            if masked:
                row = lax.broadcasted_iota(jnp.int32, scores.shape, 0)
                col = lax.broadcasted_iota(jnp.int32, scores.shape, 1)
                scores = jnp.where(col <= row, scores, NEG_LARGE)
            old_max = max_ref[m]
            new_max = jnp.maximum(old_max, jnp.max(scores, axis=1, keepdims=True))
            factor = jnp.exp(old_max - new_max)
            expo = jnp.exp(scores - new_max[:, :1])
            acc_ref[m] = acc_ref[m] * factor[:, :1] + jnp.dot(
                expo.astype(jnp.bfloat16), values, preferred_element_type=jnp.float32
            )
            max_ref[m] = new_max

    def body(g, carry):
        step(g, False)
        return carry

    lax.fori_loop(0, last, body, 0)
    step(last, True)
    first = acc_ref[0]
    second = acc_ref[1]
    mix = first[:, :vdim] / first[:, vdim:] - lam_ref[0] * (second[:, :vdim] / second[:, vdim:])
    mean_sq = jnp.mean(mix * mix, axis=1, keepdims=True)
    out_ref[0] = (mix * lax.rsqrt(mean_sq + EPSILON) * gain_ref[...]).astype(jnp.bfloat16)


def flash(q, kv, member, lam, sub_gain):
    inner, outer, rows, width = kv.shape
    qdim = q.shape[-1]
    vdim = width - qdim
    smem = pl.BlockSpec(memory_space=pltpu.SMEM)
    work = outer * rows * outer * rows * inner
    return pl.pallas_call(
        functools.partial(attend, inner, vdim, qdim // 2),
        grid=(outer,),
        out_shape=jax.ShapeDtypeStruct((outer, rows, vdim), jnp.bfloat16),
        in_specs=[
            smem,
            smem,
            pl.BlockSpec((1, rows, qdim), lambda b: (b, 0, 0)),
            pl.BlockSpec(memory_space=pltpu.VMEM),
            pl.BlockSpec(memory_space=pltpu.VMEM),
        ],
        out_specs=pl.BlockSpec((1, rows, vdim), lambda b: (b, 0, 0)),
        scratch_shapes=[
            pltpu.VMEM((2, rows, 2 * vdim), jnp.float32),
            pltpu.VMEM((2, rows, 128), jnp.float32),
        ],
        compiler_params=pltpu.CompilerParams(vmem_limit_bytes=56 * 2**20),
        cost_estimate=pl.CostEstimate(
            flops=4 * work * vdim, bytes_accessed=kv.size * 2, transcendentals=work
        ),
    )(member, lam, q, kv, sub_gain.reshape(1, -1))


def attend_members(hdim, lam_ref, q_ref, own_ref, gain_ref, out_ref, held, acc_ref, max_ref, send, recv):
    outer, rows, _ = q_ref.shape
    vdim = own_ref.shape[2] - 2 * hdim
    sp = lax.axis_index("sp")
    member = lax.rem(sp, 4)
    y = lax.div(member, 2)
    c = lax.rem(member, 2)
    y_peer = sp + 2 - 4 * y
    c_peer = sp + 1 - 2 * c
    barrier = pltpu.get_barrier_semaphore()
    for peer in (y_peer, c_peer):
        pl.semaphore_signal(
            barrier, 1, device_id={"sp": peer}, device_id_type=pl.DeviceIdType.MESH
        )
    pl.semaphore_wait(barrier, 2)

    def remote(src, index, peer):
        return pltpu.make_async_remote_copy(
            src_ref=src,
            dst_ref=held.at[index],
            send_sem=send.at[index],
            recv_sem=recv.at[index],
            device_id={"sp": peer},
            device_id_type=pl.DeviceIdType.MESH,
        )

    across = remote(own_ref, 1, y_peer)
    beside = remote(own_ref, 0, c_peer)
    onward = remote(held.at[1], 2, c_peer)
    across.start()
    beside.start()
    acc_ref[...] = jnp.zeros_like(acc_ref)
    max_ref[...] = jnp.full_like(max_ref, NEG_LARGE)
    scale = 1.0 / math.sqrt(hdim)

    def visit(ref, other):
        shift = (member - other) * rows
        for block in range(outer):
            queries = (q_ref[block].astype(jnp.float32) * scale).astype(jnp.bfloat16)
            length = (block + 1) * rows
            keys_values = ref[: block + 1].reshape(length, 2 * hdim + vdim)
            values = jnp.concatenate(
                [keys_values[:, 2 * hdim :], jnp.ones((length, vdim), jnp.bfloat16)], axis=1
            )
            for m in range(2):
                scores = lax.dot_general(
                    queries[:, m * hdim : (m + 1) * hdim],
                    keys_values[:, m * hdim : (m + 1) * hdim],
                    (((1,), (1,)), ((), ())),
                    preferred_element_type=jnp.float32,
                )
                edge = scores[:, block * rows :]
                row = lax.broadcasted_iota(jnp.int32, edge.shape, 0)
                col = lax.broadcasted_iota(jnp.int32, edge.shape, 1)
                edge = jnp.where(col <= row + shift, edge, NEG_LARGE)
                if block > 0:
                    scores = jnp.concatenate([scores[:, : block * rows], edge], axis=1)
                else:
                    scores = edge
                old_max = max_ref[block, m]
                new_max = jnp.maximum(old_max, jnp.max(scores, axis=1, keepdims=True))
                factor = jnp.exp(old_max - new_max)
                expo = jnp.exp(scores - new_max[:, :1])
                acc_ref[block, m] = acc_ref[block, m] * factor[:, :1] + jnp.dot(
                    expo.astype(jnp.bfloat16), values, preferred_element_type=jnp.float32
                )
                max_ref[block, m] = new_max

    visit(own_ref, member)

    def arrived(j, carry):
        @pl.when(j == 0)
        def _():
            beside.wait_recv()

        @pl.when(j == 1)
        def _():
            across.wait_recv()
            onward.start()

        @pl.when(j == 2)
        def _():
            onward.wait_recv()

        other_y = jnp.where(j >= 1, 1 - y, y)
        other_c = jnp.where(j == 1, c, 1 - c)
        visit(held.at[j], 2 * other_y + other_c)
        return carry

    lax.fori_loop(0, 3, arrived, 0)
    for copy in (across, beside, onward):
        copy.wait_send()
    for block in range(outer):
        first = acc_ref[block, 0]
        second = acc_ref[block, 1]
        mix = first[:, :vdim] / first[:, vdim:]
        mix = mix - lam_ref[0] * (second[:, :vdim] / second[:, vdim:])
        mean_sq = jnp.mean(mix * mix, axis=1, keepdims=True)
        normed = mix * lax.rsqrt(mean_sq + EPSILON) * gain_ref[...]
        out_ref[block] = normed.astype(jnp.bfloat16)


def flash_members(q, kv, lam, sub_gain):
    outer, rows, width = kv.shape
    qdim = q.shape[-1]
    vdim = width - qdim
    vmem = pl.BlockSpec(memory_space=pltpu.VMEM)
    work = 4 * outer * rows * outer * rows
    return pl.pallas_call(
        functools.partial(attend_members, qdim // 2),
        out_shape=jax.ShapeDtypeStruct((outer, rows, vdim), jnp.bfloat16),
        in_specs=[pl.BlockSpec(memory_space=pltpu.SMEM), vmem, vmem, vmem],
        out_specs=vmem,
        scratch_shapes=[
            pltpu.VMEM((3, outer, rows, width), jnp.bfloat16),
            pltpu.VMEM((outer, 2, rows, 2 * vdim), jnp.float32),
            pltpu.VMEM((outer, 2, rows, 128), jnp.float32),
            pltpu.SemaphoreType.DMA((3,)),
            pltpu.SemaphoreType.DMA((3,)),
        ],
        compiler_params=pltpu.CompilerParams(
            vmem_limit_bytes=56 * 2**20, collective_id=1, has_side_effects=True
        ),
        cost_estimate=pl.CostEstimate(
            flops=4 * work * vdim, bytes_accessed=4 * kv.size * 2, transcendentals=work
        ),
    )(lam, q, kv, sub_gain.reshape(1, -1))


def spread(n_sp, count, with_swap, *refs):
    weights, refs = refs[:count], refs[count:]
    mine, refs = refs[0], refs[1:]
    fulls, refs = refs[:count], refs[count:]
    theirs, refs = refs[0], refs[1:]
    up_send, up_recv, down_send, down_recv, y_send, y_recv, c_send, c_recv, own_sem, swap_sem = refs
    depth = n_sp // 4
    rows = weights[0].shape[0]
    sp = lax.axis_index("sp")
    z = lax.div(sp, 4)
    y = lax.rem(lax.div(sp, 2), 2)
    c = lax.rem(sp, 2)
    y_peer = z * 4 + (1 - y) * 2 + c
    c_peer = z * 4 + y * 2 + (1 - c)
    barrier = pltpu.get_barrier_semaphore()

    def greet(device):
        pl.semaphore_signal(barrier, 1, device_id=device, device_id_type=pl.DeviceIdType.MESH)

    greet({"sp": y_peer})
    greet({"sp": c_peer})
    greeted = 2
    if with_swap:
        greet({"tp": 1 - lax.axis_index("tp")})
        greeted = 3

    @pl.when(z > 0)
    def _():
        greet({"sp": sp - 4})

    @pl.when(z < depth - 1)
    def _():
        greet({"sp": sp + 4})

    in_line = jnp.where(z > 0, 1, 0) + jnp.where(z < depth - 1, 1, 0)
    pl.semaphore_wait(barrier, greeted + in_line)

    def slot(a, zz, yy, cc):
        start = pl.multiple_of((zz * 4 + yy * 2 + cc) * rows, rows)
        return fulls[a].at[pl.ds(start, rows), :]

    def remote(src, dst, send, recv, device):
        return pltpu.make_async_remote_copy(
            src_ref=src,
            dst_ref=dst,
            send_sem=send,
            recv_sem=recv,
            device_id=device,
            device_id_type=pl.DeviceIdType.MESH,
        )

    def line_copy(side, k, a, src):
        sends, recvs = (up_send, up_recv) if side > 0 else (down_send, down_recv)
        there = slot(a, z - side * k, y, c)
        return remote(
            there if src is None else src,
            there,
            sends.at[k, a],
            recvs.at[k + 1, a],
            {"sp": sp + 4 * side},
        )

    def y_copy(zz, yy, a, src):
        there = slot(a, zz, yy, c)
        src = there if src is None else src
        return remote(src, there, y_send.at[zz, a], y_recv.at[zz, a], {"sp": y_peer})

    def c_copy(zz, yy, cc, a, src):
        there = slot(a, zz, yy, cc)
        src = there if src is None else src
        return remote(src, there, c_send.at[zz, yy, a], c_recv.at[zz, yy, a], {"sp": c_peer})

    def can_go(side):
        return z < depth - 1 if side > 0 else z > 0

    def came(side, k):
        return z >= k if side > 0 else z + k <= depth - 1

    if with_swap:
        swap = remote(
            mine, theirs, swap_sem.at[0], swap_sem.at[1], {"tp": 1 - lax.axis_index("tp")}
        )
        swap.start()
    for a in range(count):
        for side in (1, -1):

            @pl.when(can_go(side))
            def _():
                line_copy(side, 0, a, weights[a]).start()

        y_copy(z, y, a, weights[a]).start()
    for a in range(count):
        c_copy(z, y, c, a, weights[a]).start()
        pltpu.make_async_copy(weights[a], slot(a, z, y, c), own_sem.at[a]).start()

    def from_pair(zz):
        for a in range(count):
            y_copy(zz, 1 - y, a, None).wait_recv()
            c_copy(zz, 1 - y, c, a, None).start()

    def relay(k, carry):
        for side in (1, -1):
            recvs = up_recv if side > 0 else down_recv

            @pl.when(came(side, k))
            def _():
                zz = z - side * k
                for a in range(count):
                    there = slot(a, zz, y, c)
                    remote(there, there, up_send.at[0, a], recvs.at[k, a], {"sp": y_peer}).wait_recv()

                    @pl.when(can_go(side))
                    def _():
                        line_copy(side, k, a, None).start()

                    y_copy(zz, y, a, None).start()
                    c_copy(zz, y, c, a, None).start()

        @pl.when(k == 1)
        def _():
            from_pair(z)

        for side in (1, -1):

            @pl.when((k > 1) & came(side, k - 1))
            def _():
                from_pair(z - side * (k - 1))

        return carry

    lax.fori_loop(1, depth, relay, 0)
    if depth == 1:
        from_pair(z)
    for side in (1, -1):
        if depth > 1:

            @pl.when(came(side, depth - 1))
            def _():
                from_pair(z - side * (depth - 1))

    def drain(zz, carry):
        for a in range(count):
            y_copy(zz, y, a, None).wait_send()
            for yy in range(2):
                c_copy(zz, yy, 1 - c, a, None).wait_recv()
                c_copy(zz, yy, c, a, None).wait_send()
        return carry

    lax.fori_loop(0, depth, drain, 0)

    def drain_line(k, carry):
        for side in (1, -1):

            @pl.when(came(side, k) & can_go(side))
            def _():
                for a in range(count):
                    line_copy(side, k, a, None).wait_send()

        return carry

    lax.fori_loop(0, depth, drain_line, 0)
    for a in range(count):
        pltpu.make_async_copy(weights[a], slot(a, z, y, c), own_sem.at[a]).wait()
    if with_swap:
        swap.wait()


def gather_weights(weights, mine, with_swap):
    n_sp = lax.axis_size("sp")
    count = len(weights)
    depth = n_sp // 4
    sems = pltpu.SemaphoreType.DMA
    any_spec = pl.BlockSpec(memory_space=pl.ANY)
    vmem_spec = pl.BlockSpec(memory_space=pltpu.VMEM)
    shapes = [jax.ShapeDtypeStruct((n_sp * w.shape[0], w.shape[1]), w.dtype) for w in weights]
    shapes.append(jax.ShapeDtypeStruct(mine.shape, mine.dtype))
    moved = sum(w.size for w in weights) * 2 * n_sp
    return pl.pallas_call(
        functools.partial(spread, n_sp, count, with_swap),
        out_shape=shapes,
        in_specs=[vmem_spec] * (count + 1),
        out_specs=[any_spec] * (count + 1),
        scratch_shapes=[
            sems((depth + 1, count)),
            sems((depth + 1, count)),
            sems((depth + 1, count)),
            sems((depth + 1, count)),
            sems((depth, count)),
            sems((depth, count)),
            sems((depth, 2, count)),
            sems((depth, 2, count)),
            sems((count,)),
            sems((2,)),
        ],
        compiler_params=pltpu.CompilerParams(collective_id=0, has_side_effects=True),
        cost_estimate=pl.CostEstimate(flops=10**10, bytes_accessed=moved, transcendentals=0),
    )(*weights, mine)


def arrival(z, i):
    half = z // 2
    later = jnp.where(i == 2, 2 - half, 3 - 3 * half)
    return jnp.where(i == 0, z, jnp.where(i == 1, 1 + 4 * half - z, later))


def layer(
    hdim,
    model_width,
    lam_ref,
    tok_ref,
    gain_in,
    wk_ref,
    wv_ref,
    wq_ref,
    wp_ref,
    gain_ref,
    group_ref,
    pscale_ref,
    wo_ref,
    out_ref,
    full,
    theirs,
    their_gain,
    pieces,
    product,
    inverse_sc,
    k_src,
    v_src,
    q_src,
    q_in,
    k_all,
    v_all,
    acc,
    top,
    total,
    done,
    w_pool,
    w_full,
    branch,
    pool_sc,
    halo,
    pooled_sc,
    *sems,
):
    (line_send, line_recv, y_send, y_recv, c_send, c_recv, swap_sem) = sems[:7]
    (z_send, z_recv, in_send, in_recv, back_send, back_recv) = sems[7:13]
    (py_send, py_recv, pc_send, pc_recv, edge_sem, half_sem, pool_send, pool_recv) = sems[13:21]
    (wl_send, wl_recv, wy_send, wy_recv, wx_send, wx_recv, wc_send, wc_recv) = sems[21:]
    weights = (wk_ref, wv_ref, wq_ref)
    first_pair, last_one = (0, 1), (2,)
    planes, rows, _ = q_src.shape
    vdim = v_src.shape[1]
    members = k_all.shape[1]
    w_rows, columns = wq_ref.shape
    half_width = tok_ref.shape[1]
    groups = group_ref.shape[0]
    half_rows = rows // 2
    sp = lax.axis_index("sp")
    tp = lax.axis_index("tp")
    n_sp = lax.axis_size("sp")
    z = sp // members
    m = sp % members
    y = m // 2
    c = m % 2
    y_member = (m + 2) % members
    c_member = m + 1 - 2 * c
    turned = members - 1 - m
    upper = z // 2
    between = (z > 0) & (z < planes - 1)
    turn = [jnp.where(between, 1 + i % 3, i) for i in range(planes)]
    turn[0] = 0

    def at(plane, member, half=None):
        device = {"sp": plane * members + member}
        if half is not None:
            device["tp"] = half
        return device

    y_peer = at(z, y_member)
    c_peer = at(z, c_member)
    x_peer = {"tp": 1 - tp}

    def order(i):
        return arrival(z, i)

    barrier = pltpu.get_barrier_semaphore()

    def greet(device):
        pl.semaphore_signal(barrier, 1, device_id=device, device_id_type=pl.DeviceIdType.MESH)

    for i in range(1, planes):
        greet(at(order(i), m))
    for member in range(1, members):
        greet(at(z, (m + member) % members))
    for plane in range(planes):
        greet(at(plane, m, 1 - tp))

    @pl.when((m == 0) & (z > 0))
    def _():
        greet({"sp": sp - 1})

    @pl.when((m == members - 1) & (z < planes - 1))
    def _():
        greet({"sp": sp + 1})

    beyond = jnp.where((m == 0) & (z > 0), 1, 0)
    beyond += jnp.where((m == members - 1) & (z < planes - 1), 1, 0)
    pl.semaphore_wait(barrier, 2 * planes + members - 2 + beyond)

    def remote(src, dst, send, recv, device):
        return pltpu.make_async_remote_copy(
            src_ref=src,
            dst_ref=dst,
            send_sem=send,
            recv_sem=recv,
            device_id=device,
            device_id_type=pl.DeviceIdType.MESH,
        )

    def arrived(ref, recv):
        remote(ref, ref, recv, recv, c_peer).wait_recv()

    def k_out(plane):
        return remote(k_src.at[plane], k_all.at[z, m], z_send.at[0, plane], z_recv.at[0, z], at(plane, m))

    def v_out(plane):
        return remote(v_src.at[plane], v_all.at[z, m], z_send.at[1, plane], z_recv.at[1, z], at(plane, m))

    def q_out(plane):
        return remote(
            q_src.at[plane], q_in.at[z], z_send.at[2, plane], z_recv.at[2, z], at(plane, m)
        )

    def in_plane(plane, own):
        copies = []
        for t, (mine, everyone) in enumerate(((k_src, k_all), (v_src, v_all))):
            src = mine.at[plane] if own else everyone.at[plane, m]
            there = everyone.at[plane, m]
            passed = everyone.at[plane, y_member]
            copies.append(
                [
                    remote(src, there, in_send.at[plane, 0, t], in_recv.at[plane, 0, t], y_peer),
                    remote(src, there, in_send.at[plane, 1, t], in_recv.at[plane, 1, t], c_peer),
                    remote(passed, passed, in_send.at[plane, 2, t], in_recv.at[plane, 2, t], c_peer),
                ]
            )
        return copies

    def share(plane, own):
        for copies in in_plane(plane, own):
            copies[0].start()
            copies[1].start()

    def hand_on(plane, own):
        for copies in in_plane(plane, own):
            copies[0].wait_recv()
            copies[2].start()

    def shared(plane, own):
        for copies in in_plane(plane, own):
            copies[1].wait_recv()
            copies[2].wait_recv()

    def landed(i):
        plane = order(i)
        arrived(k_all.at[plane, m], z_recv.at[0, plane])
        arrived(v_all.at[plane, m], z_recv.at[1, plane])
        share(plane, False)

    pool_rows = wp_ref.shape[0]

    def pool_slot(plane, member):
        start = pl.multiple_of((plane * members + member) * pool_rows, pool_rows)
        return w_pool.at[pl.ds(start, pool_rows), :]

    def pool_line(i):
        return remote(wp_ref, pool_slot(z, m), pool_send.at[i - 1], pool_recv.at[z], at(order(i), m))

    def pool_line_on(i):
        there = pool_slot(order(i), m)
        return remote(there, there, pool_send.at[i], pool_recv.at[order(i)], at(order(1), m))

    def pool_across(plane, own):
        there = pool_slot(plane, m)
        return remote(wp_ref if own else there, there, py_send.at[plane], py_recv.at[plane], y_peer)

    def pool_beside(plane, own):
        there = pool_slot(plane, m)
        return remote(wp_ref if own else there, there, pc_send.at[plane, 0], pc_recv.at[plane, 0], c_peer)

    def pool_onward(plane):
        passed = pool_slot(plane, y_member)
        return remote(passed, passed, pc_send.at[plane, 1], pc_recv.at[plane, 1], c_peer)

    def pool_from_line(i):
        plane = order(i)
        arrived(pool_slot(plane, m), pool_recv.at[plane])
        pool_beside(plane, False).start()

    def pool_from_pair(i):
        arrived(pool_slot(order(i), y_member), py_recv.at[order(i)])
        pool_onward(order(i)).start()

    out_rows, out_columns = wo_ref.shape

    def out_slot(half, plane, yy, cc):
        first = pl.multiple_of(half * out_rows, out_rows)
        column = pl.multiple_of((plane * members + yy * 2 + cc) * out_columns, out_columns)
        return w_full.at[pl.ds(first, out_rows), pl.ds(column, out_columns)]

    def w_line(i):
        return remote(wo_ref, out_slot(tp, z, y, c), wl_send.at[i - 1], wl_recv.at[z], at(order(i), m))

    def w_line_on(i):
        there = out_slot(tp, order(i), y, c)
        return remote(there, there, wl_send.at[i], wl_recv.at[order(i)], at(order(1), m))

    def w_across(plane, own):
        there = out_slot(tp, plane, y, c)
        return remote(wo_ref if own else there, there, wy_send.at[plane], wy_recv.at[plane], y_peer)

    def w_swap(plane, yy, own):
        there = out_slot(tp, plane, yy, c)
        return remote(wo_ref if own else there, there, wx_send.at[plane, yy], wx_recv.at[plane, yy], x_peer)

    def w_beside(half, plane, yy, own):
        there = out_slot(half, plane, yy, c)
        return remote(
            wo_ref if own else there, there, wc_send.at[half, plane, yy], wc_recv.at[half, plane, yy], c_peer
        )

    def w_from_line(i):
        plane = order(i)
        arrived(out_slot(tp, plane, y, c), wl_recv.at[plane])
        w_swap(plane, y, False).start()
        w_beside(tp, plane, y, False).start()

    def w_from_pair(i):
        plane = order(i)
        arrived(out_slot(tp, plane, 1 - y, c), wy_recv.at[plane])
        w_swap(plane, 1 - y, False).start()
        w_beside(tp, plane, 1 - y, False).start()

    def w_from_swap(i):
        plane = order(i)
        for yy in (y, 1 - y):
            arrived(out_slot(1 - tp, plane, yy, c), wx_recv.at[plane, yy])
            w_beside(1 - tp, plane, yy, False).start()

    def slot(a, zz, yy, cc):
        start = pl.multiple_of((zz * members + yy * 2 + cc) * w_rows, w_rows)
        return full.at[a, pl.ds(start, w_rows), :]

    def line(a, i):
        there = slot(a, z, y, c)
        return remote(weights[a], there, line_send.at[i - 1, a], line_recv.at[z, a], at(order(i), m))

    def line_on(a, i):
        there = slot(a, order(i), y, c)
        return remote(there, there, line_send.at[i, a], line_recv.at[order(i), a], at(order(1), m))

    def y_copy(a, i, own):
        there = slot(a, order(i), y, c)
        src = weights[a] if own else there
        return remote(src, there, y_send.at[order(i), a], y_recv.at[order(i), a], y_peer)

    def c_copy(a, zz, yy, own):
        there = slot(a, zz, yy, c)
        src = weights[a] if own else there
        return remote(src, there, c_send.at[zz, yy, a], c_recv.at[zz, yy, a], c_peer)

    def c_came(a, zz, yy):
        there = slot(a, zz, yy, 1 - c)
        return remote(there, there, c_send.at[zz, yy, a], c_recv.at[zz, yy, a], c_peer)

    def from_line(i, arrays):
        zz = order(i)
        for a in arrays:
            arrived(slot(a, zz, y, c), line_recv.at[zz, a])

            @pl.when(between & (i > 1))
            def _():
                line_on(a, i).start()

            y_copy(a, i, False).start()
            c_copy(a, zz, y, False).start()

    def from_pair(i, arrays):
        zz = order(i)
        for a in arrays:
            arrived(slot(a, zz, 1 - y, c), y_recv.at[zz, a])
            c_copy(a, zz, 1 - y, False).start()

    def multiply(i, yy, arrays):
        zz = order(i)
        for a in arrays:
            c_came(a, zz, yy).wait_recv()
        piece = zz * 2 + yy
        start = pl.multiple_of(piece * 2 * w_rows, 2 * w_rows)
        for a in arrays:
            part = jnp.dot(
                pieces[piece], full[a, pl.ds(start, 2 * w_rows), :], preferred_element_type=jnp.float32
            )
            product[a] += part

    def own_weights(arrays):
        for a in arrays:
            line(a, 2).start()
            line(a, 1).start()
            y_copy(a, 0, True).start()
            c_copy(a, z, y, True).start()
            full[a, pl.ds(pl.multiple_of(sp * w_rows, w_rows), w_rows), :] = weights[a][...]

    swaps = (
        remote(tok_ref, theirs, swap_sem.at[0], swap_sem.at[1], x_peer),
        remote(gain_in, their_gain, swap_sem.at[2], swap_sem.at[3], x_peer),
    )
    own_weights(first_pair)
    for swap in swaps:
        swap.start()
    own_weights(last_one)
    w_swap(z, y, True).start()
    w_beside(tp, z, y, True).start()
    pool_beside(z, True).start()
    w_line(2).start()
    pool_line(2).start()

    @pl.when(jnp.logical_not(between))
    def _():
        w_line(1).start()
        pool_line(1).start()

    product[...] = jnp.zeros_like(product)
    acc[...] = jnp.zeros_like(acc)
    total[...] = jnp.zeros_like(total)
    top[...] = jnp.full_like(top, NEG_LARGE)
    own_pool = pl.ds(pl.multiple_of(sp * pool_rows, pool_rows), pool_rows)
    w_pool[own_pool, :] = wp_ref[...]
    w_full[
        pl.ds(pl.multiple_of(tp * out_rows, out_rows), out_rows),
        pl.ds(pl.multiple_of(sp * out_columns, out_columns), out_columns),
    ] = wo_ref[...]

    from_line(turn[1], first_pair)
    from_line(turn[2], first_pair)
    from_pair(0, first_pair)
    from_line(turn[1], last_one)
    from_line(turn[2], last_one)
    from_pair(0, last_one)
    from_line(turn[3], first_pair)
    from_pair(turn[1], first_pair)
    for swap in swaps:
        swap.wait()
    squares = jnp.zeros((rows, 1), jnp.float32)
    per_half = half_width // (2 * w_rows)
    for ref, gains, owner in ((tok_ref, gain_in, tp), (theirs, their_gain, 1 - tp)):
        for j in range(per_half):
            chunk = pl.ds(j * 2 * w_rows, 2 * w_rows)
            features = ref[:, chunk].astype(jnp.float32)
            squares += jnp.sum(features * features, axis=1, keepdims=True)
            scaled = (features * gains[:, chunk].astype(jnp.float32)).astype(jnp.bfloat16)
            pieces[owner * per_half + j] = scaled
    inverse = lax.rsqrt(squares / model_width + EPSILON)
    inverse_sc[...] = jnp.broadcast_to(inverse, inverse_sc.shape)
    every = first_pair + last_one
    multiply(0, y, every)
    multiply(0, 1 - y, every)
    from_line(turn[3], last_one)

    @pl.when(between)
    def _():
        w_line(1).start()
        pool_line(1).start()

    from_pair(turn[1], last_one)
    multiply(turn[1], y, every)
    from_pair(turn[2], first_pair)
    multiply(turn[1], 1 - y, every)
    from_pair(turn[2], last_one)
    multiply(turn[2], y, every)
    multiply(turn[2], 1 - y, every)
    multiply(turn[3], y, first_pair)
    from_pair(turn[3], first_pair)
    multiply(turn[3], 1 - y, first_pair)
    width = columns // planes
    for p in range(planes):
        part = slice(p * width, (p + 1) * width)
        k_src[p] = (product[0, :, part] * inverse_sc[:, :1]).astype(jnp.bfloat16)
        v_src[p] = (product[1, :, part] * inverse_sc[:, :1]).T.astype(jnp.bfloat16)
    k_all[z, m] = k_src[z]
    v_all[z, m] = v_src[z]
    share(z, True)
    w_across(z, True).start()
    for i in range(1, planes):
        k_out(order(i)).start()
        v_out(order(i)).start()
    from_pair(turn[3], last_one)
    multiply(turn[3], y, last_one)
    multiply(turn[3], 1 - y, last_one)
    for p in range(planes):
        part = slice(p * width, (p + 1) * width)
        query = (product[2, :, part] * inverse_sc[:, :1]).astype(jnp.bfloat16)
        q_src[p] = query * (1.0 / math.sqrt(hdim))

    q_in[z] = q_src[z]
    for i in range(1, planes):
        q_out(order(i)).start()
    w_from_line(1)
    pool_from_line(1)

    @pl.when(between)
    def _():
        for i in (2, 3):
            w_from_line(i)
            pool_from_line(i)

    def visit(block, plane, first, count, masked):
        query = q_in[block]
        lane = lax.broadcasted_iota(jnp.int32, query.shape, 1)
        none = jnp.zeros_like(query)
        both = jnp.concatenate(
            [jnp.where(lane < hdim, query, none), jnp.where(lane < hdim, none, query)], axis=0
        )
        keys = k_all[plane, pl.ds(first, count)].reshape(count * rows, 2 * hdim)
        values = jnp.concatenate([v_all[plane, first + i] for i in range(count)], axis=1)
        scores = lax.dot_general(
            keys, both, (((1,), (1,)), ((), ())), preferred_element_type=jnp.float32
        )
        if masked:
            shift = (first - m) * rows
            key = lax.broadcasted_iota(jnp.int32, scores.shape, 0)
            col = lax.broadcasted_iota(jnp.int32, scores.shape, 1)
            col = jnp.where(col < rows, col, col - rows)
            scores = jnp.where(key + shift <= col, scores, NEG_LARGE)
        old = top[block]
        new = jnp.maximum(old, jnp.max(scores, axis=0, keepdims=True))
        factor = jnp.exp(old - new)
        expo = jnp.exp(scores - new)
        acc[block] = acc[block] * factor + jnp.dot(
            values, expo.astype(jnp.bfloat16), preferred_element_type=jnp.float32
        )
        partial = jnp.sum(expo.reshape(count * rows // 8, 8, 2 * rows), axis=0)
        total[block] = total[block] * factor + partial
        top[block] = new

    def diagonal(block):
        pair = m // 2

        @pl.when(pair > 0)
        def _():
            visit(block, block, 0, members // 2, False)

        visit(block, block, pair * (members // 2), members // 2, True)

    def result_copy(block, half):
        return remote(
            done.at[block, pl.ds(pl.multiple_of(half * half_rows, half_rows), half_rows)],
            branch.at[tp * planes + z, :, pl.ds(0, vdim)],
            back_send.at[block, half],
            back_recv.at[tp * planes + z],
            at(block, m, half),
        )

    def at_home(block):
        return block == z

    def finish(block):
        both = acc[block] / jnp.sum(total[block], axis=0, keepdims=True)
        mixed = both[:, :rows] - lam_ref[z] * both[:, rows:]
        mean_sq = jnp.mean(mixed * mixed, axis=0, keepdims=True)
        normed = (mixed * lax.rsqrt(mean_sq + EPSILON)).T * gain_ref[...]
        done[block] = normed.astype(jnp.bfloat16)

        @pl.when(at_home(block))
        def _():
            kept = pl.ds(pl.multiple_of(tp * half_rows, half_rows), half_rows)
            branch[tp * planes + z, :, :vdim] = done[block, kept]

        @pl.when(jnp.logical_not(at_home(block)))
        def _():
            result_copy(block, tp).start()

        result_copy(block, 1 - tp).start()

    edge_rows = halo.shape[0]

    def edge_out():
        return remote(
            pool_sc.at[pl.ds(rows - edge_rows, edge_rows)], halo, edge_sem.at[0], edge_sem.at[1], {"sp": sp + 1}
        )

    def half_out():
        mine = pl.ds(pl.multiple_of(tp * groups, groups), groups)
        return remote(
            pooled_sc, branch.at[mine, :, pl.ds(vdim, vdim)], half_sem.at[0], half_sem.at[1], x_peer
        )

    def pool_project():
        for plane in range(planes):
            arrived(pool_slot(plane, c_member), pc_recv.at[plane, 0])
            arrived(pool_slot(plane, turned), pc_recv.at[plane, 1])
        scaled = jnp.concatenate([pieces[j] for j in range(pieces.shape[0])], axis=1)
        pool_in = jnp.dot(scaled, w_pool[...], preferred_element_type=jnp.float32)
        pool_sc[...] = (pool_in * inverse_sc[:, :1]).astype(jnp.bfloat16)

        @pl.when(sp < n_sp - 1)
        def _():
            edge_out().start()

        @pl.when(sp == 0)
        def _():
            halo[...] = jnp.zeros_like(halo)

    def pool_mix():
        @pl.when(sp > 0)
        def _():
            arrived(halo, edge_sem.at[1])

        for g in range(groups):
            part = slice(g * vdim, (g + 1) * vdim)
            own = pool_sc[:, part].astype(jnp.float32)
            running = jnp.concatenate([halo[:, part].astype(jnp.float32), own], axis=0)
            span = WINDOWS[g % len(WINDOWS)]
            step = 1
            while step < span:
                running = running + pltpu.roll(running, step, 0)
                step *= 2
            position = sp * rows + lax.broadcasted_iota(jnp.int32, own.shape, 0)
            count = jnp.minimum(position + 1, span).astype(jnp.float32)
            differ = (running[edge_rows:] / count - own).astype(jnp.bfloat16)
            pooled = jnp.dot(differ, group_ref[g], preferred_element_type=jnp.float32)
            pooled = (pooled * pscale_ref[:, part]).astype(jnp.bfloat16)
            low, high = pooled[:half_rows], pooled[half_rows:]
            branch[tp * groups + g, :, vdim:] = jnp.where(tp == 0, low, high)
            pooled_sc[g] = jnp.where(tp == 0, high, low)
        half_out().start()

    hand_on(z, True)
    landed(1)
    shared(z, True)

    def stage(i, carry):
        block = order(i)

        diagonal(block)

        @pl.when(i == 1)
        def _():
            w_across(order(1), False).start()

        @pl.when(i < planes - 2)
        def _():
            landed(i + 2)

        @pl.when(i == 0)
        def _():
            w_from_pair(0)

        @pl.when((i == 1) & between)
        def _():
            for j in (2, 3):
                w_line_on(j).start()
                w_across(order(j), False).start()
            for j in (2, 3):
                pool_line_on(j).start()
            pool_across(z, True).start()
            for j in (1, 2, 3):
                pool_across(order(j), False).start()

        @pl.when((i == 2) & jnp.logical_not(between))
        def _():
            w_from_line(2)
            w_across(order(2), False).start()
            pool_across(z, True).start()
            pool_across(order(1), False).start()

        @pl.when(i == 2)
        def _():
            w_from_pair(1)

        @pl.when((i == 3) & between)
        def _():
            w_from_pair(2)

        @pl.when(i < planes - 2)
        def _():
            hand_on(order(i + 1), False)

        @pl.when(i == planes - 1)
        def _():
            finish(0)

        def pair(j, carry):
            other = jnp.where(i < planes - 1, order(j), j + upper)
            visit(jnp.maximum(block, other), jnp.minimum(block, other), 0, members, False)

            @pl.when(i == planes - 1)
            def _():
                finish(j + 1)

            @pl.when((i == 3) & (j == 1) & between)
            def _():
                w_from_pair(3)

            @pl.when((i == planes - 2) & (j == 0))
            def _():
                hand_on(order(i + 1), False)

            @pl.when((i == 2) & (j == 1) & jnp.logical_not(between))
            def _():
                w_from_line(3)
                w_across(order(3), False).start()

            @pl.when((i == 3) & (j == 0) & jnp.logical_not(between))
            def _():
                w_from_pair(2)

            return carry

        lax.fori_loop(0, i, pair, 0)

        @pl.when(i < planes - 1)
        def _():
            arrived(q_in.at[order(i + 1)], z_recv.at[2, order(i + 1)])
            shared(order(i + 1), False)

        return carry

    lax.fori_loop(0, planes, stage, 0)


    @pl.when(jnp.logical_not(between))
    def _():
        for i in (2, 3):
            pool_from_line(i)
            pool_across(order(i), False).start()
        w_from_pair(3)

    for i in range(planes):
        pool_from_pair(i)
    pool_project()
    w_from_swap(0)
    pool_mix()

    for head in range(2 * planes):
        own_head = tp * planes + z == head

        @pl.when(jnp.logical_not(own_head & at_home(z)))
        def _():
            arrived(branch.at[head, :, pl.ds(0, vdim)], back_recv.at[head])

    w_from_swap(1)
    w_from_swap(2)
    theirs = pl.ds(pl.multiple_of((1 - tp) * groups, groups), groups)
    arrived(branch.at[theirs, :, pl.ds(vdim, vdim)], half_sem.at[1])
    w_from_swap(3)
    left = jnp.concatenate([branch[head] for head in range(2 * planes)], axis=1)
    out_width = members * out_columns

    def column(i, carry):
        plane = order(i)

        for half in range(2):
            for yy in range(2):
                arrived(out_slot(half, plane, yy, 1 - c), wc_recv.at[half, plane, yy])
        part = pl.ds(pl.multiple_of(plane * out_width, out_width), out_width)
        out_ref[:, part] = jnp.dot(
            left, w_full[:, part], preferred_element_type=jnp.float32
        ).astype(jnp.bfloat16)
        return carry

    lax.fori_loop(0, planes, column, 0)

    for i in range(1, planes):
        k_out(order(i)).wait_send()
        v_out(order(i)).wait_send()
        q_out(order(i)).wait_send()

    for i in range(planes):
        plane = order(i)
        for copies in in_plane(plane, i == 0):
            for copy in copies:
                copy.wait_send()
        w_across(plane, False).wait_send()
        for a in first_pair + last_one:
            y_copy(a, i, False).wait_send()
            c_copy(a, plane, y, False).wait_send()
            c_copy(a, plane, 1 - y, False).wait_send()
        for yy in (y, 1 - y):
            w_swap(plane, yy, False).wait_send()
            w_beside(0, plane, yy, False).wait_send()
            w_beside(1, plane, yy, False).wait_send()

    for i in (1, 2):
        w_line(i).wait_send()
        pool_line(i).wait_send()
        for a in first_pair + last_one:
            line(a, i).wait_send()

    @pl.when(between)
    def _():
        for i in (2, 3):
            w_line_on(i).wait_send()
            pool_line_on(i).wait_send()
            for a in first_pair + last_one:
                line_on(a, i).wait_send()

    for plane in range(planes):
        pool_across(plane, False).wait_send()
        pool_beside(plane, False).wait_send()
        pool_onward(plane).wait_send()
        result_copy(plane, 1 - tp).wait_send()

        @pl.when(jnp.logical_not(at_home(plane)))
        def _():
            result_copy(plane, tp).wait_send()

    half_out().wait_send()

    @pl.when(sp < n_sp - 1)
    def _():
        edge_out().wait_send()


def whole_layer(
    tokens,
    pre_gain,
    w_query,
    w_key,
    w_value,
    w_pool,
    lambdas,
    sub_gain,
    group_weight,
    pool_scale,
    w_out,
):
    planes = lambdas.shape[0]
    rows, half_width = tokens.shape
    n_sp = lax.axis_size("sp")
    members = n_sp // planes
    w_rows, columns = w_query.shape
    model_width = n_sp * w_rows
    width = columns // planes
    groups, vdim, _ = group_weight.shape
    out_rows, out_columns = w_out.shape
    vmem = pl.BlockSpec(memory_space=pltpu.VMEM)
    dma = pltpu.SemaphoreType.DMA
    bf16, f32 = jnp.bfloat16, jnp.float32
    work = planes * rows * members * planes * rows
    return pl.pallas_call(
        functools.partial(layer, width // 2, model_width),
        out_shape=jax.ShapeDtypeStruct((rows // 2, n_sp * out_columns), bf16),
        in_specs=[pl.BlockSpec(memory_space=pltpu.SMEM)] + [vmem] * 10,
        out_specs=vmem,
        scratch_shapes=[
            pltpu.VMEM((3, model_width, columns), bf16),
            pltpu.VMEM((rows, half_width), bf16),
            pltpu.VMEM((1, half_width), bf16),
            pltpu.VMEM((model_width // (2 * w_rows), rows, 2 * w_rows), bf16),
            pltpu.VMEM((3, rows, columns), f32),
            pltpu.VMEM((rows, 128), f32),
            pltpu.VMEM((planes, rows, width), bf16),
            pltpu.VMEM((planes, vdim, rows), bf16),
            pltpu.VMEM((planes, rows, width), bf16),
            pltpu.VMEM((planes, rows, width), bf16),
            pltpu.VMEM((planes, members, rows, width), bf16),
            pltpu.VMEM((planes, members, vdim, rows), bf16),
            pltpu.VMEM((planes, vdim, 2 * rows), f32),
            pltpu.VMEM((planes, 1, 2 * rows), f32),
            pltpu.VMEM((planes, 8, 2 * rows), f32),
            pltpu.VMEM((planes, rows, vdim), bf16),
            pltpu.VMEM((model_width, groups * vdim), bf16),
            pltpu.VMEM((2 * out_rows, n_sp * out_columns), bf16),
            pltpu.VMEM((2 * planes, rows // 2, 2 * vdim), bf16),
            pltpu.VMEM((rows, groups * vdim), bf16),
            pltpu.VMEM((RIM_ROWS + 1, groups * vdim), bf16),
            pltpu.VMEM((groups, rows // 2, vdim), bf16),
            dma((planes, 3)),
            dma((planes, 3)),
            dma((planes, 3)),
            dma((planes, 3)),
            dma((planes, 2, 3)),
            dma((planes, 2, 3)),
            dma((4,)),
            dma((3, planes)),
            dma((3, planes)),
            dma((planes, 3, 2)),
            dma((planes, 3, 2)),
            dma((planes, 2)),
            dma((2 * planes,)),
            dma((planes,)),
            dma((planes,)),
            dma((planes, 2)),
            dma((planes, 2)),
            dma((2,)),
            dma((2,)),
            dma((planes,)),
            dma((planes,)),
            dma((planes,)),
            dma((planes,)),
            dma((planes,)),
            dma((planes,)),
            dma((planes, 2)),
            dma((planes, 2)),
            dma((2, planes, 2)),
            dma((2, planes, 2)),
        ],
        compiler_params=pltpu.CompilerParams(
            vmem_limit_bytes=60 * 2**20, collective_id=2, has_side_effects=True
        ),
        cost_estimate=pl.CostEstimate(
            flops=4 * work * vdim, bytes_accessed=2**24, transcendentals=work
        ),
    )(
        lambdas,
        tokens,
        pre_gain.reshape(1, -1),
        w_key,
        w_value,
        w_query,
        w_pool,
        sub_gain.reshape(1, -1),
        group_weight,
        pool_scale.reshape(1, -1),
        w_out,
    )


def trailing(x, window_ids, group_dim):
    column_window = jnp.repeat(window_ids, group_dim)[None, :]
    running = x
    picked = jnp.zeros_like(x)
    for slot, span in enumerate(WINDOWS):
        half = span // 2
        running = running + jnp.pad(running[:-half], ((half, 0), (0, 0)))
        picked = jnp.where(column_window == slot, running, picked)
    return picked


def general_attention(queries, key_rows, values, lambdas, sub_gain):
    n_sp = lax.axis_size("sp")
    sp = lax.axis_index("sp")
    tok_rows = queries.shape[0]
    heads = lambdas.shape[0]
    qdim = queries.shape[1] // heads
    vdim = values.shape[1] // heads
    head_width = 2 * qdim + vdim
    outer = math.gcd(n_sp, heads)
    inner = n_sp // outer
    per_device = heads // outer
    by_head = jnp.concatenate(
        [
            x.reshape(tok_rows, heads, -1).swapaxes(0, 1)
            for x in (queries, key_rows, values)
        ],
        axis=2,
    )
    across = [[o * inner + i for o in range(outer)] for i in range(inner)]
    within = [[o * inner + i for i in range(inner)] for o in range(outer)]
    by_head = by_head.reshape(outer, per_device, tok_rows, head_width)
    if outer > 1:
        by_head = lax.all_to_all(by_head, "sp", 0, 0, axis_index_groups=across)
    first_head = lax.div(sp, inner) * per_device
    attended = []
    if inner == 4 and per_device == 1:
        lam = lax.dynamic_slice_in_dim(lambdas, first_head, 1)
        attended.append(
            flash_members(by_head[:, 0, :, :qdim], by_head[:, 0, :, qdim:], lam, sub_gain)
        )
    else:
        kv = lax.all_gather(by_head[..., qdim:], "sp", axis=0, axis_index_groups=within)
        member = lax.rem(sp, inner).reshape(1)
        for p in range(per_device):
            lam = lax.dynamic_slice_in_dim(lambdas, first_head + p, 1)
            attended.append(flash(by_head[:, p, :, :qdim], kv[:, :, p], member, lam, sub_gain))
    attended = jnp.stack(attended, axis=1)
    if outer > 1:
        attended = lax.all_to_all(attended, "sp", 0, 0, axis_index_groups=across)
    return attended.reshape(heads, tok_rows, vdim)


def local(
    tokens,
    pre_gain,
    w_query,
    w_key,
    w_value,
    w_pool,
    lambdas,
    sub_gain,
    group_weight,
    pool_scale,
    w_out,
):
    n_tp = lax.axis_size("tp")
    n_sp = lax.axis_size("sp")
    tp = lax.axis_index("tp")
    sp = lax.axis_index("sp")
    tok_rows = tokens.shape[0]
    model_width = tokens.shape[1] * n_tp
    heads = lambdas.shape[0]
    qdim = w_query.shape[1] // heads
    vdim = w_value.shape[1] // heads
    groups = group_weight.shape[0]
    group_dim = group_weight.shape[1]

    shaped_for_mix = n_tp == 2 and heads == 4 and n_sp == 4 * heads and tok_rows % 32 == 0
    if shaped_for_mix and qdim == vdim == group_dim and groups == heads:
        return whole_layer(
            tokens,
            pre_gain,
            w_query,
            w_key,
            w_value,
            w_pool,
            lambdas,
            sub_gain,
            group_weight,
            pool_scale,
            w_out,
        )
    swap = [(0, 1), (1, 0)]
    w_sorted = w_out.reshape(heads, 2, vdim, -1).swapaxes(0, 1).reshape(w_out.shape)
    features = tokens.astype(jnp.float32)
    mine = (features * pre_gain.astype(jnp.float32)[None, :]).astype(jnp.bfloat16)
    squares = jnp.sum(features * features, axis=1, keepdims=True)
    weights = [w_query, w_key, w_value, w_pool]
    if n_sp % 4 == 0:
        *weights, theirs = gather_weights(weights, mine, n_tp == 2)
    else:
        weights = [lax.all_gather(w, "sp", axis=0, tiled=True) for w in weights]
        theirs = lax.ppermute(mine, "tp", swap) if n_tp == 2 else mine
    w_sorted, weights = lax.optimization_barrier((w_sorted, weights))
    w_out_rows = lax.all_gather(w_sorted, "sp", axis=1, tiled=True)
    if n_tp == 2:
        squares = squares + lax.ppermute(squares, "tp", swap)
        scaled = jnp.concatenate(
            [jnp.where(tp == 0, mine, theirs), jnp.where(tp == 0, theirs, mine)], axis=1
        )
    else:
        scaled = lax.all_gather(mine, "tp", axis=1, tiled=True)
        squares = lax.psum(squares, "tp")
    inverse = lax.rsqrt(squares / model_width + EPSILON)
    queries, key_rows, values, pool_in = [
        (jnp.dot(scaled, w, preferred_element_type=jnp.float32) * inverse).astype(jnp.bfloat16)
        for w in weights
    ]
    attended = general_attention(queries, key_rows, values, lambdas, sub_gain)

    halo = passed_along(pool_in[tok_rows - RIM_ROWS - 1 :], "sp", 1)
    extended = jnp.concatenate([halo, pool_in], axis=0).astype(jnp.float32)
    window_ids = (tp * groups + jnp.arange(groups, dtype=jnp.int32)) % len(WINDOWS)
    sums = trailing(extended, window_ids, group_dim)[RIM_ROWS + 1 :]
    spans = jnp.repeat(jnp.left_shift(2, window_ids), group_dim)
    positions = sp * tok_rows + jnp.arange(tok_rows, dtype=jnp.int32)
    count = jnp.minimum(positions[:, None] + 1, spans[None, :]).astype(jnp.float32)
    differ = (sums / count - pool_in.astype(jnp.float32)).astype(jnp.bfloat16)
    pooled = jnp.einsum(
        "tgc,gcd->tgd",
        differ.reshape(tok_rows, groups, group_dim),
        group_weight,
        preferred_element_type=jnp.float32,
    )
    pooled = (pooled * pool_scale.reshape(groups, group_dim)).astype(jnp.bfloat16)
    branch = jnp.concatenate(
        [attended.swapaxes(0, 1).reshape(tok_rows, -1), pooled.reshape(tok_rows, -1)], axis=1
    )
    if n_tp == 2:
        half = tok_rows // 2
        send = lax.dynamic_slice_in_dim(branch, (1 - tp) * half, half, 0)
        send = jnp.dot(send, w_out_rows, preferred_element_type=jnp.float32).astype(jnp.bfloat16)
        got = lax.ppermute(send, "tp", swap)
        keep = lax.dynamic_slice_in_dim(branch, tp * half, half, 0)
        keep = jnp.dot(keep, w_out_rows, preferred_element_type=jnp.float32)
        return (keep + got.astype(jnp.float32)).astype(jnp.bfloat16)
    partial = jnp.dot(branch, w_out_rows, preferred_element_type=jnp.float32)
    return lax.psum_scatter(partial.astype(jnp.bfloat16), "tp", scatter_dimension=0, tiled=True)


def solution(mesh):
    placed = (
        P("sp", "tp"),
        P("tp"),
        P("sp", "tp"),
        P("sp", "tp"),
        P("sp", "tp"),
        P("sp", "tp"),
        P("tp"),
        P(),
        P("tp", None, None),
        P("tp"),
        P("tp", "sp"),
    )
    return jax.shard_map(
        local, mesh=mesh, in_specs=placed, out_specs=P(("sp", "tp"), None), check_vma=False
    )
```

```python
import functools
import math

import jax
import jax.numpy as jnp
from jax import lax
from jax.experimental import pallas as pl
from jax.experimental.pallas import tpu as pltpu
from jax.sharding import PartitionSpec as P

EPSILON = 1e-06
NEG_LARGE = -1e30
WINDOWS = (2, 4, 8, 16)
RIM_ROWS = 15


def passed_along(block, axis, distance):
    devices = range(lax.axis_size(axis))
    route = [(i - distance, i) for i in devices if i - distance in devices]
    return lax.ppermute(block, axis, route)


def attend(inner, vdim, hdim, member_ref, lam_ref, q_ref, kv_ref, gain_ref, out_ref, acc_ref, max_ref):
    rows = q_ref.shape[1]
    block = pl.program_id(0)
    last = block * inner + member_ref[0]
    scale = 1.0 / math.sqrt(hdim)
    queries = (q_ref[0].astype(jnp.float32) * scale).astype(jnp.bfloat16)
    maps = (queries[:, :hdim], queries[:, hdim:])
    ones = jnp.ones((rows, vdim), jnp.bfloat16)
    acc_ref[...] = jnp.zeros_like(acc_ref)
    max_ref[...] = jnp.full_like(max_ref, NEG_LARGE)

    def step(g, masked):
        keys_values = kv_ref[lax.rem(g, inner), lax.div(g, inner)]
        values = jnp.concatenate([keys_values[:, 2 * hdim :], ones], axis=1)
        for m in range(2):
            keys = keys_values[:, m * hdim : (m + 1) * hdim]
            scores = lax.dot_general(
                maps[m], keys, (((1,), (1,)), ((), ())), preferred_element_type=jnp.float32
            )
            if masked:
                row = lax.broadcasted_iota(jnp.int32, scores.shape, 0)
                col = lax.broadcasted_iota(jnp.int32, scores.shape, 1)
                scores = jnp.where(col <= row, scores, NEG_LARGE)
            old_max = max_ref[m]
            new_max = jnp.maximum(old_max, jnp.max(scores, axis=1, keepdims=True))
            factor = jnp.exp(old_max - new_max)
            expo = jnp.exp(scores - new_max[:, :1])
            acc_ref[m] = acc_ref[m] * factor[:, :1] + jnp.dot(
                expo.astype(jnp.bfloat16), values, preferred_element_type=jnp.float32
            )
            max_ref[m] = new_max

    def body(g, carry):
        step(g, False)
        return carry

    lax.fori_loop(0, last, body, 0)
    step(last, True)
    first = acc_ref[0]
    second = acc_ref[1]
    mix = first[:, :vdim] / first[:, vdim:] - lam_ref[0] * (second[:, :vdim] / second[:, vdim:])
    mean_sq = jnp.mean(mix * mix, axis=1, keepdims=True)
    out_ref[0] = (mix * lax.rsqrt(mean_sq + EPSILON) * gain_ref[...]).astype(jnp.bfloat16)


def flash(q, kv, member, lam, sub_gain):
    inner, outer, rows, width = kv.shape
    qdim = q.shape[-1]
    vdim = width - qdim
    smem = pl.BlockSpec(memory_space=pltpu.SMEM)
    work = outer * rows * outer * rows * inner
    return pl.pallas_call(
        functools.partial(attend, inner, vdim, qdim // 2),
        grid=(outer,),
        out_shape=jax.ShapeDtypeStruct((outer, rows, vdim), jnp.bfloat16),
        in_specs=[
            smem,
            smem,
            pl.BlockSpec((1, rows, qdim), lambda b: (b, 0, 0)),
            pl.BlockSpec(memory_space=pltpu.VMEM),
            pl.BlockSpec(memory_space=pltpu.VMEM),
        ],
        out_specs=pl.BlockSpec((1, rows, vdim), lambda b: (b, 0, 0)),
        scratch_shapes=[
            pltpu.VMEM((2, rows, 2 * vdim), jnp.float32),
            pltpu.VMEM((2, rows, 128), jnp.float32),
        ],
        compiler_params=pltpu.CompilerParams(vmem_limit_bytes=56 * 2**20),
        cost_estimate=pl.CostEstimate(
            flops=4 * work * vdim, bytes_accessed=kv.size * 2, transcendentals=work
        ),
    )(member, lam, q, kv, sub_gain.reshape(1, -1))


def attend_members(hdim, lam_ref, q_ref, own_ref, gain_ref, out_ref, held, acc_ref, max_ref, send, recv):
    outer, rows, _ = q_ref.shape
    vdim = own_ref.shape[2] - 2 * hdim
    sp = lax.axis_index("sp")
    member = lax.rem(sp, 4)
    y = lax.div(member, 2)
    c = lax.rem(member, 2)
    y_peer = sp + 2 - 4 * y
    c_peer = sp + 1 - 2 * c
    barrier = pltpu.get_barrier_semaphore()
    for peer in (y_peer, c_peer):
        pl.semaphore_signal(
            barrier, 1, device_id={"sp": peer}, device_id_type=pl.DeviceIdType.MESH
        )
    pl.semaphore_wait(barrier, 2)

    def remote(src, index, peer):
        return pltpu.make_async_remote_copy(
            src_ref=src,
            dst_ref=held.at[index],
            send_sem=send.at[index],
            recv_sem=recv.at[index],
            device_id={"sp": peer},
            device_id_type=pl.DeviceIdType.MESH,
        )

    across = remote(own_ref, 1, y_peer)
    beside = remote(own_ref, 0, c_peer)
    onward = remote(held.at[1], 2, c_peer)
    across.start()
    beside.start()
    acc_ref[...] = jnp.zeros_like(acc_ref)
    max_ref[...] = jnp.full_like(max_ref, NEG_LARGE)
    scale = 1.0 / math.sqrt(hdim)

    def visit(ref, other):
        shift = (member - other) * rows
        for block in range(outer):
            queries = (q_ref[block].astype(jnp.float32) * scale).astype(jnp.bfloat16)
            length = (block + 1) * rows
            keys_values = ref[: block + 1].reshape(length, 2 * hdim + vdim)
            values = jnp.concatenate(
                [keys_values[:, 2 * hdim :], jnp.ones((length, vdim), jnp.bfloat16)], axis=1
            )
            for m in range(2):
                scores = lax.dot_general(
                    queries[:, m * hdim : (m + 1) * hdim],
                    keys_values[:, m * hdim : (m + 1) * hdim],
                    (((1,), (1,)), ((), ())),
                    preferred_element_type=jnp.float32,
                )
                edge = scores[:, block * rows :]
                row = lax.broadcasted_iota(jnp.int32, edge.shape, 0)
                col = lax.broadcasted_iota(jnp.int32, edge.shape, 1)
                edge = jnp.where(col <= row + shift, edge, NEG_LARGE)
                if block > 0:
                    scores = jnp.concatenate([scores[:, : block * rows], edge], axis=1)
                else:
                    scores = edge
                old_max = max_ref[block, m]
                new_max = jnp.maximum(old_max, jnp.max(scores, axis=1, keepdims=True))
                factor = jnp.exp(old_max - new_max)
                expo = jnp.exp(scores - new_max[:, :1])
                acc_ref[block, m] = acc_ref[block, m] * factor[:, :1] + jnp.dot(
                    expo.astype(jnp.bfloat16), values, preferred_element_type=jnp.float32
                )
                max_ref[block, m] = new_max

    visit(own_ref, member)

    def arrived(j, carry):
        @pl.when(j == 0)
        def _():
            beside.wait_recv()

        @pl.when(j == 1)
        def _():
            across.wait_recv()
            onward.start()

        @pl.when(j == 2)
        def _():
            onward.wait_recv()

        other_y = jnp.where(j >= 1, 1 - y, y)
        other_c = jnp.where(j == 1, c, 1 - c)
        visit(held.at[j], 2 * other_y + other_c)
        return carry

    lax.fori_loop(0, 3, arrived, 0)
    for copy in (across, beside, onward):
        copy.wait_send()
    for block in range(outer):
        first = acc_ref[block, 0]
        second = acc_ref[block, 1]
        mix = first[:, :vdim] / first[:, vdim:]
        mix = mix - lam_ref[0] * (second[:, :vdim] / second[:, vdim:])
        mean_sq = jnp.mean(mix * mix, axis=1, keepdims=True)
        normed = mix * lax.rsqrt(mean_sq + EPSILON) * gain_ref[...]
        out_ref[block] = normed.astype(jnp.bfloat16)


def flash_members(q, kv, lam, sub_gain):
    outer, rows, width = kv.shape
    qdim = q.shape[-1]
    vdim = width - qdim
    vmem = pl.BlockSpec(memory_space=pltpu.VMEM)
    work = 4 * outer * rows * outer * rows
    return pl.pallas_call(
        functools.partial(attend_members, qdim // 2),
        out_shape=jax.ShapeDtypeStruct((outer, rows, vdim), jnp.bfloat16),
        in_specs=[pl.BlockSpec(memory_space=pltpu.SMEM), vmem, vmem, vmem],
        out_specs=vmem,
        scratch_shapes=[
            pltpu.VMEM((3, outer, rows, width), jnp.bfloat16),
            pltpu.VMEM((outer, 2, rows, 2 * vdim), jnp.float32),
            pltpu.VMEM((outer, 2, rows, 128), jnp.float32),
            pltpu.SemaphoreType.DMA((3,)),
            pltpu.SemaphoreType.DMA((3,)),
        ],
        compiler_params=pltpu.CompilerParams(
            vmem_limit_bytes=56 * 2**20, collective_id=1, has_side_effects=True
        ),
        cost_estimate=pl.CostEstimate(
            flops=4 * work * vdim, bytes_accessed=4 * kv.size * 2, transcendentals=work
        ),
    )(lam, q, kv, sub_gain.reshape(1, -1))


def spread(n_sp, count, with_swap, *refs):
    weights, refs = refs[:count], refs[count:]
    mine, refs = refs[0], refs[1:]
    fulls, refs = refs[:count], refs[count:]
    theirs, refs = refs[0], refs[1:]
    up_send, up_recv, down_send, down_recv, y_send, y_recv, c_send, c_recv, own_sem, swap_sem = refs
    depth = n_sp // 4
    rows = weights[0].shape[0]
    sp = lax.axis_index("sp")
    z = lax.div(sp, 4)
    y = lax.rem(lax.div(sp, 2), 2)
    c = lax.rem(sp, 2)
    y_peer = z * 4 + (1 - y) * 2 + c
    c_peer = z * 4 + y * 2 + (1 - c)
    barrier = pltpu.get_barrier_semaphore()

    def greet(device):
        pl.semaphore_signal(barrier, 1, device_id=device, device_id_type=pl.DeviceIdType.MESH)

    greet({"sp": y_peer})
    greet({"sp": c_peer})
    greeted = 2
    if with_swap:
        greet({"tp": 1 - lax.axis_index("tp")})
        greeted = 3

    @pl.when(z > 0)
    def _():
        greet({"sp": sp - 4})

    @pl.when(z < depth - 1)
    def _():
        greet({"sp": sp + 4})

    in_line = jnp.where(z > 0, 1, 0) + jnp.where(z < depth - 1, 1, 0)
    pl.semaphore_wait(barrier, greeted + in_line)

    def slot(a, zz, yy, cc):
        start = pl.multiple_of((zz * 4 + yy * 2 + cc) * rows, rows)
        return fulls[a].at[pl.ds(start, rows), :]

    def remote(src, dst, send, recv, device):
        return pltpu.make_async_remote_copy(
            src_ref=src,
            dst_ref=dst,
            send_sem=send,
            recv_sem=recv,
            device_id=device,
            device_id_type=pl.DeviceIdType.MESH,
        )

    def line_copy(side, k, a, src):
        sends, recvs = (up_send, up_recv) if side > 0 else (down_send, down_recv)
        there = slot(a, z - side * k, y, c)
        return remote(
            there if src is None else src,
            there,
            sends.at[k, a],
            recvs.at[k + 1, a],
            {"sp": sp + 4 * side},
        )

    def y_copy(zz, yy, a, src):
        there = slot(a, zz, yy, c)
        src = there if src is None else src
        return remote(src, there, y_send.at[zz, a], y_recv.at[zz, a], {"sp": y_peer})

    def c_copy(zz, yy, cc, a, src):
        there = slot(a, zz, yy, cc)
        src = there if src is None else src
        return remote(src, there, c_send.at[zz, yy, a], c_recv.at[zz, yy, a], {"sp": c_peer})

    def can_go(side):
        return z < depth - 1 if side > 0 else z > 0

    def came(side, k):
        return z >= k if side > 0 else z + k <= depth - 1

    if with_swap:
        swap = remote(
            mine, theirs, swap_sem.at[0], swap_sem.at[1], {"tp": 1 - lax.axis_index("tp")}
        )
        swap.start()
    for a in range(count):
        for side in (1, -1):

            @pl.when(can_go(side))
            def _():
                line_copy(side, 0, a, weights[a]).start()

        y_copy(z, y, a, weights[a]).start()
    for a in range(count):
        c_copy(z, y, c, a, weights[a]).start()
        pltpu.make_async_copy(weights[a], slot(a, z, y, c), own_sem.at[a]).start()

    def from_pair(zz):
        for a in range(count):
            y_copy(zz, 1 - y, a, None).wait_recv()
            c_copy(zz, 1 - y, c, a, None).start()

    def relay(k, carry):
        for side in (1, -1):
            recvs = up_recv if side > 0 else down_recv

            @pl.when(came(side, k))
            def _():
                zz = z - side * k
                for a in range(count):
                    there = slot(a, zz, y, c)
                    remote(there, there, up_send.at[0, a], recvs.at[k, a], {"sp": y_peer}).wait_recv()

                    @pl.when(can_go(side))
                    def _():
                        line_copy(side, k, a, None).start()

                    y_copy(zz, y, a, None).start()
                    c_copy(zz, y, c, a, None).start()

        @pl.when(k == 1)
        def _():
            from_pair(z)

        for side in (1, -1):

            @pl.when((k > 1) & came(side, k - 1))
            def _():
                from_pair(z - side * (k - 1))

        return carry

    lax.fori_loop(1, depth, relay, 0)
    if depth == 1:
        from_pair(z)
    for side in (1, -1):
        if depth > 1:

            @pl.when(came(side, depth - 1))
            def _():
                from_pair(z - side * (depth - 1))

    def drain(zz, carry):
        for a in range(count):
            y_copy(zz, y, a, None).wait_send()
            for yy in range(2):
                c_copy(zz, yy, 1 - c, a, None).wait_recv()
                c_copy(zz, yy, c, a, None).wait_send()
        return carry

    lax.fori_loop(0, depth, drain, 0)

    def drain_line(k, carry):
        for side in (1, -1):

            @pl.when(came(side, k) & can_go(side))
            def _():
                for a in range(count):
                    line_copy(side, k, a, None).wait_send()

        return carry

    lax.fori_loop(0, depth, drain_line, 0)
    for a in range(count):
        pltpu.make_async_copy(weights[a], slot(a, z, y, c), own_sem.at[a]).wait()
    if with_swap:
        swap.wait()


def gather_weights(weights, mine, with_swap):
    n_sp = lax.axis_size("sp")
    count = len(weights)
    depth = n_sp // 4
    sems = pltpu.SemaphoreType.DMA
    any_spec = pl.BlockSpec(memory_space=pl.ANY)
    vmem_spec = pl.BlockSpec(memory_space=pltpu.VMEM)
    shapes = [jax.ShapeDtypeStruct((n_sp * w.shape[0], w.shape[1]), w.dtype) for w in weights]
    shapes.append(jax.ShapeDtypeStruct(mine.shape, mine.dtype))
    moved = sum(w.size for w in weights) * 2 * n_sp
    return pl.pallas_call(
        functools.partial(spread, n_sp, count, with_swap),
        out_shape=shapes,
        in_specs=[vmem_spec] * (count + 1),
        out_specs=[any_spec] * (count + 1),
        scratch_shapes=[
            sems((depth + 1, count)),
            sems((depth + 1, count)),
            sems((depth + 1, count)),
            sems((depth + 1, count)),
            sems((depth, count)),
            sems((depth, count)),
            sems((depth, 2, count)),
            sems((depth, 2, count)),
            sems((count,)),
            sems((2,)),
        ],
        compiler_params=pltpu.CompilerParams(collective_id=0, has_side_effects=True),
        cost_estimate=pl.CostEstimate(flops=10**10, bytes_accessed=moved, transcendentals=0),
    )(*weights, mine)


def arrival(z, i):
    half = z // 2
    later = jnp.where(i == 2, 2 - half, 3 - 3 * half)
    return jnp.where(i == 0, z, jnp.where(i == 1, 1 + 4 * half - z, later))


def layer(
    hdim,
    model_width,
    lam_ref,
    tok_ref,
    gain_in,
    wk_ref,
    wv_ref,
    wq_ref,
    wp_ref,
    gain_ref,
    group_ref,
    pscale_ref,
    wo_ref,
    out_ref,
    full,
    theirs,
    their_gain,
    pieces,
    product,
    inverse_sc,
    k_src,
    v_src,
    q_src,
    q_in,
    k_all,
    v_all,
    acc,
    top,
    total,
    done,
    w_pool,
    w_full,
    branch,
    pool_sc,
    halo,
    pooled_sc,
    *sems,
):
    (line_send, line_recv, y_send, y_recv, c_send, c_recv, swap_sem) = sems[:7]
    (z_send, z_recv, in_send, in_recv, back_send, back_recv) = sems[7:13]
    (py_send, py_recv, pc_send, pc_recv, edge_sem, half_sem, pool_send, pool_recv) = sems[13:21]
    (wl_send, wl_recv, wy_send, wy_recv, wx_send, wx_recv, wc_send, wc_recv) = sems[21:]
    weights = (wk_ref, wv_ref, wq_ref)
    first_pair, last_one = (0, 1), (2,)
    planes, rows, _ = q_src.shape
    vdim = v_src.shape[1]
    members = k_all.shape[1]
    w_rows, columns = wq_ref.shape
    half_width = tok_ref.shape[1]
    groups = group_ref.shape[0]
    half_rows = rows // 2
    sp = lax.axis_index("sp")
    tp = lax.axis_index("tp")
    n_sp = lax.axis_size("sp")
    z = sp // members
    m = sp % members
    y = m // 2
    c = m % 2
    y_member = (m + 2) % members
    c_member = m + 1 - 2 * c
    turned = members - 1 - m
    upper = z // 2
    between = (z > 0) & (z < planes - 1)
    turn = [jnp.where(between, 1 + i % 3, i) for i in range(planes)]
    turn[0] = 0

    def at(plane, member, half=None):
        device = {"sp": plane * members + member}
        if half is not None:
            device["tp"] = half
        return device

    y_peer = at(z, y_member)
    c_peer = at(z, c_member)
    x_peer = {"tp": 1 - tp}

    def order(i):
        return arrival(z, i)

    barrier = pltpu.get_barrier_semaphore()

    def greet(device):
        pl.semaphore_signal(barrier, 1, device_id=device, device_id_type=pl.DeviceIdType.MESH)

    for i in range(1, planes):
        greet(at(order(i), m))
    for member in range(1, members):
        greet(at(z, (m + member) % members))
    for plane in range(planes):
        greet(at(plane, m, 1 - tp))

    @pl.when((m == 0) & (z > 0))
    def _():
        greet({"sp": sp - 1})

    @pl.when((m == members - 1) & (z < planes - 1))
    def _():
        greet({"sp": sp + 1})

    beyond = jnp.where((m == 0) & (z > 0), 1, 0)
    beyond += jnp.where((m == members - 1) & (z < planes - 1), 1, 0)
    pl.semaphore_wait(barrier, 2 * planes + members - 2 + beyond)

    def remote(src, dst, send, recv, device):
        return pltpu.make_async_remote_copy(
            src_ref=src,
            dst_ref=dst,
            send_sem=send,
            recv_sem=recv,
            device_id=device,
            device_id_type=pl.DeviceIdType.MESH,
        )

    def arrived(ref, recv):
        remote(ref, ref, recv, recv, c_peer).wait_recv()

    def k_out(plane):
        return remote(k_src.at[plane], k_all.at[z, m], z_send.at[0, plane], z_recv.at[0, z], at(plane, m))

    def v_out(plane):
        return remote(v_src.at[plane], v_all.at[z, m], z_send.at[1, plane], z_recv.at[1, z], at(plane, m))

    def q_out(plane):
        return remote(
            q_src.at[plane], q_in.at[z], z_send.at[2, plane], z_recv.at[2, z], at(plane, m)
        )

    def in_plane(plane, own):
        copies = []
        for t, (mine, everyone) in enumerate(((k_src, k_all), (v_src, v_all))):
            src = mine.at[plane] if own else everyone.at[plane, m]
            there = everyone.at[plane, m]
            passed = everyone.at[plane, y_member]
            copies.append(
                [
                    remote(src, there, in_send.at[plane, 0, t], in_recv.at[plane, 0, t], y_peer),
                    remote(src, there, in_send.at[plane, 1, t], in_recv.at[plane, 1, t], c_peer),
                    remote(passed, passed, in_send.at[plane, 2, t], in_recv.at[plane, 2, t], c_peer),
                ]
            )
        return copies

    def share(plane, own):
        for copies in in_plane(plane, own):
            copies[0].start()
            copies[1].start()

    def hand_on(plane, own):
        for copies in in_plane(plane, own):
            copies[0].wait_recv()
            copies[2].start()

    def shared(plane, own):
        for copies in in_plane(plane, own):
            copies[1].wait_recv()
            copies[2].wait_recv()

    def landed(i):
        plane = order(i)
        arrived(k_all.at[plane, m], z_recv.at[0, plane])
        arrived(v_all.at[plane, m], z_recv.at[1, plane])
        share(plane, False)

    pool_rows = wp_ref.shape[0]

    def pool_slot(plane, member):
        start = pl.multiple_of((plane * members + member) * pool_rows, pool_rows)
        return w_pool.at[pl.ds(start, pool_rows), :]

    def pool_line(i):
        return remote(wp_ref, pool_slot(z, m), pool_send.at[i - 1], pool_recv.at[z], at(order(i), m))

    def pool_line_on(i):
        there = pool_slot(order(i), m)
        return remote(there, there, pool_send.at[i], pool_recv.at[order(i)], at(order(1), m))

    def pool_across(plane, own):
        there = pool_slot(plane, m)
        return remote(wp_ref if own else there, there, py_send.at[plane], py_recv.at[plane], y_peer)

    def pool_beside(plane, own):
        there = pool_slot(plane, m)
        return remote(wp_ref if own else there, there, pc_send.at[plane, 0], pc_recv.at[plane, 0], c_peer)

    def pool_onward(plane):
        passed = pool_slot(plane, y_member)
        return remote(passed, passed, pc_send.at[plane, 1], pc_recv.at[plane, 1], c_peer)

    def pool_from_line(i):
        plane = order(i)
        arrived(pool_slot(plane, m), pool_recv.at[plane])
        pool_beside(plane, False).start()

    def pool_from_pair(i):
        arrived(pool_slot(order(i), y_member), py_recv.at[order(i)])
        pool_onward(order(i)).start()

    out_rows, out_columns = wo_ref.shape

    def out_slot(half, plane, yy, cc):
        first = pl.multiple_of(half * out_rows, out_rows)
        column = pl.multiple_of((plane * members + yy * 2 + cc) * out_columns, out_columns)
        return w_full.at[pl.ds(first, out_rows), pl.ds(column, out_columns)]

    def w_line(i):
        return remote(wo_ref, out_slot(tp, z, y, c), wl_send.at[i - 1], wl_recv.at[z], at(order(i), m))

    def w_line_on(i):
        there = out_slot(tp, order(i), y, c)
        return remote(there, there, wl_send.at[i], wl_recv.at[order(i)], at(order(1), m))

    def w_across(plane, own):
        there = out_slot(tp, plane, y, c)
        return remote(wo_ref if own else there, there, wy_send.at[plane], wy_recv.at[plane], y_peer)

    def w_swap(plane, yy, own):
        there = out_slot(tp, plane, yy, c)
        return remote(wo_ref if own else there, there, wx_send.at[plane, yy], wx_recv.at[plane, yy], x_peer)

    def w_beside(half, plane, yy, own):
        there = out_slot(half, plane, yy, c)
        return remote(
            wo_ref if own else there, there, wc_send.at[half, plane, yy], wc_recv.at[half, plane, yy], c_peer
        )

    def w_from_line(i):
        plane = order(i)
        arrived(out_slot(tp, plane, y, c), wl_recv.at[plane])
        w_swap(plane, y, False).start()
        w_beside(tp, plane, y, False).start()

    def w_from_pair(i):
        plane = order(i)
        arrived(out_slot(tp, plane, 1 - y, c), wy_recv.at[plane])
        w_swap(plane, 1 - y, False).start()
        w_beside(tp, plane, 1 - y, False).start()

    def w_from_swap(i):
        plane = order(i)
        for yy in (y, 1 - y):
            arrived(out_slot(1 - tp, plane, yy, c), wx_recv.at[plane, yy])
            w_beside(1 - tp, plane, yy, False).start()

    def slot(a, zz, yy, cc):
        start = pl.multiple_of((zz * members + yy * 2 + cc) * w_rows, w_rows)
        return full.at[a, pl.ds(start, w_rows), :]

    def line(a, i):
        there = slot(a, z, y, c)
        return remote(weights[a], there, line_send.at[i - 1, a], line_recv.at[z, a], at(order(i), m))

    def line_on(a, i):
        there = slot(a, order(i), y, c)
        return remote(there, there, line_send.at[i, a], line_recv.at[order(i), a], at(order(1), m))

    def y_copy(a, i, own):
        there = slot(a, order(i), y, c)
        src = weights[a] if own else there
        return remote(src, there, y_send.at[order(i), a], y_recv.at[order(i), a], y_peer)

    def c_copy(a, zz, yy, own):
        there = slot(a, zz, yy, c)
        src = weights[a] if own else there
        return remote(src, there, c_send.at[zz, yy, a], c_recv.at[zz, yy, a], c_peer)

    def c_came(a, zz, yy):
        there = slot(a, zz, yy, 1 - c)
        return remote(there, there, c_send.at[zz, yy, a], c_recv.at[zz, yy, a], c_peer)

    def from_line(i, arrays):
        zz = order(i)
        for a in arrays:
            arrived(slot(a, zz, y, c), line_recv.at[zz, a])

            @pl.when(between & (i > 1))
            def _():
                line_on(a, i).start()

            y_copy(a, i, False).start()
            c_copy(a, zz, y, False).start()

    def from_pair(i, arrays):
        zz = order(i)
        for a in arrays:
            arrived(slot(a, zz, 1 - y, c), y_recv.at[zz, a])
            c_copy(a, zz, 1 - y, False).start()

    def multiply(i, yy, arrays):
        zz = order(i)
        for a in arrays:
            c_came(a, zz, yy).wait_recv()
        piece = zz * 2 + yy
        start = pl.multiple_of(piece * 2 * w_rows, 2 * w_rows)
        for a in arrays:
            part = jnp.dot(
                pieces[piece], full[a, pl.ds(start, 2 * w_rows), :], preferred_element_type=jnp.float32
            )
            product[a] += part

    def own_weights(arrays):
        for a in arrays:
            line(a, 2).start()
            line(a, 1).start()
            y_copy(a, 0, True).start()
            c_copy(a, z, y, True).start()
            full[a, pl.ds(pl.multiple_of(sp * w_rows, w_rows), w_rows), :] = weights[a][...]

    swaps = (
        remote(tok_ref, theirs, swap_sem.at[0], swap_sem.at[1], x_peer),
        remote(gain_in, their_gain, swap_sem.at[2], swap_sem.at[3], x_peer),
    )
    own_weights(first_pair)
    for swap in swaps:
        swap.start()
    own_weights(last_one)
    w_swap(z, y, True).start()
    w_beside(tp, z, y, True).start()
    pool_beside(z, True).start()
    w_line(2).start()
    pool_line(2).start()

    @pl.when(jnp.logical_not(between))
    def _():
        w_line(1).start()
        pool_line(1).start()

    product[...] = jnp.zeros_like(product)
    acc[...] = jnp.zeros_like(acc)
    total[...] = jnp.zeros_like(total)
    top[...] = jnp.full_like(top, NEG_LARGE)
    own_pool = pl.ds(pl.multiple_of(sp * pool_rows, pool_rows), pool_rows)
    w_pool[own_pool, :] = wp_ref[...]
    w_full[
        pl.ds(pl.multiple_of(tp * out_rows, out_rows), out_rows),
        pl.ds(pl.multiple_of(sp * out_columns, out_columns), out_columns),
    ] = wo_ref[...]

    from_line(turn[1], first_pair)
    from_line(turn[2], first_pair)
    from_pair(0, first_pair)
    from_line(turn[1], last_one)
    from_line(turn[2], last_one)
    from_pair(0, last_one)
    from_line(turn[3], first_pair)
    from_pair(turn[1], first_pair)
    for swap in swaps:
        swap.wait()
    squares = jnp.zeros((rows, 1), jnp.float32)
    per_half = half_width // (2 * w_rows)
    for ref, gains, owner in ((tok_ref, gain_in, tp), (theirs, their_gain, 1 - tp)):
        for j in range(per_half):
            chunk = pl.ds(j * 2 * w_rows, 2 * w_rows)
            features = ref[:, chunk].astype(jnp.float32)
            squares += jnp.sum(features * features, axis=1, keepdims=True)
            scaled = (features * gains[:, chunk].astype(jnp.float32)).astype(jnp.bfloat16)
            pieces[owner * per_half + j] = scaled
    inverse = lax.rsqrt(squares / model_width + EPSILON)
    inverse_sc[...] = jnp.broadcast_to(inverse, inverse_sc.shape)
    every = first_pair + last_one
    multiply(0, y, every)
    multiply(0, 1 - y, every)
    from_line(turn[3], last_one)

    @pl.when(between)
    def _():
        w_line(1).start()
        pool_line(1).start()

    from_pair(turn[1], last_one)
    multiply(turn[1], y, every)
    from_pair(turn[2], first_pair)
    multiply(turn[1], 1 - y, every)
    from_pair(turn[2], last_one)
    multiply(turn[2], y, every)
    multiply(turn[2], 1 - y, every)
    multiply(turn[3], y, first_pair)
    from_pair(turn[3], first_pair)
    multiply(turn[3], 1 - y, first_pair)
    width = columns // planes
    for p in range(planes):
        part = slice(p * width, (p + 1) * width)
        k_src[p] = (product[0, :, part] * inverse_sc[:, :1]).astype(jnp.bfloat16)
        v_src[p] = (product[1, :, part] * inverse_sc[:, :1]).T.astype(jnp.bfloat16)
    k_all[z, m] = k_src[z]
    v_all[z, m] = v_src[z]
    share(z, True)
    w_across(z, True).start()
    for i in range(1, planes):
        k_out(order(i)).start()
        v_out(order(i)).start()
    from_pair(turn[3], last_one)
    multiply(turn[3], y, last_one)
    multiply(turn[3], 1 - y, last_one)
    for p in range(planes):
        part = slice(p * width, (p + 1) * width)
        query = (product[2, :, part] * inverse_sc[:, :1]).astype(jnp.bfloat16)
        q_src[p] = query * (1.0 / math.sqrt(hdim))

    q_in[z] = q_src[z]
    for i in range(1, planes):
        q_out(order(i)).start()
    w_from_line(1)
    pool_from_line(1)

    @pl.when(between)
    def _():
        for i in (2, 3):
            w_from_line(i)
            pool_from_line(i)

    def visit(block, plane, first, count, masked):
        query = q_in[block]
        lane = lax.broadcasted_iota(jnp.int32, query.shape, 1)
        none = jnp.zeros_like(query)
        both = jnp.concatenate(
            [jnp.where(lane < hdim, query, none), jnp.where(lane < hdim, none, query)], axis=0
        )
        keys = k_all[plane, pl.ds(first, count)].reshape(count * rows, 2 * hdim)
        values = jnp.concatenate([v_all[plane, first + i] for i in range(count)], axis=1)
        scores = lax.dot_general(
            keys, both, (((1,), (1,)), ((), ())), preferred_element_type=jnp.float32
        )
        if masked:
            shift = (first - m) * rows
            key = lax.broadcasted_iota(jnp.int32, scores.shape, 0)
            col = lax.broadcasted_iota(jnp.int32, scores.shape, 1)
            col = jnp.where(col < rows, col, col - rows)
            scores = jnp.where(key + shift <= col, scores, NEG_LARGE)
        old = top[block]
        new = jnp.maximum(old, jnp.max(scores, axis=0, keepdims=True))
        factor = jnp.exp(old - new)
        expo = jnp.exp(scores - new)
        acc[block] = acc[block] * factor + jnp.dot(
            values, expo.astype(jnp.bfloat16), preferred_element_type=jnp.float32
        )
        partial = jnp.sum(expo.reshape(count * rows // 8, 8, 2 * rows), axis=0)
        total[block] = total[block] * factor + partial
        top[block] = new

    def diagonal(block):
        pair = m // 2

        @pl.when(pair > 0)
        def _():
            visit(block, block, 0, members // 2, False)

        visit(block, block, pair * (members // 2), members // 2, True)

    def result_copy(block, half):
        return remote(
            done.at[block, pl.ds(pl.multiple_of(half * half_rows, half_rows), half_rows)],
            branch.at[tp * planes + z, :, pl.ds(0, vdim)],
            back_send.at[block, half],
            back_recv.at[tp * planes + z],
            at(block, m, half),
        )

    def at_home(block):
        return block == z

    def finish(block):
        both = acc[block] / jnp.sum(total[block], axis=0, keepdims=True)
        mixed = both[:, :rows] - lam_ref[z] * both[:, rows:]
        mean_sq = jnp.mean(mixed * mixed, axis=0, keepdims=True)
        normed = (mixed * lax.rsqrt(mean_sq + EPSILON)).T * gain_ref[...]
        done[block] = normed.astype(jnp.bfloat16)

        @pl.when(at_home(block))
        def _():
            kept = pl.ds(pl.multiple_of(tp * half_rows, half_rows), half_rows)
            branch[tp * planes + z, :, :vdim] = done[block, kept]

        @pl.when(jnp.logical_not(at_home(block)))
        def _():
            result_copy(block, tp).start()

        result_copy(block, 1 - tp).start()

    edge_rows = halo.shape[0]

    def edge_out():
        return remote(
            pool_sc.at[pl.ds(rows - edge_rows, edge_rows)], halo, edge_sem.at[0], edge_sem.at[1], {"sp": sp + 1}
        )

    def half_out():
        mine = pl.ds(pl.multiple_of(tp * groups, groups), groups)
        return remote(
            pooled_sc, branch.at[mine, :, pl.ds(vdim, vdim)], half_sem.at[0], half_sem.at[1], x_peer
        )

    def pool_project():
        for plane in range(planes):
            arrived(pool_slot(plane, c_member), pc_recv.at[plane, 0])
            arrived(pool_slot(plane, turned), pc_recv.at[plane, 1])
        scaled = jnp.concatenate([pieces[j] for j in range(pieces.shape[0])], axis=1)
        pool_in = jnp.dot(scaled, w_pool[...], preferred_element_type=jnp.float32)
        pool_sc[...] = (pool_in * inverse_sc[:, :1]).astype(jnp.bfloat16)

        @pl.when(sp < n_sp - 1)
        def _():
            edge_out().start()

        @pl.when(sp == 0)
        def _():
            halo[...] = jnp.zeros_like(halo)

    def pool_mix():
        @pl.when(sp > 0)
        def _():
            arrived(halo, edge_sem.at[1])

        for g in range(groups):
            part = slice(g * vdim, (g + 1) * vdim)
            own = pool_sc[:, part].astype(jnp.float32)
            running = jnp.concatenate([halo[:, part].astype(jnp.float32), own], axis=0)
            span = WINDOWS[g % len(WINDOWS)]
            step = 1
            while step < span:
                running = running + pltpu.roll(running, step, 0)
                step *= 2
            position = sp * rows + lax.broadcasted_iota(jnp.int32, own.shape, 0)
            count = jnp.minimum(position + 1, span).astype(jnp.float32)
            differ = (running[edge_rows:] / count - own).astype(jnp.bfloat16)
            pooled = jnp.dot(differ, group_ref[g], preferred_element_type=jnp.float32)
            pooled = (pooled * pscale_ref[:, part]).astype(jnp.bfloat16)
            low, high = pooled[:half_rows], pooled[half_rows:]
            branch[tp * groups + g, :, vdim:] = jnp.where(tp == 0, low, high)
            pooled_sc[g] = jnp.where(tp == 0, high, low)
        half_out().start()

    hand_on(z, True)
    landed(1)
    shared(z, True)

    def stage(i, carry):
        block = order(i)

        diagonal(block)

        @pl.when(i < planes - 2)
        def _():
            landed(i + 2)

        @pl.when(i == 0)
        def _():
            w_from_pair(0)

        @pl.when(i == 0)
        def _():
            w_across(order(1), False).start()

        @pl.when((i == 1) & between)
        def _():
            for j in (2, 3):
                w_line_on(j).start()
                w_across(order(j), False).start()
            for j in (2, 3):
                pool_line_on(j).start()
            pool_across(z, True).start()
            for j in (1, 2, 3):
                pool_across(order(j), False).start()

        @pl.when((i == 2) & jnp.logical_not(between))
        def _():
            w_from_line(2)
            w_across(order(2), False).start()

        @pl.when(i == 2)
        def _():
            w_from_pair(1)

        @pl.when((i == 3) & between)
        def _():
            w_from_pair(2)

        @pl.when(i < planes - 2)
        def _():
            hand_on(order(i + 1), False)

        @pl.when(i == planes - 1)
        def _():
            finish(0)

        def pair(j, carry):
            other = jnp.where(i < planes - 1, order(j), j + upper)
            visit(jnp.maximum(block, other), jnp.minimum(block, other), 0, members, False)

            @pl.when(i == planes - 1)
            def _():
                finish(j + 1)

            @pl.when((i == 3) & (j == 1) & between)
            def _():
                w_from_pair(3)

            @pl.when((i == planes - 2) & (j == 0))
            def _():
                hand_on(order(i + 1), False)

            @pl.when((i == 2) & (j == 1) & jnp.logical_not(between))
            def _():
                w_from_line(3)
                w_across(order(3), False).start()
                pool_across(z, True).start()
                pool_across(order(1), False).start()

            @pl.when((i == 3) & (j == 0) & jnp.logical_not(between))
            def _():
                w_from_pair(2)

            return carry

        lax.fori_loop(0, i, pair, 0)

        @pl.when(i < planes - 1)
        def _():
            arrived(q_in.at[order(i + 1)], z_recv.at[2, order(i + 1)])
            shared(order(i + 1), False)

        return carry

    lax.fori_loop(0, planes, stage, 0)


    @pl.when(jnp.logical_not(between))
    def _():
        for i in (2, 3):
            pool_from_line(i)
            pool_across(order(i), False).start()
        w_from_pair(3)

    for i in range(planes):
        pool_from_pair(i)
    pool_project()
    w_from_swap(0)
    pool_mix()

    for head in range(2 * planes):
        own_head = tp * planes + z == head

        @pl.when(jnp.logical_not(own_head & at_home(z)))
        def _():
            arrived(branch.at[head, :, pl.ds(0, vdim)], back_recv.at[head])

    w_from_swap(1)
    w_from_swap(2)
    theirs = pl.ds(pl.multiple_of((1 - tp) * groups, groups), groups)
    arrived(branch.at[theirs, :, pl.ds(vdim, vdim)], half_sem.at[1])
    w_from_swap(3)
    left = jnp.concatenate([branch[head] for head in range(2 * planes)], axis=1)
    out_width = members * out_columns

    def column(i, carry):
        plane = order(i)

        for half in range(2):
            for yy in range(2):
                arrived(out_slot(half, plane, yy, 1 - c), wc_recv.at[half, plane, yy])
        part = pl.ds(pl.multiple_of(plane * out_width, out_width), out_width)
        out_ref[:, part] = jnp.dot(
            left, w_full[:, part], preferred_element_type=jnp.float32
        ).astype(jnp.bfloat16)
        return carry

    lax.fori_loop(0, planes, column, 0)

    for i in range(1, planes):
        k_out(order(i)).wait_send()
        v_out(order(i)).wait_send()
        q_out(order(i)).wait_send()

    for i in range(planes):
        plane = order(i)
        for copies in in_plane(plane, i == 0):
            for copy in copies:
                copy.wait_send()
        w_across(plane, False).wait_send()
        for a in first_pair + last_one:
            y_copy(a, i, False).wait_send()
            c_copy(a, plane, y, False).wait_send()
            c_copy(a, plane, 1 - y, False).wait_send()
        for yy in (y, 1 - y):
            w_swap(plane, yy, False).wait_send()
            w_beside(0, plane, yy, False).wait_send()
            w_beside(1, plane, yy, False).wait_send()

    for i in (1, 2):
        w_line(i).wait_send()
        pool_line(i).wait_send()
        for a in first_pair + last_one:
            line(a, i).wait_send()

    @pl.when(between)
    def _():
        for i in (2, 3):
            w_line_on(i).wait_send()
            pool_line_on(i).wait_send()
            for a in first_pair + last_one:
                line_on(a, i).wait_send()

    for plane in range(planes):
        pool_across(plane, False).wait_send()
        pool_beside(plane, False).wait_send()
        pool_onward(plane).wait_send()
        result_copy(plane, 1 - tp).wait_send()

        @pl.when(jnp.logical_not(at_home(plane)))
        def _():
            result_copy(plane, tp).wait_send()

    half_out().wait_send()

    @pl.when(sp < n_sp - 1)
    def _():
        edge_out().wait_send()


def whole_layer(
    tokens,
    pre_gain,
    w_query,
    w_key,
    w_value,
    w_pool,
    lambdas,
    sub_gain,
    group_weight,
    pool_scale,
    w_out,
):
    planes = lambdas.shape[0]
    rows, half_width = tokens.shape
    n_sp = lax.axis_size("sp")
    members = n_sp // planes
    w_rows, columns = w_query.shape
    model_width = n_sp * w_rows
    width = columns // planes
    groups, vdim, _ = group_weight.shape
    out_rows, out_columns = w_out.shape
    vmem = pl.BlockSpec(memory_space=pltpu.VMEM)
    dma = pltpu.SemaphoreType.DMA
    bf16, f32 = jnp.bfloat16, jnp.float32
    work = planes * rows * members * planes * rows
    return pl.pallas_call(
        functools.partial(layer, width // 2, model_width),
        out_shape=jax.ShapeDtypeStruct((rows // 2, n_sp * out_columns), bf16),
        in_specs=[pl.BlockSpec(memory_space=pltpu.SMEM)] + [vmem] * 10,
        out_specs=vmem,
        scratch_shapes=[
            pltpu.VMEM((3, model_width, columns), bf16),
            pltpu.VMEM((rows, half_width), bf16),
            pltpu.VMEM((1, half_width), bf16),
            pltpu.VMEM((model_width // (2 * w_rows), rows, 2 * w_rows), bf16),
            pltpu.VMEM((3, rows, columns), f32),
            pltpu.VMEM((rows, 128), f32),
            pltpu.VMEM((planes, rows, width), bf16),
            pltpu.VMEM((planes, vdim, rows), bf16),
            pltpu.VMEM((planes, rows, width), bf16),
            pltpu.VMEM((planes, rows, width), bf16),
            pltpu.VMEM((planes, members, rows, width), bf16),
            pltpu.VMEM((planes, members, vdim, rows), bf16),
            pltpu.VMEM((planes, vdim, 2 * rows), f32),
            pltpu.VMEM((planes, 1, 2 * rows), f32),
            pltpu.VMEM((planes, 8, 2 * rows), f32),
            pltpu.VMEM((planes, rows, vdim), bf16),
            pltpu.VMEM((model_width, groups * vdim), bf16),
            pltpu.VMEM((2 * out_rows, n_sp * out_columns), bf16),
            pltpu.VMEM((2 * planes, rows // 2, 2 * vdim), bf16),
            pltpu.VMEM((rows, groups * vdim), bf16),
            pltpu.VMEM((RIM_ROWS + 1, groups * vdim), bf16),
            pltpu.VMEM((groups, rows // 2, vdim), bf16),
            dma((planes, 3)),
            dma((planes, 3)),
            dma((planes, 3)),
            dma((planes, 3)),
            dma((planes, 2, 3)),
            dma((planes, 2, 3)),
            dma((4,)),
            dma((3, planes)),
            dma((3, planes)),
            dma((planes, 3, 2)),
            dma((planes, 3, 2)),
            dma((planes, 2)),
            dma((2 * planes,)),
            dma((planes,)),
            dma((planes,)),
            dma((planes, 2)),
            dma((planes, 2)),
            dma((2,)),
            dma((2,)),
            dma((planes,)),
            dma((planes,)),
            dma((planes,)),
            dma((planes,)),
            dma((planes,)),
            dma((planes,)),
            dma((planes, 2)),
            dma((planes, 2)),
            dma((2, planes, 2)),
            dma((2, planes, 2)),
        ],
        compiler_params=pltpu.CompilerParams(
            vmem_limit_bytes=60 * 2**20, collective_id=2, has_side_effects=True
        ),
        cost_estimate=pl.CostEstimate(
            flops=4 * work * vdim, bytes_accessed=2**24, transcendentals=work
        ),
    )(
        lambdas,
        tokens,
        pre_gain.reshape(1, -1),
        w_key,
        w_value,
        w_query,
        w_pool,
        sub_gain.reshape(1, -1),
        group_weight,
        pool_scale.reshape(1, -1),
        w_out,
    )


def trailing(x, window_ids, group_dim):
    column_window = jnp.repeat(window_ids, group_dim)[None, :]
    running = x
    picked = jnp.zeros_like(x)
    for slot, span in enumerate(WINDOWS):
        half = span // 2
        running = running + jnp.pad(running[:-half], ((half, 0), (0, 0)))
        picked = jnp.where(column_window == slot, running, picked)
    return picked


def general_attention(queries, key_rows, values, lambdas, sub_gain):
    n_sp = lax.axis_size("sp")
    sp = lax.axis_index("sp")
    tok_rows = queries.shape[0]
    heads = lambdas.shape[0]
    qdim = queries.shape[1] // heads
    vdim = values.shape[1] // heads
    head_width = 2 * qdim + vdim
    outer = math.gcd(n_sp, heads)
    inner = n_sp // outer
    per_device = heads // outer
    by_head = jnp.concatenate(
        [
            x.reshape(tok_rows, heads, -1).swapaxes(0, 1)
            for x in (queries, key_rows, values)
        ],
        axis=2,
    )
    across = [[o * inner + i for o in range(outer)] for i in range(inner)]
    within = [[o * inner + i for i in range(inner)] for o in range(outer)]
    by_head = by_head.reshape(outer, per_device, tok_rows, head_width)
    if outer > 1:
        by_head = lax.all_to_all(by_head, "sp", 0, 0, axis_index_groups=across)
    first_head = lax.div(sp, inner) * per_device
    attended = []
    if inner == 4 and per_device == 1:
        lam = lax.dynamic_slice_in_dim(lambdas, first_head, 1)
        attended.append(
            flash_members(by_head[:, 0, :, :qdim], by_head[:, 0, :, qdim:], lam, sub_gain)
        )
    else:
        kv = lax.all_gather(by_head[..., qdim:], "sp", axis=0, axis_index_groups=within)
        member = lax.rem(sp, inner).reshape(1)
        for p in range(per_device):
            lam = lax.dynamic_slice_in_dim(lambdas, first_head + p, 1)
            attended.append(flash(by_head[:, p, :, :qdim], kv[:, :, p], member, lam, sub_gain))
    attended = jnp.stack(attended, axis=1)
    if outer > 1:
        attended = lax.all_to_all(attended, "sp", 0, 0, axis_index_groups=across)
    return attended.reshape(heads, tok_rows, vdim)


def local(
    tokens,
    pre_gain,
    w_query,
    w_key,
    w_value,
    w_pool,
    lambdas,
    sub_gain,
    group_weight,
    pool_scale,
    w_out,
):
    n_tp = lax.axis_size("tp")
    n_sp = lax.axis_size("sp")
    tp = lax.axis_index("tp")
    sp = lax.axis_index("sp")
    tok_rows = tokens.shape[0]
    model_width = tokens.shape[1] * n_tp
    heads = lambdas.shape[0]
    qdim = w_query.shape[1] // heads
    vdim = w_value.shape[1] // heads
    groups = group_weight.shape[0]
    group_dim = group_weight.shape[1]

    shaped_for_mix = n_tp == 2 and heads == 4 and n_sp == 4 * heads and tok_rows % 32 == 0
    if shaped_for_mix and qdim == vdim == group_dim and groups == heads:
        return whole_layer(
            tokens,
            pre_gain,
            w_query,
            w_key,
            w_value,
            w_pool,
            lambdas,
            sub_gain,
            group_weight,
            pool_scale,
            w_out,
        )
    swap = [(0, 1), (1, 0)]
    w_sorted = w_out.reshape(heads, 2, vdim, -1).swapaxes(0, 1).reshape(w_out.shape)
    features = tokens.astype(jnp.float32)
    mine = (features * pre_gain.astype(jnp.float32)[None, :]).astype(jnp.bfloat16)
    squares = jnp.sum(features * features, axis=1, keepdims=True)
    weights = [w_query, w_key, w_value, w_pool]
    if n_sp % 4 == 0:
        *weights, theirs = gather_weights(weights, mine, n_tp == 2)
    else:
        weights = [lax.all_gather(w, "sp", axis=0, tiled=True) for w in weights]
        theirs = lax.ppermute(mine, "tp", swap) if n_tp == 2 else mine
    w_sorted, weights = lax.optimization_barrier((w_sorted, weights))
    w_out_rows = lax.all_gather(w_sorted, "sp", axis=1, tiled=True)
    if n_tp == 2:
        squares = squares + lax.ppermute(squares, "tp", swap)
        scaled = jnp.concatenate(
            [jnp.where(tp == 0, mine, theirs), jnp.where(tp == 0, theirs, mine)], axis=1
        )
    else:
        scaled = lax.all_gather(mine, "tp", axis=1, tiled=True)
        squares = lax.psum(squares, "tp")
    inverse = lax.rsqrt(squares / model_width + EPSILON)
    queries, key_rows, values, pool_in = [
        (jnp.dot(scaled, w, preferred_element_type=jnp.float32) * inverse).astype(jnp.bfloat16)
        for w in weights
    ]
    attended = general_attention(queries, key_rows, values, lambdas, sub_gain)

    halo = passed_along(pool_in[tok_rows - RIM_ROWS - 1 :], "sp", 1)
    extended = jnp.concatenate([halo, pool_in], axis=0).astype(jnp.float32)
    window_ids = (tp * groups + jnp.arange(groups, dtype=jnp.int32)) % len(WINDOWS)
    sums = trailing(extended, window_ids, group_dim)[RIM_ROWS + 1 :]
    spans = jnp.repeat(jnp.left_shift(2, window_ids), group_dim)
    positions = sp * tok_rows + jnp.arange(tok_rows, dtype=jnp.int32)
    count = jnp.minimum(positions[:, None] + 1, spans[None, :]).astype(jnp.float32)
    differ = (sums / count - pool_in.astype(jnp.float32)).astype(jnp.bfloat16)
    pooled = jnp.einsum(
        "tgc,gcd->tgd",
        differ.reshape(tok_rows, groups, group_dim),
        group_weight,
        preferred_element_type=jnp.float32,
    )
    pooled = (pooled * pool_scale.reshape(groups, group_dim)).astype(jnp.bfloat16)
    branch = jnp.concatenate(
        [attended.swapaxes(0, 1).reshape(tok_rows, -1), pooled.reshape(tok_rows, -1)], axis=1
    )
    if n_tp == 2:
        half = tok_rows // 2
        send = lax.dynamic_slice_in_dim(branch, (1 - tp) * half, half, 0)
        send = jnp.dot(send, w_out_rows, preferred_element_type=jnp.float32).astype(jnp.bfloat16)
        got = lax.ppermute(send, "tp", swap)
        keep = lax.dynamic_slice_in_dim(branch, tp * half, half, 0)
        keep = jnp.dot(keep, w_out_rows, preferred_element_type=jnp.float32)
        return (keep + got.astype(jnp.float32)).astype(jnp.bfloat16)
    partial = jnp.dot(branch, w_out_rows, preferred_element_type=jnp.float32)
    return lax.psum_scatter(partial.astype(jnp.bfloat16), "tp", scatter_dimension=0, tiled=True)


def solution(mesh):
    placed = (
        P("sp", "tp"),
        P("tp"),
        P("sp", "tp"),
        P("sp", "tp"),
        P("sp", "tp"),
        P("sp", "tp"),
        P("tp"),
        P(),
        P("tp", None, None),
        P("tp"),
        P("tp", "sp"),
    )
    return jax.shard_map(
        local, mesh=mesh, in_specs=placed, out_specs=P(("sp", "tp"), None), check_vma=False
    )
```
